32 devices in a mesh: rep: 2 (over x), fs: 8 (over z, y), tp: 2 (over core).
Axes of the slice: x: 2, y: 2, z: 4, core: 2. Of those that a mesh axis runs over, the one named last changes fastest.
Arguments:
- inputs: bfloat16 [8192, 2048], P(('rep', 'fs')), may hold values from -6 to 6
- cotangent: bfloat16 [8192, 2048], P(('rep', 'fs')), may hold values from -6 to 6
- gate_weight: bfloat16 [2048, 4096], P('fs', 'tp'), may hold values from -0.125 to 0.125
- up_weight: bfloat16 [2048, 4096], P('fs', 'tp'), may hold values from -0.125 to 0.125
- down_weight: bfloat16 [2048, 4096], P('fs', 'tp'), may hold values from -0.09375 to 0.09375
Outputs:
- grad_input: bfloat16 [8192, 2048], P(('rep', 'fs'))
- grad_down: float32 [2048, 4096], P('fs', 'tp')
The draws below stay inside these ranges and needn't reach their ends.
All inputs are finite; a program needn't handle non-finite values.
Results may differ from the reference program's by a relative error of at most 0.014.
Values may be sent and summed in bfloat16 or wider, within the bound.
A program may use at most 128 MiB of HBM per device.

```python
import jax
import jax.numpy as jnp
from jax import lax

D = 2048
FF = 4096
TOK_DEV = 512
TOKENS = 8192
N_TP = 2


def raised(values, key, source, target, shards_of, factor):
    owner, partner = [(jnp.arange(values.shape[axis_at]) // (values.shape[axis_at] // shards_of)).reshape([-1 if axis == axis_at else 1 for axis in range(values.ndim)]) for axis_at in (source, target)]
    chosen = jax.random.permutation(key, shards_of)[partner]
    strong = (owner == chosen) | (owner == (partner + shards_of // 2) % shards_of)
    return jnp.where(strong, factor * values, values)


def shard_levels(stream_key, shape, cuts, low, high):
    loudness, own = 1.0, jax.random.fold_in(stream_key, 6)
    for position, shards_of in cuts:
        draws = jnp.exp(jax.random.uniform(jax.random.fold_in(own, position), (shards_of,), jnp.float32, low / len(cuts), high / len(cuts)))
        loudness = loudness * jnp.repeat(draws, shape[position] // shards_of).reshape([-1 if axis == position else 1 for axis in range(len(shape))])
    return loudness


def normal_values(stream_key, dims, scale, most, split=(), held_as=jnp.bfloat16):
    entries = scale * jax.random.normal(stream_key, dims, jnp.float32)
    if split:
        entries = entries * shard_levels(stream_key, dims, split, -0.22, 0.18)
    return jnp.clip(entries, -most, most).astype(held_as)


def heavy_noise(rng, extent, width, most, cuts, heavy, kind=jnp.bfloat16):
    result = width * jax.random.normal(rng, extent, jnp.float32)
    if cuts:
        result = result * shard_levels(rng, extent, cuts, -0.22, 0.18)
    return jnp.clip(raised(result, jax.random.fold_in(rng, 3), *heavy), -most, most).astype(kind)


def setup_inputs(seed: int = 0) -> dict:
    splits = jax.random.split(jax.random.key(seed), 6)
    inputs = normal_values(splits[0], (TOKENS, D), 1.0, 6.0, ((0, 16),))
    cotangent = heavy_noise(splits[1], (TOKENS, D), 1.0, 6.0, ((0, 16),), (0, 1, 16, 2.0))
    gate_weight = normal_values(splits[2], (D, FF), D ** -0.5, 0.125, ((0, 8), (1, 2)))
    up_weight = normal_values(splits[3], (D, FF), D ** -0.5, 0.125, ((0, 8), (1, 2)))
    down_weight = normal_values(splits[4], (D, FF), FF ** -0.5, 0.09375, ((0, 8), (1, 2)))
    return dict(inputs=inputs, cotangent=cotangent, gate_weight=gate_weight, up_weight=up_weight, down_weight=down_weight)


def reference(inputs, cotangent, gate_weight, up_weight, down_weight):
    hid_width = FF // N_TP
    contract = (((1,), (1,)), ((), ()))
    contract_tok = (((0,), (0,)), ((), ()))

    def one_block(grad_acc, block_index):
        row_start = (block_index * TOK_DEV).astype(jnp.int32)
        in_rows = lax.dynamic_slice_in_dim(inputs, row_start, TOK_DEV, 0)
        cot_rows = lax.dynamic_slice_in_dim(cotangent, row_start, TOK_DEV, 0)
        gate_val = jnp.dot(in_rows, gate_weight, preferred_element_type=jnp.float32)
        up_val = jnp.dot(in_rows, up_weight, preferred_element_type=jnp.float32)
        sigmoid_gate = jax.nn.sigmoid(gate_val)
        active = gate_val * sigmoid_gate
        hidden = (active * up_val).astype(jnp.bfloat16)
        grad_hidden = jnp.dot(cot_rows, down_weight, preferred_element_type=jnp.float32)
        grad_gate = (grad_hidden * up_val * sigmoid_gate * (1.0 + gate_val * (1.0 - sigmoid_gate))).astype(jnp.bfloat16)
        grad_up = (grad_hidden * active).astype(jnp.bfloat16)
        total = jnp.zeros((TOK_DEV, D), jnp.float32)
        for blk in range(N_TP):
            lo_col = blk * hid_width
            hi_col = lo_col + hid_width
            piece = lax.dot_general(grad_gate[:, lo_col:hi_col], gate_weight[:, lo_col:hi_col], contract, preferred_element_type=jnp.float32)
            piece = piece + lax.dot_general(grad_up[:, lo_col:hi_col], up_weight[:, lo_col:hi_col], contract, preferred_element_type=jnp.float32)
            rounded = lax.optimization_barrier(piece.astype(jnp.bfloat16))
            total = total + rounded.astype(jnp.float32)
        grad_acc = grad_acc + lax.dot_general(cot_rows, hidden, contract_tok, preferred_element_type=jnp.float32)
        return grad_acc, total.astype(jnp.bfloat16)

    indices = jnp.arange(TOKENS // TOK_DEV, dtype=jnp.int32)
    grad_acc, pieces = lax.scan(one_block, jnp.zeros((D, FF), jnp.float32), indices)
    grad_input = pieces.reshape(TOKENS, D)
    grad_down = grad_acc * (float(TOKENS) ** -0.5)
    return grad_input, grad_down
```

```python
import functools
import math

import jax
import jax.numpy as jnp
from jax import lax
from jax.experimental import pallas as pl
from jax.experimental.pallas import tpu as pltpu
from jax.sharding import PartitionSpec as P

MESH = pl.DeviceIdType.MESH


def fused_kernel(
    line, gate_w, up_w, down_w, toks, cots, gi_out, gd_out,
    x, gu, dn_w, acc, hid, ggu, r1, rx, ry, s3, fin, g, u_in, d_in, gfin,
    up_s, up_r, dn_s, dn_r, wy_s, wy_r, tok_s, tok_r, d2d_s, d2d_r, loc,
    c_s, c_r, x_s, x_r, yy_s, yy_r, u_s, u_r, d_s, d_r, f_s, f_r, o_s, o_r, out_l,
):
    r = lax.axis_index("rep")
    f = lax.axis_index("fs")
    core = lax.axis_index("tp")
    z, y = f // 2, f % 2
    rows = toks.shape[0]
    half = rows // 2
    wrows = gate_w.shape[0]
    width = gate_w.shape[1] // 4
    depth = 2 * line * wrows
    zrows = 2 * wrows
    cols = depth // 2
    side = cols // 2
    frows = wrows
    last = line - 2
    has_up, has_dn = z < line - 1, z > 0
    is_end = (z == 0) | (z == line - 1)
    up = {"fs": (f + 2) % (2 * line)}
    dn = {"fs": (f + 2 * line - 2) % (2 * line)}
    ypart = {"fs": f + 1 - 2 * y}
    xpart = {"rep": 1 - r}
    cpart = {"tp": 1 - core}

    barrier = pltpu.get_barrier_semaphore()
    for dev in (ypart, xpart, cpart, up, dn):
        pl.semaphore_signal(barrier, inc=1, device_id=dev, device_id_type=MESH)
    pl.semaphore_wait(barrier, 5)

    def remote(src, dst, s, q, dev):
        return pltpu.make_async_remote_copy(
            src_ref=src, dst_ref=dst, send_sem=s, recv_sem=q,
            device_id=dev, device_id_type=MESH,
        )

    def wblk(k, zz, yy):
        row = pl.multiple_of((2 * zz + yy) * wrows, wrows)
        if k == 2:
            return dn_w.at[pl.ds(row, wrows), :]
        return gu.at[pl.ds(row, wrows), pl.ds(k * width, width)]

    def own(k, yy):
        col = pl.multiple_of((2 * r + yy) * width, width)
        return (gate_w, up_w, down_w)[k].at[:, pl.ds(col, width)]

    def to_y(k):
        return remote(own(k, 1 - y), wblk(k, z, y), wy_s.at[k], wy_r.at[k], ypart)

    def from_y(k):
        return remote(own(k, 1 - y), wblk(k, z, 1 - y), wy_s.at[k], wy_r.at[k], ypart)

    def zcopy(up_dir, d, sub, k, zz):
        yy = y if sub == 0 else 1 - y
        src = own(k, y) if (d == 0 and sub == 0) else wblk(k, zz, yy)
        s, q, dev = (up_s, up_r, up) if up_dir else (dn_s, dn_r, dn)
        return remote(src, wblk(k, zz, yy), s.at[d, sub, k], q.at[d, sub, k], dev)

    def pred_send(up_dir, d):
        return (has_up & (z - d >= 0)) if up_dir else (has_dn & (z + d <= line - 1))

    def src_z(up_dir, d):
        return jnp.maximum(z - d, 0) if up_dir else jnp.minimum(z + d, line - 1)

    def send(up_dir, d, sub, k):
        @pl.when(pred_send(up_dir, d))
        def _():
            zcopy(up_dir, d, sub, k, src_z(up_dir, d)).start()

    def await_send(up_dir, d, sub, k):
        @pl.when(pred_send(up_dir, d))
        def _():
            zcopy(up_dir, d, sub, k, src_z(up_dir, d)).wait_send()

    def await_recv(up_dir, d, sub, k):
        ok = (z - d - 1 >= 0) if up_dir else (z + d + 1 <= line - 1)

        @pl.when(ok)
        def _():
            zcopy(up_dir, d, sub, k, src_z(up_dir, d + 1)).wait_recv()

    def hop(d, sub, k):
        for up_dir in (True, False):
            await_recv(up_dir, d, sub, k)
            if d < last:
                send(up_dir, d + 1, sub, k)

    def slot(rr, yy):
        return pl.multiple_of((2 * rr + yy) * rows, rows)

    def tblk(j, rr, yy, c):
        row = pl.multiple_of((2 * rr + yy) * rows + c * half, half)
        return x.at[j, pl.ds(row, half), :]

    def mine(j):
        src = toks if j == 0 else cots
        return src.at[pl.ds(pl.multiple_of(core * half, half), half), :]

    def tcopy(i, landing):
        j = (0, 1, 0, 1, 0, 1)[i]
        dev = xpart if i in (0, 1, 4) else ypart
        if landing:
            rr = (1 - r, 1 - r, r, r, 1 - r, 1 - r)[i]
            yy = (y, y, 1 - y, 1 - y, 1 - y, 1 - y)[i]
            src = dst = tblk(j, rr, yy, core)
        else:
            rr = (r, r, r, r, r, 1 - r)[i]
            yy = (y, y, y, y, 1 - y, y)[i]
            dst = tblk(j, rr, yy, core)
            src = mine(j) if i < 4 else dst
        return remote(src, dst, tok_s.at[i], tok_r.at[i], dev)

    def dcopy(i, c):
        j = (0, 1, 0, 1, 0, 1)[i]
        rr = (1 - r, 1 - r, r, r, 1 - r, 1 - r)[i]
        yy = (y, y, 1 - y, 1 - y, 1 - y, 1 - y)[i]
        blk = tblk(j, rr, yy, c)
        return remote(blk, blk, d2d_s.at[i], d2d_r.at[i], cpart)

    def event(i):
        tcopy(i, True).wait_recv()
        if i == 2:
            tcopy(4, False).start()
        if i == 1:
            tcopy(5, False).start()
        dcopy(i, core).start()

    trow = slot(r, y)
    loads = [
        pltpu.make_async_copy(own(0, y), wblk(0, z, y), loc.at[0]),
        pltpu.make_async_copy(own(1, y), wblk(1, z, y), loc.at[1]),
        pltpu.make_async_copy(own(2, y), wblk(2, z, y), loc.at[2]),
        pltpu.make_async_copy(toks, x.at[0, pl.ds(trow, rows), :], loc.at[3]),
        pltpu.make_async_copy(cots, x.at[1, pl.ds(trow, rows), :], loc.at[4]),
    ]

    tile = 256
    z_lo = jnp.maximum(z - last, 0)
    z_hi = jnp.minimum(z + last, line - 1) + 1

    def product(j, row, k0, kk, w, wcol, acol, n):
        at = pl.ds(pl.multiple_of(row, rows), rows)
        kat = pl.ds(pl.multiple_of(k0, wrows), kk)
        for c in range(0, n, tile):
            one = jnp.dot(
                x[j, at, kat], w[kat, pl.ds(wcol + c, tile)],
                preferred_element_type=jnp.float32,
            )
            acc[at, pl.ds(acol + c, tile)] += one

    def forward(j, w, acol, n, first, count):
        @pl.loop(first, first + count)
        def _(b):
            row = ((2 * r + y) + 2 * (b % 2) * (1 - 2 * r) + (b // 2) * (1 - 2 * y)) * rows

            @pl.loop(z_lo, z_hi)
            def _(zz):
                product(j, row, zz * zrows, zrows, w, 0, acol, n)

    def forward_end(j, k, sub):
        for up_dir in (True, False):
            await_recv(up_dir, last, sub, k)

        @pl.when(is_end)
        def _():
            zz = line - 1 - z
            yy = y if sub == 0 else 1 - y
            w = dn_w if k == 2 else gu

            @pl.loop(0, 4)
            def _(b):
                product(
                    j, b * rows, (2 * zz + yy) * wrows, wrows, w,
                    0 if k == 2 else k * width, k * width, width,
                )

    def total(dst, terms, count, step=64):
        @pl.loop(0, count // step)
        def _(i):
            at = pl.multiple_of(i * step, step)
            value = None
            for ref, row, col, wide in terms:
                one = ref[pl.ds(row + at, step), pl.ds(col, wide)].astype(jnp.float32)
                value = one if value is None else value + one
            ref, row, col, wide = dst
            ref[pl.ds(row + at, step), pl.ds(col, wide)] = value.astype(ref.dtype)

    for k in (0, 1):
        to_y(k).start()
        send(True, 0, 0, k)
        send(False, 0, 0, k)
    tcopy(0, False).start()
    tcopy(2, False).start()
    to_y(2).start()
    tcopy(1, False).start()
    tcopy(3, False).start()
    for copy in loads:
        copy.start()

    @pl.loop(0, 4 * rows // 64)
    def _(i):
        at = pl.ds(pl.multiple_of(i * 64, 64), 64)
        acc[at, :] = jnp.zeros((64, 3 * width), jnp.float32)

    for k in (0, 1):
        from_y(k).wait_recv()
        send(True, 0, 1, k)
        send(False, 0, 1, k)
    for sub in range(2):
        for k in (0, 1):
            if last > 0:
                hop(0, sub, k)
    event(0)
    event(2)
    for d in range(1, last):
        for sub in range(2):
            for k in (0, 1):
                hop(d, sub, k)
    send(True, 0, 0, 2)
    send(False, 0, 0, 2)
    from_y(2).wait_recv()
    send(True, 0, 1, 2)
    send(False, 0, 1, 2)
    event(1)
    for load in loads:
        load.wait()
    dcopy(0, 1 - core).wait_recv()
    dcopy(2, 1 - core).wait_recv()
    forward(0, gu, 0, 2 * width, 0, 3)
    for d in range(last):
        for sub in range(2):
            hop(d, sub, 2)
    event(3)
    event(4)
    dcopy(4, 1 - core).wait_recv()
    forward(0, gu, 0, 2 * width, 3, 1)
    for sub in range(2):
        for k in (0, 1):
            forward_end(0, k, sub)

    @pl.loop(0, 4 * rows // 32)
    def _(i):
        at = pl.ds(pl.multiple_of(i * 32, 32), 32)
        gate = acc[at, pl.ds(0, width)]
        up_val = acc[at, pl.ds(width, width)]
        sig = jax.nn.sigmoid(gate)
        active = gate * sig
        hid[at, :] = (active * up_val).astype(hid.dtype)
        acc[at, pl.ds(0, width)] = up_val * sig * (1.0 + gate * (1.0 - sig))
        acc[at, pl.ds(width, width)] = active

    event(5)
    for i in (1, 3, 5):
        dcopy(i, 1 - core).wait_recv()

    def block(ref, zt):
        return ref.at[pl.ds(zt * zrows, zrows), :]

    def up_copy(zt, first):
        return remote(block(g if first else u_in, zt), block(u_in, zt), u_s.at[zt], u_r.at[zt], up)

    def dn_copy(zt, first):
        return remote(block(g if first else d_in, zt), block(d_in, zt), d_s.at[zt], d_r.at[zt], dn)

    for i in range(line):
        zt = jnp.where(z < line // 2, line - 1 - i, i)

        @pl.loop(0, zrows // tile)
        def _(m):
            at = pl.multiple_of(zt * zrows + m * tile, tile)
            one = lax.dot_general(
                x[1, :, pl.ds(at, tile)], hid[...], (((0,), (0,)), ((), ())),
                preferred_element_type=jnp.float32,
            )
            g[pl.ds(at, tile), :] = one.astype(g.dtype)

        if i < line - 1:
            @pl.when(z == 0)
            def _():
                up_copy(line - 1 - i, True).start()

            @pl.when(z == line - 1)
            def _():
                dn_copy(i, True).start()

    def line_step(i):
        zt = line - 1 - i
        if zt > 0:
            @pl.when((z > 0) & (z < zt))
            def _():
                up_copy(zt, False).wait_recv()
                row = zt * zrows
                total((u_in, row, 0, width), [(g, row, 0, width), (u_in, row, 0, width)], zrows)
                up_copy(zt, False).start()

            zd = i

            @pl.when((z < line - 1) & (z > zd))
            def _():
                dn_copy(zd, False).wait_recv()
                row = zd * zrows
                total((d_in, row, 0, width), [(g, row, 0, width), (d_in, row, 0, width)], zrows)
                dn_copy(zd, False).start()

    forward(1, dn_w, 2 * width, width, 0, 4)
    for sub in range(2):
        forward_end(1, 2, sub)

    for i in (0, 2, 4):
        dcopy(i, core).wait_send()
    tcopy(4, False).wait_send()
    order = [(1 - r, 1 - y), (1 - r, y), (r, 1 - y), (r, y)]
    my_col = pl.multiple_of(core * cols, cols)
    its_col = pl.multiple_of((1 - core) * cols, cols)
    part = x.at[0]

    def slopes(row):
        @pl.loop(0, rows // 32)
        def _(i):
            at = pl.ds(pl.multiple_of(row + i * 32, 32), 32)
            grad = acc[at, pl.ds(2 * width, width)]
            ggu[at, pl.ds(0, width)] = (grad * acc[at, pl.ds(0, width)]).astype(ggu.dtype)
            ggu[at, pl.ds(width, width)] = (grad * acc[at, pl.ds(width, width)]).astype(ggu.dtype)

    def back(row, col):
        @pl.loop(0, cols // tile)
        def _(n):
            at = pl.multiple_of(col + n * tile, tile)
            one = lax.dot_general(
                ggu[pl.ds(row, rows), :], gu[pl.ds(at, tile), :], (((1,), (1,)), ((), ())),
                preferred_element_type=jnp.float32,
            )
            x[0, pl.ds(row, rows), pl.ds(at, tile)] = one.astype(x.dtype)

    def core_copy(i):
        at = pl.ds(slot(*order[i]), rows)
        return remote(part.at[at, pl.ds(its_col, cols)], r1.at[at, :], c_s.at[i], c_r.at[i], cpart)

    def s1_half(i, second):
        col = pl.multiple_of(my_col + (side if second else 0), side)
        return part.at[pl.ds(slot(*order[i]), rows), pl.ds(col, side)]

    def s1(row, second):
        return (part, row, pl.multiple_of(my_col + (side if second else 0), side), side)

    def x_copy(i):
        src = s3.at[1] if i == 2 else s1_half(i, False)
        return remote(src, rx.at[i], x_s.at[i], x_r.at[i], xpart)

    def y_copy(i):
        src = s3.at[0] if i == 2 else s1_half((0, 2)[i], True)
        return remote(src, ry.at[i], yy_s.at[i], yy_r.at[i], ypart)

    for i in range(4):
        row = slot(*order[i])
        slopes(row)
        back(row, its_col)
        core_copy(i).start()
        back(row, my_col)
        core_copy(i).wait_recv()
        total((part, row, my_col, cols), [(part, row, my_col, cols), (r1, row, 0, cols)], rows)
        if i in (0, 1):
            x_copy(i).start()
        if i == 0:
            y_copy(0).start()
        if i == 2:
            y_copy(1).start()
        if i < line - 1:
            line_step(i)

    x_copy(0).wait_recv()
    total((s3.at[0], 0, 0, side), [s1(slot(r, 1 - y), False), (rx.at[0], 0, 0, side)], rows)
    y_copy(2).start()
    y_copy(0).wait_recv()
    total((s3.at[1], 0, 0, side), [s1(slot(1 - r, y), True), (ry.at[0], 0, 0, side)], rows)
    x_copy(2).start()
    for i in range(4, line - 1):
        line_step(i)

    zrow = pl.multiple_of(z * zrows, zrows)

    def here(ref):
        return (ref, zrow, 0, width)

    @pl.when(z == 0)
    def _():
        dn_copy(0, True).wait_recv()
        total((gfin, 0, 0, width), [here(g), here(d_in)], zrows)

    @pl.when(z == line - 1)
    def _():
        up_copy(line - 1, True).wait_recv()
        total((gfin, 0, 0, width), [here(g), here(u_in)], zrows)

    @pl.when((z > 0) & (z < line - 1))
    def _():
        remote(block(g, z), block(u_in, z), u_s.at[z], u_r.at[z], up).wait_recv()
        remote(block(g, z), block(d_in, z), d_s.at[z], d_r.at[z], dn).wait_recv()
        total((gfin, 0, 0, width), [here(g), here(u_in), here(d_in)], zrows)

    def gcols(rr, yy):
        return gd_out.at[:, pl.ds(pl.multiple_of((2 * rr + yy) * width, width), width)]

    def grows(yy):
        return gfin.at[pl.ds(pl.multiple_of(yy * frows, frows), frows), :]

    def f_copy(i, landing):
        if i == 0:
            dst = gcols(r, 1 - y) if landing else gcols(r, y)
            return remote(grows(1 - y), dst, f_s.at[0], f_r.at[0], ypart)
        if i == 1:
            dst = gcols(1 - r, y) if landing else gcols(r, y)
            return remote(grows(y), dst, f_s.at[1], f_r.at[1], xpart)
        dst = gcols(1 - r, 1 - y) if landing else gcols(r, 1 - y)
        return remote(gcols(r, 1 - y), dst, f_s.at[2], f_r.at[2], xpart)

    f_copy(0, False).start()
    f_copy(1, False).start()
    own_g = pltpu.make_async_copy(grows(y), gcols(r, y), out_l.at[0])
    own_g.start()

    x_copy(1).wait_recv()
    y_copy(2).wait_recv()
    here_row = slot(r, y)
    total(
        (fin, 0, 0, side),
        [s1(here_row, False), (rx.at[1], 0, 0, side), (ry.at[2], 0, 0, side)], rows,
    )

    def o_copy(i, landing):
        base = (1 - core if landing else core) * cols + i * side
        dst = gi_out.at[:, pl.ds(pl.multiple_of(base, side), side)]
        return remote(fin.at[:, pl.ds(i * side, side)], dst, o_s.at[i], o_r.at[i], cpart)

    def o_local(i):
        base = pl.multiple_of(core * cols + i * side, side)
        return pltpu.make_async_copy(
            fin.at[:, pl.ds(i * side, side)], gi_out.at[:, pl.ds(base, side)], out_l.at[1 + i]
        )

    o_copy(0, False).start()
    o_local(0).start()
    f_copy(0, True).wait_recv()
    f_copy(2, False).start()
    y_copy(1).wait_recv()
    x_copy(2).wait_recv()
    total(
        (fin, 0, side, side),
        [s1(here_row, True), (ry.at[1], 0, 0, side), (rx.at[2], 0, 0, side)], rows,
    )
    o_copy(1, False).start()
    o_local(1).start()

    for i in range(6):
        if i in (1, 3, 5):
            dcopy(i, core).wait_send()
        if i != 4:
            tcopy(i, False).wait_send()
    for k in range(3):
        to_y(k).wait_send()
        for d in range(line - 1):
            for sub in range(2):
                await_send(True, d, sub, k)
                await_send(False, d, sub, k)
    for i in range(4):
        core_copy(i).wait_send()
    for i in range(3):
        x_copy(i).wait_send()
        y_copy(i).wait_send()
        f_copy(i, False).wait_send()
    f_copy(1, True).wait_recv()
    f_copy(2, True).wait_recv()
    for i in range(2):
        o_copy(i, True).wait_recv()
        o_copy(i, False).wait_send()
        o_local(i).wait()
    own_g.wait()
    for zt in range(line):
        if zt > 0:
            pl.when(z < zt)(lambda: up_copy(zt, True).wait_send())
        if zt < line - 1:
            pl.when(z > zt)(lambda: dn_copy(zt, True).wait_send())


def fused(gate_w, up_w, down_w, toks, cots):
    line = lax.axis_size("fs") // 2
    rows, full = toks.shape
    wrows, width = gate_w.shape[0], gate_w.shape[1] // 4
    depth = 2 * line * wrows
    cols = full // 2
    kind = gate_w.dtype
    dma = pltpu.SemaphoreType.DMA
    zsem = dma((line - 1, 2, 3))
    anyspec = pl.BlockSpec(memory_space=pl.ANY)
    whole = pltpu.VMEM((depth, width), kind)
    unit = pltpu.VMEM((3, rows, cols // 2), kind)
    return pl.pallas_call(
        functools.partial(fused_kernel, line),
        out_shape=(
            jax.ShapeDtypeStruct((rows, full), kind),
            jax.ShapeDtypeStruct((wrows, 4 * width), kind),
        ),
        in_specs=[anyspec] * 5,
        out_specs=(anyspec,) * 2,
        scratch_shapes=[
            pltpu.VMEM((2, 4 * rows, full), kind),
            pltpu.VMEM((depth, 2 * width), kind),
            whole,
            pltpu.VMEM((4 * rows, 3 * width), jnp.float32),
            pltpu.VMEM((4 * rows, width), kind),
            pltpu.VMEM((4 * rows, 2 * width), kind),
            pltpu.VMEM((4 * rows, cols), kind),
            unit, unit,
            pltpu.VMEM((2, rows, cols // 2), kind),
            pltpu.VMEM((rows, cols), kind),
            whole, whole, whole,
            pltpu.VMEM((2 * wrows, width), kind),
            zsem, zsem, zsem, zsem,
            dma((3,)), dma((3,)),
            dma((6,)), dma((6,)), dma((6,)), dma((6,)), dma((5,)),
            dma((4,)), dma((4,)), dma((3,)), dma((3,)), dma((3,)), dma((3,)),
            dma((line,)), dma((line,)), dma((line,)), dma((line,)),
            dma((3,)), dma((3,)), dma((2,)), dma((2,)), dma((3,)),
        ],
        compiler_params=pltpu.CompilerParams(
            collective_id=1, has_side_effects=True, vmem_limit_bytes=67043328
        ),
        name="fused_all",
    )(gate_w, up_w, down_w, toks, cots)


def gather_kernel(
    line, units, gate_w, up_w, down_w, toks, cots, gu_out, d_out, t_out, w_tmp, t_tmp,
    up_s, up_r, dn_s, dn_r, y_s, y_r, tok_s, tok_r, d2d_s, d2d_r, loc, loc2,
):
    r = lax.axis_index("rep")
    f = lax.axis_index("fs")
    t = lax.axis_index("tp")
    z, y = f // 2, f % 2
    rows = toks.shape[0]
    half = rows // 2
    wrows = gate_w.shape[0]
    width = gate_w.shape[1] // 4
    parts = len(units)
    has_up, has_dn = z < line - 1, z > 0
    up = {"fs": (f + 2) % (2 * line)}
    dn = {"fs": (f + 2 * line - 2) % (2 * line)}
    ypart = {"fs": f + 1 - 2 * y}
    xpart = {"rep": 1 - r}
    core = t % 2
    cpart = {"tp": t + 1 - 2 * core}

    barrier = pltpu.get_barrier_semaphore()

    def greet(dev):
        pl.semaphore_signal(barrier, inc=1, device_id=dev, device_id_type=MESH)

    for dev in (ypart, xpart, cpart, up, dn):
        greet(dev)
    pl.semaphore_wait(barrier, 5)

    def remote(src, dst, s, q, dev):
        return pltpu.make_async_remote_copy(
            src_ref=src, dst_ref=dst, send_sem=s, recv_sem=q,
            device_id=dev, device_id_type=MESH,
        )

    def wblk(k, zz, yy):
        row = pl.multiple_of((2 * zz + yy) * wrows, wrows)
        which, col, wide = units[k]
        return (gu_out, d_out)[which].at[pl.ds(row, wrows), pl.ds(col, wide)]

    def own(k, yy):
        col = pl.multiple_of((2 * r + yy) * width, width)
        return (gate_w, up_w, down_w)[k].at[:, pl.ds(col, width)]

    def to_y(k):
        return remote(own(k, 1 - y), wblk(k, z, y), y_s.at[k], y_r.at[k], ypart)

    def from_y(k):
        return remote(own(k, 1 - y), wblk(k, z, 1 - y), y_s.at[k], y_r.at[k], ypart)

    def zcopy(up_dir, d, sub, k, zz):
        yy = y if sub == 0 else 1 - y
        src = own(k, y) if (d == 0 and sub == 0) else wblk(k, zz, yy)
        s, q, dev = (up_s, up_r, up) if up_dir else (dn_s, dn_r, dn)
        return remote(src, wblk(k, zz, yy), s.at[d, sub, k], q.at[d, sub, k], dev)

    def pred_send(up_dir, d):
        return (has_up & (z - d >= 0)) if up_dir else (has_dn & (z + d <= line - 1))

    def src_z(up_dir, d):
        return jnp.maximum(z - d, 0) if up_dir else jnp.minimum(z + d, line - 1)

    def send(up_dir, d, sub, k):
        @pl.when(pred_send(up_dir, d))
        def _():
            zcopy(up_dir, d, sub, k, src_z(up_dir, d)).start()

    def await_send(up_dir, d, sub, k):
        @pl.when(pred_send(up_dir, d))
        def _():
            zcopy(up_dir, d, sub, k, src_z(up_dir, d)).wait_send()

    def await_recv(up_dir, d, sub, k):
        ok = (z - d - 1 >= 0) if up_dir else (z + d + 1 <= line - 1)

        @pl.when(ok)
        def _():
            zcopy(up_dir, d, sub, k, src_z(up_dir, d + 1)).wait_recv()

    def tblk(j, rr, yy, c):
        row = pl.multiple_of((2 * rr + yy) * rows + c * half, half)
        return t_out.at[j, pl.ds(row, half), :]

    def mine(j):
        src = toks if j == 0 else cots
        return src.at[pl.ds(pl.multiple_of(core * half, half), half), :]

    def tcopy(i, landing):
        j = (0, 1, 0, 1, 0, 1)[i]
        dev = xpart if i in (0, 1, 5) else ypart
        if landing:
            rr = (1 - r, 1 - r, r, r, 1 - r, 1 - r)[i]
            yy = (y, y, 1 - y, 1 - y, 1 - y, 1 - y)[i]
            src = dst = tblk(j, rr, yy, core)
        else:
            rr = (r, r, r, r, 1 - r, r)[i]
            yy = (y, y, y, y, y, 1 - y)[i]
            dst = tblk(j, rr, yy, core)
            src = mine(j) if i < 4 else dst
        return remote(src, dst, tok_s.at[i], tok_r.at[i], dev)

    def dcopy(i, c):
        j = (0, 1, 0, 1, 0, 1)[i]
        rr = (1 - r, 1 - r, r, r, 1 - r, 1 - r)[i]
        yy = (y, y, 1 - y, 1 - y, 1 - y, 1 - y)[i]
        blk = tblk(j, rr, yy, c)
        return remote(blk, blk, d2d_s.at[i], d2d_r.at[i], cpart)

    loads = [
        pltpu.make_async_copy(own(0, y), w_tmp.at[0], loc.at[0]),
        pltpu.make_async_copy(own(1, y), w_tmp.at[1], loc.at[3]),
        pltpu.make_async_copy(own(2, y), w_tmp.at[2], loc.at[4]),
        pltpu.make_async_copy(toks, t_tmp.at[0], loc.at[1]),
        pltpu.make_async_copy(cots, t_tmp.at[1], loc.at[2]),
    ]
    trow = pl.multiple_of((2 * r + y) * rows, rows)
    stores = [
        pltpu.make_async_copy(w_tmp.at[0], wblk(0, z, y), loc2.at[0]),
        pltpu.make_async_copy(w_tmp.at[1], wblk(1, z, y), loc2.at[3]),
        pltpu.make_async_copy(w_tmp.at[2], wblk(2, z, y), loc2.at[4]),
        pltpu.make_async_copy(t_tmp.at[0], t_out.at[0, pl.ds(trow, rows), :], loc2.at[1]),
        pltpu.make_async_copy(t_tmp.at[1], t_out.at[1, pl.ds(trow, rows), :], loc2.at[2]),
    ]

    for k in range(parts):
        to_y(k).start()
        send(True, 0, 0, k)
        send(False, 0, 0, k)
    for i in (0, 1, 3, 2):
        tcopy(i, False).start()
    for copy in loads:
        copy.start()
    for load, store in zip(loads, stores):
        load.wait()
        store.start()
    for k in range(parts):
        from_y(k).wait_recv()
        send(True, 0, 1, k)
        send(False, 0, 1, k)

    def event(i):
        tcopy(i, True).wait_recv()
        if i == 0:
            tcopy(4, False).start()
        if i == 3:
            tcopy(5, False).start()
        dcopy(i, core).start()

    events = [0, 3, 1, 2, 5, 4]
    for d in range(line - 1):
        for sub in range(2):
            if events:
                event(events.pop(0))
            for k in range(parts):
                for up_dir in (True, False):
                    await_recv(up_dir, d, sub, k)
                    if d + 1 < line - 1:
                        send(up_dir, d + 1, sub, k)
    for i in events:
        event(i)
    for i in range(6):
        dcopy(i, 1 - core).wait_recv()
        dcopy(i, core).wait_send()
        tcopy(i, False).wait_send()
    for k in range(parts):
        to_y(k).wait_send()
        for d in range(line - 1):
            for sub in range(2):
                await_send(True, d, sub, k)
                await_send(False, d, sub, k)
    for store in stores:
        store.wait()


def gather(gate_w, up_w, down_w, toks, cots):
    line = lax.axis_size("fs") // 2
    wrows, width = gate_w.shape[0], gate_w.shape[1] // 4
    units = [(0, 0, width), (0, width, width), (1, 0, width)]
    parts = len(units)
    depth = 2 * line * wrows
    kind = gate_w.dtype
    dma = pltpu.SemaphoreType.DMA
    zsem = dma((line - 1, 2, parts))
    anyspec = pl.BlockSpec(memory_space=pl.ANY)
    return pl.pallas_call(
        functools.partial(gather_kernel, line, units),
        out_shape=(
            jax.ShapeDtypeStruct((depth, 2 * width), kind),
            jax.ShapeDtypeStruct((depth, width), kind),
            jax.ShapeDtypeStruct((2, 4 * toks.shape[0], toks.shape[1]), toks.dtype),
        ),
        in_specs=[anyspec] * 5,
        out_specs=(anyspec,) * 3,
        scratch_shapes=[
            pltpu.VMEM((parts, wrows, width), kind),
            pltpu.VMEM((2,) + toks.shape, toks.dtype),
            zsem, zsem, zsem, zsem,
            dma((parts,)), dma((parts,)),
            dma((6,)), dma((6,)), dma((6,)), dma((6,)),
            dma((5,)), dma((5,)),
        ],
        compiler_params=pltpu.CompilerParams(collective_id=0, has_side_effects=True),
        name="gather_all",
    )(gate_w, up_w, down_w, toks, cots)


def on_device(inputs, cotangent, gate_weight, up_weight, down_weight):
    tok_rows = inputs.shape[0]
    fs_size = lax.axis_size("fs")
    rep_size = lax.axis_size("rep")
    grad_scale = 1.0 / math.sqrt(tok_rows * fs_size * rep_size)
    if lax.axis_size("tp") == 2:
        grad_input, grad_down = fused(
            gate_weight, up_weight, down_weight, inputs, cotangent
        )
        return (grad_input, grad_down.astype(jnp.float32) * grad_scale)
    contract = (((1,), (1,)), ((), ()))
    contract_tok = (((0,), (0,)), ((), ()))
    width = gate_weight.shape[1] // 4
    gate_up, down_full, tokens = gather(
        gate_weight, up_weight, down_weight, inputs, cotangent
    )
    gate_up_val = jnp.dot(tokens[0], gate_up, preferred_element_type=jnp.float32)
    gate_val, up_val = gate_up_val[:, :width], gate_up_val[:, width:]
    grad_hidden = jnp.dot(tokens[1], down_full, preferred_element_type=jnp.float32)
    sigmoid_gate = jax.nn.sigmoid(gate_val)
    active = gate_val * sigmoid_gate
    hidden = (active * up_val).astype(jnp.bfloat16)
    grad_gate = (
        grad_hidden * up_val * sigmoid_gate * (1.0 + gate_val * (1.0 - sigmoid_gate))
    ).astype(jnp.bfloat16)
    grad_up = (grad_hidden * active).astype(jnp.bfloat16)
    pairs = [[i, i + 1] for i in range(0, fs_size, 2)]
    lines = [list(range(i, fs_size, 2)) for i in range(2)]
    grad_part = lax.dot_general(
        tokens[1], hidden, contract_tok, preferred_element_type=jnp.float32
    )
    part = lax.dot_general(
        jnp.concatenate([grad_gate, grad_up], axis=1), gate_up, contract,
        preferred_element_type=jnp.float32,
    )
    shard = lax.psum_scatter(
        grad_part.astype(jnp.bfloat16), "fs", scatter_dimension=0, tiled=True,
        axis_index_groups=lines,
    ).astype(jnp.float32) * grad_scale
    shard = lax.all_to_all(
        shard, "fs", split_axis=0, concat_axis=1, tiled=True, axis_index_groups=pairs
    )
    grad_down = lax.all_gather(shard, "rep", axis=1, tiled=True)
    part = lax.psum_scatter(
        part.astype(jnp.bfloat16), "rep", scatter_dimension=0, tiled=True
    )
    part = lax.psum_scatter(
        part, "fs", scatter_dimension=0, tiled=True, axis_index_groups=pairs
    )
    grad_input = lax.psum(part, "tp")
    return (grad_input, grad_down)


def solution(mesh):
    placed = (
        P(("rep", "fs"), None),
        P(("rep", "fs"), None),
        P("fs", "tp"),
        P("fs", "tp"),
        P("fs", "tp"),
    )
    return jax.shard_map(
        on_device,
        mesh=mesh,
        in_specs=placed,
        out_specs=(P(("rep", "fs"), None), P("fs", "tp")),
        check_vma=False,
    )
```

```python
import functools
import math

import jax
import jax.numpy as jnp
from jax import lax
from jax.experimental import pallas as pl
from jax.experimental.pallas import tpu as pltpu
from jax.sharding import PartitionSpec as P

MESH = pl.DeviceIdType.MESH


def fused_kernel(
    line, grad_scale, gate_w, up_w, down_w, toks, cots, gi_out, gd_out,
    x, gu, dn_w, acc, hid, ggu, r1, rx, ry, s3, fin, g, u_in, d_in, gfin, gl, gs,
    up_s, up_r, dn_s, dn_r, wy_s, wy_r, tok_s, tok_r, d2d_s, d2d_r, loc,
    c_s, c_r, x_s, x_r, yy_s, yy_r, u_s, u_r, d_s, d_r, f_s, f_r, o_s, o_r, out_l, gl_s,
):
    r = lax.axis_index("rep")
    f = lax.axis_index("fs")
    core = lax.axis_index("tp")
    z, y = f // 2, f % 2
    rows = toks.shape[0]
    half = rows // 2
    wrows = gate_w.shape[0]
    width = gate_w.shape[1] // 4
    depth = 2 * line * wrows
    zrows = 2 * wrows
    cols = depth // 2
    side = cols // 2
    frows = wrows
    last = line - 2
    has_up, has_dn = z < line - 1, z > 0
    is_end = (z == 0) | (z == line - 1)
    up = {"fs": (f + 2) % (2 * line)}
    dn = {"fs": (f + 2 * line - 2) % (2 * line)}
    ypart = {"fs": f + 1 - 2 * y}
    xpart = {"rep": 1 - r}
    cpart = {"tp": 1 - core}

    barrier = pltpu.get_barrier_semaphore()
    for dev in (ypart, xpart, cpart, up, dn):
        pl.semaphore_signal(barrier, inc=1, device_id=dev, device_id_type=MESH)
    pl.semaphore_wait(barrier, 5)

    def remote(src, dst, s, q, dev):
        return pltpu.make_async_remote_copy(
            src_ref=src, dst_ref=dst, send_sem=s, recv_sem=q,
            device_id=dev, device_id_type=MESH,
        )

    def wblk(k, zz, yy):
        row = pl.multiple_of((2 * zz + yy) * wrows, wrows)
        if k == 2:
            return dn_w.at[pl.ds(row, wrows), :]
        return gu.at[pl.ds(row, wrows), pl.ds(k * width, width)]

    def own(k, yy):
        col = pl.multiple_of((2 * r + yy) * width, width)
        return (gate_w, up_w, down_w)[k].at[:, pl.ds(col, width)]

    def to_y(k):
        return remote(own(k, 1 - y), wblk(k, z, y), wy_s.at[k], wy_r.at[k], ypart)

    def from_y(k):
        return remote(own(k, 1 - y), wblk(k, z, 1 - y), wy_s.at[k], wy_r.at[k], ypart)

    def zcopy(up_dir, d, sub, k, zz):
        yy = y if sub == 0 else 1 - y
        src = own(k, y) if (d == 0 and sub == 0) else wblk(k, zz, yy)
        s, q, dev = (up_s, up_r, up) if up_dir else (dn_s, dn_r, dn)
        return remote(src, wblk(k, zz, yy), s.at[d, sub, k], q.at[d, sub, k], dev)

    def pred_send(up_dir, d):
        return (has_up & (z - d >= 0)) if up_dir else (has_dn & (z + d <= line - 1))

    def src_z(up_dir, d):
        return jnp.maximum(z - d, 0) if up_dir else jnp.minimum(z + d, line - 1)

    def send(up_dir, d, sub, k):
        @pl.when(pred_send(up_dir, d))
        def _():
            zcopy(up_dir, d, sub, k, src_z(up_dir, d)).start()

    def await_send(up_dir, d, sub, k):
        @pl.when(pred_send(up_dir, d))
        def _():
            zcopy(up_dir, d, sub, k, src_z(up_dir, d)).wait_send()

    def await_recv(up_dir, d, sub, k):
        ok = (z - d - 1 >= 0) if up_dir else (z + d + 1 <= line - 1)

        @pl.when(ok)
        def _():
            zcopy(up_dir, d, sub, k, src_z(up_dir, d + 1)).wait_recv()

    def relay(d, sub, k):
        for up_dir in (True, False):
            @pl.when(pred_send(up_dir, d + 1))
            def _():
                zcopy(up_dir, d, sub, k, src_z(up_dir, d + 1)).wait_recv()
                zcopy(up_dir, d + 1, sub, k, src_z(up_dir, d + 1)).start()

    def settle(d, sub, k):
        for up_dir in (True, False):
            ok = (z - d - 1 >= 0) if up_dir else (z + d + 1 <= line - 1)
            onward = has_up if up_dir else has_dn

            @pl.when(ok & jnp.logical_not(onward))
            def _():
                zcopy(up_dir, d, sub, k, src_z(up_dir, d + 1)).wait_recv()

    def slot(rr, yy):
        return pl.multiple_of((2 * rr + yy) * rows, rows)

    kinds = (0, 1, 1, 0, 1, 0, 1, 1)
    over_x = (True, True, True, False, False, True, False, True)
    parts = (2, 0, 1, 2, 2, 2, 0, 1)
    ntok = len(kinds)

    def span(c, p):
        if p == 2:
            return c * half, half
        return c * half + p * (half // 2), half // 2

    def tblk(i, rr, yy, c):
        at, count = span(c, parts[i])
        row = pl.multiple_of((2 * rr + yy) * rows + at, half // 2)
        return x.at[kinds[i], pl.ds(row, count), :]

    def mine(i):
        at, count = span(core, parts[i])
        src = toks if kinds[i] == 0 else cots
        return src.at[pl.ds(pl.multiple_of(at, half // 2), count), :]

    def landing(i, c):
        rr = (1 - r, 1 - r, 1 - r, r, r, 1 - r, 1 - r, 1 - r)[i]
        yy = (y, y, y, 1 - y, 1 - y, 1 - y, 1 - y, 1 - y)[i]
        return tblk(i, rr, yy, c)

    def tcopy(i, land):
        dev = xpart if over_x[i] else ypart
        if land:
            src = dst = landing(i, core)
        else:
            rr = (r, r, r, r, r, r, 1 - r, r)[i]
            yy = (y, y, y, y, y, 1 - y, y, 1 - y)[i]
            dst = tblk(i, rr, yy, core)
            src = mine(i) if i < 5 else dst
        return remote(src, dst, tok_s.at[i], tok_r.at[i], dev)

    def dcopy(i, c):
        blk = landing(i, c)
        return remote(blk, blk, d2d_s.at[i], d2d_r.at[i], cpart)

    def event(i):
        tcopy(i, True).wait_recv()
        onward = {1: 6, 3: 5, 4: 7}.get(i)
        if onward is not None:
            tcopy(onward, False).start()
        dcopy(i, core).start()

    trow = slot(r, y)
    loads = [
        pltpu.make_async_copy(own(0, y), wblk(0, z, y), loc.at[0]),
        pltpu.make_async_copy(own(1, y), wblk(1, z, y), loc.at[1]),
        pltpu.make_async_copy(own(2, y), wblk(2, z, y), loc.at[2]),
        pltpu.make_async_copy(toks, x.at[0, pl.ds(trow, rows), :], loc.at[3]),
        pltpu.make_async_copy(cots, x.at[1, pl.ds(trow, rows), :], loc.at[4]),
    ]

    tile = 256
    z_lo = jnp.maximum(z - last, 0)
    z_hi = jnp.minimum(z + last, line - 1) + 1

    def product(j, row, k0, kk, w, wcol, acol, n):
        at = pl.ds(pl.multiple_of(row, rows), rows)
        kat = pl.ds(pl.multiple_of(k0, wrows), kk)
        for c in range(0, n, tile):
            one = jnp.dot(
                x[j, at, kat], w[kat, pl.ds(wcol + c, tile)],
                preferred_element_type=jnp.float32,
            )
            acc[at, pl.ds(acol + c, tile)] += one

    def forward(j, w, acol, n, first, count):
        @pl.loop(first, first + count)
        def _(b):
            row = ((2 * r + y) + 2 * (b % 2) * (1 - 2 * r) + (b // 2) * (1 - 2 * y)) * rows

            @pl.loop(z_lo, z_hi)
            def _(zz):
                product(j, row, zz * zrows, zrows, w, 0, acol, n)

    def forward_end(j, k, sub):
        for up_dir in (True, False):
            await_recv(up_dir, last, sub, k)

        @pl.when(is_end)
        def _():
            zz = line - 1 - z
            yy = y if sub == 0 else 1 - y
            w = dn_w if k == 2 else gu

            @pl.loop(0, 4)
            def _(b):
                product(
                    j, b * rows, (2 * zz + yy) * wrows, wrows, w,
                    0 if k == 2 else k * width, k * width, width,
                )

    def total(dst, terms, count, step=64):
        @pl.loop(0, count // step)
        def _(i):
            at = pl.multiple_of(i * step, step)
            value = None
            for ref, row, col, wide in terms:
                one = ref[pl.ds(row + at, step), pl.ds(col, wide)].astype(jnp.float32)
                value = one if value is None else value + one
            ref, row, col, wide = dst
            ref[pl.ds(row + at, step), pl.ds(col, wide)] = value.astype(ref.dtype)

    for k in (0, 1):
        to_y(k).start()
        send(True, 0, 0, k)
        send(False, 0, 0, k)
    for i in (0, 1, 3):
        tcopy(i, False).start()
    to_y(2).start()
    tcopy(4, False).start()
    for copy in loads:
        copy.start()

    @pl.loop(0, 4 * rows // 64)
    def _(i):
        at = pl.ds(pl.multiple_of(i * 64, 64), 64)
        acc[at, :] = jnp.zeros((64, 3 * width), jnp.float32)

    for k in (0, 1):
        from_y(k).wait_recv()
        send(True, 0, 1, k)
        send(False, 0, 1, k)
    if last > 0:
        for sub in range(2):
            for k in (0, 1):
                relay(0, sub, k)
    event(0)
    event(3)
    tcopy(2, False).start()
    event(1)
    for d in range(1, last):
        for sub in range(2):
            for k in (0, 1):
                relay(d, sub, k)
    send(True, 0, 0, 2)
    send(False, 0, 0, 2)
    from_y(2).wait_recv()
    send(True, 0, 1, 2)
    send(False, 0, 1, 2)
    for load in loads:
        load.wait()
    for d in range(last):
        for sub in range(2):
            for k in (0, 1):
                settle(d, sub, k)
    dcopy(0, 1 - core).wait_recv()
    dcopy(3, 1 - core).wait_recv()
    forward(0, gu, 0, 2 * width, 0, 3)
    if last > 0:
        for sub in range(2):
            relay(0, sub, 2)
    event(5)
    event(4)
    dcopy(5, 1 - core).wait_recv()
    forward(0, gu, 0, 2 * width, 3, 1)
    for d in range(1, last):
        for sub in range(2):
            relay(d, sub, 2)
    for sub in range(2):
        for k in (0, 1):
            forward_end(0, k, sub)

    @pl.loop(0, 4 * rows // 32)
    def _(i):
        at = pl.ds(pl.multiple_of(i * 32, 32), 32)
        gate = acc[at, pl.ds(0, width)]
        up_val = acc[at, pl.ds(width, width)]
        sig = jax.nn.sigmoid(gate)
        active = gate * sig
        hid[at, :] = (active * up_val).astype(hid.dtype)
        acc[at, pl.ds(0, width)] = up_val * sig * (1.0 + gate * (1.0 - sig))
        acc[at, pl.ds(width, width)] = active

    for i in (2, 6, 7):
        event(i)
    for i in (1, 2, 4, 6, 7):
        dcopy(i, 1 - core).wait_recv()

    def block(ref, zt):
        return ref.at[pl.ds(zt * zrows, zrows), :]

    def up_copy(zt, first):
        return remote(block(g if first else u_in, zt), block(u_in, zt), u_s.at[zt], u_r.at[zt], up)

    def dn_copy(zt, first):
        return remote(block(g if first else d_in, zt), block(d_in, zt), d_s.at[zt], d_r.at[zt], dn)

    for i in range(line):
        zt = jnp.where(z < line // 2, line - 1 - i, i)

        at = pl.multiple_of(zt * zrows, zrows)
        one = lax.dot_general(
            x[1, :, pl.ds(at, zrows)], hid[...], (((0,), (0,)), ((), ())),
            preferred_element_type=jnp.float32,
        )
        g[pl.ds(at, zrows), :] = one.astype(g.dtype)

        if i < line - 1:
            @pl.when(z == 0)
            def _():
                up_copy(line - 1 - i, True).start()

            @pl.when(z == line - 1)
            def _():
                dn_copy(i, True).start()

    def line_step(t):
        zt = line - 1 + z - t

        @pl.when((z > 0) & (zt <= line - 1) & (zt > z))
        def _():
            up_copy(zt, False).wait_recv()
            row = pl.multiple_of(zt * zrows, zrows)
            total((u_in, row, 0, width), [(g, row, 0, width), (u_in, row, 0, width)], zrows)
            up_copy(zt, False).start()

        zd = t - (line - 1 - z)

        @pl.when((z < line - 1) & (zd >= 0) & (zd < z))
        def _():
            dn_copy(zd, False).wait_recv()
            row = pl.multiple_of(zd * zrows, zrows)
            total((d_in, row, 0, width), [(g, row, 0, width), (d_in, row, 0, width)], zrows)
            dn_copy(zd, False).start()

    for d in range(last):
        for sub in range(2):
            settle(d, sub, 2)
    forward(1, dn_w, 2 * width, width, 0, 4)
    for sub in range(2):
        forward_end(1, 2, sub)

    for i in (0, 3, 5):
        dcopy(i, core).wait_send()
    tcopy(5, False).wait_send()
    line_step(1)
    order = [(1 - r, 1 - y), (1 - r, y), (r, 1 - y), (r, y)]
    my_col = pl.multiple_of(core * cols, cols)
    its_col = pl.multiple_of((1 - core) * cols, cols)
    part = x.at[0]

    def slopes(row):
        @pl.loop(0, rows // 32)
        def _(i):
            at = pl.ds(pl.multiple_of(row + i * 32, 32), 32)
            grad = acc[at, pl.ds(2 * width, width)]
            ggu[at, pl.ds(0, width)] = (grad * acc[at, pl.ds(0, width)]).astype(ggu.dtype)
            ggu[at, pl.ds(width, width)] = (grad * acc[at, pl.ds(width, width)]).astype(ggu.dtype)

    def back(row, col):
        @pl.loop(0, cols // side)
        def _(n):
            at = pl.multiple_of(col + n * side, side)
            one = lax.dot_general(
                ggu[pl.ds(row, rows), :], gu[pl.ds(at, side), :], (((1,), (1,)), ((), ())),
                preferred_element_type=jnp.float32,
            )
            x[0, pl.ds(row, rows), pl.ds(at, side)] = one.astype(x.dtype)

    def core_copy(i):
        at = pl.ds(slot(*order[i]), rows)
        return remote(part.at[at, pl.ds(its_col, cols)], r1.at[at, :], c_s.at[i], c_r.at[i], cpart)

    def s1_half(i, second):
        col = pl.multiple_of(my_col + (side if second else 0), side)
        return part.at[pl.ds(slot(*order[i]), rows), pl.ds(col, side)]

    def s1(row, second):
        return (part, row, pl.multiple_of(my_col + (side if second else 0), side), side)

    def x_copy(i):
        src = s3.at[1] if i == 2 else s1_half(i, False)
        return remote(src, rx.at[i], x_s.at[i], x_r.at[i], xpart)

    def y_copy(i):
        src = s3.at[0] if i == 2 else s1_half((0, 2)[i], True)
        return remote(src, ry.at[i], yy_s.at[i], yy_r.at[i], ypart)

    for i in range(4):
        row = slot(*order[i])
        slopes(row)
        back(row, its_col)
        core_copy(i).start()
        back(row, my_col)
        core_copy(i).wait_recv()
        total((part, row, my_col, cols), [(part, row, my_col, cols), (r1, row, 0, cols)], rows)
        if i in (0, 1):
            x_copy(i).start()
        if i == 0:
            y_copy(0).start()
        if i == 2:
            y_copy(1).start()
        if i == 2:
            for t in range(2, line - 1):
                line_step(t)

    zrow = pl.multiple_of(z * zrows, zrows)

    def here(ref):
        return (ref, zrow, 0, width)

    @pl.when(z == 0)
    def _():
        dn_copy(0, True).wait_recv()
        total((gfin, 0, 0, width), [here(g), here(d_in)], zrows)

    @pl.when(z == line - 1)
    def _():
        up_copy(line - 1, True).wait_recv()
        total((gfin, 0, 0, width), [here(g), here(u_in)], zrows)

    @pl.when((z > 0) & (z < line - 1))
    def _():
        remote(block(g, z), block(u_in, z), u_s.at[z], u_r.at[z], up).wait_recv()
        remote(block(g, z), block(d_in, z), d_s.at[z], d_r.at[z], dn).wait_recv()
        total((gfin, 0, 0, width), [here(g), here(u_in), here(d_in)], zrows)

    def gcol(rr, yy):
        return pl.multiple_of((2 * rr + yy) * width, width)

    def gcols(rr, yy):
        return gl.at[:, pl.ds(gcol(rr, yy), width)]

    def grows(yy):
        return gfin.at[pl.ds(pl.multiple_of(yy * frows, frows), frows), :]

    def f_copy(i, land):
        if i == 0:
            src, dst, dev = grows(1 - y), gcols(r, 1 - y) if land else gcols(r, y), ypart
        elif i == 1:
            src, dst, dev = grows(y), gcols(1 - r, y) if land else gcols(r, y), xpart
        else:
            src, dev = gcols(r, 1 - y), xpart
            dst = gcols(1 - r, 1 - y) if land else src
        return remote(src, dst, f_s.at[i], f_r.at[i], dev)

    def scaled(i, ref, row, col, rr, yy):
        at_col = gcol(rr, yy)

        @pl.loop(0, frows // 64)
        def _(m):
            at = pl.multiple_of(m * 64, 64)
            one = ref[pl.ds(row + at, 64), pl.ds(col, width)].astype(jnp.float32)
            gs[pl.ds(at, 64), pl.ds(at_col, width)] = one * grad_scale

        g_local(i, rr, yy).start()

    def g_local(i, rr, yy):
        at = gcol(rr, yy)
        return pltpu.make_async_copy(
            gs.at[:, pl.ds(at, width)], gd_out.at[:, pl.ds(at, width)], gl_s.at[i]
        )

    f_copy(0, False).start()
    f_copy(1, False).start()
    scaled(0, gfin, pl.multiple_of(y * frows, frows), 0, r, y)

    x_copy(0).wait_recv()
    total((s3.at[0], 0, 0, side), [s1(slot(r, 1 - y), False), (rx.at[0], 0, 0, side)], rows)
    y_copy(2).start()
    y_copy(0).wait_recv()
    total((s3.at[1], 0, 0, side), [s1(slot(1 - r, y), True), (ry.at[0], 0, 0, side)], rows)
    x_copy(2).start()
    f_copy(0, True).wait_recv()
    f_copy(2, False).start()
    scaled(1, gl, 0, gcol(r, 1 - y), r, 1 - y)
    f_copy(1, True).wait_recv()
    scaled(2, gl, 0, gcol(1 - r, y), 1 - r, y)

    x_copy(1).wait_recv()
    y_copy(2).wait_recv()
    here_row = slot(r, y)
    total(
        (fin, 0, 0, side),
        [s1(here_row, False), (rx.at[1], 0, 0, side), (ry.at[2], 0, 0, side)], rows,
    )

    def o_copy(i, land):
        base = (1 - core if land else core) * cols + i * side
        dst = gi_out.at[:, pl.ds(pl.multiple_of(base, side), side)]
        return remote(fin.at[:, pl.ds(i * side, side)], dst, o_s.at[i], o_r.at[i], cpart)

    def o_local(i):
        base = pl.multiple_of(core * cols + i * side, side)
        return pltpu.make_async_copy(
            fin.at[:, pl.ds(i * side, side)], gi_out.at[:, pl.ds(base, side)], out_l.at[i]
        )

    o_copy(0, False).start()
    o_local(0).start()
    y_copy(1).wait_recv()
    x_copy(2).wait_recv()
    total(
        (fin, 0, side, side),
        [s1(here_row, True), (ry.at[1], 0, 0, side), (rx.at[2], 0, 0, side)], rows,
    )
    o_copy(1, False).start()
    o_local(1).start()
    f_copy(2, True).wait_recv()
    scaled(3, gl, 0, gcol(1 - r, 1 - y), 1 - r, 1 - y)

    for i in range(ntok):
        if kinds[i] == 1:
            dcopy(i, core).wait_send()
        if i != 5:
            tcopy(i, False).wait_send()
    for k in range(3):
        to_y(k).wait_send()
        for d in range(line - 1):
            for sub in range(2):
                await_send(True, d, sub, k)
                await_send(False, d, sub, k)
    for i in range(4):
        core_copy(i).wait_send()
    for i in range(3):
        x_copy(i).wait_send()
        y_copy(i).wait_send()
        f_copy(i, False).wait_send()
    for i in range(2):
        o_copy(i, True).wait_recv()
        o_copy(i, False).wait_send()
        o_local(i).wait()
    for i, (rr, yy) in enumerate(((r, y), (r, 1 - y), (1 - r, y), (1 - r, 1 - y))):
        g_local(i, rr, yy).wait()
    for zt in range(line):
        if zt > 0:
            pl.when(z < zt)(lambda: up_copy(zt, True).wait_send())
        if zt < line - 1:
            pl.when(z > zt)(lambda: dn_copy(zt, True).wait_send())


def fused(grad_scale, gate_w, up_w, down_w, toks, cots):
    line = lax.axis_size("fs") // 2
    rows, full = toks.shape
    wrows, width = gate_w.shape[0], gate_w.shape[1] // 4
    depth = 2 * line * wrows
    cols = full // 2
    kind = gate_w.dtype
    dma = pltpu.SemaphoreType.DMA
    zsem = dma((line - 1, 2, 3))
    anyspec = pl.BlockSpec(memory_space=pl.ANY)
    whole = pltpu.VMEM((depth, width), kind)
    unit = pltpu.VMEM((3, rows, cols // 2), kind)
    return pl.pallas_call(
        functools.partial(fused_kernel, line, grad_scale),
        out_shape=(
            jax.ShapeDtypeStruct((rows, full), kind),
            jax.ShapeDtypeStruct((wrows, 4 * width), jnp.float32),
        ),
        in_specs=[anyspec] * 5,
        out_specs=(anyspec,) * 2,
        scratch_shapes=[
            pltpu.VMEM((2, 4 * rows, full), kind),
            pltpu.VMEM((depth, 2 * width), kind),
            whole,
            pltpu.VMEM((4 * rows, 3 * width), jnp.float32),
            pltpu.VMEM((4 * rows, width), kind),
            pltpu.VMEM((4 * rows, 2 * width), kind),
            pltpu.VMEM((4 * rows, cols), kind),
            unit, unit,
            pltpu.VMEM((2, rows, cols // 2), kind),
            pltpu.VMEM((rows, cols), kind),
            whole, whole, whole,
            pltpu.VMEM((2 * wrows, width), kind),
            pltpu.VMEM((wrows, 4 * width), kind),
            pltpu.VMEM((wrows, 4 * width), jnp.float32),
            zsem, zsem, zsem, zsem,
            dma((3,)), dma((3,)),
            dma((8,)), dma((8,)), dma((8,)), dma((8,)), dma((5,)),
            dma((4,)), dma((4,)), dma((3,)), dma((3,)), dma((3,)), dma((3,)),
            dma((line,)), dma((line,)), dma((line,)), dma((line,)),
            dma((3,)), dma((3,)), dma((2,)), dma((2,)), dma((2,)), dma((4,)),
        ],
        compiler_params=pltpu.CompilerParams(
            collective_id=1, has_side_effects=True, vmem_limit_bytes=67043328
        ),
        name="fused_all",
    )(gate_w, up_w, down_w, toks, cots)


def gather_kernel(
    line, units, gate_w, up_w, down_w, toks, cots, gu_out, d_out, t_out, w_tmp, t_tmp,
    up_s, up_r, dn_s, dn_r, y_s, y_r, tok_s, tok_r, d2d_s, d2d_r, loc, loc2,
):
    r = lax.axis_index("rep")
    f = lax.axis_index("fs")
    t = lax.axis_index("tp")
    z, y = f // 2, f % 2
    rows = toks.shape[0]
    half = rows // 2
    wrows = gate_w.shape[0]
    width = gate_w.shape[1] // 4
    parts = len(units)
    has_up, has_dn = z < line - 1, z > 0
    up = {"fs": (f + 2) % (2 * line)}
    dn = {"fs": (f + 2 * line - 2) % (2 * line)}
    ypart = {"fs": f + 1 - 2 * y}
    xpart = {"rep": 1 - r}
    core = t % 2
    cpart = {"tp": t + 1 - 2 * core}

    barrier = pltpu.get_barrier_semaphore()

    def greet(dev):
        pl.semaphore_signal(barrier, inc=1, device_id=dev, device_id_type=MESH)

    for dev in (ypart, xpart, cpart, up, dn):
        greet(dev)
    pl.semaphore_wait(barrier, 5)

    def remote(src, dst, s, q, dev):
        return pltpu.make_async_remote_copy(
            src_ref=src, dst_ref=dst, send_sem=s, recv_sem=q,
            device_id=dev, device_id_type=MESH,
        )

    def wblk(k, zz, yy):
        row = pl.multiple_of((2 * zz + yy) * wrows, wrows)
        which, col, wide = units[k]
        return (gu_out, d_out)[which].at[pl.ds(row, wrows), pl.ds(col, wide)]

    def own(k, yy):
        col = pl.multiple_of((2 * r + yy) * width, width)
        return (gate_w, up_w, down_w)[k].at[:, pl.ds(col, width)]

    def to_y(k):
        return remote(own(k, 1 - y), wblk(k, z, y), y_s.at[k], y_r.at[k], ypart)

    def from_y(k):
        return remote(own(k, 1 - y), wblk(k, z, 1 - y), y_s.at[k], y_r.at[k], ypart)

    def zcopy(up_dir, d, sub, k, zz):
        yy = y if sub == 0 else 1 - y
        src = own(k, y) if (d == 0 and sub == 0) else wblk(k, zz, yy)
        s, q, dev = (up_s, up_r, up) if up_dir else (dn_s, dn_r, dn)
        return remote(src, wblk(k, zz, yy), s.at[d, sub, k], q.at[d, sub, k], dev)

    def pred_send(up_dir, d):
        return (has_up & (z - d >= 0)) if up_dir else (has_dn & (z + d <= line - 1))

    def src_z(up_dir, d):
        return jnp.maximum(z - d, 0) if up_dir else jnp.minimum(z + d, line - 1)

    def send(up_dir, d, sub, k):
        @pl.when(pred_send(up_dir, d))
        def _():
            zcopy(up_dir, d, sub, k, src_z(up_dir, d)).start()

    def await_send(up_dir, d, sub, k):
        @pl.when(pred_send(up_dir, d))
        def _():
            zcopy(up_dir, d, sub, k, src_z(up_dir, d)).wait_send()

    def await_recv(up_dir, d, sub, k):
        ok = (z - d - 1 >= 0) if up_dir else (z + d + 1 <= line - 1)

        @pl.when(ok)
        def _():
            zcopy(up_dir, d, sub, k, src_z(up_dir, d + 1)).wait_recv()

    def tblk(j, rr, yy, c):
        row = pl.multiple_of((2 * rr + yy) * rows + c * half, half)
        return t_out.at[j, pl.ds(row, half), :]

    def mine(j):
        src = toks if j == 0 else cots
        return src.at[pl.ds(pl.multiple_of(core * half, half), half), :]

    def tcopy(i, landing):
        j = (0, 1, 0, 1, 0, 1)[i]
        dev = xpart if i in (0, 1, 5) else ypart
        if landing:
            rr = (1 - r, 1 - r, r, r, 1 - r, 1 - r)[i]
            yy = (y, y, 1 - y, 1 - y, 1 - y, 1 - y)[i]
            src = dst = tblk(j, rr, yy, core)
        else:
            rr = (r, r, r, r, 1 - r, r)[i]
            yy = (y, y, y, y, y, 1 - y)[i]
            dst = tblk(j, rr, yy, core)
            src = mine(j) if i < 4 else dst
        return remote(src, dst, tok_s.at[i], tok_r.at[i], dev)

    def dcopy(i, c):
        j = (0, 1, 0, 1, 0, 1)[i]
        rr = (1 - r, 1 - r, r, r, 1 - r, 1 - r)[i]
        yy = (y, y, 1 - y, 1 - y, 1 - y, 1 - y)[i]
        blk = tblk(j, rr, yy, c)
        return remote(blk, blk, d2d_s.at[i], d2d_r.at[i], cpart)

    loads = [
        pltpu.make_async_copy(own(0, y), w_tmp.at[0], loc.at[0]),
        pltpu.make_async_copy(own(1, y), w_tmp.at[1], loc.at[3]),
        pltpu.make_async_copy(own(2, y), w_tmp.at[2], loc.at[4]),
        pltpu.make_async_copy(toks, t_tmp.at[0], loc.at[1]),
        pltpu.make_async_copy(cots, t_tmp.at[1], loc.at[2]),
    ]
    trow = pl.multiple_of((2 * r + y) * rows, rows)
    stores = [
        pltpu.make_async_copy(w_tmp.at[0], wblk(0, z, y), loc2.at[0]),
        pltpu.make_async_copy(w_tmp.at[1], wblk(1, z, y), loc2.at[3]),
        pltpu.make_async_copy(w_tmp.at[2], wblk(2, z, y), loc2.at[4]),
        pltpu.make_async_copy(t_tmp.at[0], t_out.at[0, pl.ds(trow, rows), :], loc2.at[1]),
        pltpu.make_async_copy(t_tmp.at[1], t_out.at[1, pl.ds(trow, rows), :], loc2.at[2]),
    ]

    for k in range(parts):
        to_y(k).start()
        send(True, 0, 0, k)
        send(False, 0, 0, k)
    for i in (0, 1, 3, 2):
        tcopy(i, False).start()
    for copy in loads:
        copy.start()
    for load, store in zip(loads, stores):
        load.wait()
        store.start()
    for k in range(parts):
        from_y(k).wait_recv()
        send(True, 0, 1, k)
        send(False, 0, 1, k)

    def event(i):
        tcopy(i, True).wait_recv()
        if i == 0:
            tcopy(4, False).start()
        if i == 3:
            tcopy(5, False).start()
        dcopy(i, core).start()

    events = [0, 3, 1, 2, 5, 4]
    for d in range(line - 1):
        for sub in range(2):
            if events:
                event(events.pop(0))
            for k in range(parts):
                for up_dir in (True, False):
                    await_recv(up_dir, d, sub, k)
                    if d + 1 < line - 1:
                        send(up_dir, d + 1, sub, k)
    for i in events:
        event(i)
    for i in range(6):
        dcopy(i, 1 - core).wait_recv()
        dcopy(i, core).wait_send()
        tcopy(i, False).wait_send()
    for k in range(parts):
        to_y(k).wait_send()
        for d in range(line - 1):
            for sub in range(2):
                await_send(True, d, sub, k)
                await_send(False, d, sub, k)
    for store in stores:
        store.wait()


def gather(gate_w, up_w, down_w, toks, cots):
    line = lax.axis_size("fs") // 2
    wrows, width = gate_w.shape[0], gate_w.shape[1] // 4
    units = [(0, 0, width), (0, width, width), (1, 0, width)]
    parts = len(units)
    depth = 2 * line * wrows
    kind = gate_w.dtype
    dma = pltpu.SemaphoreType.DMA
    zsem = dma((line - 1, 2, parts))
    anyspec = pl.BlockSpec(memory_space=pl.ANY)
    return pl.pallas_call(
        functools.partial(gather_kernel, line, units),
        out_shape=(
            jax.ShapeDtypeStruct((depth, 2 * width), kind),
            jax.ShapeDtypeStruct((depth, width), kind),
            jax.ShapeDtypeStruct((2, 4 * toks.shape[0], toks.shape[1]), toks.dtype),
        ),
        in_specs=[anyspec] * 5,
        out_specs=(anyspec,) * 3,
        scratch_shapes=[
            pltpu.VMEM((parts, wrows, width), kind),
            pltpu.VMEM((2,) + toks.shape, toks.dtype),
            zsem, zsem, zsem, zsem,
            dma((parts,)), dma((parts,)),
            dma((6,)), dma((6,)), dma((6,)), dma((6,)),
            dma((5,)), dma((5,)),
        ],
        compiler_params=pltpu.CompilerParams(collective_id=0, has_side_effects=True),
        name="gather_all",
    )(gate_w, up_w, down_w, toks, cots)


def on_device(inputs, cotangent, gate_weight, up_weight, down_weight):
    tok_rows = inputs.shape[0]
    fs_size = lax.axis_size("fs")
    rep_size = lax.axis_size("rep")
    grad_scale = 1.0 / math.sqrt(tok_rows * fs_size * rep_size)
    if lax.axis_size("tp") == 2:
        return fused(
            grad_scale, gate_weight, up_weight, down_weight, inputs, cotangent
        )
    contract = (((1,), (1,)), ((), ()))
    contract_tok = (((0,), (0,)), ((), ()))
    width = gate_weight.shape[1] // 4
    gate_up, down_full, tokens = gather(
        gate_weight, up_weight, down_weight, inputs, cotangent
    )
    gate_up_val = jnp.dot(tokens[0], gate_up, preferred_element_type=jnp.float32)
    gate_val, up_val = gate_up_val[:, :width], gate_up_val[:, width:]
    grad_hidden = jnp.dot(tokens[1], down_full, preferred_element_type=jnp.float32)
    sigmoid_gate = jax.nn.sigmoid(gate_val)
    active = gate_val * sigmoid_gate
    hidden = (active * up_val).astype(jnp.bfloat16)
    grad_gate = (
        grad_hidden * up_val * sigmoid_gate * (1.0 + gate_val * (1.0 - sigmoid_gate))
    ).astype(jnp.bfloat16)
    grad_up = (grad_hidden * active).astype(jnp.bfloat16)
    pairs = [[i, i + 1] for i in range(0, fs_size, 2)]
    lines = [list(range(i, fs_size, 2)) for i in range(2)]
    grad_part = lax.dot_general(
        tokens[1], hidden, contract_tok, preferred_element_type=jnp.float32
    )
    part = lax.dot_general(
        jnp.concatenate([grad_gate, grad_up], axis=1), gate_up, contract,
        preferred_element_type=jnp.float32,
    )
    shard = lax.psum_scatter(
        grad_part.astype(jnp.bfloat16), "fs", scatter_dimension=0, tiled=True,
        axis_index_groups=lines,
    ).astype(jnp.float32) * grad_scale
    shard = lax.all_to_all(
        shard, "fs", split_axis=0, concat_axis=1, tiled=True, axis_index_groups=pairs
    )
    grad_down = lax.all_gather(shard, "rep", axis=1, tiled=True)
    part = lax.psum_scatter(
        part.astype(jnp.bfloat16), "rep", scatter_dimension=0, tiled=True
    )
    part = lax.psum_scatter(
        part, "fs", scatter_dimension=0, tiled=True, axis_index_groups=pairs
    )
    grad_input = lax.psum(part, "tp")
    return (grad_input, grad_down)


def solution(mesh):
    placed = (
        P(("rep", "fs"), None),
        P(("rep", "fs"), None),
        P("fs", "tp"),
        P("fs", "tp"),
        P("fs", "tp"),
    )
    return jax.shard_map(
        on_device,
        mesh=mesh,
        in_specs=placed,
        out_specs=(P(("rep", "fs"), None), P("fs", "tp")),
        check_vma=False,
    )
```

```python
import functools
import math

import jax
import jax.numpy as jnp
from jax import lax
from jax.experimental import pallas as pl
from jax.experimental.pallas import tpu as pltpu
from jax.sharding import PartitionSpec as P

MESH = pl.DeviceIdType.MESH


def fused_kernel(
    line, grad_scale, gate_w, up_w, down_w, toks, cots, gi_out, gd_out,
    x, gu, dn_w, acc, hid, ggu, r1, rxa, rxb, rya, ryb, s3a, s3b, g, u_in, d_in, gfin, gl,
    up_s, up_r, dn_s, dn_r, wy_s, wy_r, tok_s, tok_r, d2d_s, d2d_r, loc,
    c_s, c_r, x_s, x_r, yy_s, yy_r, u_s, u_r, d_s, d_r, f_s, f_r, o_s, o_r,
):
    r = lax.axis_index("rep")
    f = lax.axis_index("fs")
    core = lax.axis_index("tp")
    z, y = f // 2, f % 2
    rows = toks.shape[0]
    half = rows // 2
    wrows = gate_w.shape[0]
    width = gate_w.shape[1] // 4
    depth = 2 * line * wrows
    zrows = 2 * wrows
    cols = depth // 2
    wide = cols // 2
    parts_a = rxa.shape[2]
    parts_b = cols - parts_a
    frows = wrows
    last = line - 2
    has_up, has_dn = z < line - 1, z > 0
    is_end = (z == 0) | (z == line - 1)
    up = {"fs": (f + 2) % (2 * line)}
    dn = {"fs": (f + 2 * line - 2) % (2 * line)}
    ypart = {"fs": f + 1 - 2 * y}
    xpart = {"rep": 1 - r}
    cpart = {"tp": 1 - core}

    barrier = pltpu.get_barrier_semaphore()
    for dev in (ypart, xpart, cpart, up, dn):
        pl.semaphore_signal(barrier, inc=1, device_id=dev, device_id_type=MESH)
    pl.semaphore_wait(barrier, 5)

    def remote(src, dst, s, q, dev):
        return pltpu.make_async_remote_copy(
            src_ref=src, dst_ref=dst, send_sem=s, recv_sem=q,
            device_id=dev, device_id_type=MESH,
        )

    def wblk(k, zz, yy):
        row = pl.multiple_of((2 * zz + yy) * wrows, wrows)
        if k == 2:
            return dn_w.at[pl.ds(row, wrows), :]
        return gu.at[pl.ds(row, wrows), pl.ds(k * width, width)]

    def own(k, yy):
        col = pl.multiple_of((2 * r + yy) * width, width)
        return (gate_w, up_w, down_w)[k].at[:, pl.ds(col, width)]

    def to_y(k):
        return remote(own(k, 1 - y), wblk(k, z, y), wy_s.at[k], wy_r.at[k], ypart)

    def from_y(k):
        return remote(own(k, 1 - y), wblk(k, z, 1 - y), wy_s.at[k], wy_r.at[k], ypart)

    def zcopy(up_dir, d, sub, k, zz):
        yy = y if sub == 0 else 1 - y
        src = own(k, y) if (d == 0 and sub == 0) else wblk(k, zz, yy)
        s, q, dev = (up_s, up_r, up) if up_dir else (dn_s, dn_r, dn)
        return remote(src, wblk(k, zz, yy), s.at[d, sub, k], q.at[d, sub, k], dev)

    def pred_send(up_dir, d):
        return (has_up & (z - d >= 0)) if up_dir else (has_dn & (z + d <= line - 1))

    def src_z(up_dir, d):
        return jnp.maximum(z - d, 0) if up_dir else jnp.minimum(z + d, line - 1)

    def send(up_dir, d, sub, k):
        @pl.when(pred_send(up_dir, d))
        def _():
            zcopy(up_dir, d, sub, k, src_z(up_dir, d)).start()

    def await_send(up_dir, d, sub, k):
        @pl.when(pred_send(up_dir, d))
        def _():
            zcopy(up_dir, d, sub, k, src_z(up_dir, d)).wait_send()

    def await_recv(up_dir, d, sub, k):
        ok = (z - d - 1 >= 0) if up_dir else (z + d + 1 <= line - 1)

        @pl.when(ok)
        def _():
            zcopy(up_dir, d, sub, k, src_z(up_dir, d + 1)).wait_recv()

    def relay(d, sub, k):
        for up_dir in (True, False):
            @pl.when(pred_send(up_dir, d + 1))
            def _():
                zcopy(up_dir, d, sub, k, src_z(up_dir, d + 1)).wait_recv()
                zcopy(up_dir, d + 1, sub, k, src_z(up_dir, d + 1)).start()

    def settle(d, sub, k):
        for up_dir in (True, False):
            ok = (z - d - 1 >= 0) if up_dir else (z + d + 1 <= line - 1)
            onward = has_up if up_dir else has_dn

            @pl.when(ok & jnp.logical_not(onward))
            def _():
                zcopy(up_dir, d, sub, k, src_z(up_dir, d + 1)).wait_recv()

    def slot(rr, yy):
        return pl.multiple_of((2 * rr + yy) * rows, rows)

    kinds = (0, 1, 1, 0, 1, 0, 1, 1)
    over_x = (True, True, True, False, False, True, False, True)
    parts = (2, 0, 1, 2, 2, 2, 0, 1)
    ntok = len(kinds)

    def span(c, p):
        if p == 2:
            return c * half, half
        return c * half + p * (half // 2), half // 2

    def tblk(i, rr, yy, c):
        at, count = span(c, parts[i])
        row = pl.multiple_of((2 * rr + yy) * rows + at, half // 2)
        return x.at[kinds[i], pl.ds(row, count), :]

    def mine(i):
        at, count = span(core, parts[i])
        src = toks if kinds[i] == 0 else cots
        return src.at[pl.ds(pl.multiple_of(at, half // 2), count), :]

    def landing(i, c):
        rr = (1 - r, 1 - r, 1 - r, r, r, 1 - r, 1 - r, 1 - r)[i]
        yy = (y, y, y, 1 - y, 1 - y, 1 - y, 1 - y, 1 - y)[i]
        return tblk(i, rr, yy, c)

    def tcopy(i, land):
        dev = xpart if over_x[i] else ypart
        if land:
            src = dst = landing(i, core)
        else:
            rr = (r, r, r, r, r, r, 1 - r, r)[i]
            yy = (y, y, y, y, y, 1 - y, y, 1 - y)[i]
            dst = tblk(i, rr, yy, core)
            src = mine(i) if i < 5 else dst
        return remote(src, dst, tok_s.at[i], tok_r.at[i], dev)

    def dcopy(i, c):
        blk = landing(i, c)
        return remote(blk, blk, d2d_s.at[i], d2d_r.at[i], cpart)

    def event(i):
        tcopy(i, True).wait_recv()
        onward = {1: 6, 3: 5, 4: 7}.get(i)
        if onward is not None:
            tcopy(onward, False).start()
        dcopy(i, core).start()

    trow = slot(r, y)
    loads = [
        pltpu.make_async_copy(own(0, y), wblk(0, z, y), loc.at[0]),
        pltpu.make_async_copy(own(1, y), wblk(1, z, y), loc.at[1]),
        pltpu.make_async_copy(own(2, y), wblk(2, z, y), loc.at[2]),
        pltpu.make_async_copy(toks, x.at[0, pl.ds(trow, rows), :], loc.at[3]),
        pltpu.make_async_copy(cots, x.at[1, pl.ds(trow, rows), :], loc.at[4]),
    ]

    tile = 256
    z_lo = jnp.maximum(z - last, 0)
    z_hi = jnp.minimum(z + last, line - 1) + 1

    def product(j, row, k0, kk, w, wcol, acol, n):
        at = pl.ds(pl.multiple_of(row, rows), rows)
        kat = pl.ds(pl.multiple_of(k0, wrows), kk)
        for c in range(0, n, tile):
            one = jnp.dot(
                x[j, at, kat], w[kat, pl.ds(wcol + c, tile)],
                preferred_element_type=jnp.float32,
            )
            acc[at, pl.ds(acol + c, tile)] += one

    def forward(j, w, acol, n, first, count):
        @pl.loop(first, first + count)
        def _(b):
            row = ((2 * r + y) + 2 * (b % 2) * (1 - 2 * r) + (b // 2) * (1 - 2 * y)) * rows

            @pl.loop(z_lo, z_hi)
            def _(zz):
                product(j, row, zz * zrows, zrows, w, 0, acol, n)

    def forward_end(j, k, sub):
        for up_dir in (True, False):
            await_recv(up_dir, last, sub, k)

        @pl.when(is_end)
        def _():
            zz = line - 1 - z
            yy = y if sub == 0 else 1 - y
            w = dn_w if k == 2 else gu

            @pl.loop(0, 4)
            def _(b):
                product(
                    j, b * rows, (2 * zz + yy) * wrows, wrows, w,
                    0 if k == 2 else k * width, k * width, width,
                )

    def total(dst, terms, count, step=64):
        @pl.loop(0, count // step)
        def _(i):
            at = pl.multiple_of(i * step, step)
            value = None
            for ref, row, col, wide in terms:
                one = ref[pl.ds(row + at, step), pl.ds(col, wide)].astype(jnp.float32)
                value = one if value is None else value + one
            ref, row, col, wide = dst
            ref[pl.ds(row + at, step), pl.ds(col, wide)] = value.astype(ref.dtype)

    for k in (0, 1):
        to_y(k).start()
        send(True, 0, 0, k)
        send(False, 0, 0, k)
    for i in (0, 1, 3):
        tcopy(i, False).start()
    to_y(2).start()
    tcopy(4, False).start()
    for copy in loads:
        copy.start()

    @pl.loop(0, 4 * rows // 64)
    def _(i):
        at = pl.ds(pl.multiple_of(i * 64, 64), 64)
        acc[at, :] = jnp.zeros((64, 3 * width), jnp.float32)

    for k in (0, 1):
        from_y(k).wait_recv()
        send(True, 0, 1, k)
        send(False, 0, 1, k)
    if last > 0:
        for sub in range(2):
            for k in (0, 1):
                relay(0, sub, k)
    event(0)
    event(3)
    tcopy(2, False).start()
    event(1)
    for d in range(1, last):
        for sub in range(2):
            for k in (0, 1):
                relay(d, sub, k)
    send(True, 0, 0, 2)
    send(False, 0, 0, 2)
    from_y(2).wait_recv()
    send(True, 0, 1, 2)
    send(False, 0, 1, 2)
    for load in loads:
        load.wait()
    for d in range(last):
        for sub in range(2):
            for k in (0, 1):
                settle(d, sub, k)
    dcopy(0, 1 - core).wait_recv()
    dcopy(3, 1 - core).wait_recv()
    forward(0, gu, 0, 2 * width, 0, 3)
    if last > 0:
        for sub in range(2):
            relay(0, sub, 2)
    event(5)
    event(4)
    dcopy(5, 1 - core).wait_recv()
    forward(0, gu, 0, 2 * width, 3, 1)
    for d in range(1, last):
        for sub in range(2):
            relay(d, sub, 2)
    for sub in range(2):
        for k in (0, 1):
            forward_end(0, k, sub)

    @pl.loop(0, 4 * rows // 32)
    def _(i):
        at = pl.ds(pl.multiple_of(i * 32, 32), 32)
        gate = acc[at, pl.ds(0, width)]
        up_val = acc[at, pl.ds(width, width)]
        sig = jax.nn.sigmoid(gate)
        active = gate * sig
        hid[at, :] = (active * up_val).astype(hid.dtype)
        acc[at, pl.ds(0, width)] = up_val * sig * (1.0 + gate * (1.0 - sig))
        acc[at, pl.ds(width, width)] = active

    for i in (2, 6, 7):
        event(i)
    for i in (1, 2, 4, 6, 7):
        dcopy(i, 1 - core).wait_recv()

    def block(ref, zt):
        return ref.at[pl.ds(zt * zrows, zrows), :]

    def up_copy(zt, first):
        return remote(block(g if first else u_in, zt), block(u_in, zt), u_s.at[zt], u_r.at[zt], up)

    def dn_copy(zt, first):
        return remote(block(g if first else d_in, zt), block(d_in, zt), d_s.at[zt], d_r.at[zt], dn)

    for i in range(line):
        zt = jnp.where(z < line // 2, line - 1 - i, i)

        at = pl.multiple_of(zt * zrows, zrows)
        one = lax.dot_general(
            x[1, :, pl.ds(at, zrows)], hid[...], (((0,), (0,)), ((), ())),
            preferred_element_type=jnp.float32,
        )
        g[pl.ds(at, zrows), :] = one.astype(g.dtype)

        if i < line - 1:
            @pl.when(z == 0)
            def _():
                up_copy(line - 1 - i, True).start()

            @pl.when(z == line - 1)
            def _():
                dn_copy(i, True).start()

    def line_step(t):
        zt = line - 1 + z - t

        @pl.when((z > 0) & (zt <= line - 1) & (zt > z))
        def _():
            up_copy(zt, False).wait_recv()
            row = pl.multiple_of(zt * zrows, zrows)
            total((u_in, row, 0, width), [(g, row, 0, width), (u_in, row, 0, width)], zrows)
            up_copy(zt, False).start()

        zd = t - (line - 1 - z)

        @pl.when((z < line - 1) & (zd >= 0) & (zd < z))
        def _():
            dn_copy(zd, False).wait_recv()
            row = pl.multiple_of(zd * zrows, zrows)
            total((d_in, row, 0, width), [(g, row, 0, width), (d_in, row, 0, width)], zrows)
            dn_copy(zd, False).start()

    for d in range(last):
        for sub in range(2):
            settle(d, sub, 2)
    forward(1, dn_w, 2 * width, width, 0, 4)
    forward_end(1, 2, 0)
    for up_dir in (True, False):
        await_recv(up_dir, last, 1, 2)

    for i in (0, 3, 5):
        dcopy(i, core).wait_send()
    tcopy(5, False).wait_send()
    line_step(1)
    order = [(1 - r, 1 - y), (1 - r, y), (r, 1 - y), (r, y)]
    my_col = pl.multiple_of(core * cols, cols)
    its_col = pl.multiple_of((1 - core) * cols, cols)
    part = x.at[0]

    def slopes(row, count):
        @pl.loop(0, count // 32)
        def _(i):
            at = pl.ds(pl.multiple_of(row + i * 32, 32), 32)
            grad = acc[at, pl.ds(2 * width, width)]
            ggu[at, pl.ds(0, width)] = (grad * acc[at, pl.ds(0, width)]).astype(ggu.dtype)
            ggu[at, pl.ds(width, width)] = (grad * acc[at, pl.ds(width, width)]).astype(ggu.dtype)

    def back(row, count, col):
        @pl.loop(0, cols // wide)
        def _(n):
            at = pl.multiple_of(col + n * wide, wide)
            one = lax.dot_general(
                ggu[pl.ds(row, count), :], gu[pl.ds(at, wide), :], (((1,), (1,)), ((), ())),
                preferred_element_type=jnp.float32,
            )
            x[0, pl.ds(row, count), pl.ds(at, wide)] = one.astype(x.dtype)

    hrows = rows // 2
    units = [(0, 0, hrows), (0, hrows, hrows), (1, 0, rows), (2, 0, rows), (3, 0, rows)]

    def urow(i):
        b, at, count = units[i]
        return pl.multiple_of(slot(*order[b]) + at, hrows)

    def core_copy(i):
        at = pl.ds(urow(i), units[i][2])
        return remote(part.at[at, pl.ds(its_col, cols)], r1.at[at, :], c_s.at[i], c_r.at[i], cpart)

    first_col = my_col
    second_col = pl.multiple_of(my_col + parts_a, 128)

    def mine_a(row, count):
        return part.at[pl.ds(row, count), pl.ds(first_col, parts_a)]

    def mine_b(row, count):
        return part.at[pl.ds(row, count), pl.ds(second_col, parts_b)]

    def x_copy(i):
        if i == 3:
            src, dst = s3b, rxb
        elif i == 2:
            src, dst = mine_a(slot(*order[1]), rows), rxa.at[1]
        else:
            src, dst = mine_a(urow(i), hrows), rxa.at[0, pl.ds(i * hrows, hrows), :]
        return remote(src, dst, x_s.at[i], x_r.at[i], xpart)

    def y_copy(i):
        if i == 4:
            src, dst = s3a, ryb
        elif i in (2, 3):
            at = (i - 2) * hrows
            row = pl.multiple_of(slot(*order[2]) + at, hrows)
            src, dst = mine_b(row, hrows), rya.at[1, pl.ds(at, hrows), :]
        else:
            src, dst = mine_b(urow(i), hrows), rya.at[0, pl.ds(i * hrows, hrows), :]
        return remote(src, dst, yy_s.at[i], yy_r.at[i], ypart)

    def finish(b):
        @pl.when(is_end)
        def _():
            product(
                1, slot(*order[b]), (2 * (line - 1 - z) + 1 - y) * wrows, wrows,
                dn_w, 0, 2 * width, width,
            )

    def theirs(i):
        slopes(urow(i), units[i][2])
        back(urow(i), units[i][2], its_col)
        core_copy(i).start()

    def summed(i):
        back(urow(i), units[i][2], my_col)
        core_copy(i).wait_recv()
        total(
            (part, urow(i), my_col, cols),
            [(part, urow(i), my_col, cols), (r1, urow(i), 0, cols)], units[i][2],
        )

    finish(0)
    theirs(0)
    theirs(1)
    for i in (0, 1):
        summed(i)
        x_copy(i).start()
        y_copy(i).start()
    finish(1)
    theirs(2)
    summed(2)
    x_copy(2).start()
    finish(2)
    theirs(3)
    summed(3)
    y_copy(2).start()
    for t in range(2, line - 1):
        line_step(t)
    finish(3)
    theirs(4)
    summed(4)

    for i in (0, 1):
        x_copy(i).wait_recv()
    total(
        (s3a, 0, 0, parts_a),
        [(part, slot(r, 1 - y), first_col, parts_a), (rxa.at[0], 0, 0, parts_a)], rows,
    )
    y_copy(4).start()
    for i in (0, 1):
        y_copy(i).wait_recv()
    total(
        (s3b, 0, 0, parts_b),
        [(part, slot(1 - r, y), second_col, parts_b), (rya.at[0], 0, 0, parts_b)], rows,
    )
    x_copy(3).start()

    zrow = pl.multiple_of(z * zrows, zrows)

    def here(ref):
        return (ref, zrow, 0, width)

    @pl.when(z == 0)
    def _():
        dn_copy(0, True).wait_recv()
        total((gfin, 0, 0, width), [here(g), here(d_in)], zrows)

    @pl.when(z == line - 1)
    def _():
        up_copy(line - 1, True).wait_recv()
        total((gfin, 0, 0, width), [here(g), here(u_in)], zrows)

    @pl.when((z > 0) & (z < line - 1))
    def _():
        remote(block(g, z), block(u_in, z), u_s.at[z], u_r.at[z], up).wait_recv()
        remote(block(g, z), block(d_in, z), d_s.at[z], d_r.at[z], dn).wait_recv()
        total((gfin, 0, 0, width), [here(g), here(u_in), here(d_in)], zrows)

    def gcol(rr, yy):
        return pl.multiple_of((2 * rr + yy) * width, width)

    def gcols(rr, yy):
        return gl.at[:, pl.ds(gcol(rr, yy), width)]

    def grows(yy):
        return gfin.at[pl.ds(pl.multiple_of(yy * frows, frows), frows), :]

    def f_copy(i, land):
        if i == 0:
            src, dst, dev = grows(1 - y), gcols(r, 1 - y) if land else gcols(r, y), ypart
        elif i == 1:
            src, dst, dev = grows(y), gcols(1 - r, y) if land else gcols(r, y), xpart
        else:
            src, dev = gcols(r, 1 - y), xpart
            dst = gcols(1 - r, 1 - y) if land else src
        return remote(src, dst, f_s.at[i], f_r.at[i], dev)

    def scaled(ref, row, col, rr, yy):
        at_col = gcol(rr, yy)

        @pl.loop(0, frows // 64)
        def _(m):
            at = pl.multiple_of(m * 64, 64)
            one = ref[pl.ds(row + at, 64), pl.ds(col, width)].astype(jnp.float32)
            gd_out[pl.ds(at, 64), pl.ds(at_col, width)] = one * grad_scale

    f_copy(0, False).start()
    f_copy(1, False).start()
    y_copy(3).start()
    scaled(gfin, pl.multiple_of(y * frows, frows), 0, r, y)

    here_row = slot(r, y)

    def o_copy(i, land):
        base = (1 - core if land else core) * cols
        if i == 0:
            at = gi_out.at[:, pl.ds(pl.multiple_of(base, 128), parts_a)]
        else:
            at = gi_out.at[
                pl.ds((i - 1) * hrows, hrows), pl.ds(pl.multiple_of(base + parts_a, 128), parts_b)
            ]
        return remote(at, at, o_s.at[i], o_r.at[i], cpart)

    def final_b(at):
        total(
            (gi_out, at, second_col, parts_b),
            [
                (part, here_row + at, second_col, parts_b),
                (rya.at[1], at, 0, parts_b), (rxb, at, 0, parts_b),
            ], hrows,
        )

    x_copy(2).wait_recv()
    y_copy(4).wait_recv()
    total(
        (gi_out, 0, first_col, parts_a),
        [
            (part, here_row, first_col, parts_a),
            (rxa.at[1], 0, 0, parts_a), (ryb, 0, 0, parts_a),
        ], rows,
    )
    o_copy(0, False).start()
    x_copy(3).wait_recv()
    y_copy(2).wait_recv()
    final_b(0)
    o_copy(1, False).start()
    f_copy(0, True).wait_recv()
    f_copy(2, False).start()
    scaled(gl, 0, gcol(r, 1 - y), r, 1 - y)
    f_copy(1, True).wait_recv()
    scaled(gl, 0, gcol(1 - r, y), 1 - r, y)
    y_copy(3).wait_recv()
    final_b(hrows)
    o_copy(2, False).start()
    f_copy(2, True).wait_recv()
    scaled(gl, 0, gcol(1 - r, 1 - y), 1 - r, 1 - y)

    for i in range(ntok):
        if kinds[i] == 1:
            dcopy(i, core).wait_send()
        if i != 5:
            tcopy(i, False).wait_send()
    for k in range(3):
        to_y(k).wait_send()
        for d in range(line - 1):
            for sub in range(2):
                await_send(True, d, sub, k)
                await_send(False, d, sub, k)
    for i in range(5):
        core_copy(i).wait_send()
        y_copy(i).wait_send()
    for i in range(4):
        x_copy(i).wait_send()
    for i in range(3):
        f_copy(i, False).wait_send()
    for i in range(3):
        o_copy(i, True).wait_recv()
        o_copy(i, False).wait_send()
    for zt in range(line):
        if zt > 0:
            pl.when(z < zt)(lambda: up_copy(zt, True).wait_send())
        if zt < line - 1:
            pl.when(z > zt)(lambda: dn_copy(zt, True).wait_send())


def fused(grad_scale, gate_w, up_w, down_w, toks, cots):
    line = lax.axis_size("fs") // 2
    rows, full = toks.shape
    wrows, width = gate_w.shape[0], gate_w.shape[1] // 4
    depth = 2 * line * wrows
    cols = full // 2
    kind = gate_w.dtype
    dma = pltpu.SemaphoreType.DMA
    zsem = dma((line - 1, 2, 3))
    anyspec = pl.BlockSpec(memory_space=pl.ANY)
    whole = pltpu.VMEM((depth, width), kind)
    parts_a = cols * 3 // 8 // 128 * 128
    parts_b = cols - parts_a
    return pl.pallas_call(
        functools.partial(fused_kernel, line, grad_scale),
        out_shape=(
            pltpu.VMEM((rows, full), kind),
            pltpu.VMEM((wrows, 4 * width), jnp.float32),
        ),
        in_specs=[anyspec] * 5,
        out_specs=(pl.BlockSpec(memory_space=pltpu.VMEM),) * 2,
        scratch_shapes=[
            pltpu.VMEM((2, 4 * rows, full), kind),
            pltpu.VMEM((depth, 2 * width), kind),
            whole,
            pltpu.VMEM((4 * rows, 3 * width), jnp.float32),
            pltpu.VMEM((4 * rows, width), kind),
            pltpu.VMEM((4 * rows, 2 * width), kind),
            pltpu.VMEM((4 * rows, cols), kind),
            pltpu.VMEM((2, rows, parts_a), kind), pltpu.VMEM((rows, parts_b), kind),
            pltpu.VMEM((2, rows, parts_b), kind), pltpu.VMEM((rows, parts_a), kind),
            pltpu.VMEM((rows, parts_a), kind), pltpu.VMEM((rows, parts_b), kind),
            whole, whole, whole,
            pltpu.VMEM((2 * wrows, width), kind),
            pltpu.VMEM((wrows, 4 * width), kind),
            zsem, zsem, zsem, zsem,
            dma((3,)), dma((3,)),
            dma((8,)), dma((8,)), dma((8,)), dma((8,)), dma((5,)),
            dma((5,)), dma((5,)), dma((4,)), dma((4,)), dma((5,)), dma((5,)),
            dma((line,)), dma((line,)), dma((line,)), dma((line,)),
            dma((3,)), dma((3,)), dma((3,)), dma((3,)),
        ],
        compiler_params=pltpu.CompilerParams(
            collective_id=1, has_side_effects=True, vmem_limit_bytes=59 * 2**20
        ),
        name="fused_all",
    )(gate_w, up_w, down_w, toks, cots)


def gather_kernel(
    line, units, gate_w, up_w, down_w, toks, cots, gu_out, d_out, t_out, w_tmp, t_tmp,
    up_s, up_r, dn_s, dn_r, y_s, y_r, tok_s, tok_r, d2d_s, d2d_r, loc, loc2,
):
    r = lax.axis_index("rep")
    f = lax.axis_index("fs")
    t = lax.axis_index("tp")
    z, y = f // 2, f % 2
    rows = toks.shape[0]
    half = rows // 2
    wrows = gate_w.shape[0]
    width = gate_w.shape[1] // 4
    parts = len(units)
    has_up, has_dn = z < line - 1, z > 0
    up = {"fs": (f + 2) % (2 * line)}
    dn = {"fs": (f + 2 * line - 2) % (2 * line)}
    ypart = {"fs": f + 1 - 2 * y}
    xpart = {"rep": 1 - r}
    core = t % 2
    cpart = {"tp": t + 1 - 2 * core}

    barrier = pltpu.get_barrier_semaphore()

    def greet(dev):
        pl.semaphore_signal(barrier, inc=1, device_id=dev, device_id_type=MESH)

    for dev in (ypart, xpart, cpart, up, dn):
        greet(dev)
    pl.semaphore_wait(barrier, 5)

    def remote(src, dst, s, q, dev):
        return pltpu.make_async_remote_copy(
            src_ref=src, dst_ref=dst, send_sem=s, recv_sem=q,
            device_id=dev, device_id_type=MESH,
        )

    def wblk(k, zz, yy):
        row = pl.multiple_of((2 * zz + yy) * wrows, wrows)
        which, col, wide = units[k]
        return (gu_out, d_out)[which].at[pl.ds(row, wrows), pl.ds(col, wide)]

    def own(k, yy):
        col = pl.multiple_of((2 * r + yy) * width, width)
        return (gate_w, up_w, down_w)[k].at[:, pl.ds(col, width)]

    def to_y(k):
        return remote(own(k, 1 - y), wblk(k, z, y), y_s.at[k], y_r.at[k], ypart)

    def from_y(k):
        return remote(own(k, 1 - y), wblk(k, z, 1 - y), y_s.at[k], y_r.at[k], ypart)

    def zcopy(up_dir, d, sub, k, zz):
        yy = y if sub == 0 else 1 - y
        src = own(k, y) if (d == 0 and sub == 0) else wblk(k, zz, yy)
        s, q, dev = (up_s, up_r, up) if up_dir else (dn_s, dn_r, dn)
        return remote(src, wblk(k, zz, yy), s.at[d, sub, k], q.at[d, sub, k], dev)

    def pred_send(up_dir, d):
        return (has_up & (z - d >= 0)) if up_dir else (has_dn & (z + d <= line - 1))

    def src_z(up_dir, d):
        return jnp.maximum(z - d, 0) if up_dir else jnp.minimum(z + d, line - 1)

    def send(up_dir, d, sub, k):
        @pl.when(pred_send(up_dir, d))
        def _():
            zcopy(up_dir, d, sub, k, src_z(up_dir, d)).start()

    def await_send(up_dir, d, sub, k):
        @pl.when(pred_send(up_dir, d))
        def _():
            zcopy(up_dir, d, sub, k, src_z(up_dir, d)).wait_send()

    def await_recv(up_dir, d, sub, k):
        ok = (z - d - 1 >= 0) if up_dir else (z + d + 1 <= line - 1)

        @pl.when(ok)
        def _():
            zcopy(up_dir, d, sub, k, src_z(up_dir, d + 1)).wait_recv()

    def tblk(j, rr, yy, c):
        row = pl.multiple_of((2 * rr + yy) * rows + c * half, half)
        return t_out.at[j, pl.ds(row, half), :]

    def mine(j):
        src = toks if j == 0 else cots
        return src.at[pl.ds(pl.multiple_of(core * half, half), half), :]

    def tcopy(i, landing):
        j = (0, 1, 0, 1, 0, 1)[i]
        dev = xpart if i in (0, 1, 5) else ypart
        if landing:
            rr = (1 - r, 1 - r, r, r, 1 - r, 1 - r)[i]
            yy = (y, y, 1 - y, 1 - y, 1 - y, 1 - y)[i]
            src = dst = tblk(j, rr, yy, core)
        else:
            rr = (r, r, r, r, 1 - r, r)[i]
            yy = (y, y, y, y, y, 1 - y)[i]
            dst = tblk(j, rr, yy, core)
            src = mine(j) if i < 4 else dst
        return remote(src, dst, tok_s.at[i], tok_r.at[i], dev)

    def dcopy(i, c):
        j = (0, 1, 0, 1, 0, 1)[i]
        rr = (1 - r, 1 - r, r, r, 1 - r, 1 - r)[i]
        yy = (y, y, 1 - y, 1 - y, 1 - y, 1 - y)[i]
        blk = tblk(j, rr, yy, c)
        return remote(blk, blk, d2d_s.at[i], d2d_r.at[i], cpart)

    loads = [
        pltpu.make_async_copy(own(0, y), w_tmp.at[0], loc.at[0]),
        pltpu.make_async_copy(own(1, y), w_tmp.at[1], loc.at[3]),
        pltpu.make_async_copy(own(2, y), w_tmp.at[2], loc.at[4]),
        pltpu.make_async_copy(toks, t_tmp.at[0], loc.at[1]),
        pltpu.make_async_copy(cots, t_tmp.at[1], loc.at[2]),
    ]
    trow = pl.multiple_of((2 * r + y) * rows, rows)
    stores = [
        pltpu.make_async_copy(w_tmp.at[0], wblk(0, z, y), loc2.at[0]),
        pltpu.make_async_copy(w_tmp.at[1], wblk(1, z, y), loc2.at[3]),
        pltpu.make_async_copy(w_tmp.at[2], wblk(2, z, y), loc2.at[4]),
        pltpu.make_async_copy(t_tmp.at[0], t_out.at[0, pl.ds(trow, rows), :], loc2.at[1]),
        pltpu.make_async_copy(t_tmp.at[1], t_out.at[1, pl.ds(trow, rows), :], loc2.at[2]),
    ]

    for k in range(parts):
        to_y(k).start()
        send(True, 0, 0, k)
        send(False, 0, 0, k)
    for i in (0, 1, 3, 2):
        tcopy(i, False).start()
    for copy in loads:
        copy.start()
    for load, store in zip(loads, stores):
        load.wait()
        store.start()
    for k in range(parts):
        from_y(k).wait_recv()
        send(True, 0, 1, k)
        send(False, 0, 1, k)

    def event(i):
        tcopy(i, True).wait_recv()
        if i == 0:
            tcopy(4, False).start()
        if i == 3:
            tcopy(5, False).start()
        dcopy(i, core).start()

    events = [0, 3, 1, 2, 5, 4]
    for d in range(line - 1):
        for sub in range(2):
            if events:
                event(events.pop(0))
            for k in range(parts):
                for up_dir in (True, False):
                    await_recv(up_dir, d, sub, k)
                    if d + 1 < line - 1:
                        send(up_dir, d + 1, sub, k)
    for i in events:
        event(i)
    for i in range(6):
        dcopy(i, 1 - core).wait_recv()
        dcopy(i, core).wait_send()
        tcopy(i, False).wait_send()
    for k in range(parts):
        to_y(k).wait_send()
        for d in range(line - 1):
            for sub in range(2):
                await_send(True, d, sub, k)
                await_send(False, d, sub, k)
    for store in stores:
        store.wait()


def gather(gate_w, up_w, down_w, toks, cots):
    line = lax.axis_size("fs") // 2
    wrows, width = gate_w.shape[0], gate_w.shape[1] // 4
    units = [(0, 0, width), (0, width, width), (1, 0, width)]
    parts = len(units)
    depth = 2 * line * wrows
    kind = gate_w.dtype
    dma = pltpu.SemaphoreType.DMA
    zsem = dma((line - 1, 2, parts))
    anyspec = pl.BlockSpec(memory_space=pl.ANY)
    return pl.pallas_call(
        functools.partial(gather_kernel, line, units),
        out_shape=(
            jax.ShapeDtypeStruct((depth, 2 * width), kind),
            jax.ShapeDtypeStruct((depth, width), kind),
            jax.ShapeDtypeStruct((2, 4 * toks.shape[0], toks.shape[1]), toks.dtype),
        ),
        in_specs=[anyspec] * 5,
        out_specs=(anyspec,) * 3,
        scratch_shapes=[
            pltpu.VMEM((parts, wrows, width), kind),
            pltpu.VMEM((2,) + toks.shape, toks.dtype),
            zsem, zsem, zsem, zsem,
            dma((parts,)), dma((parts,)),
            dma((6,)), dma((6,)), dma((6,)), dma((6,)),
            dma((5,)), dma((5,)),
        ],
        compiler_params=pltpu.CompilerParams(collective_id=0, has_side_effects=True),
        name="gather_all",
    )(gate_w, up_w, down_w, toks, cots)


def on_device(inputs, cotangent, gate_weight, up_weight, down_weight):
    tok_rows = inputs.shape[0]
    fs_size = lax.axis_size("fs")
    rep_size = lax.axis_size("rep")
    grad_scale = 1.0 / math.sqrt(tok_rows * fs_size * rep_size)
    if lax.axis_size("tp") == 2:
        return fused(
            grad_scale, gate_weight, up_weight, down_weight, inputs, cotangent
        )
    contract = (((1,), (1,)), ((), ()))
    contract_tok = (((0,), (0,)), ((), ()))
    width = gate_weight.shape[1] // 4
    gate_up, down_full, tokens = gather(
        gate_weight, up_weight, down_weight, inputs, cotangent
    )
    gate_up_val = jnp.dot(tokens[0], gate_up, preferred_element_type=jnp.float32)
    gate_val, up_val = gate_up_val[:, :width], gate_up_val[:, width:]
    grad_hidden = jnp.dot(tokens[1], down_full, preferred_element_type=jnp.float32)
    sigmoid_gate = jax.nn.sigmoid(gate_val)
    active = gate_val * sigmoid_gate
    hidden = (active * up_val).astype(jnp.bfloat16)
    grad_gate = (
        grad_hidden * up_val * sigmoid_gate * (1.0 + gate_val * (1.0 - sigmoid_gate))
    ).astype(jnp.bfloat16)
    grad_up = (grad_hidden * active).astype(jnp.bfloat16)
    pairs = [[i, i + 1] for i in range(0, fs_size, 2)]
    lines = [list(range(i, fs_size, 2)) for i in range(2)]
    grad_part = lax.dot_general(
        tokens[1], hidden, contract_tok, preferred_element_type=jnp.float32
    )
    part = lax.dot_general(
        jnp.concatenate([grad_gate, grad_up], axis=1), gate_up, contract,
        preferred_element_type=jnp.float32,
    )
    shard = lax.psum_scatter(
        grad_part.astype(jnp.bfloat16), "fs", scatter_dimension=0, tiled=True,
        axis_index_groups=lines,
    ).astype(jnp.float32) * grad_scale
    shard = lax.all_to_all(
        shard, "fs", split_axis=0, concat_axis=1, tiled=True, axis_index_groups=pairs
    )
    grad_down = lax.all_gather(shard, "rep", axis=1, tiled=True)
    part = lax.psum_scatter(
        part.astype(jnp.bfloat16), "rep", scatter_dimension=0, tiled=True
    )
    part = lax.psum_scatter(
        part, "fs", scatter_dimension=0, tiled=True, axis_index_groups=pairs
    )
    grad_input = lax.psum(part, "tp")
    return (grad_input, grad_down)


def solution(mesh):
    placed = (
        P(("rep", "fs"), None),
        P(("rep", "fs"), None),
        P("fs", "tp"),
        P("fs", "tp"),
        P("fs", "tp"),
    )
    return jax.shard_map(
        on_device,
        mesh=mesh,
        in_specs=placed,
        out_specs=(P(("rep", "fs"), None), P("fs", "tp")),
        check_vma=False,
    )
```

```python
import functools
import math

import jax
import jax.numpy as jnp
from jax import lax
from jax.experimental import pallas as pl
from jax.experimental.pallas import tpu as pltpu
from jax.sharding import PartitionSpec as P

MESH = pl.DeviceIdType.MESH


def fused_kernel(
    line, grad_scale, gate_w, up_w, down_w, toks, cots, gi_out, gd_out,
    x, gu, dn_w, acc, hid, ggu, r1, rxa, rxb, rya, ryb, s3a, s3b, g, u_in, d_in, gfin, gl, hl,
    up_s, up_r, dn_s, dn_r, wy_s, wy_r, tok_s, tok_r, d2d_s, d2d_r, loc,
    c_s, c_r, x_s, x_r, yy_s, yy_r, u_s, u_r, d_s, d_r, f_s, f_r, o_s, o_r, e_s, e_r, h_s, h_r,
):
    r = lax.axis_index("rep")
    f = lax.axis_index("fs")
    core = lax.axis_index("tp")
    z, y = f // 2, f % 2
    rows = toks.shape[0]
    half = rows // 2
    wrows = gate_w.shape[0]
    width = gate_w.shape[1] // 4
    depth = 2 * line * wrows
    zrows = 2 * wrows
    cols = depth // 2
    wide = cols // 2
    parts_a = rxa.shape[2]
    parts_b = cols - parts_a
    frows = wrows
    last = line - 2
    has_up, has_dn = z < line - 1, z > 0
    is_end = (z == 0) | (z == line - 1)
    up = {"fs": (f + 2) % (2 * line)}
    dn = {"fs": (f + 2 * line - 2) % (2 * line)}
    ypart = {"fs": f + 1 - 2 * y}
    xpart = {"rep": 1 - r}
    cpart = {"tp": 1 - core}

    barrier = pltpu.get_barrier_semaphore()
    for dev in (ypart, xpart, cpart, up, dn):
        pl.semaphore_signal(barrier, inc=1, device_id=dev, device_id_type=MESH)
    pl.semaphore_wait(barrier, 5)

    def remote(src, dst, s, q, dev):
        return pltpu.make_async_remote_copy(
            src_ref=src, dst_ref=dst, send_sem=s, recv_sem=q,
            device_id=dev, device_id_type=MESH,
        )

    def wblk(k, zz, yy):
        row = pl.multiple_of((2 * zz + yy) * wrows, wrows)
        if k == 2:
            return dn_w.at[pl.ds(row, wrows), :]
        return gu.at[pl.ds(row, wrows), pl.ds(k * width, width)]

    def own(k, yy):
        col = pl.multiple_of((2 * r + yy) * width, width)
        return (gate_w, up_w, down_w)[k].at[:, pl.ds(col, width)]

    def to_y(k):
        return remote(own(k, 1 - y), wblk(k, z, y), wy_s.at[k], wy_r.at[k], ypart)

    def from_y(k):
        return remote(own(k, 1 - y), wblk(k, z, 1 - y), wy_s.at[k], wy_r.at[k], ypart)

    def zcopy(up_dir, d, sub, k, zz):
        yy = y if sub == 0 else 1 - y
        src = own(k, y) if (d == 0 and sub == 0) else wblk(k, zz, yy)
        s, q, dev = (up_s, up_r, up) if up_dir else (dn_s, dn_r, dn)
        return remote(src, wblk(k, zz, yy), s.at[d, sub, k], q.at[d, sub, k], dev)

    def pred_send(up_dir, d):
        return (has_up & (z - d >= 0)) if up_dir else (has_dn & (z + d <= line - 1))

    def src_z(up_dir, d):
        return jnp.maximum(z - d, 0) if up_dir else jnp.minimum(z + d, line - 1)

    def send(up_dir, d, sub, k):
        @pl.when(pred_send(up_dir, d))
        def _():
            zcopy(up_dir, d, sub, k, src_z(up_dir, d)).start()

    def await_send(up_dir, d, sub, k):
        @pl.when(pred_send(up_dir, d))
        def _():
            zcopy(up_dir, d, sub, k, src_z(up_dir, d)).wait_send()

    def await_recv(up_dir, d, sub, k):
        ok = (z - d - 1 >= 0) if up_dir else (z + d + 1 <= line - 1)

        @pl.when(ok)
        def _():
            zcopy(up_dir, d, sub, k, src_z(up_dir, d + 1)).wait_recv()

    def relay(d, sub, k):
        for up_dir in (True, False):
            @pl.when(pred_send(up_dir, d + 1))
            def _():
                zcopy(up_dir, d, sub, k, src_z(up_dir, d + 1)).wait_recv()
                zcopy(up_dir, d + 1, sub, k, src_z(up_dir, d + 1)).start()

    def settle(d, sub, k):
        for up_dir in (True, False):
            ok = (z - d - 1 >= 0) if up_dir else (z + d + 1 <= line - 1)
            onward = has_up if up_dir else has_dn

            @pl.when(ok & jnp.logical_not(onward))
            def _():
                zcopy(up_dir, d, sub, k, src_z(up_dir, d + 1)).wait_recv()

    def slot(rr, yy):
        return pl.multiple_of((2 * rr + yy) * rows, rows)

    kinds = (0, 1, 1, 0, 1, 0, 1, 1)
    over_x = (True, True, True, False, False, True, False, True)
    parts = (2, 0, 1, 2, 2, 2, 0, 1)
    ntok = len(kinds)

    def span(c, p):
        if p == 2:
            return c * half, half
        return c * half + p * (half // 2), half // 2

    def tblk(i, rr, yy, c):
        at, count = span(c, parts[i])
        row = pl.multiple_of((2 * rr + yy) * rows + at, half // 2)
        return x.at[kinds[i], pl.ds(row, count), :]

    def mine(i):
        at, count = span(core, parts[i])
        src = toks if kinds[i] == 0 else cots
        return src.at[pl.ds(pl.multiple_of(at, half // 2), count), :]

    def landing(i, c):
        rr = (1 - r, 1 - r, 1 - r, r, r, 1 - r, 1 - r, 1 - r)[i]
        yy = (y, y, y, 1 - y, 1 - y, 1 - y, 1 - y, 1 - y)[i]
        return tblk(i, rr, yy, c)

    def tcopy(i, land):
        dev = xpart if over_x[i] else ypart
        if land:
            src = dst = landing(i, core)
        else:
            rr = (r, r, r, r, r, r, 1 - r, r)[i]
            yy = (y, y, y, y, y, 1 - y, y, 1 - y)[i]
            dst = tblk(i, rr, yy, core)
            src = mine(i) if i < 5 else dst
        return remote(src, dst, tok_s.at[i], tok_r.at[i], dev)

    def dcopy(i, c):
        blk = landing(i, c)
        return remote(blk, blk, d2d_s.at[i], d2d_r.at[i], cpart)

    def event(i):
        tcopy(i, True).wait_recv()
        onward = {1: 6, 3: 5, 4: 7}.get(i)
        if onward is not None:
            tcopy(onward, False).start()
        dcopy(i, core).start()

    trow = slot(r, y)
    loads = [
        pltpu.make_async_copy(own(0, y), wblk(0, z, y), loc.at[0]),
        pltpu.make_async_copy(own(1, y), wblk(1, z, y), loc.at[1]),
        pltpu.make_async_copy(own(2, y), wblk(2, z, y), loc.at[2]),
        pltpu.make_async_copy(toks, x.at[0, pl.ds(trow, rows), :], loc.at[3]),
        pltpu.make_async_copy(cots, x.at[1, pl.ds(trow, rows), :], loc.at[4]),
    ]

    tile = 256
    z_lo = jnp.maximum(z - last, 0)
    z_hi = jnp.minimum(z + last, line - 1) + 1

    def product(j, row, k0, kk, w, wcol, acol, n):
        at = pl.ds(pl.multiple_of(row, rows), rows)
        kat = pl.ds(pl.multiple_of(k0, wrows), kk)
        for c in range(0, n, tile):
            one = jnp.dot(
                x[j, at, kat], w[kat, pl.ds(wcol + c, tile)],
                preferred_element_type=jnp.float32,
            )
            acc[at, pl.ds(acol + c, tile)] += one

    def forward(j, w, acol, n, first, count):
        @pl.loop(first, first + count)
        def _(b):
            row = ((2 * r + y) + 2 * (b % 2) * (1 - 2 * r) + (b // 2) * (1 - 2 * y)) * rows

            @pl.loop(z_lo, z_hi)
            def _(zz):
                product(j, row, zz * zrows, zrows, w, 0, acol, n)

    def forward_end(j, k, sub):
        for up_dir in (True, False):
            await_recv(up_dir, last, sub, k)

        @pl.when(is_end)
        def _():
            zz = line - 1 - z
            yy = y if sub == 0 else 1 - y
            w = dn_w if k == 2 else gu

            @pl.loop(0, 4)
            def _(b):
                product(
                    j, b * rows, (2 * zz + yy) * wrows, wrows, w,
                    0 if k == 2 else k * width, k * width, width,
                )

    def total(dst, terms, count, step=64):
        @pl.loop(0, count // step)
        def _(i):
            at = pl.multiple_of(i * step, step)
            value = None
            for ref, row, col, wide in terms:
                one = ref[pl.ds(row + at, step), pl.ds(col, wide)].astype(jnp.float32)
                value = one if value is None else value + one
            ref, row, col, wide = dst
            ref[pl.ds(row + at, step), pl.ds(col, wide)] = value.astype(ref.dtype)

    for k in (0, 1):
        to_y(k).start()
        send(True, 0, 0, k)
        send(False, 0, 0, k)
    for i in (0, 1, 3):
        tcopy(i, False).start()
    to_y(2).start()
    tcopy(4, False).start()
    for copy in loads:
        copy.start()

    @pl.loop(0, 4 * rows // 64)
    def _(i):
        at = pl.ds(pl.multiple_of(i * 64, 64), 64)
        acc[at, :] = jnp.zeros((64, 3 * width), jnp.float32)

    for k in (0, 1):
        from_y(k).wait_recv()
        send(True, 0, 1, k)
        send(False, 0, 1, k)
    if last > 0:
        for sub in range(2):
            for k in (0, 1):
                relay(0, sub, k)
    event(0)
    event(3)
    tcopy(2, False).start()
    event(1)
    for d in range(1, last):
        for sub in range(2):
            for k in (0, 1):
                relay(d, sub, k)
    send(True, 0, 0, 2)
    send(False, 0, 0, 2)
    from_y(2).wait_recv()
    send(True, 0, 1, 2)
    send(False, 0, 1, 2)
    for load in loads:
        load.wait()
    for d in range(last):
        for sub in range(2):
            for k in (0, 1):
                settle(d, sub, k)
    dcopy(0, 1 - core).wait_recv()
    dcopy(3, 1 - core).wait_recv()
    forward(0, gu, 0, 2 * width, 0, 3)
    if last > 0:
        for sub in range(2):
            relay(0, sub, 2)
    event(5)
    event(4)
    dcopy(5, 1 - core).wait_recv()
    forward(0, gu, 0, 2 * width, 3, 1)
    for d in range(1, last):
        for sub in range(2):
            relay(d, sub, 2)
    for sub in range(2):
        for k in (0, 1):
            forward_end(0, k, sub)

    @pl.loop(0, 4 * rows // 32)
    def _(i):
        at = pl.ds(pl.multiple_of(i * 32, 32), 32)
        gate = acc[at, pl.ds(0, width)]
        up_val = acc[at, pl.ds(width, width)]
        sig = jax.nn.sigmoid(gate)
        active = gate * sig
        hid[at, :] = (active * up_val).astype(hid.dtype)
        acc[at, pl.ds(0, width)] = up_val * sig * (1.0 + gate * (1.0 - sig))
        acc[at, pl.ds(width, width)] = active

    for i in (2, 6, 7):
        event(i)
    for i in (1, 2, 4, 6, 7):
        dcopy(i, 1 - core).wait_recv()

    zrow = pl.multiple_of(z * zrows, zrows)
    lower = z < line // 2

    def block(ref, zt):
        return ref.at[pl.ds(zt * zrows, zrows), :]

    def up_copy(zt, first):
        return remote(block(g if first else u_in, zt), block(u_in, zt), u_s.at[zt], u_r.at[zt], up)

    def dn_copy(zt, first):
        return remote(block(g if first else d_in, zt), block(d_in, zt), d_s.at[zt], d_r.at[zt], dn)

    def g_block(zt):
        at = pl.multiple_of(zt * zrows, zrows)
        one = lax.dot_general(
            x[1, :, pl.ds(at, zrows)], hid[...], (((0,), (0,)), ((), ())),
            preferred_element_type=jnp.float32,
        )
        g[pl.ds(at, zrows), :] = one.astype(g.dtype)

    def gcol(rr, yy):
        return pl.multiple_of((2 * rr + yy) * width, width)

    def gcols(ref, rr, yy):
        return ref.at[:, pl.ds(gcol(rr, yy), width)]

    def half_rows(ref, row, yy):
        return ref.at[pl.ds(pl.multiple_of(row + yy * frows, frows), frows), :]

    def f_copy(i, land, ref=gfin, row=0):
        if i == 0:
            src, dst, dev = half_rows(ref, row, 1 - y), gcols(gl, r, 1 - y if land else y), ypart
        elif i == 1:
            src, dst, dev = half_rows(ref, row, y), gcols(gl, 1 - r if land else r, y), xpart
        else:
            src, dst, dev = gcols(gl, r, 1 - y), gcols(gl, 1 - r if land else r, 1 - y), xpart
        return remote(src, dst, f_s.at[i], f_r.at[i], dev)

    def e_copy(i, land, ref=gfin, row=0):
        if i == 0:
            src, dst, dev = half_rows(ref, row, 1 - y), gcols(hl, r, 1 - y if land else y), ypart
        else:
            src, dst, dev = half_rows(ref, row, y), gcols(hl, 1 - r if land else r, y), xpart
        return remote(src, dst, e_s.at[i], e_r.at[i], dev)

    end_z = jnp.where((z == 1) | (z == line - 1), 0, line - 1)
    end_dev = {"fs": 2 * end_z + y}
    next_to_end = (z == 1) | (z == line - 2)

    def h_copy(i, ref=gfin, row=0):
        rr, yy = ((r, y), (r, 1 - y), (1 - r, y))[i]
        dst = gcols(hl, rr, yy)
        src = half_rows(ref, row, y) if i == 0 else dst
        return remote(src, dst, h_s.at[i], h_r.at[i], end_dev)

    def share(ref, row):
        h_copy(0, ref, row).start()
        e_copy(0, False, ref, row).start()
        e_copy(1, False, ref, row).start()

    def line_step(t):
        zt = line - 1 + z - t
        row_u = pl.multiple_of(zt * zrows, zrows)
        is_u = (z > 0) & (zt <= line - 1) & (zt > z)
        zd = t - (line - 1 - z)
        row_d = pl.multiple_of(zd * zrows, zrows)
        is_d = (z < line - 1) & (zd >= 0) & (zd < z)
        final = t == line - 2

        @pl.when(is_u)
        def _():
            up_copy(zt, False).wait_recv()
            total((u_in, row_u, 0, width), [(g, row_u, 0, width), (u_in, row_u, 0, width)], zrows)

        @pl.when((is_u & (z < line - 2)) if final else is_u)
        def _():
            up_copy(zt, False).start()

        @pl.when(is_d)
        def _():
            dn_copy(zd, False).wait_recv()
            total((d_in, row_d, 0, width), [(g, row_d, 0, width), (d_in, row_d, 0, width)], zrows)

        @pl.when((is_d & (z > 1)) if final else is_d)
        def _():
            dn_copy(zd, False).start()

        if final:
            @pl.when(z == line - 2)
            def _():
                share(u_in, (line - 1) * zrows)

            @pl.when(z == 1)
            def _():
                share(d_in, 0)

    order = [(1 - r, 1 - y), (1 - r, y), (r, 1 - y), (r, y)]
    my_col = pl.multiple_of(core * cols, cols)
    its_col = pl.multiple_of((1 - core) * cols, cols)
    part = x.at[0]

    def slopes(row, count):
        @pl.loop(0, count // 32)
        def _(i):
            at = pl.ds(pl.multiple_of(row + i * 32, 32), 32)
            grad = acc[at, pl.ds(2 * width, width)]
            ggu[at, pl.ds(0, width)] = (grad * acc[at, pl.ds(0, width)]).astype(ggu.dtype)
            ggu[at, pl.ds(width, width)] = (grad * acc[at, pl.ds(width, width)]).astype(ggu.dtype)

    def back(row, count, col):
        @pl.loop(0, cols // wide)
        def _(n):
            at = pl.multiple_of(col + n * wide, wide)
            one = lax.dot_general(
                ggu[pl.ds(row, count), :], gu[pl.ds(at, wide), :], (((1,), (1,)), ((), ())),
                preferred_element_type=jnp.float32,
            )
            x[0, pl.ds(row, count), pl.ds(at, wide)] = one.astype(x.dtype)

    hrows = rows // 2
    units = [(0, 0, hrows), (0, hrows, hrows), (1, 0, rows), (2, 0, rows), (3, 0, rows)]

    def urow(i):
        b, at, count = units[i]
        return pl.multiple_of(slot(*order[b]) + at, hrows)

    def core_copy(i):
        at = pl.ds(urow(i), units[i][2])
        return remote(part.at[at, pl.ds(its_col, cols)], r1.at[at, :], c_s.at[i], c_r.at[i], cpart)

    first_col = my_col
    second_col = pl.multiple_of(my_col + parts_a, 128)

    def mine_a(row, count):
        return part.at[pl.ds(row, count), pl.ds(first_col, parts_a)]

    def mine_b(row, count):
        return part.at[pl.ds(row, count), pl.ds(second_col, parts_b)]

    def x_copy(i):
        if i == 3:
            src, dst = s3b, rxb
        elif i == 2:
            src, dst = mine_a(slot(*order[1]), rows), rxa.at[1]
        else:
            src, dst = mine_a(urow(i), hrows), rxa.at[0, pl.ds(i * hrows, hrows), :]
        return remote(src, dst, x_s.at[i], x_r.at[i], xpart)

    def y_copy(i):
        if i == 4:
            src, dst = s3a, ryb
        elif i in (2, 3):
            at = (i - 2) * hrows
            row = pl.multiple_of(slot(*order[2]) + at, hrows)
            src, dst = mine_b(row, hrows), rya.at[1, pl.ds(at, hrows), :]
        else:
            src, dst = mine_b(urow(i), hrows), rya.at[0, pl.ds(i * hrows, hrows), :]
        return remote(src, dst, yy_s.at[i], yy_r.at[i], ypart)

    def finish(b):
        @pl.when(is_end)
        def _():
            product(
                1, slot(*order[b]), (2 * (line - 1 - z) + 1 - y) * wrows, wrows,
                dn_w, 0, 2 * width, width,
            )

    def theirs(i):
        slopes(urow(i), units[i][2])
        back(urow(i), units[i][2], its_col)
        core_copy(i).start()

    def summed(i):
        back(urow(i), units[i][2], my_col)
        core_copy(i).wait_recv()
        total(
            (part, urow(i), my_col, cols),
            [(part, urow(i), my_col, cols), (r1, urow(i), 0, cols)], units[i][2],
        )

    def relay_a():
        for i in (0, 1):
            x_copy(i).wait_recv()
        total(
            (s3a, 0, 0, parts_a),
            [(part, slot(r, 1 - y), first_col, parts_a), (rxa.at[0], 0, 0, parts_a)], rows,
        )
        y_copy(4).start()

    def relay_b():
        for i in (0, 1):
            y_copy(i).wait_recv()
        total(
            (s3b, 0, 0, parts_b),
            [(part, slot(1 - r, y), second_col, parts_b), (rya.at[0], 0, 0, parts_b)], rows,
        )
        x_copy(3).start()

    here_row = slot(r, y)

    def o_copy(i, land):
        base = (1 - core if land else core) * cols
        if i == 0:
            at = gi_out.at[:, pl.ds(pl.multiple_of(base, 128), parts_a)]
        else:
            at = gi_out.at[
                pl.ds((i - 1) * hrows, hrows), pl.ds(pl.multiple_of(base + parts_a, 128), parts_b)
            ]
        return remote(at, at, o_s.at[i], o_r.at[i], cpart)

    def final_a():
        x_copy(2).wait_recv()
        y_copy(4).wait_recv()
        total(
            (gi_out, 0, first_col, parts_a),
            [
                (part, here_row, first_col, parts_a),
                (rxa.at[1], 0, 0, parts_a), (ryb, 0, 0, parts_a),
            ], rows,
        )
        o_copy(0, False).start()

    def final_b(i):
        at = i * hrows
        if i == 0:
            x_copy(3).wait_recv()
        y_copy(2 + i).wait_recv()
        total(
            (gi_out, at, second_col, parts_b),
            [
                (part, here_row + at, second_col, parts_b),
                (rya.at[1], at, 0, parts_b), (rxb, at, 0, parts_b),
            ], hrows,
        )
        o_copy(1 + i, False).start()

    def scaled(terms, rr, yy, keep=None):
        at_col = gcol(rr, yy)

        @pl.loop(0, frows // 64)
        def _(m):
            at = pl.multiple_of(m * 64, 64)
            value = None
            for ref, row, col in terms:
                one = ref[pl.ds(row + at, 64), pl.ds(col, width)].astype(jnp.float32)
                value = one if value is None else value + one
            if keep is not None:
                keep[pl.ds(at, 64), pl.ds(at_col, width)] = value.astype(keep.dtype)
            gd_out[pl.ds(at, 64), pl.ds(at_col, width)] = value * grad_scale

    def inputs_sent():
        for i in (0, 3, 5):
            dcopy(i, core).wait_send()
        tcopy(5, False).wait_send()

    @pl.when(is_end)
    def _():
        for i in range(line):
            g_block(jnp.where(lower, line - 1 - i, i))
            if i < line - 1:
                @pl.when(lower)
                def _():
                    up_copy(line - 1 - i, True).start()

                @pl.when(jnp.logical_not(lower))
                def _():
                    dn_copy(i, True).start()
        f_copy(0, False, g, zrow).start()
        f_copy(1, False, g, zrow).start()
        for d in range(last):
            for sub in range(2):
                settle(d, sub, 2)
        forward(1, dn_w, 2 * width, width, 0, 4)
        forward_end(1, 2, 0)
        for up_dir in (True, False):
            await_recv(up_dir, last, 1, 2)
        inputs_sent()
        finish(0)
        theirs(0)
        theirs(1)
        for i in (0, 1):
            summed(i)
            x_copy(i).start()
            y_copy(i).start()
        finish(1)
        theirs(2)
        summed(2)
        x_copy(2).start()
        finish(2)
        theirs(3)
        summed(3)
        y_copy(2).start()
        finish(3)
        theirs(4)
        summed(4)
        relay_a()
        y_copy(3).start()
        relay_b()
        f_copy(0, True).wait_recv()
        h_copy(1).wait_recv()
        scaled([(gl, 0, gcol(r, 1 - y)), (hl, 0, gcol(r, 1 - y))], r, 1 - y, gl)
        f_copy(2, False).start()
        h_copy(0).wait_recv()
        scaled([(g, pl.multiple_of(zrow + y * frows, frows), 0), (hl, 0, gcol(r, y))], r, y)
        final_a()
        final_b(0)
        f_copy(1, True).wait_recv()
        h_copy(2).wait_recv()
        scaled([(gl, 0, gcol(1 - r, y)), (hl, 0, gcol(1 - r, y))], 1 - r, y)
        final_b(1)
        f_copy(2, True).wait_recv()
        scaled([(gl, 0, gcol(1 - r, 1 - y))], 1 - r, 1 - y)

    @pl.when(jnp.logical_not(is_end))
    def _():
        inputs_sent()
        forward(1, dn_w, 2 * width, width, 3, 1)
        theirs(0)
        theirs(1)
        for i in (0, 1):
            summed(i)
            x_copy(i).start()
            y_copy(i).start()
        g_block(jnp.where(lower, line - 1, 0))
        forward(1, dn_w, 2 * width, width, 1, 1)
        theirs(2)
        summed(2)
        x_copy(2).start()
        line_step(1)
        forward(1, dn_w, 2 * width, width, 2, 1)
        theirs(3)
        summed(3)
        y_copy(2).start()
        relay_a()
        relay_b()
        for i in range(1, line):
            g_block(jnp.where(lower, line - 1 - i, i))
        for t in range(2, line - 1):
            line_step(t)
        forward(1, dn_w, 2 * width, width, 0, 1)
        theirs(4)
        summed(4)
        up_copy(z, False).wait_recv()
        dn_copy(z, False).wait_recv()
        total(
            (gfin, 0, 0, width),
            [(g, zrow, 0, width), (u_in, zrow, 0, width), (d_in, zrow, 0, width)], zrows,
        )
        f_copy(0, False).start()
        f_copy(1, False).start()
        y_copy(3).start()
        scaled([(gfin, pl.multiple_of(y * frows, frows), 0)], r, y)
        final_a()
        final_b(0)

        @pl.when(next_to_end)
        def _():
            for i in (0, 1):
                e_copy(i, True).wait_recv()
                h_copy(1 + i).start()

        f_copy(0, True).wait_recv()
        f_copy(2, False).start()
        scaled([(gl, 0, gcol(r, 1 - y))], r, 1 - y)
        f_copy(1, True).wait_recv()
        scaled([(gl, 0, gcol(1 - r, y))], 1 - r, y)
        final_b(1)
        f_copy(2, True).wait_recv()
        scaled([(gl, 0, gcol(1 - r, 1 - y))], 1 - r, 1 - y)

        @pl.when(next_to_end)
        def _():
            for i in (0, 1):
                e_copy(i, False).wait_send()
            for i in (0, 1, 2):
                h_copy(i).wait_send()

    for i in range(ntok):
        if kinds[i] == 1:
            dcopy(i, core).wait_send()
        if i != 5:
            tcopy(i, False).wait_send()
    for k in range(3):
        to_y(k).wait_send()
        for d in range(line - 1):
            for sub in range(2):
                await_send(True, d, sub, k)
                await_send(False, d, sub, k)
    for i in range(5):
        core_copy(i).wait_send()
        y_copy(i).wait_send()
    for i in range(4):
        x_copy(i).wait_send()
    for i in range(3):
        f_copy(i, False).wait_send()
    for i in range(3):
        o_copy(i, True).wait_recv()
        o_copy(i, False).wait_send()
    for zt in range(line):
        if zt > 0:
            far = line - 2 if zt == line - 1 else zt
            pl.when(z < far)(lambda: up_copy(zt, True).wait_send())
        if zt < line - 1:
            near = 1 if zt == 0 else zt
            pl.when(z > near)(lambda: dn_copy(zt, True).wait_send())


def fused(grad_scale, gate_w, up_w, down_w, toks, cots):
    line = lax.axis_size("fs") // 2
    rows, full = toks.shape
    wrows, width = gate_w.shape[0], gate_w.shape[1] // 4
    depth = 2 * line * wrows
    cols = full // 2
    kind = gate_w.dtype
    dma = pltpu.SemaphoreType.DMA
    zsem = dma((line - 1, 2, 3))
    anyspec = pl.BlockSpec(memory_space=pl.ANY)
    whole = pltpu.VMEM((depth, width), kind)
    parts_a = cols * 3 // 8 // 128 * 128
    parts_b = cols - parts_a
    return pl.pallas_call(
        functools.partial(fused_kernel, line, grad_scale),
        out_shape=(
            pltpu.VMEM((rows, full), kind),
            pltpu.VMEM((wrows, 4 * width), jnp.float32),
        ),
        in_specs=[anyspec] * 5,
        out_specs=(pl.BlockSpec(memory_space=pltpu.VMEM),) * 2,
        scratch_shapes=[
            pltpu.VMEM((2, 4 * rows, full), kind),
            pltpu.VMEM((depth, 2 * width), kind),
            whole,
            pltpu.VMEM((4 * rows, 3 * width), jnp.float32),
            pltpu.VMEM((4 * rows, width), kind),
            pltpu.VMEM((4 * rows, 2 * width), kind),
            pltpu.VMEM((4 * rows, cols), kind),
            pltpu.VMEM((2, rows, parts_a), kind), pltpu.VMEM((rows, parts_b), kind),
            pltpu.VMEM((2, rows, parts_b), kind), pltpu.VMEM((rows, parts_a), kind),
            pltpu.VMEM((rows, parts_a), kind), pltpu.VMEM((rows, parts_b), kind),
            whole, whole, whole,
            pltpu.VMEM((2 * wrows, width), kind),
            pltpu.VMEM((wrows, 4 * width), kind),
            pltpu.VMEM((wrows, 4 * width), kind),
            zsem, zsem, zsem, zsem,
            dma((3,)), dma((3,)),
            dma((8,)), dma((8,)), dma((8,)), dma((8,)), dma((5,)),
            dma((5,)), dma((5,)), dma((4,)), dma((4,)), dma((5,)), dma((5,)),
            dma((line,)), dma((line,)), dma((line,)), dma((line,)),
            dma((3,)), dma((3,)), dma((3,)), dma((3,)),
            dma((2,)), dma((2,)), dma((3,)), dma((3,)),
        ],
        compiler_params=pltpu.CompilerParams(
            collective_id=1, has_side_effects=True, vmem_limit_bytes=59 * 2**20
        ),
        name="fused_all",
    )(gate_w, up_w, down_w, toks, cots)


def gather_kernel(
    line, units, gate_w, up_w, down_w, toks, cots, gu_out, d_out, t_out, w_tmp, t_tmp,
    up_s, up_r, dn_s, dn_r, y_s, y_r, tok_s, tok_r, d2d_s, d2d_r, loc, loc2,
):
    r = lax.axis_index("rep")
    f = lax.axis_index("fs")
    t = lax.axis_index("tp")
    z, y = f // 2, f % 2
    rows = toks.shape[0]
    half = rows // 2
    wrows = gate_w.shape[0]
    width = gate_w.shape[1] // 4
    parts = len(units)
    has_up, has_dn = z < line - 1, z > 0
    up = {"fs": (f + 2) % (2 * line)}
    dn = {"fs": (f + 2 * line - 2) % (2 * line)}
    ypart = {"fs": f + 1 - 2 * y}
    xpart = {"rep": 1 - r}
    core = t % 2
    cpart = {"tp": t + 1 - 2 * core}

    barrier = pltpu.get_barrier_semaphore()

    def greet(dev):
        pl.semaphore_signal(barrier, inc=1, device_id=dev, device_id_type=MESH)

    for dev in (ypart, xpart, cpart, up, dn):
        greet(dev)
    pl.semaphore_wait(barrier, 5)

    def remote(src, dst, s, q, dev):
        return pltpu.make_async_remote_copy(
            src_ref=src, dst_ref=dst, send_sem=s, recv_sem=q,
            device_id=dev, device_id_type=MESH,
        )

    def wblk(k, zz, yy):
        row = pl.multiple_of((2 * zz + yy) * wrows, wrows)
        which, col, wide = units[k]
        return (gu_out, d_out)[which].at[pl.ds(row, wrows), pl.ds(col, wide)]

    def own(k, yy):
        col = pl.multiple_of((2 * r + yy) * width, width)
        return (gate_w, up_w, down_w)[k].at[:, pl.ds(col, width)]

    def to_y(k):
        return remote(own(k, 1 - y), wblk(k, z, y), y_s.at[k], y_r.at[k], ypart)

    def from_y(k):
        return remote(own(k, 1 - y), wblk(k, z, 1 - y), y_s.at[k], y_r.at[k], ypart)

    def zcopy(up_dir, d, sub, k, zz):
        yy = y if sub == 0 else 1 - y
        src = own(k, y) if (d == 0 and sub == 0) else wblk(k, zz, yy)
        s, q, dev = (up_s, up_r, up) if up_dir else (dn_s, dn_r, dn)
        return remote(src, wblk(k, zz, yy), s.at[d, sub, k], q.at[d, sub, k], dev)

    def pred_send(up_dir, d):
        return (has_up & (z - d >= 0)) if up_dir else (has_dn & (z + d <= line - 1))

    def src_z(up_dir, d):
        return jnp.maximum(z - d, 0) if up_dir else jnp.minimum(z + d, line - 1)

    def send(up_dir, d, sub, k):
        @pl.when(pred_send(up_dir, d))
        def _():
            zcopy(up_dir, d, sub, k, src_z(up_dir, d)).start()

    def await_send(up_dir, d, sub, k):
        @pl.when(pred_send(up_dir, d))
        def _():
            zcopy(up_dir, d, sub, k, src_z(up_dir, d)).wait_send()

    def await_recv(up_dir, d, sub, k):
        ok = (z - d - 1 >= 0) if up_dir else (z + d + 1 <= line - 1)

        @pl.when(ok)
        def _():
            zcopy(up_dir, d, sub, k, src_z(up_dir, d + 1)).wait_recv()

    def tblk(j, rr, yy, c):
        row = pl.multiple_of((2 * rr + yy) * rows + c * half, half)
        return t_out.at[j, pl.ds(row, half), :]

    def mine(j):
        src = toks if j == 0 else cots
        return src.at[pl.ds(pl.multiple_of(core * half, half), half), :]

    def tcopy(i, landing):
        j = (0, 1, 0, 1, 0, 1)[i]
        dev = xpart if i in (0, 1, 5) else ypart
        if landing:
            rr = (1 - r, 1 - r, r, r, 1 - r, 1 - r)[i]
            yy = (y, y, 1 - y, 1 - y, 1 - y, 1 - y)[i]
            src = dst = tblk(j, rr, yy, core)
        else:
            rr = (r, r, r, r, 1 - r, r)[i]
            yy = (y, y, y, y, y, 1 - y)[i]
            dst = tblk(j, rr, yy, core)
            src = mine(j) if i < 4 else dst
        return remote(src, dst, tok_s.at[i], tok_r.at[i], dev)

    def dcopy(i, c):
        j = (0, 1, 0, 1, 0, 1)[i]
        rr = (1 - r, 1 - r, r, r, 1 - r, 1 - r)[i]
        yy = (y, y, 1 - y, 1 - y, 1 - y, 1 - y)[i]
        blk = tblk(j, rr, yy, c)
        return remote(blk, blk, d2d_s.at[i], d2d_r.at[i], cpart)

    loads = [
        pltpu.make_async_copy(own(0, y), w_tmp.at[0], loc.at[0]),
        pltpu.make_async_copy(own(1, y), w_tmp.at[1], loc.at[3]),
        pltpu.make_async_copy(own(2, y), w_tmp.at[2], loc.at[4]),
        pltpu.make_async_copy(toks, t_tmp.at[0], loc.at[1]),
        pltpu.make_async_copy(cots, t_tmp.at[1], loc.at[2]),
    ]
    trow = pl.multiple_of((2 * r + y) * rows, rows)
    stores = [
        pltpu.make_async_copy(w_tmp.at[0], wblk(0, z, y), loc2.at[0]),
        pltpu.make_async_copy(w_tmp.at[1], wblk(1, z, y), loc2.at[3]),
        pltpu.make_async_copy(w_tmp.at[2], wblk(2, z, y), loc2.at[4]),
        pltpu.make_async_copy(t_tmp.at[0], t_out.at[0, pl.ds(trow, rows), :], loc2.at[1]),
        pltpu.make_async_copy(t_tmp.at[1], t_out.at[1, pl.ds(trow, rows), :], loc2.at[2]),
    ]

    for k in range(parts):
        to_y(k).start()
        send(True, 0, 0, k)
        send(False, 0, 0, k)
    for i in (0, 1, 3, 2):
        tcopy(i, False).start()
    for copy in loads:
        copy.start()
    for load, store in zip(loads, stores):
        load.wait()
        store.start()
    for k in range(parts):
        from_y(k).wait_recv()
        send(True, 0, 1, k)
        send(False, 0, 1, k)

    def event(i):
        tcopy(i, True).wait_recv()
        if i == 0:
            tcopy(4, False).start()
        if i == 3:
            tcopy(5, False).start()
        dcopy(i, core).start()

    events = [0, 3, 1, 2, 5, 4]
    for d in range(line - 1):
        for sub in range(2):
            if events:
                event(events.pop(0))
            for k in range(parts):
                for up_dir in (True, False):
                    await_recv(up_dir, d, sub, k)
                    if d + 1 < line - 1:
                        send(up_dir, d + 1, sub, k)
    for i in events:
        event(i)
    for i in range(6):
        dcopy(i, 1 - core).wait_recv()
        dcopy(i, core).wait_send()
        tcopy(i, False).wait_send()
    for k in range(parts):
        to_y(k).wait_send()
        for d in range(line - 1):
            for sub in range(2):
                await_send(True, d, sub, k)
                await_send(False, d, sub, k)
    for store in stores:
        store.wait()


def gather(gate_w, up_w, down_w, toks, cots):
    line = lax.axis_size("fs") // 2
    wrows, width = gate_w.shape[0], gate_w.shape[1] // 4
    units = [(0, 0, width), (0, width, width), (1, 0, width)]
    parts = len(units)
    depth = 2 * line * wrows
    kind = gate_w.dtype
    dma = pltpu.SemaphoreType.DMA
    zsem = dma((line - 1, 2, parts))
    anyspec = pl.BlockSpec(memory_space=pl.ANY)
    return pl.pallas_call(
        functools.partial(gather_kernel, line, units),
        out_shape=(
            jax.ShapeDtypeStruct((depth, 2 * width), kind),
            jax.ShapeDtypeStruct((depth, width), kind),
            jax.ShapeDtypeStruct((2, 4 * toks.shape[0], toks.shape[1]), toks.dtype),
        ),
        in_specs=[anyspec] * 5,
        out_specs=(anyspec,) * 3,
        scratch_shapes=[
            pltpu.VMEM((parts, wrows, width), kind),
            pltpu.VMEM((2,) + toks.shape, toks.dtype),
            zsem, zsem, zsem, zsem,
            dma((parts,)), dma((parts,)),
            dma((6,)), dma((6,)), dma((6,)), dma((6,)),
            dma((5,)), dma((5,)),
        ],
        compiler_params=pltpu.CompilerParams(collective_id=0, has_side_effects=True),
        name="gather_all",
    )(gate_w, up_w, down_w, toks, cots)


def on_device(inputs, cotangent, gate_weight, up_weight, down_weight):
    tok_rows = inputs.shape[0]
    fs_size = lax.axis_size("fs")
    rep_size = lax.axis_size("rep")
    grad_scale = 1.0 / math.sqrt(tok_rows * fs_size * rep_size)
    if lax.axis_size("tp") == 2 and rep_size == 2 and fs_size >= 8:
        return fused(
            grad_scale, gate_weight, up_weight, down_weight, inputs, cotangent
        )
    contract = (((1,), (1,)), ((), ()))
    contract_tok = (((0,), (0,)), ((), ()))
    width = gate_weight.shape[1] // 4
    gate_up, down_full, tokens = gather(
        gate_weight, up_weight, down_weight, inputs, cotangent
    )
    gate_up_val = jnp.dot(tokens[0], gate_up, preferred_element_type=jnp.float32)
    gate_val, up_val = gate_up_val[:, :width], gate_up_val[:, width:]
    grad_hidden = jnp.dot(tokens[1], down_full, preferred_element_type=jnp.float32)
    sigmoid_gate = jax.nn.sigmoid(gate_val)
    active = gate_val * sigmoid_gate
    hidden = (active * up_val).astype(jnp.bfloat16)
    grad_gate = (
        grad_hidden * up_val * sigmoid_gate * (1.0 + gate_val * (1.0 - sigmoid_gate))
    ).astype(jnp.bfloat16)
    grad_up = (grad_hidden * active).astype(jnp.bfloat16)
    pairs = [[i, i + 1] for i in range(0, fs_size, 2)]
    lines = [list(range(i, fs_size, 2)) for i in range(2)]
    grad_part = lax.dot_general(
        tokens[1], hidden, contract_tok, preferred_element_type=jnp.float32
    )
    part = lax.dot_general(
        jnp.concatenate([grad_gate, grad_up], axis=1), gate_up, contract,
        preferred_element_type=jnp.float32,
    )
    shard = lax.psum_scatter(
        grad_part.astype(jnp.bfloat16), "fs", scatter_dimension=0, tiled=True,
        axis_index_groups=lines,
    ).astype(jnp.float32) * grad_scale
    shard = lax.all_to_all(
        shard, "fs", split_axis=0, concat_axis=1, tiled=True, axis_index_groups=pairs
    )
    grad_down = lax.all_gather(shard, "rep", axis=1, tiled=True)
    part = lax.psum_scatter(
        part.astype(jnp.bfloat16), "rep", scatter_dimension=0, tiled=True
    )
    part = lax.psum_scatter(
        part, "fs", scatter_dimension=0, tiled=True, axis_index_groups=pairs
    )
    grad_input = lax.psum(part, "tp")
    return (grad_input, grad_down)


def solution(mesh):
    placed = (
        P(("rep", "fs"), None),
        P(("rep", "fs"), None),
        P("fs", "tp"),
        P("fs", "tp"),
        P("fs", "tp"),
    )
    return jax.shard_map(
        on_device,
        mesh=mesh,
        in_specs=placed,
        out_specs=(P(("rep", "fs"), None), P("fs", "tp")),
        check_vma=False,
    )
```

```python
import functools
import math

import jax
import jax.numpy as jnp
from jax import lax
from jax.experimental import pallas as pl
from jax.experimental.pallas import tpu as pltpu
from jax.sharding import PartitionSpec as P

MESH = pl.DeviceIdType.MESH


def fused_kernel(
    line, grad_scale, end_a, mid_a, gate_w, up_w, down_w, toks, cots, gi_out, gd_out,
    x, gu, dn_w, acc, hid, ggu, r1, rxa, rxb, rya, ryb, s3a, s3b, g, u_in, d_in, gfin, gl, hl,
    up_s, up_r, dn_s, dn_r, wy_s, wy_r, tok_s, tok_r, d2d_s, d2d_r, loc,
    c_s, c_r, x_s, x_r, yy_s, yy_r, u_s, u_r, d_s, d_r, f_s, f_r, o_s, o_r, e_s, e_r, h_s, h_r,
):
    r = lax.axis_index("rep")
    f = lax.axis_index("fs")
    core = lax.axis_index("tp")
    z, y = f // 2, f % 2
    rows = toks.shape[0]
    half = rows // 2
    wrows = gate_w.shape[0]
    width = gate_w.shape[1] // 4
    depth = 2 * line * wrows
    zrows = 2 * wrows
    cols = depth // 2
    wide = cols // 2
    frows = wrows
    last = line - 2
    has_up, has_dn = z < line - 1, z > 0
    is_end = (z == 0) | (z == line - 1)
    up = {"fs": (f + 2) % (2 * line)}
    dn = {"fs": (f + 2 * line - 2) % (2 * line)}
    ypart = {"fs": f + 1 - 2 * y}
    xpart = {"rep": 1 - r}
    cpart = {"tp": 1 - core}

    barrier = pltpu.get_barrier_semaphore()
    for dev in (ypart, xpart, cpart, up, dn):
        pl.semaphore_signal(barrier, inc=1, device_id=dev, device_id_type=MESH)
    pl.semaphore_wait(barrier, 5)

    def remote(src, dst, s, q, dev):
        return pltpu.make_async_remote_copy(
            src_ref=src, dst_ref=dst, send_sem=s, recv_sem=q,
            device_id=dev, device_id_type=MESH,
        )

    def wblk(k, zz, yy):
        row = pl.multiple_of((2 * zz + yy) * wrows, wrows)
        if k == 2:
            return dn_w.at[pl.ds(row, wrows), :]
        return gu.at[pl.ds(row, wrows), pl.ds(k * width, width)]

    def own(k, yy):
        col = pl.multiple_of((2 * r + yy) * width, width)
        return (gate_w, up_w, down_w)[k].at[:, pl.ds(col, width)]

    def to_y(k):
        return remote(own(k, 1 - y), wblk(k, z, y), wy_s.at[k], wy_r.at[k], ypart)

    def from_y(k):
        return remote(own(k, 1 - y), wblk(k, z, 1 - y), wy_s.at[k], wy_r.at[k], ypart)

    def zcopy(up_dir, d, sub, k, zz):
        yy = y if sub == 0 else 1 - y
        src = own(k, y) if (d == 0 and sub == 0) else wblk(k, zz, yy)
        s, q, dev = (up_s, up_r, up) if up_dir else (dn_s, dn_r, dn)
        return remote(src, wblk(k, zz, yy), s.at[d, sub, k], q.at[d, sub, k], dev)

    def pred_send(up_dir, d):
        return (has_up & (z - d >= 0)) if up_dir else (has_dn & (z + d <= line - 1))

    def src_z(up_dir, d):
        return jnp.maximum(z - d, 0) if up_dir else jnp.minimum(z + d, line - 1)

    def send(up_dir, d, sub, k):
        @pl.when(pred_send(up_dir, d))
        def _():
            zcopy(up_dir, d, sub, k, src_z(up_dir, d)).start()

    def await_send(up_dir, d, sub, k):
        @pl.when(pred_send(up_dir, d))
        def _():
            zcopy(up_dir, d, sub, k, src_z(up_dir, d)).wait_send()

    def await_recv(up_dir, d, sub, k):
        ok = (z - d - 1 >= 0) if up_dir else (z + d + 1 <= line - 1)

        @pl.when(ok)
        def _():
            zcopy(up_dir, d, sub, k, src_z(up_dir, d + 1)).wait_recv()

    def relay(d, sub, k):
        for up_dir in (True, False):
            @pl.when(pred_send(up_dir, d + 1))
            def _():
                zcopy(up_dir, d, sub, k, src_z(up_dir, d + 1)).wait_recv()
                zcopy(up_dir, d + 1, sub, k, src_z(up_dir, d + 1)).start()

    def settle(d, sub, k):
        for up_dir in (True, False):
            ok = (z - d - 1 >= 0) if up_dir else (z + d + 1 <= line - 1)
            onward = has_up if up_dir else has_dn

            @pl.when(ok & jnp.logical_not(onward))
            def _():
                zcopy(up_dir, d, sub, k, src_z(up_dir, d + 1)).wait_recv()

    def slot(rr, yy):
        return pl.multiple_of((2 * rr + yy) * rows, rows)

    kinds = (0, 1, 1, 0, 1, 0, 1, 1)
    over_x = (True, True, True, False, False, True, False, True)
    parts = (2, 0, 1, 2, 2, 2, 0, 1)
    ntok = len(kinds)

    def span(c, p):
        if p == 2:
            return c * half, half
        return c * half + p * (half // 2), half // 2

    def tblk(i, rr, yy, c):
        at, count = span(c, parts[i])
        row = pl.multiple_of((2 * rr + yy) * rows + at, half // 2)
        return x.at[kinds[i], pl.ds(row, count), :]

    def mine(i):
        at, count = span(core, parts[i])
        src = toks if kinds[i] == 0 else cots
        return src.at[pl.ds(pl.multiple_of(at, half // 2), count), :]

    def landing(i, c):
        rr = (1 - r, 1 - r, 1 - r, r, r, 1 - r, 1 - r, 1 - r)[i]
        yy = (y, y, y, 1 - y, 1 - y, 1 - y, 1 - y, 1 - y)[i]
        return tblk(i, rr, yy, c)

    def tcopy(i, land):
        dev = xpart if over_x[i] else ypart
        if land:
            src = dst = landing(i, core)
        else:
            rr = (r, r, r, r, r, r, 1 - r, r)[i]
            yy = (y, y, y, y, y, 1 - y, y, 1 - y)[i]
            dst = tblk(i, rr, yy, core)
            src = mine(i) if i < 5 else dst
        return remote(src, dst, tok_s.at[i], tok_r.at[i], dev)

    def dcopy(i, c):
        blk = landing(i, c)
        return remote(blk, blk, d2d_s.at[i], d2d_r.at[i], cpart)

    def event(i):
        tcopy(i, True).wait_recv()
        onward = {1: 6, 3: 5, 4: 7}.get(i)
        if onward is not None:
            tcopy(onward, False).start()
        dcopy(i, core).start()

    trow = slot(r, y)
    loads = [
        pltpu.make_async_copy(own(0, y), wblk(0, z, y), loc.at[0]),
        pltpu.make_async_copy(own(1, y), wblk(1, z, y), loc.at[1]),
        pltpu.make_async_copy(own(2, y), wblk(2, z, y), loc.at[2]),
        pltpu.make_async_copy(toks, x.at[0, pl.ds(trow, rows), :], loc.at[3]),
        pltpu.make_async_copy(cots, x.at[1, pl.ds(trow, rows), :], loc.at[4]),
    ]

    tile = 256
    z_lo = jnp.maximum(z - last, 0)
    z_hi = jnp.minimum(z + last, line - 1) + 1

    def product(j, row, k0, kk, w, wcol, acol, n):
        at = pl.ds(pl.multiple_of(row, rows), rows)
        kat = pl.ds(pl.multiple_of(k0, wrows), kk)
        for c in range(0, n, tile):
            one = jnp.dot(
                x[j, at, kat], w[kat, pl.ds(wcol + c, tile)],
                preferred_element_type=jnp.float32,
            )
            acc[at, pl.ds(acol + c, tile)] += one

    def forward(j, w, acol, n, first, count):
        @pl.loop(first, first + count)
        def _(b):
            row = ((2 * r + y) + 2 * (b % 2) * (1 - 2 * r) + (b // 2) * (1 - 2 * y)) * rows

            @pl.loop(z_lo, z_hi)
            def _(zz):
                product(j, row, zz * zrows, zrows, w, 0, acol, n)

    def forward_end(j, k, sub):
        for up_dir in (True, False):
            await_recv(up_dir, last, sub, k)

        @pl.when(is_end)
        def _():
            zz = line - 1 - z
            yy = y if sub == 0 else 1 - y
            w = dn_w if k == 2 else gu

            @pl.loop(0, 4)
            def _(b):
                product(
                    j, b * rows, (2 * zz + yy) * wrows, wrows, w,
                    0 if k == 2 else k * width, k * width, width,
                )

    def total(dst, terms, count, step=64):
        @pl.loop(0, count // step)
        def _(i):
            at = pl.multiple_of(i * step, step)
            value = None
            for ref, row, col, wide in terms:
                one = ref[pl.ds(row + at, step), pl.ds(col, wide)].astype(jnp.float32)
                value = one if value is None else value + one
            ref, row, col, wide = dst
            ref[pl.ds(row + at, step), pl.ds(col, wide)] = value.astype(ref.dtype)

    for k in (0, 1):
        to_y(k).start()
        send(True, 0, 0, k)
        send(False, 0, 0, k)
    for i in (0, 1, 3):
        tcopy(i, False).start()
    to_y(2).start()
    tcopy(4, False).start()
    for copy in loads:
        copy.start()

    @pl.loop(0, 4 * rows // 64)
    def _(i):
        at = pl.ds(pl.multiple_of(i * 64, 64), 64)
        acc[at, :] = jnp.zeros((64, 3 * width), jnp.float32)

    for k in (0, 1):
        from_y(k).wait_recv()
        send(True, 0, 1, k)
        send(False, 0, 1, k)
    if last > 0:
        for sub in range(2):
            for k in (0, 1):
                relay(0, sub, k)
    event(0)
    event(3)
    tcopy(2, False).start()
    event(1)
    for d in range(1, last):
        for sub in range(2):
            for k in (0, 1):
                relay(d, sub, k)
    send(True, 0, 0, 2)
    send(False, 0, 0, 2)
    from_y(2).wait_recv()
    send(True, 0, 1, 2)
    send(False, 0, 1, 2)
    for load in loads:
        load.wait()
    for d in range(last):
        for sub in range(2):
            for k in (0, 1):
                settle(d, sub, k)
    dcopy(0, 1 - core).wait_recv()
    dcopy(3, 1 - core).wait_recv()
    forward(0, gu, 0, 2 * width, 0, 3)
    if last > 0:
        for sub in range(2):
            relay(0, sub, 2)
    event(5)
    event(4)
    dcopy(5, 1 - core).wait_recv()
    forward(0, gu, 0, 2 * width, 3, 1)
    for d in range(1, last):
        for sub in range(2):
            relay(d, sub, 2)
    for sub in range(2):
        for k in (0, 1):
            forward_end(0, k, sub)

    @pl.loop(0, 4 * rows // 32)
    def _(i):
        at = pl.ds(pl.multiple_of(i * 32, 32), 32)
        gate = acc[at, pl.ds(0, width)]
        up_val = acc[at, pl.ds(width, width)]
        sig = jax.nn.sigmoid(gate)
        active = gate * sig
        hid[at, :] = (active * up_val).astype(hid.dtype)
        acc[at, pl.ds(0, width)] = up_val * sig * (1.0 + gate * (1.0 - sig))
        acc[at, pl.ds(width, width)] = active

    for i in (2, 6, 7):
        event(i)
    for i in (1, 2, 4, 6, 7):
        dcopy(i, 1 - core).wait_recv()

    zrow = pl.multiple_of(z * zrows, zrows)
    lower = z < line // 2

    def block(ref, zt):
        return ref.at[pl.ds(zt * zrows, zrows), :]

    def up_copy(zt, first):
        return remote(block(g if first else u_in, zt), block(u_in, zt), u_s.at[zt], u_r.at[zt], up)

    def dn_copy(zt, first):
        return remote(block(g if first else d_in, zt), block(d_in, zt), d_s.at[zt], d_r.at[zt], dn)

    def g_block(zt):
        at = pl.multiple_of(zt * zrows, zrows)
        one = lax.dot_general(
            x[1, :, pl.ds(at, zrows)], hid[...], (((0,), (0,)), ((), ())),
            preferred_element_type=jnp.float32,
        )
        g[pl.ds(at, zrows), :] = one.astype(g.dtype)

    def gcol(rr, yy):
        return pl.multiple_of((2 * rr + yy) * width, width)

    def gcols(ref, rr, yy):
        return ref.at[:, pl.ds(gcol(rr, yy), width)]

    def half_rows(ref, row, yy):
        return ref.at[pl.ds(pl.multiple_of(row + yy * frows, frows), frows), :]

    def f_copy(i, land, ref=gfin, row=0):
        if i == 0:
            src, dst, dev = half_rows(ref, row, 1 - y), gcols(gl, r, 1 - y if land else y), ypart
        elif i == 1:
            src, dst, dev = half_rows(ref, row, y), gcols(gl, 1 - r if land else r, y), xpart
        else:
            src, dst, dev = gcols(gl, r, 1 - y), gcols(gl, 1 - r if land else r, 1 - y), xpart
        return remote(src, dst, f_s.at[i], f_r.at[i], dev)

    def e_copy(i, land, ref=gfin, row=0):
        if i == 0:
            src, dst, dev = half_rows(ref, row, 1 - y), gcols(hl, r, 1 - y if land else y), ypart
        elif i == 1:
            src, dst, dev = half_rows(ref, row, y), gcols(hl, 1 - r if land else r, y), xpart
        else:
            src, dst, dev = gcols(hl, r, 1 - y), gcols(hl, 1 - r if land else r, 1 - y), xpart
        return remote(src, dst, e_s.at[i], e_r.at[i], dev)

    end_z = jnp.where((z == 1) | (z == line - 1), 0, line - 1)
    end_dev = {"fs": 2 * end_z + y}
    next_to_end = (z == 1) | (z == line - 2)

    def h_copy(i, ref=gfin, row=0):
        rr, yy = ((r, y), (r, 1 - y), (1 - r, y), (1 - r, 1 - y))[i]
        dst = gcols(hl, rr, yy)
        src = half_rows(ref, row, y) if i == 0 else dst
        return remote(src, dst, h_s.at[i], h_r.at[i], end_dev)

    def share(ref, row):
        h_copy(0, ref, row).start()
        e_copy(0, False, ref, row).start()
        e_copy(1, False, ref, row).start()

    def line_step(t):
        zt = line - 1 + z - t
        row_u = pl.multiple_of(zt * zrows, zrows)
        is_u = (z > 0) & (zt <= line - 1) & (zt > z)
        zd = t - (line - 1 - z)
        row_d = pl.multiple_of(zd * zrows, zrows)
        is_d = (z < line - 1) & (zd >= 0) & (zd < z)
        final = t == line - 2

        @pl.when(is_u)
        def _():
            up_copy(zt, False).wait_recv()
            total((u_in, row_u, 0, width), [(g, row_u, 0, width), (u_in, row_u, 0, width)], zrows)

        @pl.when((is_u & (z < line - 2)) if final else is_u)
        def _():
            up_copy(zt, False).start()

        @pl.when(is_d)
        def _():
            dn_copy(zd, False).wait_recv()
            total((d_in, row_d, 0, width), [(g, row_d, 0, width), (d_in, row_d, 0, width)], zrows)

        @pl.when((is_d & (z > 1)) if final else is_d)
        def _():
            dn_copy(zd, False).start()

        if final:
            @pl.when(z == line - 2)
            def _():
                share(u_in, (line - 1) * zrows)

            @pl.when(z == 1)
            def _():
                share(d_in, 0)

    order = [(1 - r, 1 - y), (1 - r, y), (r, 1 - y), (r, y)]
    my_col = pl.multiple_of(core * cols, cols)
    its_col = pl.multiple_of((1 - core) * cols, cols)
    part = x.at[0]

    def slopes(row, count):
        @pl.loop(0, count // 32)
        def _(i):
            at = pl.ds(pl.multiple_of(row + i * 32, 32), 32)
            grad = acc[at, pl.ds(2 * width, width)]
            ggu[at, pl.ds(0, width)] = (grad * acc[at, pl.ds(0, width)]).astype(ggu.dtype)
            ggu[at, pl.ds(width, width)] = (grad * acc[at, pl.ds(width, width)]).astype(ggu.dtype)

    def back(row, count, col):
        @pl.loop(0, cols // wide)
        def _(n):
            at = pl.multiple_of(col + n * wide, wide)
            one = lax.dot_general(
                ggu[pl.ds(row, count), :], gu[pl.ds(at, wide), :], (((1,), (1,)), ((), ())),
                preferred_element_type=jnp.float32,
            )
            x[0, pl.ds(row, count), pl.ds(at, wide)] = one.astype(x.dtype)

    hrows = rows // 2
    units = [(0, 0, hrows), (0, hrows, hrows), (1, 0, rows), (2, 0, rows), (3, 0, rows)]

    def urow(i):
        b, at, count = units[i]
        return pl.multiple_of(slot(*order[b]) + at, hrows)

    def core_copy(i):
        at = pl.ds(urow(i), units[i][2])
        return remote(part.at[at, pl.ds(its_col, cols)], r1.at[at, :], c_s.at[i], c_r.at[i], cpart)

    def finish(b):
        @pl.when(is_end)
        def _():
            product(
                1, slot(*order[b]), (2 * (line - 1 - z) + 1 - y) * wrows, wrows,
                dn_w, 0, 2 * width, width,
            )

    def theirs(i):
        slopes(urow(i), units[i][2])
        back(urow(i), units[i][2], its_col)
        core_copy(i).start()

    def summed(i):
        back(urow(i), units[i][2], my_col)
        core_copy(i).wait_recv()
        total(
            (part, urow(i), my_col, cols),
            [(part, urow(i), my_col, cols), (r1, urow(i), 0, cols)], units[i][2],
        )

    here_row = slot(r, y)

    def plane_sums(pa):
        pb = cols - pa
        second_col = pl.multiple_of(my_col + pa, 128)

        def mine_a(row, count):
            return part.at[pl.ds(row, count), pl.ds(my_col, pa)]

        def mine_b(row, count):
            return part.at[pl.ds(row, count), pl.ds(second_col, pb)]

        def x_copy(i):
            if i == 3:
                src, dst = s3b.at[:, pl.ds(0, pb)], rxb.at[:, pl.ds(0, pb)]
            elif i == 2:
                src, dst = mine_a(slot(*order[1]), rows), rxa.at[1, :, pl.ds(0, pa)]
            else:
                src, dst = mine_a(urow(i), hrows), rxa.at[0, pl.ds(i * hrows, hrows), pl.ds(0, pa)]
            return remote(src, dst, x_s.at[i], x_r.at[i], xpart)

        def y_copy(i):
            if i == 4:
                src, dst = s3a.at[:, pl.ds(0, pa)], ryb.at[:, pl.ds(0, pa)]
            elif i in (2, 3):
                at = (i - 2) * hrows
                row = pl.multiple_of(slot(*order[2]) + at, hrows)
                src, dst = mine_b(row, hrows), rya.at[1, pl.ds(at, hrows), pl.ds(0, pb)]
            else:
                src, dst = mine_b(urow(i), hrows), rya.at[0, pl.ds(i * hrows, hrows), pl.ds(0, pb)]
            return remote(src, dst, yy_s.at[i], yy_r.at[i], ypart)

        def relay_a():
            for i in (0, 1):
                x_copy(i).wait_recv()
            total(
                (s3a, 0, 0, pa),
                [(part, slot(r, 1 - y), my_col, pa), (rxa.at[0], 0, 0, pa)], rows,
            )
            y_copy(4).start()

        def relay_b():
            for i in (0, 1):
                y_copy(i).wait_recv()
            total(
                (s3b, 0, 0, pb),
                [(part, slot(1 - r, y), second_col, pb), (rya.at[0], 0, 0, pb)], rows,
            )
            x_copy(3).start()

        def o_copy(i, land):
            base = (1 - core if land else core) * cols
            if i == 0:
                at = gi_out.at[:, pl.ds(pl.multiple_of(base, 128), pa)]
            else:
                at = gi_out.at[
                    pl.ds((i - 1) * hrows, hrows), pl.ds(pl.multiple_of(base + pa, 128), pb)
                ]
            return remote(at, at, o_s.at[i], o_r.at[i], cpart)

        def final_a():
            x_copy(2).wait_recv()
            y_copy(4).wait_recv()
            total(
                (gi_out, 0, my_col, pa),
                [
                    (part, here_row, my_col, pa),
                    (rxa.at[1], 0, 0, pa), (ryb, 0, 0, pa),
                ], rows,
            )
            o_copy(0, False).start()

        def final_b(i):
            at = i * hrows
            if i == 0:
                x_copy(3).wait_recv()
            y_copy(2 + i).wait_recv()
            total(
                (gi_out, at, second_col, pb),
                [
                    (part, here_row + at, second_col, pb),
                    (rya.at[1], at, 0, pb), (rxb, at, 0, pb),
                ], hrows,
            )
            o_copy(1 + i, False).start()

        def settled():
            for i in range(5):
                y_copy(i).wait_send()
            for i in range(4):
                x_copy(i).wait_send()
            for i in range(3):
                o_copy(i, True).wait_recv()
                o_copy(i, False).wait_send()

        return x_copy, y_copy, relay_a, relay_b, final_a, final_b, settled

    def scaled(terms, rr, yy):
        at_col = gcol(rr, yy)

        @pl.loop(0, frows // 64)
        def _(m):
            at = pl.multiple_of(m * 64, 64)
            value = None
            for ref, row, col in terms:
                one = ref[pl.ds(row + at, 64), pl.ds(col, width)].astype(jnp.float32)
                value = one if value is None else value + one
            gd_out[pl.ds(at, 64), pl.ds(at_col, width)] = value * grad_scale

    def inputs_sent():
        for i in (0, 3, 5):
            dcopy(i, core).wait_send()
        tcopy(5, False).wait_send()

    @pl.when(is_end)
    def _():
        x_copy, y_copy, relay_a, relay_b, final_a, final_b, settled = plane_sums(end_a)
        for i in range(line):
            g_block(jnp.where(lower, line - 1 - i, i))
            if i < line - 1:
                @pl.when(lower)
                def _():
                    up_copy(line - 1 - i, True).start()

                @pl.when(jnp.logical_not(lower))
                def _():
                    dn_copy(i, True).start()
        f_copy(0, False, g, zrow).start()
        f_copy(1, False, g, zrow).start()
        for d in range(last):
            for sub in range(2):
                settle(d, sub, 2)
        forward(1, dn_w, 2 * width, width, 0, 4)
        f_copy(0, True).wait_recv()
        f_copy(2, False).start()
        forward_end(1, 2, 0)
        for up_dir in (True, False):
            await_recv(up_dir, last, 1, 2)
        inputs_sent()
        finish(0)
        theirs(0)
        theirs(1)
        for i in (0, 1):
            summed(i)
            x_copy(i).start()
            y_copy(i).start()
        finish(1)
        theirs(2)
        summed(2)
        x_copy(2).start()
        finish(2)
        theirs(3)
        summed(3)
        y_copy(2).start()
        finish(3)
        theirs(4)
        summed(4)
        relay_a()
        y_copy(3).start()
        relay_b()
        h_copy(0).wait_recv()
        scaled([(g, pl.multiple_of(zrow + y * frows, frows), 0), (hl, 0, gcol(r, y))], r, y)
        final_a()
        final_b(0)
        for i, (rr, yy) in enumerate(((r, 1 - y), (1 - r, y))):
            if i == 1:
                f_copy(1, True).wait_recv()
            h_copy(1 + i).wait_recv()
            scaled([(gl, 0, gcol(rr, yy)), (hl, 0, gcol(rr, yy))], rr, yy)
        final_b(1)
        f_copy(2, True).wait_recv()
        h_copy(3).wait_recv()
        diag = gcol(1 - r, 1 - y)
        scaled([(gl, 0, diag), (hl, 0, diag)], 1 - r, 1 - y)
        settled()

    @pl.when(jnp.logical_not(is_end))
    def _():
        x_copy, y_copy, relay_a, relay_b, final_a, final_b, settled = plane_sums(mid_a)
        inputs_sent()
        forward(1, dn_w, 2 * width, width, 3, 1)
        theirs(0)
        theirs(1)
        for i in (0, 1):
            summed(i)
            x_copy(i).start()
            y_copy(i).start()
        g_block(jnp.where(lower, line - 1, 0))
        forward(1, dn_w, 2 * width, width, 1, 1)
        theirs(2)
        summed(2)
        x_copy(2).start()
        line_step(1)
        forward(1, dn_w, 2 * width, width, 2, 1)
        theirs(3)
        summed(3)
        y_copy(2).start()
        relay_a()
        relay_b()
        for i in range(1, line):
            g_block(jnp.where(lower, line - 1 - i, i))
        for t in range(2, line - 1):
            line_step(t)
        forward(1, dn_w, 2 * width, width, 0, 1)
        theirs(4)
        summed(4)
        up_copy(z, False).wait_recv()
        dn_copy(z, False).wait_recv()
        total(
            (gfin, 0, 0, width),
            [(g, zrow, 0, width), (u_in, zrow, 0, width), (d_in, zrow, 0, width)], zrows,
        )
        f_copy(0, False).start()
        y_copy(3).start()
        scaled([(gfin, pl.multiple_of(y * frows, frows), 0)], r, y)

        @pl.when(next_to_end)
        def _():
            e_copy(0, True).wait_recv()
            e_copy(2, False).start()
            h_copy(1).start()
            e_copy(1, True).wait_recv()
            h_copy(2).start()

        f_copy(1, False).start()
        final_a()
        final_b(0)

        @pl.when(next_to_end)
        def _():
            e_copy(2, True).wait_recv()
            h_copy(3).start()

        f_copy(0, True).wait_recv()
        f_copy(2, False).start()
        scaled([(gl, 0, gcol(r, 1 - y))], r, 1 - y)
        f_copy(1, True).wait_recv()
        scaled([(gl, 0, gcol(1 - r, y))], 1 - r, y)
        final_b(1)
        f_copy(2, True).wait_recv()
        scaled([(gl, 0, gcol(1 - r, 1 - y))], 1 - r, 1 - y)

        @pl.when(next_to_end)
        def _():
            for i in range(3):
                e_copy(i, False).wait_send()
            for i in range(4):
                h_copy(i).wait_send()

        settled()

    for i in range(ntok):
        if kinds[i] == 1:
            dcopy(i, core).wait_send()
        if i != 5:
            tcopy(i, False).wait_send()
    for k in range(3):
        to_y(k).wait_send()
        for d in range(line - 1):
            for sub in range(2):
                await_send(True, d, sub, k)
                await_send(False, d, sub, k)
    for i in range(5):
        core_copy(i).wait_send()
    for i in range(3):
        f_copy(i, False).wait_send()
    for zt in range(line):
        if zt > 0:
            far = line - 2 if zt == line - 1 else zt
            pl.when(z < far)(lambda: up_copy(zt, True).wait_send())
        if zt < line - 1:
            near = 1 if zt == 0 else zt
            pl.when(z > near)(lambda: dn_copy(zt, True).wait_send())


def fused(grad_scale, gate_w, up_w, down_w, toks, cots):
    line = lax.axis_size("fs") // 2
    rows, full = toks.shape
    wrows, width = gate_w.shape[0], gate_w.shape[1] // 4
    depth = 2 * line * wrows
    cols = full // 2
    kind = gate_w.dtype
    dma = pltpu.SemaphoreType.DMA
    zsem = dma((line - 1, 2, 3))
    anyspec = pl.BlockSpec(memory_space=pl.ANY)
    whole = pltpu.VMEM((depth, width), kind)
    end_a, mid_a = cols // 2, cols // 4
    most_b = cols - mid_a
    return pl.pallas_call(
        functools.partial(fused_kernel, line, grad_scale, end_a, mid_a),
        out_shape=(
            pltpu.VMEM((rows, full), kind),
            pltpu.VMEM((wrows, 4 * width), jnp.float32),
        ),
        in_specs=[anyspec] * 5,
        out_specs=(pl.BlockSpec(memory_space=pltpu.VMEM),) * 2,
        scratch_shapes=[
            pltpu.VMEM((2, 4 * rows, full), kind),
            pltpu.VMEM((depth, 2 * width), kind),
            whole,
            pltpu.VMEM((4 * rows, 3 * width), jnp.float32),
            pltpu.VMEM((4 * rows, width), kind),
            pltpu.VMEM((4 * rows, 2 * width), kind),
            pltpu.VMEM((4 * rows, cols), kind),
            pltpu.VMEM((2, rows, end_a), kind), pltpu.VMEM((rows, most_b), kind),
            pltpu.VMEM((2, rows, most_b), kind), pltpu.VMEM((rows, end_a), kind),
            pltpu.VMEM((rows, end_a), kind), pltpu.VMEM((rows, most_b), kind),
            whole, whole, whole,
            pltpu.VMEM((2 * wrows, width), kind),
            pltpu.VMEM((wrows, 4 * width), kind),
            pltpu.VMEM((wrows, 4 * width), kind),
            zsem, zsem, zsem, zsem,
            dma((3,)), dma((3,)),
            dma((8,)), dma((8,)), dma((8,)), dma((8,)), dma((5,)),
            dma((5,)), dma((5,)), dma((4,)), dma((4,)), dma((5,)), dma((5,)),
            dma((line,)), dma((line,)), dma((line,)), dma((line,)),
            dma((3,)), dma((3,)), dma((3,)), dma((3,)),
            dma((3,)), dma((3,)), dma((4,)), dma((4,)),
        ],
        compiler_params=pltpu.CompilerParams(
            collective_id=1, has_side_effects=True, vmem_limit_bytes=59 * 2**20
        ),
        name="fused_all",
    )(gate_w, up_w, down_w, toks, cots)


def gather_kernel(
    line, units, gate_w, up_w, down_w, toks, cots, gu_out, d_out, t_out, w_tmp, t_tmp,
    up_s, up_r, dn_s, dn_r, y_s, y_r, tok_s, tok_r, d2d_s, d2d_r, loc, loc2,
):
    r = lax.axis_index("rep")
    f = lax.axis_index("fs")
    t = lax.axis_index("tp")
    z, y = f // 2, f % 2
    rows = toks.shape[0]
    half = rows // 2
    wrows = gate_w.shape[0]
    width = gate_w.shape[1] // 4
    parts = len(units)
    has_up, has_dn = z < line - 1, z > 0
    up = {"fs": (f + 2) % (2 * line)}
    dn = {"fs": (f + 2 * line - 2) % (2 * line)}
    ypart = {"fs": f + 1 - 2 * y}
    xpart = {"rep": 1 - r}
    core = t % 2
    cpart = {"tp": t + 1 - 2 * core}

    barrier = pltpu.get_barrier_semaphore()

    def greet(dev):
        pl.semaphore_signal(barrier, inc=1, device_id=dev, device_id_type=MESH)

    for dev in (ypart, xpart, cpart, up, dn):
        greet(dev)
    pl.semaphore_wait(barrier, 5)

    def remote(src, dst, s, q, dev):
        return pltpu.make_async_remote_copy(
            src_ref=src, dst_ref=dst, send_sem=s, recv_sem=q,
            device_id=dev, device_id_type=MESH,
        )

    def wblk(k, zz, yy):
        row = pl.multiple_of((2 * zz + yy) * wrows, wrows)
        which, col, wide = units[k]
        return (gu_out, d_out)[which].at[pl.ds(row, wrows), pl.ds(col, wide)]

    def own(k, yy):
        col = pl.multiple_of((2 * r + yy) * width, width)
        return (gate_w, up_w, down_w)[k].at[:, pl.ds(col, width)]

    def to_y(k):
        return remote(own(k, 1 - y), wblk(k, z, y), y_s.at[k], y_r.at[k], ypart)

    def from_y(k):
        return remote(own(k, 1 - y), wblk(k, z, 1 - y), y_s.at[k], y_r.at[k], ypart)

    def zcopy(up_dir, d, sub, k, zz):
        yy = y if sub == 0 else 1 - y
        src = own(k, y) if (d == 0 and sub == 0) else wblk(k, zz, yy)
        s, q, dev = (up_s, up_r, up) if up_dir else (dn_s, dn_r, dn)
        return remote(src, wblk(k, zz, yy), s.at[d, sub, k], q.at[d, sub, k], dev)

    def pred_send(up_dir, d):
        return (has_up & (z - d >= 0)) if up_dir else (has_dn & (z + d <= line - 1))

    def src_z(up_dir, d):
        return jnp.maximum(z - d, 0) if up_dir else jnp.minimum(z + d, line - 1)

    def send(up_dir, d, sub, k):
        @pl.when(pred_send(up_dir, d))
        def _():
            zcopy(up_dir, d, sub, k, src_z(up_dir, d)).start()

    def await_send(up_dir, d, sub, k):
        @pl.when(pred_send(up_dir, d))
        def _():
            zcopy(up_dir, d, sub, k, src_z(up_dir, d)).wait_send()

    def await_recv(up_dir, d, sub, k):
        ok = (z - d - 1 >= 0) if up_dir else (z + d + 1 <= line - 1)

        @pl.when(ok)
        def _():
            zcopy(up_dir, d, sub, k, src_z(up_dir, d + 1)).wait_recv()

    def tblk(j, rr, yy, c):
        row = pl.multiple_of((2 * rr + yy) * rows + c * half, half)
        return t_out.at[j, pl.ds(row, half), :]

    def mine(j):
        src = toks if j == 0 else cots
        return src.at[pl.ds(pl.multiple_of(core * half, half), half), :]

    def tcopy(i, landing):
        j = (0, 1, 0, 1, 0, 1)[i]
        dev = xpart if i in (0, 1, 5) else ypart
        if landing:
            rr = (1 - r, 1 - r, r, r, 1 - r, 1 - r)[i]
            yy = (y, y, 1 - y, 1 - y, 1 - y, 1 - y)[i]
            src = dst = tblk(j, rr, yy, core)
        else:
            rr = (r, r, r, r, 1 - r, r)[i]
            yy = (y, y, y, y, y, 1 - y)[i]
            dst = tblk(j, rr, yy, core)
            src = mine(j) if i < 4 else dst
        return remote(src, dst, tok_s.at[i], tok_r.at[i], dev)

    def dcopy(i, c):
        j = (0, 1, 0, 1, 0, 1)[i]
        rr = (1 - r, 1 - r, r, r, 1 - r, 1 - r)[i]
        yy = (y, y, 1 - y, 1 - y, 1 - y, 1 - y)[i]
        blk = tblk(j, rr, yy, c)
        return remote(blk, blk, d2d_s.at[i], d2d_r.at[i], cpart)

    loads = [
        pltpu.make_async_copy(own(0, y), w_tmp.at[0], loc.at[0]),
        pltpu.make_async_copy(own(1, y), w_tmp.at[1], loc.at[3]),
        pltpu.make_async_copy(own(2, y), w_tmp.at[2], loc.at[4]),
        pltpu.make_async_copy(toks, t_tmp.at[0], loc.at[1]),
        pltpu.make_async_copy(cots, t_tmp.at[1], loc.at[2]),
    ]
    trow = pl.multiple_of((2 * r + y) * rows, rows)
    stores = [
        pltpu.make_async_copy(w_tmp.at[0], wblk(0, z, y), loc2.at[0]),
        pltpu.make_async_copy(w_tmp.at[1], wblk(1, z, y), loc2.at[3]),
        pltpu.make_async_copy(w_tmp.at[2], wblk(2, z, y), loc2.at[4]),
        pltpu.make_async_copy(t_tmp.at[0], t_out.at[0, pl.ds(trow, rows), :], loc2.at[1]),
        pltpu.make_async_copy(t_tmp.at[1], t_out.at[1, pl.ds(trow, rows), :], loc2.at[2]),
    ]

    for k in range(parts):
        to_y(k).start()
        send(True, 0, 0, k)
        send(False, 0, 0, k)
    for i in (0, 1, 3, 2):
        tcopy(i, False).start()
    for copy in loads:
        copy.start()
    for load, store in zip(loads, stores):
        load.wait()
        store.start()
    for k in range(parts):
        from_y(k).wait_recv()
        send(True, 0, 1, k)
        send(False, 0, 1, k)

    def event(i):
        tcopy(i, True).wait_recv()
        if i == 0:
            tcopy(4, False).start()
        if i == 3:
            tcopy(5, False).start()
        dcopy(i, core).start()

    events = [0, 3, 1, 2, 5, 4]
    for d in range(line - 1):
        for sub in range(2):
            if events:
                event(events.pop(0))
            for k in range(parts):
                for up_dir in (True, False):
                    await_recv(up_dir, d, sub, k)
                    if d + 1 < line - 1:
                        send(up_dir, d + 1, sub, k)
    for i in events:
        event(i)
    for i in range(6):
        dcopy(i, 1 - core).wait_recv()
        dcopy(i, core).wait_send()
        tcopy(i, False).wait_send()
    for k in range(parts):
        to_y(k).wait_send()
        for d in range(line - 1):
            for sub in range(2):
                await_send(True, d, sub, k)
                await_send(False, d, sub, k)
    for store in stores:
        store.wait()


def gather(gate_w, up_w, down_w, toks, cots):
    line = lax.axis_size("fs") // 2
    wrows, width = gate_w.shape[0], gate_w.shape[1] // 4
    units = [(0, 0, width), (0, width, width), (1, 0, width)]
    parts = len(units)
    depth = 2 * line * wrows
    kind = gate_w.dtype
    dma = pltpu.SemaphoreType.DMA
    zsem = dma((line - 1, 2, parts))
    anyspec = pl.BlockSpec(memory_space=pl.ANY)
    return pl.pallas_call(
        functools.partial(gather_kernel, line, units),
        out_shape=(
            jax.ShapeDtypeStruct((depth, 2 * width), kind),
            jax.ShapeDtypeStruct((depth, width), kind),
            jax.ShapeDtypeStruct((2, 4 * toks.shape[0], toks.shape[1]), toks.dtype),
        ),
        in_specs=[anyspec] * 5,
        out_specs=(anyspec,) * 3,
        scratch_shapes=[
            pltpu.VMEM((parts, wrows, width), kind),
            pltpu.VMEM((2,) + toks.shape, toks.dtype),
            zsem, zsem, zsem, zsem,
            dma((parts,)), dma((parts,)),
            dma((6,)), dma((6,)), dma((6,)), dma((6,)),
            dma((5,)), dma((5,)),
        ],
        compiler_params=pltpu.CompilerParams(collective_id=0, has_side_effects=True),
        name="gather_all",
    )(gate_w, up_w, down_w, toks, cots)


def on_device(inputs, cotangent, gate_weight, up_weight, down_weight):
    tok_rows = inputs.shape[0]
    fs_size = lax.axis_size("fs")
    rep_size = lax.axis_size("rep")
    grad_scale = 1.0 / math.sqrt(tok_rows * fs_size * rep_size)
    if lax.axis_size("tp") == 2 and rep_size == 2 and fs_size >= 8:
        return fused(
            grad_scale, gate_weight, up_weight, down_weight, inputs, cotangent
        )
    contract = (((1,), (1,)), ((), ()))
    contract_tok = (((0,), (0,)), ((), ()))
    width = gate_weight.shape[1] // 4
    gate_up, down_full, tokens = gather(
        gate_weight, up_weight, down_weight, inputs, cotangent
    )
    gate_up_val = jnp.dot(tokens[0], gate_up, preferred_element_type=jnp.float32)
    gate_val, up_val = gate_up_val[:, :width], gate_up_val[:, width:]
    grad_hidden = jnp.dot(tokens[1], down_full, preferred_element_type=jnp.float32)
    sigmoid_gate = jax.nn.sigmoid(gate_val)
    active = gate_val * sigmoid_gate
    hidden = (active * up_val).astype(jnp.bfloat16)
    grad_gate = (
        grad_hidden * up_val * sigmoid_gate * (1.0 + gate_val * (1.0 - sigmoid_gate))
    ).astype(jnp.bfloat16)
    grad_up = (grad_hidden * active).astype(jnp.bfloat16)
    pairs = [[i, i + 1] for i in range(0, fs_size, 2)]
    lines = [list(range(i, fs_size, 2)) for i in range(2)]
    grad_part = lax.dot_general(
        tokens[1], hidden, contract_tok, preferred_element_type=jnp.float32
    )
    part = lax.dot_general(
        jnp.concatenate([grad_gate, grad_up], axis=1), gate_up, contract,
        preferred_element_type=jnp.float32,
    )
    shard = lax.psum_scatter(
        grad_part.astype(jnp.bfloat16), "fs", scatter_dimension=0, tiled=True,
        axis_index_groups=lines,
    ).astype(jnp.float32) * grad_scale
    shard = lax.all_to_all(
        shard, "fs", split_axis=0, concat_axis=1, tiled=True, axis_index_groups=pairs
    )
    grad_down = lax.all_gather(shard, "rep", axis=1, tiled=True)
    part = lax.psum_scatter(
        part.astype(jnp.bfloat16), "rep", scatter_dimension=0, tiled=True
    )
    part = lax.psum_scatter(
        part, "fs", scatter_dimension=0, tiled=True, axis_index_groups=pairs
    )
    grad_input = lax.psum(part, "tp")
    return (grad_input, grad_down)


def solution(mesh):
    placed = (
        P(("rep", "fs"), None),
        P(("rep", "fs"), None),
        P("fs", "tp"),
        P("fs", "tp"),
        P("fs", "tp"),
    )
    return jax.shard_map(
        on_device,
        mesh=mesh,
        in_specs=placed,
        out_specs=(P(("rep", "fs"), None), P("fs", "tp")),
        check_vma=False,
    )
```

```python
import functools
import math

import jax
import jax.numpy as jnp
from jax import lax
from jax.experimental import pallas as pl
from jax.experimental.pallas import tpu as pltpu
from jax.sharding import PartitionSpec as P

MESH = pl.DeviceIdType.MESH


def fused_kernel(
    line, grad_scale, end_a, mid_a, gate_w, up_w, down_w, toks, cots, gi_out, gd_out,
    x, gu, dn_w, acc, hid, ggu, r1, rxa, rxb, rya, ryb, s3a, s3b, g, u_in, d_in, gfin, gl, hl,
    up_s, up_r, dn_s, dn_r, wy_s, wy_r, tok_s, tok_r, d2d_s, d2d_r, loc,
    c_s, c_r, x_s, x_r, yy_s, yy_r, u_s, u_r, d_s, d_r, f_s, f_r, o_s, o_r, e_s, e_r, h_s, h_r,
):
    r = lax.axis_index("rep")
    f = lax.axis_index("fs")
    core = lax.axis_index("tp")
    z, y = f // 2, f % 2
    rows = toks.shape[0]
    half = rows // 2
    wrows = gate_w.shape[0]
    width = gate_w.shape[1] // 4
    depth = 2 * line * wrows
    zrows = 2 * wrows
    cols = depth // 2
    wide = cols // 2
    frows = wrows
    last = line - 2
    has_up, has_dn = z < line - 1, z > 0
    is_end = (z == 0) | (z == line - 1)
    up = {"fs": (f + 2) % (2 * line)}
    dn = {"fs": (f + 2 * line - 2) % (2 * line)}
    ypart = {"fs": f + 1 - 2 * y}
    xpart = {"rep": 1 - r}
    cpart = {"tp": 1 - core}

    barrier = pltpu.get_barrier_semaphore()
    for dev in (ypart, xpart, cpart, up, dn):
        pl.semaphore_signal(barrier, inc=1, device_id=dev, device_id_type=MESH)
    pl.semaphore_wait(barrier, 5)

    def remote(src, dst, s, q, dev):
        return pltpu.make_async_remote_copy(
            src_ref=src, dst_ref=dst, send_sem=s, recv_sem=q,
            device_id=dev, device_id_type=MESH,
        )

    def wblk(k, zz, yy):
        row = pl.multiple_of((2 * zz + yy) * wrows, wrows)
        if k == 2:
            return dn_w.at[pl.ds(row, wrows), :]
        return gu.at[pl.ds(row, wrows), pl.ds(k * width, width)]

    def own(k, yy):
        col = pl.multiple_of((2 * r + yy) * width, width)
        return (gate_w, up_w, down_w)[k].at[:, pl.ds(col, width)]

    def to_y(k):
        return remote(own(k, 1 - y), wblk(k, z, y), wy_s.at[k], wy_r.at[k], ypart)

    def from_y(k):
        return remote(own(k, 1 - y), wblk(k, z, 1 - y), wy_s.at[k], wy_r.at[k], ypart)

    def zcopy(up_dir, d, sub, k, zz):
        yy = y if sub == 0 else 1 - y
        src = own(k, y) if (d == 0 and sub == 0) else wblk(k, zz, yy)
        s, q, dev = (up_s, up_r, up) if up_dir else (dn_s, dn_r, dn)
        return remote(src, wblk(k, zz, yy), s.at[d, sub, k], q.at[d, sub, k], dev)

    def pred_send(up_dir, d):
        return (has_up & (z - d >= 0)) if up_dir else (has_dn & (z + d <= line - 1))

    def src_z(up_dir, d):
        return jnp.maximum(z - d, 0) if up_dir else jnp.minimum(z + d, line - 1)

    def send(up_dir, d, sub, k):
        @pl.when(pred_send(up_dir, d))
        def _():
            zcopy(up_dir, d, sub, k, src_z(up_dir, d)).start()

    def await_send(up_dir, d, sub, k):
        @pl.when(pred_send(up_dir, d))
        def _():
            zcopy(up_dir, d, sub, k, src_z(up_dir, d)).wait_send()

    def await_recv(up_dir, d, sub, k):
        ok = (z - d - 1 >= 0) if up_dir else (z + d + 1 <= line - 1)

        @pl.when(ok)
        def _():
            zcopy(up_dir, d, sub, k, src_z(up_dir, d + 1)).wait_recv()

    def relay(d, sub, k):
        for up_dir in (True, False):
            @pl.when(pred_send(up_dir, d + 1))
            def _():
                zcopy(up_dir, d, sub, k, src_z(up_dir, d + 1)).wait_recv()
                zcopy(up_dir, d + 1, sub, k, src_z(up_dir, d + 1)).start()

    def settle(d, sub, k):
        for up_dir in (True, False):
            ok = (z - d - 1 >= 0) if up_dir else (z + d + 1 <= line - 1)
            onward = has_up if up_dir else has_dn

            @pl.when(ok & jnp.logical_not(onward))
            def _():
                zcopy(up_dir, d, sub, k, src_z(up_dir, d + 1)).wait_recv()

    def slot(rr, yy):
        return pl.multiple_of((2 * rr + yy) * rows, rows)

    kinds = (0, 1, 1, 0, 1, 0, 1, 1)
    over_x = (True, True, True, False, False, True, False, True)
    parts = (2, 0, 1, 2, 2, 2, 0, 1)
    ntok = len(kinds)

    def span(c, p):
        if p == 2:
            return c * half, half
        return c * half + p * (half // 2), half // 2

    def tblk(i, rr, yy, c):
        at, count = span(c, parts[i])
        row = pl.multiple_of((2 * rr + yy) * rows + at, half // 2)
        return x.at[kinds[i], pl.ds(row, count), :]

    def mine(i):
        at, count = span(core, parts[i])
        src = toks if kinds[i] == 0 else cots
        return src.at[pl.ds(pl.multiple_of(at, half // 2), count), :]

    def landing(i, c):
        rr = (1 - r, 1 - r, 1 - r, r, r, 1 - r, 1 - r, 1 - r)[i]
        yy = (y, y, y, 1 - y, 1 - y, 1 - y, 1 - y, 1 - y)[i]
        return tblk(i, rr, yy, c)

    def tcopy(i, land):
        dev = xpart if over_x[i] else ypart
        if land:
            src = dst = landing(i, core)
        else:
            rr = (r, r, r, r, r, r, 1 - r, r)[i]
            yy = (y, y, y, y, y, 1 - y, y, 1 - y)[i]
            dst = tblk(i, rr, yy, core)
            src = mine(i) if i < 5 else dst
        return remote(src, dst, tok_s.at[i], tok_r.at[i], dev)

    def dcopy(i, c):
        blk = landing(i, c)
        return remote(blk, blk, d2d_s.at[i], d2d_r.at[i], cpart)

    def event(i):
        tcopy(i, True).wait_recv()
        onward = {1: 6, 3: 5, 4: 7}.get(i)
        if onward is not None:
            tcopy(onward, False).start()
        dcopy(i, core).start()

    trow = slot(r, y)
    loads = [
        pltpu.make_async_copy(own(0, y), wblk(0, z, y), loc.at[0]),
        pltpu.make_async_copy(own(1, y), wblk(1, z, y), loc.at[1]),
        pltpu.make_async_copy(own(2, y), wblk(2, z, y), loc.at[2]),
        pltpu.make_async_copy(toks, x.at[0, pl.ds(trow, rows), :], loc.at[3]),
        pltpu.make_async_copy(cots, x.at[1, pl.ds(trow, rows), :], loc.at[4]),
    ]

    tile = 256
    z_lo = jnp.maximum(z - last, 0)
    z_hi = jnp.minimum(z + last, line - 1) + 1

    def product(j, row, k0, kk, w, wcol, acol, n):
        at = pl.ds(pl.multiple_of(row, rows), rows)
        kat = pl.ds(pl.multiple_of(k0, wrows), kk)
        for c in range(0, n, tile):
            one = jnp.dot(
                x[j, at, kat], w[kat, pl.ds(wcol + c, tile)],
                preferred_element_type=jnp.float32,
            )
            acc[at, pl.ds(acol + c, tile)] += one

    def forward(j, w, acol, n, first, count):
        @pl.loop(first, first + count)
        def _(b):
            row = ((2 * r + y) + 2 * (b % 2) * (1 - 2 * r) + (b // 2) * (1 - 2 * y)) * rows

            @pl.loop(z_lo, z_hi)
            def _(zz):
                product(j, row, zz * zrows, zrows, w, 0, acol, n)

    def forward_end(j, k, sub):
        for up_dir in (True, False):
            await_recv(up_dir, last, sub, k)

        @pl.when(is_end)
        def _():
            zz = line - 1 - z
            yy = y if sub == 0 else 1 - y
            w = dn_w if k == 2 else gu

            @pl.loop(0, 4)
            def _(b):
                product(
                    j, b * rows, (2 * zz + yy) * wrows, wrows, w,
                    0 if k == 2 else k * width, k * width, width,
                )

    def total(dst, terms, count, step=64):
        @pl.loop(0, count // step)
        def _(i):
            at = pl.multiple_of(i * step, step)
            value = None
            for ref, row, col, wide in terms:
                one = ref[pl.ds(row + at, step), pl.ds(col, wide)].astype(jnp.float32)
                value = one if value is None else value + one
            ref, row, col, wide = dst
            ref[pl.ds(row + at, step), pl.ds(col, wide)] = value.astype(ref.dtype)

    for k in (0, 1):
        to_y(k).start()
        send(True, 0, 0, k)
        send(False, 0, 0, k)
    for i in (0, 1, 3):
        tcopy(i, False).start()
    to_y(2).start()
    tcopy(4, False).start()
    for copy in loads:
        copy.start()

    @pl.loop(0, 4 * rows // 64)
    def _(i):
        at = pl.ds(pl.multiple_of(i * 64, 64), 64)
        acc[at, :] = jnp.zeros((64, 3 * width), jnp.float32)

    for k in (0, 1):
        from_y(k).wait_recv()
        send(True, 0, 1, k)
        send(False, 0, 1, k)
    if last > 0:
        for sub in range(2):
            for k in (0, 1):
                relay(0, sub, k)
    event(0)
    event(3)
    tcopy(2, False).start()
    event(1)
    for d in range(1, last):
        for sub in range(2):
            for k in (0, 1):
                relay(d, sub, k)
    send(True, 0, 0, 2)
    send(False, 0, 0, 2)
    from_y(2).wait_recv()
    send(True, 0, 1, 2)
    send(False, 0, 1, 2)
    for load in loads:
        load.wait()
    for d in range(last):
        for sub in range(2):
            for k in (0, 1):
                settle(d, sub, k)
    dcopy(0, 1 - core).wait_recv()
    dcopy(3, 1 - core).wait_recv()
    forward(0, gu, 0, 2 * width, 0, 3)
    if last > 0:
        for sub in range(2):
            relay(0, sub, 2)
    event(5)
    event(4)
    dcopy(5, 1 - core).wait_recv()
    forward(0, gu, 0, 2 * width, 3, 1)
    for d in range(1, last):
        for sub in range(2):
            relay(d, sub, 2)
    for sub in range(2):
        for k in (0, 1):
            forward_end(0, k, sub)

    @pl.loop(0, 4 * rows // 32)
    def _(i):
        at = pl.ds(pl.multiple_of(i * 32, 32), 32)
        gate = acc[at, pl.ds(0, width)]
        up_val = acc[at, pl.ds(width, width)]
        sig = jax.nn.sigmoid(gate)
        active = gate * sig
        hid[at, :] = (active * up_val).astype(hid.dtype)
        acc[at, pl.ds(0, width)] = up_val * sig * (1.0 + gate * (1.0 - sig))
        acc[at, pl.ds(width, width)] = active

    for i in (2, 6, 7):
        event(i)
    for i in (1, 2, 4, 6, 7):
        dcopy(i, 1 - core).wait_recv()

    zrow = pl.multiple_of(z * zrows, zrows)
    lower = z < line // 2

    def block(ref, zt):
        return ref.at[pl.ds(zt * zrows, zrows), :]

    def up_copy(zt, first):
        return remote(block(g if first else u_in, zt), block(u_in, zt), u_s.at[zt], u_r.at[zt], up)

    def dn_copy(zt, first):
        return remote(block(g if first else d_in, zt), block(d_in, zt), d_s.at[zt], d_r.at[zt], dn)

    def g_block(zt):
        at = pl.multiple_of(zt * zrows, zrows)
        one = lax.dot_general(
            x[1, :, pl.ds(at, zrows)], hid[...], (((0,), (0,)), ((), ())),
            preferred_element_type=jnp.float32,
        )
        g[pl.ds(at, zrows), :] = one.astype(g.dtype)

    def gcol(rr, yy):
        return pl.multiple_of((2 * rr + yy) * width, width)

    def gcols(ref, rr, yy):
        return ref.at[:, pl.ds(gcol(rr, yy), width)]

    def half_rows(ref, row, yy):
        return ref.at[pl.ds(pl.multiple_of(row + yy * frows, frows), frows), :]

    def f_copy(i, land, ref=gfin, row=0):
        if i == 0:
            src, dst, dev = half_rows(ref, row, 1 - y), gcols(gl, r, 1 - y if land else y), ypart
        elif i == 1:
            src, dst, dev = half_rows(ref, row, y), gcols(gl, 1 - r if land else r, y), xpart
        else:
            src, dst, dev = gcols(gl, r, 1 - y), gcols(gl, 1 - r if land else r, 1 - y), xpart
        return remote(src, dst, f_s.at[i], f_r.at[i], dev)

    def e_copy(i, land, ref=gfin, row=0):
        if i == 0:
            src, dst, dev = half_rows(ref, row, 1 - y), gcols(hl, r, 1 - y if land else y), ypart
        elif i == 1:
            src, dst, dev = half_rows(ref, row, y), gcols(hl, 1 - r if land else r, y), xpart
        else:
            src, dst, dev = gcols(hl, r, 1 - y), gcols(hl, 1 - r if land else r, 1 - y), xpart
        return remote(src, dst, e_s.at[i], e_r.at[i], dev)

    end_z = jnp.where((z == 1) | (z == line - 1), 0, line - 1)
    end_dev = {"fs": 2 * end_z + y}
    next_to_end = (z == 1) | (z == line - 2)

    def h_copy(i, ref=gfin, row=0):
        rr, yy = ((r, y), (r, 1 - y), (1 - r, y), (1 - r, 1 - y))[i]
        dst = gcols(hl, rr, yy)
        src = half_rows(ref, row, y) if i == 0 else dst
        return remote(src, dst, h_s.at[i], h_r.at[i], end_dev)

    def share(ref, row):
        h_copy(0, ref, row).start()
        e_copy(0, False, ref, row).start()
        e_copy(1, False, ref, row).start()

    def line_step(t):
        zt = line - 1 + z - t
        row_u = pl.multiple_of(zt * zrows, zrows)
        is_u = (z > 0) & (zt <= line - 1) & (zt > z)
        zd = t - (line - 1 - z)
        row_d = pl.multiple_of(zd * zrows, zrows)
        is_d = (z < line - 1) & (zd >= 0) & (zd < z)
        final = t == line - 2

        @pl.when(is_u)
        def _():
            up_copy(zt, False).wait_recv()
            total((u_in, row_u, 0, width), [(g, row_u, 0, width), (u_in, row_u, 0, width)], zrows)

        @pl.when((is_u & (z < line - 2)) if final else is_u)
        def _():
            up_copy(zt, False).start()

        @pl.when(is_d)
        def _():
            dn_copy(zd, False).wait_recv()
            total((d_in, row_d, 0, width), [(g, row_d, 0, width), (d_in, row_d, 0, width)], zrows)

        @pl.when((is_d & (z > 1)) if final else is_d)
        def _():
            dn_copy(zd, False).start()

        if final:
            @pl.when(z == line - 2)
            def _():
                share(u_in, (line - 1) * zrows)

            @pl.when(z == 1)
            def _():
                share(d_in, 0)

    order = [(1 - r, 1 - y), (1 - r, y), (r, 1 - y), (r, y)]
    my_col = pl.multiple_of(core * cols, cols)
    its_col = pl.multiple_of((1 - core) * cols, cols)
    part = x.at[0]

    def slopes(row, count):
        @pl.loop(0, count // 32)
        def _(i):
            at = pl.ds(pl.multiple_of(row + i * 32, 32), 32)
            grad = acc[at, pl.ds(2 * width, width)]
            ggu[at, pl.ds(0, width)] = (grad * acc[at, pl.ds(0, width)]).astype(ggu.dtype)
            ggu[at, pl.ds(width, width)] = (grad * acc[at, pl.ds(width, width)]).astype(ggu.dtype)

    def back(row, count, col):
        @pl.loop(0, cols // wide)
        def _(n):
            at = pl.multiple_of(col + n * wide, wide)
            one = lax.dot_general(
                ggu[pl.ds(row, count), :], gu[pl.ds(at, wide), :], (((1,), (1,)), ((), ())),
                preferred_element_type=jnp.float32,
            )
            x[0, pl.ds(row, count), pl.ds(at, wide)] = one.astype(x.dtype)

    hrows = rows // 2
    units = [(0, 0, hrows), (0, hrows, hrows), (1, 0, rows), (2, 0, rows), (3, 0, rows)]

    def urow(i):
        b, at, count = units[i]
        return pl.multiple_of(slot(*order[b]) + at, hrows)

    def core_copy(i):
        at = pl.ds(urow(i), units[i][2])
        return remote(part.at[at, pl.ds(its_col, cols)], r1.at[at, :], c_s.at[i], c_r.at[i], cpart)

    def finish(b):
        @pl.when(is_end)
        def _():
            product(
                1, slot(*order[b]), (2 * (line - 1 - z) + 1 - y) * wrows, wrows,
                dn_w, 0, 2 * width, width,
            )

    def theirs(i):
        slopes(urow(i), units[i][2])
        back(urow(i), units[i][2], its_col)
        core_copy(i).start()

    def summed(i):
        back(urow(i), units[i][2], my_col)
        core_copy(i).wait_recv()
        total(
            (part, urow(i), my_col, cols),
            [(part, urow(i), my_col, cols), (r1, urow(i), 0, cols)], units[i][2],
        )

    here_row = slot(r, y)

    def plane_sums(pa):
        pb = cols - pa
        second_col = pl.multiple_of(my_col + pa, 128)

        def mine_a(row, count):
            return part.at[pl.ds(row, count), pl.ds(my_col, pa)]

        def mine_b(row, count):
            return part.at[pl.ds(row, count), pl.ds(second_col, pb)]

        def x_copy(i):
            if i == 3:
                src, dst = s3b.at[:, pl.ds(0, pb)], rxb.at[:, pl.ds(0, pb)]
            elif i == 2:
                src, dst = mine_a(slot(*order[1]), rows), rxa.at[1, :, pl.ds(0, pa)]
            else:
                src, dst = mine_a(urow(i), hrows), rxa.at[0, pl.ds(i * hrows, hrows), pl.ds(0, pa)]
            return remote(src, dst, x_s.at[i], x_r.at[i], xpart)

        def y_copy(i):
            if i == 4:
                src, dst = s3a.at[:, pl.ds(0, pa)], ryb.at[:, pl.ds(0, pa)]
            elif i in (2, 3):
                at = (i - 2) * hrows
                row = pl.multiple_of(slot(*order[2]) + at, hrows)
                src, dst = mine_b(row, hrows), rya.at[1, pl.ds(at, hrows), pl.ds(0, pb)]
            else:
                src, dst = mine_b(urow(i), hrows), rya.at[0, pl.ds(i * hrows, hrows), pl.ds(0, pb)]
            return remote(src, dst, yy_s.at[i], yy_r.at[i], ypart)

        def relay_a():
            for i in (0, 1):
                x_copy(i).wait_recv()
            total(
                (s3a, 0, 0, pa),
                [(part, slot(r, 1 - y), my_col, pa), (rxa.at[0], 0, 0, pa)], rows,
            )
            y_copy(4).start()

        def relay_b():
            for i in (0, 1):
                y_copy(i).wait_recv()
            total(
                (s3b, 0, 0, pb),
                [(part, slot(1 - r, y), second_col, pb), (rya.at[0], 0, 0, pb)], rows,
            )
            x_copy(3).start()

        def o_copy(i, land):
            base = (1 - core if land else core) * cols
            if i == 0:
                at = gi_out.at[:, pl.ds(pl.multiple_of(base, 128), pa)]
            else:
                at = gi_out.at[
                    pl.ds((i - 1) * hrows, hrows), pl.ds(pl.multiple_of(base + pa, 128), pb)
                ]
            return remote(at, at, o_s.at[i], o_r.at[i], cpart)

        def final_a():
            x_copy(2).wait_recv()
            y_copy(4).wait_recv()
            total(
                (gi_out, 0, my_col, pa),
                [
                    (part, here_row, my_col, pa),
                    (rxa.at[1], 0, 0, pa), (ryb, 0, 0, pa),
                ], rows,
            )
            o_copy(0, False).start()

        def final_b(i):
            at = i * hrows
            if i == 0:
                x_copy(3).wait_recv()
            y_copy(2 + i).wait_recv()
            total(
                (gi_out, at, second_col, pb),
                [
                    (part, here_row + at, second_col, pb),
                    (rya.at[1], at, 0, pb), (rxb, at, 0, pb),
                ], hrows,
            )
            o_copy(1 + i, False).start()

        def settled():
            for i in range(5):
                y_copy(i).wait_send()
            for i in range(4):
                x_copy(i).wait_send()
            for i in range(3):
                o_copy(i, True).wait_recv()
                o_copy(i, False).wait_send()

        return x_copy, y_copy, relay_a, relay_b, final_a, final_b, settled

    def scaled(terms, rr, yy):
        at_col = gcol(rr, yy)

        @pl.loop(0, frows // 64)
        def _(m):
            at = pl.multiple_of(m * 64, 64)
            value = None
            for ref, row, col in terms:
                one = ref[pl.ds(row + at, 64), pl.ds(col, width)].astype(jnp.float32)
                value = one if value is None else value + one
            gd_out[pl.ds(at, 64), pl.ds(at_col, width)] = value * grad_scale

    def inputs_sent():
        for i in (0, 3, 5):
            dcopy(i, core).wait_send()
        tcopy(5, False).wait_send()

    @pl.when(is_end)
    def _():
        x_copy, y_copy, relay_a, relay_b, final_a, final_b, settled = plane_sums(end_a)
        for i in range(line):
            g_block(jnp.where(lower, line - 1 - i, i))
            if i < line - 1:
                @pl.when(lower)
                def _():
                    up_copy(line - 1 - i, True).start()

                @pl.when(jnp.logical_not(lower))
                def _():
                    dn_copy(i, True).start()
        f_copy(0, False, g, zrow).start()
        f_copy(1, False, g, zrow).start()
        for d in range(last):
            for sub in range(2):
                settle(d, sub, 2)
        forward(1, dn_w, 2 * width, width, 0, 4)
        f_copy(0, True).wait_recv()
        f_copy(2, False).start()
        forward_end(1, 2, 0)
        for up_dir in (True, False):
            await_recv(up_dir, last, 1, 2)
        inputs_sent()
        finish(0)
        theirs(0)
        theirs(1)
        for i in (0, 1):
            summed(i)
            x_copy(i).start()
            y_copy(i).start()
        finish(1)
        theirs(2)
        summed(2)
        x_copy(2).start()
        finish(2)
        theirs(3)
        summed(3)
        y_copy(2).start()
        finish(3)
        theirs(4)
        summed(4)
        relay_a()
        y_copy(3).start()
        relay_b()
        h_copy(0).wait_recv()
        scaled([(g, pl.multiple_of(zrow + y * frows, frows), 0), (hl, 0, gcol(r, y))], r, y)
        final_a()
        final_b(0)
        for i, (rr, yy) in enumerate(((r, 1 - y), (1 - r, y))):
            if i == 1:
                f_copy(1, True).wait_recv()
            h_copy(1 + i).wait_recv()
            scaled([(gl, 0, gcol(rr, yy)), (hl, 0, gcol(rr, yy))], rr, yy)
        final_b(1)
        f_copy(2, True).wait_recv()
        h_copy(3).wait_recv()
        diag = gcol(1 - r, 1 - y)
        scaled([(gl, 0, diag), (hl, 0, diag)], 1 - r, 1 - y)
        settled()

    @pl.when(jnp.logical_not(is_end))
    def _():
        x_copy, y_copy, relay_a, relay_b, final_a, final_b, settled = plane_sums(mid_a)
        inputs_sent()
        forward(1, dn_w, 2 * width, width, 3, 1)
        theirs(0)
        theirs(1)
        for i in (0, 1):
            summed(i)
            x_copy(i).start()
            y_copy(i).start()
        g_block(jnp.where(lower, line - 1, 0))
        forward(1, dn_w, 2 * width, width, 1, 1)
        theirs(2)
        summed(2)
        x_copy(2).start()
        line_step(1)
        forward(1, dn_w, 2 * width, width, 2, 1)
        theirs(3)
        summed(3)
        y_copy(2).start()
        relay_a()
        relay_b()
        for i in range(1, line):
            g_block(jnp.where(lower, line - 1 - i, i))
        for t in range(2, line - 1):
            line_step(t)
        forward(1, dn_w, 2 * width, width, 0, 1)
        theirs(4)
        summed(4)
        up_copy(z, False).wait_recv()
        dn_copy(z, False).wait_recv()
        total(
            (gfin, 0, 0, width),
            [(g, zrow, 0, width), (u_in, zrow, 0, width), (d_in, zrow, 0, width)], zrows,
        )
        f_copy(0, False).start()
        y_copy(3).start()
        scaled([(gfin, pl.multiple_of(y * frows, frows), 0)], r, y)

        @pl.when(next_to_end)
        def _():
            e_copy(0, True).wait_recv()
            e_copy(2, False).start()
            h_copy(1).start()
            e_copy(1, True).wait_recv()
            h_copy(2).start()

        f_copy(1, False).start()
        final_a()
        final_b(0)

        @pl.when(next_to_end)
        def _():
            e_copy(2, True).wait_recv()
            h_copy(3).start()

        f_copy(0, True).wait_recv()
        f_copy(2, False).start()
        scaled([(gl, 0, gcol(r, 1 - y))], r, 1 - y)
        f_copy(1, True).wait_recv()
        scaled([(gl, 0, gcol(1 - r, y))], 1 - r, y)
        final_b(1)
        f_copy(2, True).wait_recv()
        scaled([(gl, 0, gcol(1 - r, 1 - y))], 1 - r, 1 - y)

        @pl.when(next_to_end)
        def _():
            for i in range(3):
                e_copy(i, False).wait_send()
            for i in range(4):
                h_copy(i).wait_send()

        settled()

    for i in range(ntok):
        if kinds[i] == 1:
            dcopy(i, core).wait_send()
        if i != 5:
            tcopy(i, False).wait_send()
    for k in range(3):
        to_y(k).wait_send()
        for d in range(line - 1):
            for sub in range(2):
                await_send(True, d, sub, k)
                await_send(False, d, sub, k)
    for i in range(5):
        core_copy(i).wait_send()
    for i in range(3):
        f_copy(i, False).wait_send()
    for zt in range(line):
        if zt > 0:
            far = line - 2 if zt == line - 1 else zt
            pl.when(z < far)(lambda: up_copy(zt, True).wait_send())
        if zt < line - 1:
            near = 1 if zt == 0 else zt
            pl.when(z > near)(lambda: dn_copy(zt, True).wait_send())


def fused(grad_scale, gate_w, up_w, down_w, toks, cots):
    line = lax.axis_size("fs") // 2
    rows, full = toks.shape
    wrows, width = gate_w.shape[0], gate_w.shape[1] // 4
    depth = 2 * line * wrows
    cols = full // 2
    kind = gate_w.dtype
    dma = pltpu.SemaphoreType.DMA
    zsem = dma((line - 1, 2, 3))
    anyspec = pl.BlockSpec(memory_space=pl.ANY)
    whole = pltpu.VMEM((depth, width), kind)
    end_a, mid_a = cols // 2, cols * 3 // 8 // 128 * 128
    most_b = cols - mid_a
    return pl.pallas_call(
        functools.partial(fused_kernel, line, grad_scale, end_a, mid_a),
        out_shape=(
            pltpu.VMEM((rows, full), kind),
            pltpu.VMEM((wrows, 4 * width), jnp.float32),
        ),
        in_specs=[anyspec] * 5,
        out_specs=(pl.BlockSpec(memory_space=pltpu.VMEM),) * 2,
        scratch_shapes=[
            pltpu.VMEM((2, 4 * rows, full), kind),
            pltpu.VMEM((depth, 2 * width), kind),
            whole,
            pltpu.VMEM((4 * rows, 3 * width), jnp.float32),
            pltpu.VMEM((4 * rows, width), kind),
            pltpu.VMEM((4 * rows, 2 * width), kind),
            pltpu.VMEM((4 * rows, cols), kind),
            pltpu.VMEM((2, rows, end_a), kind), pltpu.VMEM((rows, most_b), kind),
            pltpu.VMEM((2, rows, most_b), kind), pltpu.VMEM((rows, end_a), kind),
            pltpu.VMEM((rows, end_a), kind), pltpu.VMEM((rows, most_b), kind),
            whole, whole, whole,
            pltpu.VMEM((2 * wrows, width), kind),
            pltpu.VMEM((wrows, 4 * width), kind),
            pltpu.VMEM((wrows, 4 * width), kind),
            zsem, zsem, zsem, zsem,
            dma((3,)), dma((3,)),
            dma((8,)), dma((8,)), dma((8,)), dma((8,)), dma((5,)),
            dma((5,)), dma((5,)), dma((4,)), dma((4,)), dma((5,)), dma((5,)),
            dma((line,)), dma((line,)), dma((line,)), dma((line,)),
            dma((3,)), dma((3,)), dma((3,)), dma((3,)),
            dma((3,)), dma((3,)), dma((4,)), dma((4,)),
        ],
        compiler_params=pltpu.CompilerParams(
            collective_id=1, has_side_effects=True, vmem_limit_bytes=59 * 2**20
        ),
        name="fused_all",
    )(gate_w, up_w, down_w, toks, cots)


def place_kernel(a, b, a_out, b_out, sems):
    copies = [
        pltpu.make_async_copy(a, a_out, sems.at[0]),
        pltpu.make_async_copy(b, b_out, sems.at[1]),
    ]
    for copy in copies:
        copy.start()
    for copy in copies:
        copy.wait()


def place(a, b):
    anyspec = pl.BlockSpec(memory_space=pl.ANY)
    return pl.pallas_call(
        place_kernel,
        out_shape=(
            jax.ShapeDtypeStruct(a.shape, a.dtype), jax.ShapeDtypeStruct(b.shape, b.dtype),
        ),
        in_specs=[pl.BlockSpec(memory_space=pltpu.VMEM)] * 2,
        out_specs=(anyspec,) * 2,
        scratch_shapes=[pltpu.SemaphoreType.DMA((2,))],
        compiler_params=pltpu.CompilerParams(vmem_limit_bytes=16 * 2**20),
        name="place",
    )(a, b)


def gather_kernel(
    line, units, gate_w, up_w, down_w, toks, cots, gu_out, d_out, t_out, w_tmp, t_tmp,
    up_s, up_r, dn_s, dn_r, y_s, y_r, tok_s, tok_r, d2d_s, d2d_r, loc, loc2,
):
    r = lax.axis_index("rep")
    f = lax.axis_index("fs")
    t = lax.axis_index("tp")
    z, y = f // 2, f % 2
    rows = toks.shape[0]
    half = rows // 2
    wrows = gate_w.shape[0]
    width = gate_w.shape[1] // 4
    parts = len(units)
    has_up, has_dn = z < line - 1, z > 0
    up = {"fs": (f + 2) % (2 * line)}
    dn = {"fs": (f + 2 * line - 2) % (2 * line)}
    ypart = {"fs": f + 1 - 2 * y}
    xpart = {"rep": 1 - r}
    core = t % 2
    cpart = {"tp": t + 1 - 2 * core}

    barrier = pltpu.get_barrier_semaphore()

    def greet(dev):
        pl.semaphore_signal(barrier, inc=1, device_id=dev, device_id_type=MESH)

    for dev in (ypart, xpart, cpart, up, dn):
        greet(dev)
    pl.semaphore_wait(barrier, 5)

    def remote(src, dst, s, q, dev):
        return pltpu.make_async_remote_copy(
            src_ref=src, dst_ref=dst, send_sem=s, recv_sem=q,
            device_id=dev, device_id_type=MESH,
        )

    def wblk(k, zz, yy):
        row = pl.multiple_of((2 * zz + yy) * wrows, wrows)
        which, col, wide = units[k]
        return (gu_out, d_out)[which].at[pl.ds(row, wrows), pl.ds(col, wide)]

    def own(k, yy):
        col = pl.multiple_of((2 * r + yy) * width, width)
        return (gate_w, up_w, down_w)[k].at[:, pl.ds(col, width)]

    def to_y(k):
        return remote(own(k, 1 - y), wblk(k, z, y), y_s.at[k], y_r.at[k], ypart)

    def from_y(k):
        return remote(own(k, 1 - y), wblk(k, z, 1 - y), y_s.at[k], y_r.at[k], ypart)

    def zcopy(up_dir, d, sub, k, zz):
        yy = y if sub == 0 else 1 - y
        src = own(k, y) if (d == 0 and sub == 0) else wblk(k, zz, yy)
        s, q, dev = (up_s, up_r, up) if up_dir else (dn_s, dn_r, dn)
        return remote(src, wblk(k, zz, yy), s.at[d, sub, k], q.at[d, sub, k], dev)

    def pred_send(up_dir, d):
        return (has_up & (z - d >= 0)) if up_dir else (has_dn & (z + d <= line - 1))

    def src_z(up_dir, d):
        return jnp.maximum(z - d, 0) if up_dir else jnp.minimum(z + d, line - 1)

    def send(up_dir, d, sub, k):
        @pl.when(pred_send(up_dir, d))
        def _():
            zcopy(up_dir, d, sub, k, src_z(up_dir, d)).start()

    def await_send(up_dir, d, sub, k):
        @pl.when(pred_send(up_dir, d))
        def _():
            zcopy(up_dir, d, sub, k, src_z(up_dir, d)).wait_send()

    def await_recv(up_dir, d, sub, k):
        ok = (z - d - 1 >= 0) if up_dir else (z + d + 1 <= line - 1)

        @pl.when(ok)
        def _():
            zcopy(up_dir, d, sub, k, src_z(up_dir, d + 1)).wait_recv()

    def tblk(j, rr, yy, c):
        row = pl.multiple_of((2 * rr + yy) * rows + c * half, half)
        return t_out.at[j, pl.ds(row, half), :]

    def mine(j):
        src = toks if j == 0 else cots
        return src.at[pl.ds(pl.multiple_of(core * half, half), half), :]

    def tcopy(i, landing):
        j = (0, 1, 0, 1, 0, 1)[i]
        dev = xpart if i in (0, 1, 5) else ypart
        if landing:
            rr = (1 - r, 1 - r, r, r, 1 - r, 1 - r)[i]
            yy = (y, y, 1 - y, 1 - y, 1 - y, 1 - y)[i]
            src = dst = tblk(j, rr, yy, core)
        else:
            rr = (r, r, r, r, 1 - r, r)[i]
            yy = (y, y, y, y, y, 1 - y)[i]
            dst = tblk(j, rr, yy, core)
            src = mine(j) if i < 4 else dst
        return remote(src, dst, tok_s.at[i], tok_r.at[i], dev)

    def dcopy(i, c):
        j = (0, 1, 0, 1, 0, 1)[i]
        rr = (1 - r, 1 - r, r, r, 1 - r, 1 - r)[i]
        yy = (y, y, 1 - y, 1 - y, 1 - y, 1 - y)[i]
        blk = tblk(j, rr, yy, c)
        return remote(blk, blk, d2d_s.at[i], d2d_r.at[i], cpart)

    loads = [
        pltpu.make_async_copy(own(0, y), w_tmp.at[0], loc.at[0]),
        pltpu.make_async_copy(own(1, y), w_tmp.at[1], loc.at[3]),
        pltpu.make_async_copy(own(2, y), w_tmp.at[2], loc.at[4]),
        pltpu.make_async_copy(toks, t_tmp.at[0], loc.at[1]),
        pltpu.make_async_copy(cots, t_tmp.at[1], loc.at[2]),
    ]
    trow = pl.multiple_of((2 * r + y) * rows, rows)
    stores = [
        pltpu.make_async_copy(w_tmp.at[0], wblk(0, z, y), loc2.at[0]),
        pltpu.make_async_copy(w_tmp.at[1], wblk(1, z, y), loc2.at[3]),
        pltpu.make_async_copy(w_tmp.at[2], wblk(2, z, y), loc2.at[4]),
        pltpu.make_async_copy(t_tmp.at[0], t_out.at[0, pl.ds(trow, rows), :], loc2.at[1]),
        pltpu.make_async_copy(t_tmp.at[1], t_out.at[1, pl.ds(trow, rows), :], loc2.at[2]),
    ]

    for k in range(parts):
        to_y(k).start()
        send(True, 0, 0, k)
        send(False, 0, 0, k)
    for i in (0, 1, 3, 2):
        tcopy(i, False).start()
    for copy in loads:
        copy.start()
    for load, store in zip(loads, stores):
        load.wait()
        store.start()
    for k in range(parts):
        from_y(k).wait_recv()
        send(True, 0, 1, k)
        send(False, 0, 1, k)

    def event(i):
        tcopy(i, True).wait_recv()
        if i == 0:
            tcopy(4, False).start()
        if i == 3:
            tcopy(5, False).start()
        dcopy(i, core).start()

    events = [0, 3, 1, 2, 5, 4]
    for d in range(line - 1):
        for sub in range(2):
            if events:
                event(events.pop(0))
            for k in range(parts):
                for up_dir in (True, False):
                    await_recv(up_dir, d, sub, k)
                    if d + 1 < line - 1:
                        send(up_dir, d + 1, sub, k)
    for i in events:
        event(i)
    for i in range(6):
        dcopy(i, 1 - core).wait_recv()
        dcopy(i, core).wait_send()
        tcopy(i, False).wait_send()
    for k in range(parts):
        to_y(k).wait_send()
        for d in range(line - 1):
            for sub in range(2):
                await_send(True, d, sub, k)
                await_send(False, d, sub, k)
    for store in stores:
        store.wait()


def gather(gate_w, up_w, down_w, toks, cots):
    line = lax.axis_size("fs") // 2
    wrows, width = gate_w.shape[0], gate_w.shape[1] // 4
    units = [(0, 0, width), (0, width, width), (1, 0, width)]
    parts = len(units)
    depth = 2 * line * wrows
    kind = gate_w.dtype
    dma = pltpu.SemaphoreType.DMA
    zsem = dma((line - 1, 2, parts))
    anyspec = pl.BlockSpec(memory_space=pl.ANY)
    return pl.pallas_call(
        functools.partial(gather_kernel, line, units),
        out_shape=(
            jax.ShapeDtypeStruct((depth, 2 * width), kind),
            jax.ShapeDtypeStruct((depth, width), kind),
            jax.ShapeDtypeStruct((2, 4 * toks.shape[0], toks.shape[1]), toks.dtype),
        ),
        in_specs=[anyspec] * 5,
        out_specs=(anyspec,) * 3,
        scratch_shapes=[
            pltpu.VMEM((parts, wrows, width), kind),
            pltpu.VMEM((2,) + toks.shape, toks.dtype),
            zsem, zsem, zsem, zsem,
            dma((parts,)), dma((parts,)),
            dma((6,)), dma((6,)), dma((6,)), dma((6,)),
            dma((5,)), dma((5,)),
        ],
        compiler_params=pltpu.CompilerParams(collective_id=0, has_side_effects=True),
        name="gather_all",
    )(gate_w, up_w, down_w, toks, cots)


def on_device(inputs, cotangent, gate_weight, up_weight, down_weight):
    tok_rows = inputs.shape[0]
    fs_size = lax.axis_size("fs")
    rep_size = lax.axis_size("rep")
    grad_scale = 1.0 / math.sqrt(tok_rows * fs_size * rep_size)
    if lax.axis_size("tp") == 2 and rep_size == 2 and fs_size >= 8:
        return place(*fused(
            grad_scale, gate_weight, up_weight, down_weight, inputs, cotangent
        ))
    contract = (((1,), (1,)), ((), ()))
    contract_tok = (((0,), (0,)), ((), ()))
    width = gate_weight.shape[1] // 4
    gate_up, down_full, tokens = gather(
        gate_weight, up_weight, down_weight, inputs, cotangent
    )
    gate_up_val = jnp.dot(tokens[0], gate_up, preferred_element_type=jnp.float32)
    gate_val, up_val = gate_up_val[:, :width], gate_up_val[:, width:]
    grad_hidden = jnp.dot(tokens[1], down_full, preferred_element_type=jnp.float32)
    sigmoid_gate = jax.nn.sigmoid(gate_val)
    active = gate_val * sigmoid_gate
    hidden = (active * up_val).astype(jnp.bfloat16)
    grad_gate = (
        grad_hidden * up_val * sigmoid_gate * (1.0 + gate_val * (1.0 - sigmoid_gate))
    ).astype(jnp.bfloat16)
    grad_up = (grad_hidden * active).astype(jnp.bfloat16)
    pairs = [[i, i + 1] for i in range(0, fs_size, 2)]
    lines = [list(range(i, fs_size, 2)) for i in range(2)]
    grad_part = lax.dot_general(
        tokens[1], hidden, contract_tok, preferred_element_type=jnp.float32
    )
    part = lax.dot_general(
        jnp.concatenate([grad_gate, grad_up], axis=1), gate_up, contract,
        preferred_element_type=jnp.float32,
    )
    shard = lax.psum_scatter(
        grad_part.astype(jnp.bfloat16), "fs", scatter_dimension=0, tiled=True,
        axis_index_groups=lines,
    ).astype(jnp.float32) * grad_scale
    shard = lax.all_to_all(
        shard, "fs", split_axis=0, concat_axis=1, tiled=True, axis_index_groups=pairs
    )
    grad_down = lax.all_gather(shard, "rep", axis=1, tiled=True)
    part = lax.psum_scatter(
        part.astype(jnp.bfloat16), "rep", scatter_dimension=0, tiled=True
    )
    part = lax.psum_scatter(
        part, "fs", scatter_dimension=0, tiled=True, axis_index_groups=pairs
    )
    grad_input = lax.psum(part, "tp")
    return (grad_input, grad_down)


def solution(mesh):
    placed = (
        P(("rep", "fs"), None),
        P(("rep", "fs"), None),
        P("fs", "tp"),
        P("fs", "tp"),
        P("fs", "tp"),
    )
    return jax.shard_map(
        on_device,
        mesh=mesh,
        in_specs=placed,
        out_specs=(P(("rep", "fs"), None), P("fs", "tp")),
        check_vma=False,
    )
```

```python
import functools
import math

import jax
import jax.numpy as jnp
from jax import lax
from jax.experimental import pallas as pl
from jax.experimental.pallas import tpu as pltpu
from jax.sharding import PartitionSpec as P

MESH = pl.DeviceIdType.MESH


def fused_kernel(
    line, grad_scale, end_a, mid_a, gate_w, up_w, down_w, toks, cots, gi_out, gd_out,
    x, gu, dn_w, acc, hid, ggu, r1, rxa, rxb, rya, ryb, s3a, s3b, g, u_in, d_in, gfin, gl, hl,
    up_s, up_r, dn_s, dn_r, wy_s, wy_r, tok_s, tok_r, d2d_s, d2d_r, loc,
    c_s, c_r, x_s, x_r, yy_s, yy_r, u_s, u_r, d_s, d_r, f_s, f_r, o_s, o_r, e_s, e_r, h_s, h_r,
):
    r = lax.axis_index("rep")
    f = lax.axis_index("fs")
    core = lax.axis_index("tp")
    z, y = f // 2, f % 2
    rows = toks.shape[0]
    half = rows // 2
    wrows = gate_w.shape[0]
    width = gate_w.shape[1] // 4
    depth = 2 * line * wrows
    zrows = 2 * wrows
    cols = depth // 2
    wide = cols // 2
    frows = wrows
    last = line - 2
    has_up, has_dn = z < line - 1, z > 0
    is_end = (z == 0) | (z == line - 1)
    up = {"fs": (f + 2) % (2 * line)}
    dn = {"fs": (f + 2 * line - 2) % (2 * line)}
    ypart = {"fs": f + 1 - 2 * y}
    xpart = {"rep": 1 - r}
    cpart = {"tp": 1 - core}

    barrier = pltpu.get_barrier_semaphore()
    for dev in (ypart, xpart, cpart, up, dn):
        pl.semaphore_signal(barrier, inc=1, device_id=dev, device_id_type=MESH)
    pl.semaphore_wait(barrier, 5)

    def remote(src, dst, s, q, dev):
        return pltpu.make_async_remote_copy(
            src_ref=src, dst_ref=dst, send_sem=s, recv_sem=q,
            device_id=dev, device_id_type=MESH,
        )

    def wblk(k, zz, yy):
        row = pl.multiple_of((2 * zz + yy) * wrows, wrows)
        if k == 2:
            return dn_w.at[pl.ds(row, wrows), :]
        return gu.at[pl.ds(row, wrows), pl.ds(k * width, width)]

    def own(k, yy):
        col = pl.multiple_of((2 * r + yy) * width, width)
        return (gate_w, up_w, down_w)[k].at[:, pl.ds(col, width)]

    def to_y(k):
        return remote(own(k, 1 - y), wblk(k, z, y), wy_s.at[k], wy_r.at[k], ypart)

    def from_y(k):
        return remote(own(k, 1 - y), wblk(k, z, 1 - y), wy_s.at[k], wy_r.at[k], ypart)

    def zcopy(up_dir, d, sub, k, zz):
        yy = y if sub == 0 else 1 - y
        src = own(k, y) if (d == 0 and sub == 0) else wblk(k, zz, yy)
        s, q, dev = (up_s, up_r, up) if up_dir else (dn_s, dn_r, dn)
        return remote(src, wblk(k, zz, yy), s.at[d, sub, k], q.at[d, sub, k], dev)

    def pred_send(up_dir, d):
        return (has_up & (z - d >= 0)) if up_dir else (has_dn & (z + d <= line - 1))

    def src_z(up_dir, d):
        return jnp.maximum(z - d, 0) if up_dir else jnp.minimum(z + d, line - 1)

    def send(up_dir, d, sub, k):
        @pl.when(pred_send(up_dir, d))
        def _():
            zcopy(up_dir, d, sub, k, src_z(up_dir, d)).start()

    def await_send(up_dir, d, sub, k):
        @pl.when(pred_send(up_dir, d))
        def _():
            zcopy(up_dir, d, sub, k, src_z(up_dir, d)).wait_send()

    def await_recv(up_dir, d, sub, k):
        ok = (z - d - 1 >= 0) if up_dir else (z + d + 1 <= line - 1)

        @pl.when(ok)
        def _():
            zcopy(up_dir, d, sub, k, src_z(up_dir, d + 1)).wait_recv()

    def relay(d, sub, k):
        for up_dir in (True, False):
            @pl.when(pred_send(up_dir, d + 1))
            def _():
                zcopy(up_dir, d, sub, k, src_z(up_dir, d + 1)).wait_recv()
                zcopy(up_dir, d + 1, sub, k, src_z(up_dir, d + 1)).start()

    def settle(d, sub, k):
        for up_dir in (True, False):
            ok = (z - d - 1 >= 0) if up_dir else (z + d + 1 <= line - 1)
            onward = has_up if up_dir else has_dn

            @pl.when(ok & jnp.logical_not(onward))
            def _():
                zcopy(up_dir, d, sub, k, src_z(up_dir, d + 1)).wait_recv()

    def slot(rr, yy):
        return pl.multiple_of((2 * rr + yy) * rows, rows)

    kinds = (0, 1, 1, 0, 1, 0, 1, 1)
    over_x = (True, True, True, False, False, True, False, True)
    parts = (2, 0, 1, 2, 2, 2, 0, 1)
    ntok = len(kinds)

    def span(c, p):
        if p == 2:
            return c * half, half
        return c * half + p * (half // 2), half // 2

    def tblk(i, rr, yy, c):
        at, count = span(c, parts[i])
        row = pl.multiple_of((2 * rr + yy) * rows + at, half // 2)
        return x.at[kinds[i], pl.ds(row, count), :]

    def mine(i):
        at, count = span(core, parts[i])
        src = toks if kinds[i] == 0 else cots
        return src.at[pl.ds(pl.multiple_of(at, half // 2), count), :]

    def landing(i, c):
        rr = (1 - r, 1 - r, 1 - r, r, r, 1 - r, 1 - r, 1 - r)[i]
        yy = (y, y, y, 1 - y, 1 - y, 1 - y, 1 - y, 1 - y)[i]
        return tblk(i, rr, yy, c)

    def tcopy(i, land):
        dev = xpart if over_x[i] else ypart
        if land:
            src = dst = landing(i, core)
        else:
            rr = (r, r, r, r, r, r, 1 - r, r)[i]
            yy = (y, y, y, y, y, 1 - y, y, 1 - y)[i]
            dst = tblk(i, rr, yy, core)
            src = mine(i) if i < 5 else dst
        return remote(src, dst, tok_s.at[i], tok_r.at[i], dev)

    def dcopy(i, c):
        blk = landing(i, c)
        return remote(blk, blk, d2d_s.at[i], d2d_r.at[i], cpart)

    def event(i):
        tcopy(i, True).wait_recv()
        onward = {1: 6, 3: 5, 4: 7}.get(i)
        if onward is not None:
            tcopy(onward, False).start()
        dcopy(i, core).start()

    trow = slot(r, y)
    loads = [
        pltpu.make_async_copy(own(0, y), wblk(0, z, y), loc.at[0]),
        pltpu.make_async_copy(own(1, y), wblk(1, z, y), loc.at[1]),
        pltpu.make_async_copy(own(2, y), wblk(2, z, y), loc.at[2]),
        pltpu.make_async_copy(toks, x.at[0, pl.ds(trow, rows), :], loc.at[3]),
        pltpu.make_async_copy(cots, x.at[1, pl.ds(trow, rows), :], loc.at[4]),
    ]

    tile = 256
    z_lo = jnp.maximum(z - last, 0)
    z_hi = jnp.minimum(z + last, line - 1) + 1

    def product(j, row, k0, kk, w, wcol, acol, n):
        at = pl.ds(pl.multiple_of(row, rows), rows)
        kat = pl.ds(pl.multiple_of(k0, wrows), kk)
        for c in range(0, n, tile):
            one = jnp.dot(
                x[j, at, kat], w[kat, pl.ds(wcol + c, tile)],
                preferred_element_type=jnp.float32,
            )
            acc[at, pl.ds(acol + c, tile)] += one

    def forward(j, w, acol, n, first, count):
        @pl.loop(first, first + count)
        def _(b):
            row = ((2 * r + y) + 2 * (b % 2) * (1 - 2 * r) + (b // 2) * (1 - 2 * y)) * rows

            @pl.loop(z_lo, z_hi)
            def _(zz):
                product(j, row, zz * zrows, zrows, w, 0, acol, n)

    def forward_end(j, k, sub):
        for up_dir in (True, False):
            await_recv(up_dir, last, sub, k)

        @pl.when(is_end)
        def _():
            zz = line - 1 - z
            yy = y if sub == 0 else 1 - y
            w = dn_w if k == 2 else gu

            @pl.loop(0, 4)
            def _(b):
                product(
                    j, b * rows, (2 * zz + yy) * wrows, wrows, w,
                    0 if k == 2 else k * width, k * width, width,
                )

    def total(dst, terms, count, step=64):
        @pl.loop(0, count // step)
        def _(i):
            at = pl.multiple_of(i * step, step)
            value = None
            for ref, row, col, wide in terms:
                one = ref[pl.ds(row + at, step), pl.ds(col, wide)].astype(jnp.float32)
                value = one if value is None else value + one
            ref, row, col, wide = dst
            ref[pl.ds(row + at, step), pl.ds(col, wide)] = value.astype(ref.dtype)

    for k in (0, 1):
        to_y(k).start()
        send(True, 0, 0, k)
        send(False, 0, 0, k)
    for i in (0, 1, 3):
        tcopy(i, False).start()
    to_y(2).start()
    tcopy(4, False).start()
    for copy in loads:
        copy.start()

    @pl.loop(0, 4 * rows // 64)
    def _(i):
        at = pl.ds(pl.multiple_of(i * 64, 64), 64)
        acc[at, :] = jnp.zeros((64, 3 * width), jnp.float32)

    for k in (0, 1):
        from_y(k).wait_recv()
        send(True, 0, 1, k)
        send(False, 0, 1, k)
    if last > 0:
        for sub in range(2):
            for k in (0, 1):
                relay(0, sub, k)
    event(0)
    event(3)
    tcopy(2, False).start()
    event(1)
    for d in range(1, last):
        for sub in range(2):
            for k in (0, 1):
                relay(d, sub, k)
    send(True, 0, 0, 2)
    send(False, 0, 0, 2)
    from_y(2).wait_recv()
    send(True, 0, 1, 2)
    send(False, 0, 1, 2)
    for load in loads:
        load.wait()
    for d in range(last):
        for sub in range(2):
            for k in (0, 1):
                settle(d, sub, k)
    dcopy(0, 1 - core).wait_recv()
    dcopy(3, 1 - core).wait_recv()
    forward(0, gu, 0, 2 * width, 0, 3)
    if last > 0:
        for sub in range(2):
            relay(0, sub, 2)
    event(5)
    event(4)
    dcopy(5, 1 - core).wait_recv()
    forward(0, gu, 0, 2 * width, 3, 1)
    for d in range(1, last):
        for sub in range(2):
            relay(d, sub, 2)
    for sub in range(2):
        for k in (0, 1):
            forward_end(0, k, sub)

    @pl.loop(0, 4 * rows // 32)
    def _(i):
        at = pl.ds(pl.multiple_of(i * 32, 32), 32)
        gate = acc[at, pl.ds(0, width)]
        up_val = acc[at, pl.ds(width, width)]
        sig = jax.nn.sigmoid(gate)
        active = gate * sig
        hid[at, :] = (active * up_val).astype(hid.dtype)
        acc[at, pl.ds(0, width)] = up_val * sig * (1.0 + gate * (1.0 - sig))
        acc[at, pl.ds(width, width)] = active

    for i in (2, 6, 7):
        event(i)
    for i in (1, 2, 4, 6, 7):
        dcopy(i, 1 - core).wait_recv()

    zrow = pl.multiple_of(z * zrows, zrows)
    lower = z < line // 2

    def block(ref, zt):
        return ref.at[pl.ds(zt * zrows, zrows), :]

    def up_copy(zt, first):
        return remote(block(g if first else u_in, zt), block(u_in, zt), u_s.at[zt], u_r.at[zt], up)

    def dn_copy(zt, first):
        return remote(block(g if first else d_in, zt), block(d_in, zt), d_s.at[zt], d_r.at[zt], dn)

    def g_block(zt):
        at = pl.multiple_of(zt * zrows, zrows)
        one = lax.dot_general(
            x[1, :, pl.ds(at, zrows)], hid[...], (((0,), (0,)), ((), ())),
            preferred_element_type=jnp.float32,
        )
        g[pl.ds(at, zrows), :] = one.astype(g.dtype)

    def gcol(rr, yy):
        return pl.multiple_of((2 * rr + yy) * width, width)

    def gcols(ref, rr, yy):
        return ref.at[:, pl.ds(gcol(rr, yy), width)]

    def half_rows(ref, row, yy):
        return ref.at[pl.ds(pl.multiple_of(row + yy * frows, frows), frows), :]

    def f_copy(i, land, ref=gfin, row=0):
        if i == 0:
            src, dst, dev = half_rows(ref, row, 1 - y), gcols(gl, r, 1 - y if land else y), ypart
        elif i == 1:
            src, dst, dev = half_rows(ref, row, y), gcols(gl, 1 - r if land else r, y), xpart
        else:
            src, dst, dev = gcols(gl, r, 1 - y), gcols(gl, 1 - r if land else r, 1 - y), xpart
        return remote(src, dst, f_s.at[i], f_r.at[i], dev)

    def e_copy(i, land, ref=gfin, row=0):
        if i == 0:
            src, dst, dev = half_rows(ref, row, 1 - y), gcols(hl, r, 1 - y if land else y), ypart
        elif i == 1:
            src, dst, dev = half_rows(ref, row, y), gcols(hl, 1 - r if land else r, y), xpart
        else:
            src, dst, dev = gcols(hl, r, 1 - y), gcols(hl, 1 - r if land else r, 1 - y), xpart
        return remote(src, dst, e_s.at[i], e_r.at[i], dev)

    end_z = jnp.where((z == 1) | (z == line - 1), 0, line - 1)
    end_dev = {"fs": 2 * end_z + y}
    next_to_end = (z == 1) | (z == line - 2)

    def h_copy(i, ref=gfin, row=0):
        rr, yy = ((r, y), (r, 1 - y), (1 - r, y), (1 - r, 1 - y))[i]
        dst = gcols(hl, rr, yy)
        src = half_rows(ref, row, y) if i == 0 else dst
        return remote(src, dst, h_s.at[i], h_r.at[i], end_dev)

    def share(ref, row):
        h_copy(0, ref, row).start()
        e_copy(0, False, ref, row).start()
        e_copy(1, False, ref, row).start()

    def line_step(t):
        zt = line - 1 + z - t
        row_u = pl.multiple_of(zt * zrows, zrows)
        is_u = (z > 0) & (zt <= line - 1) & (zt > z)
        zd = t - (line - 1 - z)
        row_d = pl.multiple_of(zd * zrows, zrows)
        is_d = (z < line - 1) & (zd >= 0) & (zd < z)
        final = t == line - 2

        @pl.when(is_u)
        def _():
            up_copy(zt, False).wait_recv()
            total((u_in, row_u, 0, width), [(g, row_u, 0, width), (u_in, row_u, 0, width)], zrows)

        @pl.when((is_u & (z < line - 2)) if final else is_u)
        def _():
            up_copy(zt, False).start()

        @pl.when(is_d)
        def _():
            dn_copy(zd, False).wait_recv()
            total((d_in, row_d, 0, width), [(g, row_d, 0, width), (d_in, row_d, 0, width)], zrows)

        @pl.when((is_d & (z > 1)) if final else is_d)
        def _():
            dn_copy(zd, False).start()

        if final:
            @pl.when(z == line - 2)
            def _():
                share(u_in, (line - 1) * zrows)

            @pl.when(z == 1)
            def _():
                share(d_in, 0)

    order = [(1 - r, 1 - y), (1 - r, y), (r, 1 - y), (r, y)]
    my_col = pl.multiple_of(core * cols, cols)
    its_col = pl.multiple_of((1 - core) * cols, cols)
    part = x.at[0]

    def slopes(row, count):
        @pl.loop(0, count // 32)
        def _(i):
            at = pl.ds(pl.multiple_of(row + i * 32, 32), 32)
            grad = acc[at, pl.ds(2 * width, width)]
            ggu[at, pl.ds(0, width)] = (grad * acc[at, pl.ds(0, width)]).astype(ggu.dtype)
            ggu[at, pl.ds(width, width)] = (grad * acc[at, pl.ds(width, width)]).astype(ggu.dtype)

    def back(row, count, col, n):
        step = min(n, wide) if n % wide == 0 else n

        @pl.loop(0, n // step)
        def _(i):
            at = pl.multiple_of(col + i * step, 128)
            one = lax.dot_general(
                ggu[pl.ds(row, count), :], gu[pl.ds(at, step), :], (((1,), (1,)), ((), ())),
                preferred_element_type=jnp.float32,
            )
            x[0, pl.ds(row, count), pl.ds(at, step)] = one.astype(x.dtype)

    hrows = rows // 2

    def finish(b):
        @pl.when(is_end)
        def _():
            product(
                1, slot(*order[b]), (2 * (line - 1 - z) + 1 - y) * wrows, wrows,
                dn_w, 0, 2 * width, width,
            )

    here_row = slot(r, y)

    def plane_sums(pa):
        pb = cols - pa
        pieces = [
            (0, 0, hrows, 0, pa), (0, 0, hrows, pa, pb),
            (0, hrows, hrows, 0, pa), (0, hrows, hrows, pa, pb),
            (1, 0, rows, 0, cols), (2, 0, rows, 0, cols), (3, 0, rows, 0, cols),
        ]

        def place_of(i, col):
            b, at, count, c0, n = pieces[i]
            row = pl.multiple_of(slot(*order[b]) + at, hrows)
            return row, count, pl.multiple_of(col + c0, 128), c0, n

        def core_copy(i):
            row, count, col, c0, n = place_of(i, its_col)
            return remote(
                part.at[pl.ds(row, count), pl.ds(col, n)],
                r1.at[pl.ds(row, count), pl.ds(c0, n)], c_s.at[i], c_r.at[i], cpart,
            )

        def theirs(i):
            row, count, col, c0, n = place_of(i, its_col)
            if c0 == 0:
                slopes(row, count)
            back(row, count, col, n)
            core_copy(i).start()

        def summed(i):
            row, count, col, c0, n = place_of(i, my_col)
            back(row, count, col, n)
            core_copy(i).wait_recv()
            total((part, row, col, n), [(part, row, col, n), (r1, row, c0, n)], count)

        def first_block():
            for u in (0, 1):
                theirs(2 * u)
                theirs(2 * u + 1)
                summed(2 * u)
                x_copy(u).start()
                summed(2 * u + 1)
                y_copy(u).start()

        def urow(u):
            return pl.multiple_of(slot(*order[0]) + u * hrows, hrows)

        second_col = pl.multiple_of(my_col + pa, 128)

        def mine_a(row, count):
            return part.at[pl.ds(row, count), pl.ds(my_col, pa)]

        def mine_b(row, count):
            return part.at[pl.ds(row, count), pl.ds(second_col, pb)]

        def x_copy(i):
            if i >= 3:
                at = pl.ds((i - 3) * hrows, hrows)
                src, dst = s3b.at[at, pl.ds(0, pb)], rxb.at[at, pl.ds(0, pb)]
            elif i == 2:
                src, dst = mine_a(slot(*order[1]), rows), rxa.at[1, :, pl.ds(0, pa)]
            else:
                src, dst = mine_a(urow(i), hrows), rxa.at[0, pl.ds(i * hrows, hrows), pl.ds(0, pa)]
            return remote(src, dst, x_s.at[i], x_r.at[i], xpart)

        def y_copy(i):
            if i == 4:
                src, dst = s3a.at[:, pl.ds(0, pa)], ryb.at[:, pl.ds(0, pa)]
            elif i in (2, 3):
                at = (i - 2) * hrows
                row = pl.multiple_of(slot(*order[2]) + at, hrows)
                src, dst = mine_b(row, hrows), rya.at[1, pl.ds(at, hrows), pl.ds(0, pb)]
            else:
                src, dst = mine_b(urow(i), hrows), rya.at[0, pl.ds(i * hrows, hrows), pl.ds(0, pb)]
            return remote(src, dst, yy_s.at[i], yy_r.at[i], ypart)

        def relay_a():
            for i in (0, 1):
                x_copy(i).wait_recv()
            total(
                (s3a, 0, 0, pa),
                [(part, slot(r, 1 - y), my_col, pa), (rxa.at[0], 0, 0, pa)], rows,
            )

        def relay_b():
            for i in (0, 1):
                y_copy(i).wait_recv()
            total(
                (s3b, 0, 0, pb),
                [(part, slot(1 - r, y), second_col, pb), (rya.at[0], 0, 0, pb)], rows,
            )
            x_copy(3).start()

        def o_copy(i, land):
            base = (1 - core if land else core) * cols
            if i == 0:
                at = gi_out.at[:, pl.ds(pl.multiple_of(base, 128), pa)]
            else:
                at = gi_out.at[
                    pl.ds((i - 1) * hrows, hrows), pl.ds(pl.multiple_of(base + pa, 128), pb)
                ]
            return remote(at, at, o_s.at[i], o_r.at[i], cpart)

        def final_a():
            x_copy(2).wait_recv()
            y_copy(4).wait_recv()
            total(
                (gi_out, 0, my_col, pa),
                [
                    (part, here_row, my_col, pa),
                    (rxa.at[1], 0, 0, pa), (ryb, 0, 0, pa),
                ], rows,
            )
            o_copy(0, False).start()

        def final_b(i):
            at = i * hrows
            x_copy(3 + i).wait_recv()
            y_copy(2 + i).wait_recv()
            total(
                (gi_out, at, second_col, pb),
                [
                    (part, here_row + at, second_col, pb),
                    (rya.at[1], at, 0, pb), (rxb, at, 0, pb),
                ], hrows,
            )
            o_copy(1 + i, False).start()

        def settled():
            for i in range(7):
                core_copy(i).wait_send()
            for i in range(5):
                y_copy(i).wait_send()
                x_copy(i).wait_send()
            for i in range(3):
                o_copy(i, True).wait_recv()
                o_copy(i, False).wait_send()

        return (
            first_block, theirs, summed, x_copy, y_copy, relay_a, relay_b,
            final_a, final_b, settled,
        )

    def scaled(terms, rr, yy):
        at_col = gcol(rr, yy)

        @pl.loop(0, frows // 64)
        def _(m):
            at = pl.multiple_of(m * 64, 64)
            value = None
            for ref, row, col in terms:
                one = ref[pl.ds(row + at, 64), pl.ds(col, width)].astype(jnp.float32)
                value = one if value is None else value + one
            gd_out[pl.ds(at, 64), pl.ds(at_col, width)] = value * grad_scale

    def inputs_sent():
        for i in (0, 3, 5):
            dcopy(i, core).wait_send()
        tcopy(5, False).wait_send()

    @pl.when(is_end)
    def _():
        (
            first_block, theirs, summed, x_copy, y_copy, relay_a, relay_b,
            final_a, final_b, settled,
        ) = plane_sums(end_a)
        for i in range(line):
            g_block(jnp.where(lower, line - 1 - i, i))
            if i < line - 1:
                @pl.when(lower)
                def _():
                    up_copy(line - 1 - i, True).start()

                @pl.when(jnp.logical_not(lower))
                def _():
                    dn_copy(i, True).start()
        f_copy(0, False, g, zrow).start()
        f_copy(1, False, g, zrow).start()
        for d in range(last):
            for sub in range(2):
                settle(d, sub, 2)
        forward(1, dn_w, 2 * width, width, 0, 4)
        f_copy(0, True).wait_recv()
        f_copy(2, False).start()
        forward_end(1, 2, 0)
        for up_dir in (True, False):
            await_recv(up_dir, last, 1, 2)
        inputs_sent()
        finish(0)
        first_block()
        finish(1)
        theirs(4)
        summed(4)
        x_copy(2).start()
        finish(2)
        theirs(5)
        summed(5)
        y_copy(2).start()
        finish(3)
        theirs(6)
        summed(6)
        relay_a()
        y_copy(4).start()
        y_copy(3).start()
        relay_b()
        x_copy(4).start()
        h_copy(0).wait_recv()
        scaled([(g, pl.multiple_of(zrow + y * frows, frows), 0), (hl, 0, gcol(r, y))], r, y)
        final_a()
        final_b(0)
        for i, (rr, yy) in enumerate(((r, 1 - y), (1 - r, y))):
            if i == 1:
                f_copy(1, True).wait_recv()
            h_copy(1 + i).wait_recv()
            scaled([(gl, 0, gcol(rr, yy)), (hl, 0, gcol(rr, yy))], rr, yy)
        final_b(1)
        f_copy(2, True).wait_recv()
        h_copy(3).wait_recv()
        diag = gcol(1 - r, 1 - y)
        scaled([(gl, 0, diag), (hl, 0, diag)], 1 - r, 1 - y)
        settled()

    @pl.when(jnp.logical_not(is_end))
    def _():
        (
            first_block, theirs, summed, x_copy, y_copy, relay_a, relay_b,
            final_a, final_b, settled,
        ) = plane_sums(mid_a)
        inputs_sent()
        forward(1, dn_w, 2 * width, width, 3, 1)
        first_block()
        g_block(jnp.where(lower, line - 1, 0))
        forward(1, dn_w, 2 * width, width, 1, 1)
        theirs(4)
        summed(4)
        x_copy(2).start()
        line_step(1)
        forward(1, dn_w, 2 * width, width, 2, 1)
        theirs(5)
        summed(5)
        y_copy(2).start()
        relay_a()
        relay_b()
        for i in range(1, line):
            g_block(jnp.where(lower, line - 1 - i, i))
        for t in range(2, line - 1):
            line_step(t)
        y_copy(4).start()
        x_copy(4).start()
        forward(1, dn_w, 2 * width, width, 0, 1)
        theirs(6)
        summed(6)
        up_copy(z, False).wait_recv()
        dn_copy(z, False).wait_recv()
        total(
            (gfin, 0, 0, width),
            [(g, zrow, 0, width), (u_in, zrow, 0, width), (d_in, zrow, 0, width)], zrows,
        )
        f_copy(0, False).start()
        y_copy(3).start()
        scaled([(gfin, pl.multiple_of(y * frows, frows), 0)], r, y)

        @pl.when(next_to_end)
        def _():
            e_copy(0, True).wait_recv()
            e_copy(2, False).start()
            h_copy(1).start()
            e_copy(1, True).wait_recv()
            h_copy(2).start()

        f_copy(1, False).start()
        final_a()
        final_b(0)

        @pl.when(next_to_end)
        def _():
            e_copy(2, True).wait_recv()
            h_copy(3).start()

        f_copy(0, True).wait_recv()
        f_copy(2, False).start()
        scaled([(gl, 0, gcol(r, 1 - y))], r, 1 - y)
        f_copy(1, True).wait_recv()
        scaled([(gl, 0, gcol(1 - r, y))], 1 - r, y)
        final_b(1)
        f_copy(2, True).wait_recv()
        scaled([(gl, 0, gcol(1 - r, 1 - y))], 1 - r, 1 - y)

        @pl.when(next_to_end)
        def _():
            for i in range(3):
                e_copy(i, False).wait_send()
            for i in range(4):
                h_copy(i).wait_send()

        settled()

    for i in range(ntok):
        if kinds[i] == 1:
            dcopy(i, core).wait_send()
        if i != 5:
            tcopy(i, False).wait_send()
    for k in range(3):
        to_y(k).wait_send()
        for d in range(line - 1):
            for sub in range(2):
                await_send(True, d, sub, k)
                await_send(False, d, sub, k)
    for i in range(3):
        f_copy(i, False).wait_send()
    for zt in range(line):
        if zt > 0:
            far = line - 2 if zt == line - 1 else zt
            pl.when(z < far)(lambda: up_copy(zt, True).wait_send())
        if zt < line - 1:
            near = 1 if zt == 0 else zt
            pl.when(z > near)(lambda: dn_copy(zt, True).wait_send())


def fused(grad_scale, gate_w, up_w, down_w, toks, cots):
    line = lax.axis_size("fs") // 2
    rows, full = toks.shape
    wrows, width = gate_w.shape[0], gate_w.shape[1] // 4
    depth = 2 * line * wrows
    cols = full // 2
    kind = gate_w.dtype
    dma = pltpu.SemaphoreType.DMA
    zsem = dma((line - 1, 2, 3))
    anyspec = pl.BlockSpec(memory_space=pl.ANY)
    whole = pltpu.VMEM((depth, width), kind)
    end_a, mid_a = cols // 2, cols * 3 // 8 // 128 * 128
    most_b = cols - mid_a
    return pl.pallas_call(
        functools.partial(fused_kernel, line, grad_scale, end_a, mid_a),
        out_shape=(
            pltpu.VMEM((rows, full), kind),
            pltpu.VMEM((wrows, 4 * width), jnp.float32),
        ),
        in_specs=[anyspec] * 5,
        out_specs=(pl.BlockSpec(memory_space=pltpu.VMEM),) * 2,
        scratch_shapes=[
            pltpu.VMEM((2, 4 * rows, full), kind),
            pltpu.VMEM((depth, 2 * width), kind),
            whole,
            pltpu.VMEM((4 * rows, 3 * width), jnp.float32),
            pltpu.VMEM((4 * rows, width), kind),
            pltpu.VMEM((4 * rows, 2 * width), kind),
            pltpu.VMEM((4 * rows, cols), kind),
            pltpu.VMEM((2, rows, end_a), kind), pltpu.VMEM((rows, most_b), kind),
            pltpu.VMEM((2, rows, most_b), kind), pltpu.VMEM((rows, end_a), kind),
            pltpu.VMEM((rows, end_a), kind), pltpu.VMEM((rows, most_b), kind),
            whole, whole, whole,
            pltpu.VMEM((2 * wrows, width), kind),
            pltpu.VMEM((wrows, 4 * width), kind),
            pltpu.VMEM((wrows, 4 * width), kind),
            zsem, zsem, zsem, zsem,
            dma((3,)), dma((3,)),
            dma((8,)), dma((8,)), dma((8,)), dma((8,)), dma((5,)),
            dma((7,)), dma((7,)), dma((5,)), dma((5,)), dma((5,)), dma((5,)),
            dma((line,)), dma((line,)), dma((line,)), dma((line,)),
            dma((3,)), dma((3,)), dma((3,)), dma((3,)),
            dma((3,)), dma((3,)), dma((4,)), dma((4,)),
        ],
        compiler_params=pltpu.CompilerParams(
            collective_id=1, has_side_effects=True, vmem_limit_bytes=59 * 2**20
        ),
        name="fused_all",
    )(gate_w, up_w, down_w, toks, cots)


def place_kernel(a, b, a_out, b_out, sems):
    copies = [
        pltpu.make_async_copy(a, a_out, sems.at[0]),
        pltpu.make_async_copy(b, b_out, sems.at[1]),
    ]
    for copy in copies:
        copy.start()
    for copy in copies:
        copy.wait()


def place(a, b):
    anyspec = pl.BlockSpec(memory_space=pl.ANY)
    return pl.pallas_call(
        place_kernel,
        out_shape=(
            jax.ShapeDtypeStruct(a.shape, a.dtype), jax.ShapeDtypeStruct(b.shape, b.dtype),
        ),
        in_specs=[pl.BlockSpec(memory_space=pltpu.VMEM)] * 2,
        out_specs=(anyspec,) * 2,
        scratch_shapes=[pltpu.SemaphoreType.DMA((2,))],
        compiler_params=pltpu.CompilerParams(vmem_limit_bytes=16 * 2**20),
        name="place",
    )(a, b)


def gather_kernel(
    line, units, gate_w, up_w, down_w, toks, cots, gu_out, d_out, t_out, w_tmp, t_tmp,
    up_s, up_r, dn_s, dn_r, y_s, y_r, tok_s, tok_r, d2d_s, d2d_r, loc, loc2,
):
    r = lax.axis_index("rep")
    f = lax.axis_index("fs")
    t = lax.axis_index("tp")
    z, y = f // 2, f % 2
    rows = toks.shape[0]
    half = rows // 2
    wrows = gate_w.shape[0]
    width = gate_w.shape[1] // 4
    parts = len(units)
    has_up, has_dn = z < line - 1, z > 0
    up = {"fs": (f + 2) % (2 * line)}
    dn = {"fs": (f + 2 * line - 2) % (2 * line)}
    ypart = {"fs": f + 1 - 2 * y}
    xpart = {"rep": 1 - r}
    core = t % 2
    cpart = {"tp": t + 1 - 2 * core}

    barrier = pltpu.get_barrier_semaphore()

    def greet(dev):
        pl.semaphore_signal(barrier, inc=1, device_id=dev, device_id_type=MESH)

    for dev in (ypart, xpart, cpart, up, dn):
        greet(dev)
    pl.semaphore_wait(barrier, 5)

    def remote(src, dst, s, q, dev):
        return pltpu.make_async_remote_copy(
            src_ref=src, dst_ref=dst, send_sem=s, recv_sem=q,
            device_id=dev, device_id_type=MESH,
        )

    def wblk(k, zz, yy):
        row = pl.multiple_of((2 * zz + yy) * wrows, wrows)
        which, col, wide = units[k]
        return (gu_out, d_out)[which].at[pl.ds(row, wrows), pl.ds(col, wide)]

    def own(k, yy):
        col = pl.multiple_of((2 * r + yy) * width, width)
        return (gate_w, up_w, down_w)[k].at[:, pl.ds(col, width)]

    def to_y(k):
        return remote(own(k, 1 - y), wblk(k, z, y), y_s.at[k], y_r.at[k], ypart)

    def from_y(k):
        return remote(own(k, 1 - y), wblk(k, z, 1 - y), y_s.at[k], y_r.at[k], ypart)

    def zcopy(up_dir, d, sub, k, zz):
        yy = y if sub == 0 else 1 - y
        src = own(k, y) if (d == 0 and sub == 0) else wblk(k, zz, yy)
        s, q, dev = (up_s, up_r, up) if up_dir else (dn_s, dn_r, dn)
        return remote(src, wblk(k, zz, yy), s.at[d, sub, k], q.at[d, sub, k], dev)

    def pred_send(up_dir, d):
        return (has_up & (z - d >= 0)) if up_dir else (has_dn & (z + d <= line - 1))

    def src_z(up_dir, d):
        return jnp.maximum(z - d, 0) if up_dir else jnp.minimum(z + d, line - 1)

    def send(up_dir, d, sub, k):
        @pl.when(pred_send(up_dir, d))
        def _():
            zcopy(up_dir, d, sub, k, src_z(up_dir, d)).start()

    def await_send(up_dir, d, sub, k):
        @pl.when(pred_send(up_dir, d))
        def _():
            zcopy(up_dir, d, sub, k, src_z(up_dir, d)).wait_send()

    def await_recv(up_dir, d, sub, k):
        ok = (z - d - 1 >= 0) if up_dir else (z + d + 1 <= line - 1)

        @pl.when(ok)
        def _():
            zcopy(up_dir, d, sub, k, src_z(up_dir, d + 1)).wait_recv()

    def tblk(j, rr, yy, c):
        row = pl.multiple_of((2 * rr + yy) * rows + c * half, half)
        return t_out.at[j, pl.ds(row, half), :]

    def mine(j):
        src = toks if j == 0 else cots
        return src.at[pl.ds(pl.multiple_of(core * half, half), half), :]

    def tcopy(i, landing):
        j = (0, 1, 0, 1, 0, 1)[i]
        dev = xpart if i in (0, 1, 5) else ypart
        if landing:
            rr = (1 - r, 1 - r, r, r, 1 - r, 1 - r)[i]
            yy = (y, y, 1 - y, 1 - y, 1 - y, 1 - y)[i]
            src = dst = tblk(j, rr, yy, core)
        else:
            rr = (r, r, r, r, 1 - r, r)[i]
            yy = (y, y, y, y, y, 1 - y)[i]
            dst = tblk(j, rr, yy, core)
            src = mine(j) if i < 4 else dst
        return remote(src, dst, tok_s.at[i], tok_r.at[i], dev)

    def dcopy(i, c):
        j = (0, 1, 0, 1, 0, 1)[i]
        rr = (1 - r, 1 - r, r, r, 1 - r, 1 - r)[i]
        yy = (y, y, 1 - y, 1 - y, 1 - y, 1 - y)[i]
        blk = tblk(j, rr, yy, c)
        return remote(blk, blk, d2d_s.at[i], d2d_r.at[i], cpart)

    loads = [
        pltpu.make_async_copy(own(0, y), w_tmp.at[0], loc.at[0]),
        pltpu.make_async_copy(own(1, y), w_tmp.at[1], loc.at[3]),
        pltpu.make_async_copy(own(2, y), w_tmp.at[2], loc.at[4]),
        pltpu.make_async_copy(toks, t_tmp.at[0], loc.at[1]),
        pltpu.make_async_copy(cots, t_tmp.at[1], loc.at[2]),
    ]
    trow = pl.multiple_of((2 * r + y) * rows, rows)
    stores = [
        pltpu.make_async_copy(w_tmp.at[0], wblk(0, z, y), loc2.at[0]),
        pltpu.make_async_copy(w_tmp.at[1], wblk(1, z, y), loc2.at[3]),
        pltpu.make_async_copy(w_tmp.at[2], wblk(2, z, y), loc2.at[4]),
        pltpu.make_async_copy(t_tmp.at[0], t_out.at[0, pl.ds(trow, rows), :], loc2.at[1]),
        pltpu.make_async_copy(t_tmp.at[1], t_out.at[1, pl.ds(trow, rows), :], loc2.at[2]),
    ]

    for k in range(parts):
        to_y(k).start()
        send(True, 0, 0, k)
        send(False, 0, 0, k)
    for i in (0, 1, 3, 2):
        tcopy(i, False).start()
    for copy in loads:
        copy.start()
    for load, store in zip(loads, stores):
        load.wait()
        store.start()
    for k in range(parts):
        from_y(k).wait_recv()
        send(True, 0, 1, k)
        send(False, 0, 1, k)

    def event(i):
        tcopy(i, True).wait_recv()
        if i == 0:
            tcopy(4, False).start()
        if i == 3:
            tcopy(5, False).start()
        dcopy(i, core).start()

    events = [0, 3, 1, 2, 5, 4]
    for d in range(line - 1):
        for sub in range(2):
            if events:
                event(events.pop(0))
            for k in range(parts):
                for up_dir in (True, False):
                    await_recv(up_dir, d, sub, k)
                    if d + 1 < line - 1:
                        send(up_dir, d + 1, sub, k)
    for i in events:
        event(i)
    for i in range(6):
        dcopy(i, 1 - core).wait_recv()
        dcopy(i, core).wait_send()
        tcopy(i, False).wait_send()
    for k in range(parts):
        to_y(k).wait_send()
        for d in range(line - 1):
            for sub in range(2):
                await_send(True, d, sub, k)
                await_send(False, d, sub, k)
    for store in stores:
        store.wait()


def gather(gate_w, up_w, down_w, toks, cots):
    line = lax.axis_size("fs") // 2
    wrows, width = gate_w.shape[0], gate_w.shape[1] // 4
    units = [(0, 0, width), (0, width, width), (1, 0, width)]
    parts = len(units)
    depth = 2 * line * wrows
    kind = gate_w.dtype
    dma = pltpu.SemaphoreType.DMA
    zsem = dma((line - 1, 2, parts))
    anyspec = pl.BlockSpec(memory_space=pl.ANY)
    return pl.pallas_call(
        functools.partial(gather_kernel, line, units),
        out_shape=(
            jax.ShapeDtypeStruct((depth, 2 * width), kind),
            jax.ShapeDtypeStruct((depth, width), kind),
            jax.ShapeDtypeStruct((2, 4 * toks.shape[0], toks.shape[1]), toks.dtype),
        ),
        in_specs=[anyspec] * 5,
        out_specs=(anyspec,) * 3,
        scratch_shapes=[
            pltpu.VMEM((parts, wrows, width), kind),
            pltpu.VMEM((2,) + toks.shape, toks.dtype),
            zsem, zsem, zsem, zsem,
            dma((parts,)), dma((parts,)),
            dma((6,)), dma((6,)), dma((6,)), dma((6,)),
            dma((5,)), dma((5,)),
        ],
        compiler_params=pltpu.CompilerParams(collective_id=0, has_side_effects=True),
        name="gather_all",
    )(gate_w, up_w, down_w, toks, cots)


def on_device(inputs, cotangent, gate_weight, up_weight, down_weight):
    tok_rows = inputs.shape[0]
    fs_size = lax.axis_size("fs")
    rep_size = lax.axis_size("rep")
    grad_scale = 1.0 / math.sqrt(tok_rows * fs_size * rep_size)
    if lax.axis_size("tp") == 2 and rep_size == 2 and fs_size >= 8:
        return place(*fused(
            grad_scale, gate_weight, up_weight, down_weight, inputs, cotangent
        ))
    contract = (((1,), (1,)), ((), ()))
    contract_tok = (((0,), (0,)), ((), ()))
    width = gate_weight.shape[1] // 4
    gate_up, down_full, tokens = gather(
        gate_weight, up_weight, down_weight, inputs, cotangent
    )
    gate_up_val = jnp.dot(tokens[0], gate_up, preferred_element_type=jnp.float32)
    gate_val, up_val = gate_up_val[:, :width], gate_up_val[:, width:]
    grad_hidden = jnp.dot(tokens[1], down_full, preferred_element_type=jnp.float32)
    sigmoid_gate = jax.nn.sigmoid(gate_val)
    active = gate_val * sigmoid_gate
    hidden = (active * up_val).astype(jnp.bfloat16)
    grad_gate = (
        grad_hidden * up_val * sigmoid_gate * (1.0 + gate_val * (1.0 - sigmoid_gate))
    ).astype(jnp.bfloat16)
    grad_up = (grad_hidden * active).astype(jnp.bfloat16)
    pairs = [[i, i + 1] for i in range(0, fs_size, 2)]
    lines = [list(range(i, fs_size, 2)) for i in range(2)]
    grad_part = lax.dot_general(
        tokens[1], hidden, contract_tok, preferred_element_type=jnp.float32
    )
    part = lax.dot_general(
        jnp.concatenate([grad_gate, grad_up], axis=1), gate_up, contract,
        preferred_element_type=jnp.float32,
    )
    shard = lax.psum_scatter(
        grad_part.astype(jnp.bfloat16), "fs", scatter_dimension=0, tiled=True,
        axis_index_groups=lines,
    ).astype(jnp.float32) * grad_scale
    shard = lax.all_to_all(
        shard, "fs", split_axis=0, concat_axis=1, tiled=True, axis_index_groups=pairs
    )
    grad_down = lax.all_gather(shard, "rep", axis=1, tiled=True)
    part = lax.psum_scatter(
        part.astype(jnp.bfloat16), "rep", scatter_dimension=0, tiled=True
    )
    part = lax.psum_scatter(
        part, "fs", scatter_dimension=0, tiled=True, axis_index_groups=pairs
    )
    grad_input = lax.psum(part, "tp")
    return (grad_input, grad_down)


def solution(mesh):
    placed = (
        P(("rep", "fs"), None),
        P(("rep", "fs"), None),
        P("fs", "tp"),
        P("fs", "tp"),
        P("fs", "tp"),
    )
    return jax.shard_map(
        on_device,
        mesh=mesh,
        in_specs=placed,
        out_specs=(P(("rep", "fs"), None), P("fs", "tp")),
        check_vma=False,
    )
```

```python
import functools
import math

import jax
import jax.numpy as jnp
from jax import lax
from jax.experimental import pallas as pl
from jax.experimental.pallas import tpu as pltpu
from jax.sharding import PartitionSpec as P

MESH = pl.DeviceIdType.MESH


def fused_kernel(
    line, grad_scale, end_a, mid_a, gate_w, up_w, down_w, toks, cots, gi_out, gd_out,
    x, gu, dn_w, acc, hid, ggu, r1, rxa, rxb, rya, ryb, s3a, s3b, g, u_in, d_in, gfin, gl, hl,
    up_s, up_r, dn_s, dn_r, wy_s, wy_r, tok_s, tok_r, d2d_s, d2d_r, loc,
    c_s, c_r, x_s, x_r, yy_s, yy_r, u_s, u_r, d_s, d_r, f_s, f_r, o_s, o_r, e_s, e_r, h_s, h_r,
):
    r = lax.axis_index("rep")
    f = lax.axis_index("fs")
    core = lax.axis_index("tp")
    z, y = f // 2, f % 2
    rows = toks.shape[0]
    half = rows // 2
    wrows = gate_w.shape[0]
    width = gate_w.shape[1] // 4
    depth = 2 * line * wrows
    zrows = 2 * wrows
    cols = depth // 2
    wide = cols // 2
    frows = wrows
    last = line - 2
    has_up, has_dn = z < line - 1, z > 0
    is_end = (z == 0) | (z == line - 1)
    up = {"fs": (f + 2) % (2 * line)}
    dn = {"fs": (f + 2 * line - 2) % (2 * line)}
    ypart = {"fs": f + 1 - 2 * y}
    xpart = {"rep": 1 - r}
    cpart = {"tp": 1 - core}

    barrier = pltpu.get_barrier_semaphore()
    for dev in (ypart, xpart, cpart, up, dn):
        pl.semaphore_signal(barrier, inc=1, device_id=dev, device_id_type=MESH)
    pl.semaphore_wait(barrier, 5)

    def remote(src, dst, s, q, dev):
        return pltpu.make_async_remote_copy(
            src_ref=src, dst_ref=dst, send_sem=s, recv_sem=q,
            device_id=dev, device_id_type=MESH,
        )

    def wblk(k, zz, yy):
        row = pl.multiple_of((2 * zz + yy) * wrows, wrows)
        if k == 2:
            return dn_w.at[pl.ds(row, wrows), :]
        return gu.at[pl.ds(row, wrows), pl.ds(k * width, width)]

    def own(k, yy):
        col = pl.multiple_of((2 * r + yy) * width, width)
        return (gate_w, up_w, down_w)[k].at[:, pl.ds(col, width)]

    def to_y(k):
        return remote(own(k, 1 - y), wblk(k, z, y), wy_s.at[k], wy_r.at[k], ypart)

    def from_y(k):
        return remote(own(k, 1 - y), wblk(k, z, 1 - y), wy_s.at[k], wy_r.at[k], ypart)

    def zcopy(up_dir, d, sub, k, zz):
        yy = y if sub == 0 else 1 - y
        src = own(k, y) if (d == 0 and sub == 0) else wblk(k, zz, yy)
        s, q, dev = (up_s, up_r, up) if up_dir else (dn_s, dn_r, dn)
        return remote(src, wblk(k, zz, yy), s.at[d, sub, k], q.at[d, sub, k], dev)

    def pred_send(up_dir, d):
        return (has_up & (z - d >= 0)) if up_dir else (has_dn & (z + d <= line - 1))

    def src_z(up_dir, d):
        return jnp.maximum(z - d, 0) if up_dir else jnp.minimum(z + d, line - 1)

    def send(up_dir, d, sub, k):
        @pl.when(pred_send(up_dir, d))
        def _():
            zcopy(up_dir, d, sub, k, src_z(up_dir, d)).start()

    def await_send(up_dir, d, sub, k):
        @pl.when(pred_send(up_dir, d))
        def _():
            zcopy(up_dir, d, sub, k, src_z(up_dir, d)).wait_send()

    def await_recv(up_dir, d, sub, k):
        ok = (z - d - 1 >= 0) if up_dir else (z + d + 1 <= line - 1)

        @pl.when(ok)
        def _():
            zcopy(up_dir, d, sub, k, src_z(up_dir, d + 1)).wait_recv()

    def relay(d, sub, k):
        for up_dir in (True, False):
            @pl.when(pred_send(up_dir, d + 1))
            def _():
                zcopy(up_dir, d, sub, k, src_z(up_dir, d + 1)).wait_recv()
                zcopy(up_dir, d + 1, sub, k, src_z(up_dir, d + 1)).start()

    def settle(d, sub, k):
        for up_dir in (True, False):
            ok = (z - d - 1 >= 0) if up_dir else (z + d + 1 <= line - 1)
            onward = has_up if up_dir else has_dn

            @pl.when(ok & jnp.logical_not(onward))
            def _():
                zcopy(up_dir, d, sub, k, src_z(up_dir, d + 1)).wait_recv()

    def slot(rr, yy):
        return pl.multiple_of((2 * rr + yy) * rows, rows)

    kinds = (0, 1, 1, 0, 1, 0, 1, 1)
    over_x = (True, True, True, False, False, True, False, True)
    parts = (2, 0, 1, 2, 2, 2, 0, 1)
    ntok = len(kinds)

    def span(c, p):
        if p == 2:
            return c * half, half
        return c * half + p * (half // 2), half // 2

    def tblk(i, rr, yy, c):
        at, count = span(c, parts[i])
        row = pl.multiple_of((2 * rr + yy) * rows + at, half // 2)
        return x.at[kinds[i], pl.ds(row, count), :]

    def mine(i):
        at, count = span(core, parts[i])
        src = toks if kinds[i] == 0 else cots
        return src.at[pl.ds(pl.multiple_of(at, half // 2), count), :]

    def landing(i, c):
        rr = (1 - r, 1 - r, 1 - r, r, r, 1 - r, 1 - r, 1 - r)[i]
        yy = (y, y, y, 1 - y, 1 - y, 1 - y, 1 - y, 1 - y)[i]
        return tblk(i, rr, yy, c)

    def tcopy(i, land):
        dev = xpart if over_x[i] else ypart
        if land:
            src = dst = landing(i, core)
        else:
            rr = (r, r, r, r, r, r, 1 - r, r)[i]
            yy = (y, y, y, y, y, 1 - y, y, 1 - y)[i]
            dst = tblk(i, rr, yy, core)
            src = mine(i) if i < 5 else dst
        return remote(src, dst, tok_s.at[i], tok_r.at[i], dev)

    def dcopy(i, c):
        blk = landing(i, c)
        return remote(blk, blk, d2d_s.at[i], d2d_r.at[i], cpart)

    def event(i):
        tcopy(i, True).wait_recv()
        onward = {1: 6, 3: 5, 4: 7}.get(i)
        if onward is not None:
            tcopy(onward, False).start()
        dcopy(i, core).start()

    trow = slot(r, y)
    loads = [
        pltpu.make_async_copy(own(0, y), wblk(0, z, y), loc.at[0]),
        pltpu.make_async_copy(own(1, y), wblk(1, z, y), loc.at[1]),
        pltpu.make_async_copy(own(2, y), wblk(2, z, y), loc.at[2]),
        pltpu.make_async_copy(toks, x.at[0, pl.ds(trow, rows), :], loc.at[3]),
        pltpu.make_async_copy(cots, x.at[1, pl.ds(trow, rows), :], loc.at[4]),
    ]

    tile = 256
    z_lo = jnp.maximum(z - last, 0)
    z_hi = jnp.minimum(z + last, line - 1) + 1

    def product(j, row, k0, kk, w, wcol, acol, n):
        at = pl.ds(pl.multiple_of(row, rows), rows)
        kat = pl.ds(pl.multiple_of(k0, wrows), kk)
        for c in range(0, n, tile):
            one = jnp.dot(
                x[j, at, kat], w[kat, pl.ds(wcol + c, tile)],
                preferred_element_type=jnp.float32,
            )
            acc[at, pl.ds(acol + c, tile)] += one

    def forward(j, w, acol, n, first, count):
        @pl.loop(first, first + count)
        def _(b):
            row = ((2 * r + y) + 2 * (b % 2) * (1 - 2 * r) + (b // 2) * (1 - 2 * y)) * rows

            @pl.loop(z_lo, z_hi)
            def _(zz):
                product(j, row, zz * zrows, zrows, w, 0, acol, n)

    def forward_end(j, k, sub):
        for up_dir in (True, False):
            await_recv(up_dir, last, sub, k)

        @pl.when(is_end)
        def _():
            zz = line - 1 - z
            yy = y if sub == 0 else 1 - y
            w = dn_w if k == 2 else gu

            @pl.loop(0, 4)
            def _(b):
                product(
                    j, b * rows, (2 * zz + yy) * wrows, wrows, w,
                    0 if k == 2 else k * width, k * width, width,
                )

    def total(dst, terms, count, step=64):
        @pl.loop(0, count // step)
        def _(i):
            at = pl.multiple_of(i * step, step)
            value = None
            for ref, row, col, wide in terms:
                one = ref[pl.ds(row + at, step), pl.ds(col, wide)].astype(jnp.float32)
                value = one if value is None else value + one
            ref, row, col, wide = dst
            ref[pl.ds(row + at, step), pl.ds(col, wide)] = value.astype(ref.dtype)

    for k in (0, 1):
        to_y(k).start()
        send(True, 0, 0, k)
        send(False, 0, 0, k)
    for i in (0, 1, 3):
        tcopy(i, False).start()
    to_y(2).start()
    tcopy(4, False).start()
    for copy in loads:
        copy.start()

    @pl.loop(0, 4 * rows // 64)
    def _(i):
        at = pl.ds(pl.multiple_of(i * 64, 64), 64)
        acc[at, :] = jnp.zeros((64, 3 * width), jnp.float32)

    for k in (0, 1):
        from_y(k).wait_recv()
        send(True, 0, 1, k)
        send(False, 0, 1, k)
    if last > 0:
        for sub in range(2):
            for k in (0, 1):
                relay(0, sub, k)
    event(0)
    event(3)
    tcopy(2, False).start()
    event(1)
    for d in range(1, last):
        for sub in range(2):
            for k in (0, 1):
                relay(d, sub, k)
    send(True, 0, 0, 2)
    send(False, 0, 0, 2)
    from_y(2).wait_recv()
    send(True, 0, 1, 2)
    send(False, 0, 1, 2)
    for load in loads:
        load.wait()
    for d in range(last):
        for sub in range(2):
            for k in (0, 1):
                settle(d, sub, k)
    dcopy(0, 1 - core).wait_recv()
    dcopy(3, 1 - core).wait_recv()
    forward(0, gu, 0, 2 * width, 0, 3)
    if last > 0:
        for sub in range(2):
            relay(0, sub, 2)
    event(5)
    event(4)
    dcopy(5, 1 - core).wait_recv()
    forward(0, gu, 0, 2 * width, 3, 1)
    for d in range(1, last):
        for sub in range(2):
            relay(d, sub, 2)
    for sub in range(2):
        for k in (0, 1):
            forward_end(0, k, sub)

    @pl.loop(0, 4 * rows // 32)
    def _(i):
        at = pl.ds(pl.multiple_of(i * 32, 32), 32)
        gate = acc[at, pl.ds(0, width)]
        up_val = acc[at, pl.ds(width, width)]
        sig = jax.nn.sigmoid(gate)
        active = gate * sig
        hid[at, :] = (active * up_val).astype(hid.dtype)
        acc[at, pl.ds(0, width)] = up_val * sig * (1.0 + gate * (1.0 - sig))
        acc[at, pl.ds(width, width)] = active

    for i in (2, 6, 7):
        event(i)
    for i in (1, 2, 4, 6, 7):
        dcopy(i, 1 - core).wait_recv()

    zrow = pl.multiple_of(z * zrows, zrows)
    lower = z < line // 2

    def block(ref, zt):
        return ref.at[pl.ds(zt * zrows, zrows), :]

    def up_copy(zt, first):
        return remote(block(g if first else u_in, zt), block(u_in, zt), u_s.at[zt], u_r.at[zt], up)

    def dn_copy(zt, first):
        return remote(block(g if first else d_in, zt), block(d_in, zt), d_s.at[zt], d_r.at[zt], dn)

    def g_block(zt):
        at = pl.multiple_of(zt * zrows, zrows)
        one = lax.dot_general(
            x[1, :, pl.ds(at, zrows)], hid[...], (((0,), (0,)), ((), ())),
            preferred_element_type=jnp.float32,
        )
        g[pl.ds(at, zrows), :] = one.astype(g.dtype)

    def gcol(rr, yy):
        return pl.multiple_of((2 * rr + yy) * width, width)

    def gcols(ref, rr, yy):
        return ref.at[:, pl.ds(gcol(rr, yy), width)]

    def half_rows(ref, row, yy):
        return ref.at[pl.ds(pl.multiple_of(row + yy * frows, frows), frows), :]

    def f_copy(i, land, ref=gfin, row=0):
        if i == 0:
            src, dst, dev = half_rows(ref, row, 1 - y), gcols(gl, r, 1 - y if land else y), ypart
        elif i == 1:
            src, dst, dev = half_rows(ref, row, y), gcols(gl, 1 - r if land else r, y), xpart
        else:
            src, dst, dev = gcols(gl, r, 1 - y), gcols(gl, 1 - r if land else r, 1 - y), xpart
        return remote(src, dst, f_s.at[i], f_r.at[i], dev)

    def e_copy(i, land, ref=gfin, row=0):
        if i == 0:
            src, dst, dev = half_rows(ref, row, 1 - y), gcols(hl, r, 1 - y if land else y), ypart
        elif i == 1:
            src, dst, dev = half_rows(ref, row, y), gcols(hl, 1 - r if land else r, y), xpart
        else:
            src, dst, dev = gcols(hl, r, 1 - y), gcols(hl, 1 - r if land else r, 1 - y), xpart
        return remote(src, dst, e_s.at[i], e_r.at[i], dev)

    end_z = jnp.where((z == 1) | (z == line - 1), 0, line - 1)
    end_dev = {"fs": 2 * end_z + y}
    next_to_end = (z == 1) | (z == line - 2)

    def h_copy(i, ref=gfin, row=0):
        rr, yy = ((r, y), (r, 1 - y), (1 - r, y), (1 - r, 1 - y))[i]
        dst = gcols(hl, rr, yy)
        src = half_rows(ref, row, y) if i == 0 else dst
        return remote(src, dst, h_s.at[i], h_r.at[i], end_dev)

    def share(ref, row):
        h_copy(0, ref, row).start()
        e_copy(0, False, ref, row).start()
        e_copy(1, False, ref, row).start()

    def line_step(t):
        zt = line - 1 + z - t
        row_u = pl.multiple_of(zt * zrows, zrows)
        is_u = (z > 0) & (zt <= line - 1) & (zt > z)
        zd = t - (line - 1 - z)
        row_d = pl.multiple_of(zd * zrows, zrows)
        is_d = (z < line - 1) & (zd >= 0) & (zd < z)
        final = t == line - 2

        def add_u():
            up_copy(zt, False).wait_recv()
            total((u_in, row_u, 0, width), [(g, row_u, 0, width), (u_in, row_u, 0, width)], zrows)

        def add_d():
            dn_copy(zd, False).wait_recv()
            total((d_in, row_d, 0, width), [(g, row_d, 0, width), (d_in, row_d, 0, width)], zrows)

        @pl.when((is_u & (z < line - 2)) if final else is_u)
        def _():
            add_u()
            up_copy(zt, False).start()

        @pl.when((is_d & (z > 1)) if final else is_d)
        def _():
            add_d()
            dn_copy(zd, False).start()

        if final:
            @pl.when(z == line - 2)
            def _():
                add_u()
                share(u_in, (line - 1) * zrows)

            @pl.when(z == 1)
            def _():
                add_d()
                share(d_in, 0)

    order = [(1 - r, 1 - y), (1 - r, y), (r, 1 - y), (r, y)]
    my_col = pl.multiple_of(core * cols, cols)
    its_col = pl.multiple_of((1 - core) * cols, cols)
    part = x.at[0]

    def slopes(row, count):
        @pl.loop(0, count // 32)
        def _(i):
            at = pl.ds(pl.multiple_of(row + i * 32, 32), 32)
            grad = acc[at, pl.ds(2 * width, width)]
            ggu[at, pl.ds(0, width)] = (grad * acc[at, pl.ds(0, width)]).astype(ggu.dtype)
            ggu[at, pl.ds(width, width)] = (grad * acc[at, pl.ds(width, width)]).astype(ggu.dtype)

    def back(row, count, col, n):
        step = min(n, wide) if n % wide == 0 else n

        @pl.loop(0, n // step)
        def _(i):
            at = pl.multiple_of(col + i * step, 128)
            one = lax.dot_general(
                ggu[pl.ds(row, count), :], gu[pl.ds(at, step), :], (((1,), (1,)), ((), ())),
                preferred_element_type=jnp.float32,
            )
            x[0, pl.ds(row, count), pl.ds(at, step)] = one.astype(x.dtype)

    hrows = rows // 2

    def finish(b):
        @pl.when(is_end)
        def _():
            product(
                1, slot(*order[b]), (2 * (line - 1 - z) + 1 - y) * wrows, wrows,
                dn_w, 0, 2 * width, width,
            )

    here_row = slot(r, y)

    def plane_sums(pa):
        pb = cols - pa
        pieces = [
            (0, 0, hrows, 0, pa), (0, 0, hrows, pa, pb),
            (0, hrows, hrows, 0, pa), (0, hrows, hrows, pa, pb),
            (1, 0, rows, 0, cols), (2, 0, rows, 0, cols), (3, 0, rows, 0, cols),
        ]

        def place_of(i, col):
            b, at, count, c0, n = pieces[i]
            row = pl.multiple_of(slot(*order[b]) + at, hrows)
            return row, count, pl.multiple_of(col + c0, 128), c0, n

        def core_copy(i):
            row, count, col, c0, n = place_of(i, its_col)
            return remote(
                part.at[pl.ds(row, count), pl.ds(col, n)],
                r1.at[pl.ds(row, count), pl.ds(c0, n)], c_s.at[i], c_r.at[i], cpart,
            )

        def theirs(i):
            row, count, col, c0, n = place_of(i, its_col)
            if c0 == 0:
                slopes(row, count)
            back(row, count, col, n)
            core_copy(i).start()

        def summed(i):
            row, count, col, c0, n = place_of(i, my_col)
            back(row, count, col, n)
            core_copy(i).wait_recv()
            total((part, row, col, n), [(part, row, col, n), (r1, row, c0, n)], count)

        def first_block():
            theirs(0)
            theirs(1)
            theirs(2)
            summed(0)
            x_copy(0).start()
            summed(1)
            y_copy(0).start()
            theirs(3)
            summed(2)
            x_copy(1).start()
            summed(3)
            y_copy(1).start()

        def urow(u):
            return pl.multiple_of(slot(*order[0]) + u * hrows, hrows)

        second_col = pl.multiple_of(my_col + pa, 128)

        def mine_a(row, count):
            return part.at[pl.ds(row, count), pl.ds(my_col, pa)]

        def mine_b(row, count):
            return part.at[pl.ds(row, count), pl.ds(second_col, pb)]

        def x_copy(i):
            if i >= 3:
                at = pl.ds((i - 3) * hrows, hrows)
                src, dst = s3b.at[at, pl.ds(0, pb)], rxb.at[at, pl.ds(0, pb)]
            elif i == 2:
                src, dst = mine_a(slot(*order[1]), rows), rxa.at[1, :, pl.ds(0, pa)]
            else:
                src, dst = mine_a(urow(i), hrows), rxa.at[0, pl.ds(i * hrows, hrows), pl.ds(0, pa)]
            return remote(src, dst, x_s.at[i], x_r.at[i], xpart)

        def y_copy(i):
            if i == 4:
                src, dst = s3a.at[:, pl.ds(0, pa)], ryb.at[:, pl.ds(0, pa)]
            elif i in (2, 3):
                at = (i - 2) * hrows
                row = pl.multiple_of(slot(*order[2]) + at, hrows)
                src, dst = mine_b(row, hrows), rya.at[1, pl.ds(at, hrows), pl.ds(0, pb)]
            else:
                src, dst = mine_b(urow(i), hrows), rya.at[0, pl.ds(i * hrows, hrows), pl.ds(0, pb)]
            return remote(src, dst, yy_s.at[i], yy_r.at[i], ypart)

        def relay_a():
            for i in (0, 1):
                x_copy(i).wait_recv()
            total(
                (s3a, 0, 0, pa),
                [(part, slot(r, 1 - y), my_col, pa), (rxa.at[0], 0, 0, pa)], rows,
            )

        def relay_b():
            for i in (0, 1):
                y_copy(i).wait_recv()
            total(
                (s3b, 0, 0, pb),
                [(part, slot(1 - r, y), second_col, pb), (rya.at[0], 0, 0, pb)], rows,
            )
            x_copy(3).start()

        def o_copy(i, land):
            base = (1 - core if land else core) * cols
            if i == 0:
                at = gi_out.at[:, pl.ds(pl.multiple_of(base, 128), pa)]
            else:
                at = gi_out.at[
                    pl.ds((i - 1) * hrows, hrows), pl.ds(pl.multiple_of(base + pa, 128), pb)
                ]
            return remote(at, at, o_s.at[i], o_r.at[i], cpart)

        def final_a():
            x_copy(2).wait_recv()
            y_copy(4).wait_recv()
            total(
                (gi_out, 0, my_col, pa),
                [
                    (part, here_row, my_col, pa),
                    (rxa.at[1], 0, 0, pa), (ryb, 0, 0, pa),
                ], rows,
            )
            o_copy(0, False).start()

        def final_b(i):
            at = i * hrows
            x_copy(3 + i).wait_recv()
            y_copy(2 + i).wait_recv()
            total(
                (gi_out, at, second_col, pb),
                [
                    (part, here_row + at, second_col, pb),
                    (rya.at[1], at, 0, pb), (rxb, at, 0, pb),
                ], hrows,
            )
            o_copy(1 + i, False).start()

        def settled():
            for i in range(7):
                core_copy(i).wait_send()
            for i in range(5):
                y_copy(i).wait_send()
                x_copy(i).wait_send()
            for i in range(3):
                o_copy(i, True).wait_recv()
                o_copy(i, False).wait_send()

        return (
            first_block, theirs, summed, x_copy, y_copy, relay_a, relay_b,
            final_a, final_b, settled,
        )

    def scaled(terms, rr, yy):
        at_col = gcol(rr, yy)

        @pl.loop(0, frows // 64)
        def _(m):
            at = pl.multiple_of(m * 64, 64)
            value = None
            for ref, row, col in terms:
                one = ref[pl.ds(row + at, 64), pl.ds(col, width)].astype(jnp.float32)
                value = one if value is None else value + one
            gd_out[pl.ds(at, 64), pl.ds(at_col, width)] = value * grad_scale

    def inputs_sent():
        for i in (0, 3, 5):
            dcopy(i, core).wait_send()
        tcopy(5, False).wait_send()

    @pl.when(is_end)
    def _():
        (
            first_block, theirs, summed, x_copy, y_copy, relay_a, relay_b,
            final_a, final_b, settled,
        ) = plane_sums(end_a)
        for i in range(line):
            g_block(jnp.where(lower, line - 1 - i, i))
            if i < line - 1:
                @pl.when(lower)
                def _():
                    up_copy(line - 1 - i, True).start()

                @pl.when(jnp.logical_not(lower))
                def _():
                    dn_copy(i, True).start()
        f_copy(0, False, g, zrow).start()
        f_copy(1, False, g, zrow).start()
        for d in range(last):
            for sub in range(2):
                settle(d, sub, 2)
        forward(1, dn_w, 2 * width, width, 0, 4)
        f_copy(0, True).wait_recv()
        f_copy(2, False).start()
        forward_end(1, 2, 0)
        for up_dir in (True, False):
            await_recv(up_dir, last, 1, 2)
        inputs_sent()
        finish(0)
        first_block()
        finish(1)
        theirs(4)
        summed(4)
        x_copy(2).start()
        finish(2)
        theirs(5)
        summed(5)
        y_copy(2).start()
        finish(3)
        theirs(6)
        summed(6)
        relay_a()
        y_copy(4).start()
        y_copy(3).start()
        relay_b()
        x_copy(4).start()
        h_copy(0).wait_recv()
        scaled([(g, pl.multiple_of(zrow + y * frows, frows), 0), (hl, 0, gcol(r, y))], r, y)
        final_a()
        final_b(0)
        for i, (rr, yy) in enumerate(((r, 1 - y), (1 - r, y))):
            if i == 1:
                f_copy(1, True).wait_recv()
            h_copy(1 + i).wait_recv()
            scaled([(gl, 0, gcol(rr, yy)), (hl, 0, gcol(rr, yy))], rr, yy)
        final_b(1)
        f_copy(2, True).wait_recv()
        h_copy(3).wait_recv()
        diag = gcol(1 - r, 1 - y)
        scaled([(gl, 0, diag), (hl, 0, diag)], 1 - r, 1 - y)
        settled()

    @pl.when(jnp.logical_not(is_end))
    def _():
        (
            first_block, theirs, summed, x_copy, y_copy, relay_a, relay_b,
            final_a, final_b, settled,
        ) = plane_sums(mid_a)
        inputs_sent()
        forward(1, dn_w, 2 * width, width, 3, 1)
        first_block()
        g_block(jnp.where(lower, line - 1, 0))
        forward(1, dn_w, 2 * width, width, 1, 1)
        theirs(4)
        line_step(1)
        summed(4)
        x_copy(2).start()
        forward(1, dn_w, 2 * width, width, 2, 1)
        theirs(5)
        summed(5)
        y_copy(2).start()
        relay_a()
        relay_b()
        for i in range(1, line):
            g_block(jnp.where(lower, line - 1 - i, i))
        for t in range(2, line - 1):
            line_step(t)
        y_copy(4).start()
        x_copy(4).start()
        forward(1, dn_w, 2 * width, width, 0, 1)
        theirs(6)
        summed(6)

        @pl.when(next_to_end)
        def _():
            e_copy(0, True).wait_recv()
            e_copy(2, False).start()
            h_copy(1).start()
            e_copy(1, True).wait_recv()
            h_copy(2).start()

        up_copy(z, False).wait_recv()
        dn_copy(z, False).wait_recv()
        total(
            (gfin, 0, 0, width),
            [(g, zrow, 0, width), (u_in, zrow, 0, width), (d_in, zrow, 0, width)], zrows,
        )
        f_copy(0, False).start()
        y_copy(3).start()
        scaled([(gfin, pl.multiple_of(y * frows, frows), 0)], r, y)
        f_copy(1, False).start()
        final_a()
        final_b(0)

        @pl.when(next_to_end)
        def _():
            e_copy(2, True).wait_recv()
            h_copy(3).start()

        f_copy(0, True).wait_recv()
        f_copy(2, False).start()
        scaled([(gl, 0, gcol(r, 1 - y))], r, 1 - y)
        f_copy(1, True).wait_recv()
        scaled([(gl, 0, gcol(1 - r, y))], 1 - r, y)
        final_b(1)
        f_copy(2, True).wait_recv()
        scaled([(gl, 0, gcol(1 - r, 1 - y))], 1 - r, 1 - y)

        @pl.when(next_to_end)
        def _():
            for i in range(3):
                e_copy(i, False).wait_send()
            for i in range(4):
                h_copy(i).wait_send()

        settled()

    for i in range(ntok):
        if kinds[i] == 1:
            dcopy(i, core).wait_send()
        if i != 5:
            tcopy(i, False).wait_send()
    for k in range(3):
        to_y(k).wait_send()
        for d in range(line - 1):
            for sub in range(2):
                await_send(True, d, sub, k)
                await_send(False, d, sub, k)
    for i in range(3):
        f_copy(i, False).wait_send()
    for zt in range(line):
        if zt > 0:
            far = line - 2 if zt == line - 1 else zt
            pl.when(z < far)(lambda: up_copy(zt, True).wait_send())
        if zt < line - 1:
            near = 1 if zt == 0 else zt
            pl.when(z > near)(lambda: dn_copy(zt, True).wait_send())


def fused(grad_scale, gate_w, up_w, down_w, toks, cots):
    line = lax.axis_size("fs") // 2
    rows, full = toks.shape
    wrows, width = gate_w.shape[0], gate_w.shape[1] // 4
    depth = 2 * line * wrows
    cols = full // 2
    kind = gate_w.dtype
    dma = pltpu.SemaphoreType.DMA
    zsem = dma((line - 1, 2, 3))
    anyspec = pl.BlockSpec(memory_space=pl.ANY)
    whole = pltpu.VMEM((depth, width), kind)
    end_a, mid_a = cols // 2, cols * 3 // 8 // 128 * 128
    most_b = cols - mid_a
    return pl.pallas_call(
        functools.partial(fused_kernel, line, grad_scale, end_a, mid_a),
        out_shape=(
            pltpu.VMEM((rows, full), kind),
            pltpu.VMEM((wrows, 4 * width), jnp.float32),
        ),
        in_specs=[anyspec] * 5,
        out_specs=(pl.BlockSpec(memory_space=pltpu.VMEM),) * 2,
        scratch_shapes=[
            pltpu.VMEM((2, 4 * rows, full), kind),
            pltpu.VMEM((depth, 2 * width), kind),
            whole,
            pltpu.VMEM((4 * rows, 3 * width), jnp.float32),
            pltpu.VMEM((4 * rows, width), kind),
            pltpu.VMEM((4 * rows, 2 * width), kind),
            pltpu.VMEM((4 * rows, cols), kind),
            pltpu.VMEM((2, rows, end_a), kind), pltpu.VMEM((rows, most_b), kind),
            pltpu.VMEM((2, rows, most_b), kind), pltpu.VMEM((rows, end_a), kind),
            pltpu.VMEM((rows, end_a), kind), pltpu.VMEM((rows, most_b), kind),
            whole, whole, whole,
            pltpu.VMEM((2 * wrows, width), kind),
            pltpu.VMEM((wrows, 4 * width), kind),
            pltpu.VMEM((wrows, 4 * width), kind),
            zsem, zsem, zsem, zsem,
            dma((3,)), dma((3,)),
            dma((8,)), dma((8,)), dma((8,)), dma((8,)), dma((5,)),
            dma((7,)), dma((7,)), dma((5,)), dma((5,)), dma((5,)), dma((5,)),
            dma((line,)), dma((line,)), dma((line,)), dma((line,)),
            dma((3,)), dma((3,)), dma((3,)), dma((3,)),
            dma((3,)), dma((3,)), dma((4,)), dma((4,)),
        ],
        compiler_params=pltpu.CompilerParams(
            collective_id=1, has_side_effects=True, vmem_limit_bytes=59 * 2**20
        ),
        name="fused_all",
    )(gate_w, up_w, down_w, toks, cots)


def place_kernel(a, b, a_out, b_out, sems):
    copies = [
        pltpu.make_async_copy(a, a_out, sems.at[0]),
        pltpu.make_async_copy(b, b_out, sems.at[1]),
    ]
    for copy in copies:
        copy.start()
    for copy in copies:
        copy.wait()


def place(a, b):
    anyspec = pl.BlockSpec(memory_space=pl.ANY)
    return pl.pallas_call(
        place_kernel,
        out_shape=(
            jax.ShapeDtypeStruct(a.shape, a.dtype), jax.ShapeDtypeStruct(b.shape, b.dtype),
        ),
        in_specs=[pl.BlockSpec(memory_space=pltpu.VMEM)] * 2,
        out_specs=(anyspec,) * 2,
        scratch_shapes=[pltpu.SemaphoreType.DMA((2,))],
        compiler_params=pltpu.CompilerParams(vmem_limit_bytes=16 * 2**20),
        name="place",
    )(a, b)


def gather_kernel(
    line, units, gate_w, up_w, down_w, toks, cots, gu_out, d_out, t_out, w_tmp, t_tmp,
    up_s, up_r, dn_s, dn_r, y_s, y_r, tok_s, tok_r, d2d_s, d2d_r, loc, loc2,
):
    r = lax.axis_index("rep")
    f = lax.axis_index("fs")
    t = lax.axis_index("tp")
    z, y = f // 2, f % 2
    rows = toks.shape[0]
    half = rows // 2
    wrows = gate_w.shape[0]
    width = gate_w.shape[1] // 4
    parts = len(units)
    has_up, has_dn = z < line - 1, z > 0
    up = {"fs": (f + 2) % (2 * line)}
    dn = {"fs": (f + 2 * line - 2) % (2 * line)}
    ypart = {"fs": f + 1 - 2 * y}
    xpart = {"rep": 1 - r}
    core = t % 2
    cpart = {"tp": t + 1 - 2 * core}

    barrier = pltpu.get_barrier_semaphore()

    def greet(dev):
        pl.semaphore_signal(barrier, inc=1, device_id=dev, device_id_type=MESH)

    for dev in (ypart, xpart, cpart, up, dn):
        greet(dev)
    pl.semaphore_wait(barrier, 5)

    def remote(src, dst, s, q, dev):
        return pltpu.make_async_remote_copy(
            src_ref=src, dst_ref=dst, send_sem=s, recv_sem=q,
            device_id=dev, device_id_type=MESH,
        )

    def wblk(k, zz, yy):
        row = pl.multiple_of((2 * zz + yy) * wrows, wrows)
        which, col, wide = units[k]
        return (gu_out, d_out)[which].at[pl.ds(row, wrows), pl.ds(col, wide)]

    def own(k, yy):
        col = pl.multiple_of((2 * r + yy) * width, width)
        return (gate_w, up_w, down_w)[k].at[:, pl.ds(col, width)]

    def to_y(k):
        return remote(own(k, 1 - y), wblk(k, z, y), y_s.at[k], y_r.at[k], ypart)

    def from_y(k):
        return remote(own(k, 1 - y), wblk(k, z, 1 - y), y_s.at[k], y_r.at[k], ypart)

    def zcopy(up_dir, d, sub, k, zz):
        yy = y if sub == 0 else 1 - y
        src = own(k, y) if (d == 0 and sub == 0) else wblk(k, zz, yy)
        s, q, dev = (up_s, up_r, up) if up_dir else (dn_s, dn_r, dn)
        return remote(src, wblk(k, zz, yy), s.at[d, sub, k], q.at[d, sub, k], dev)

    def pred_send(up_dir, d):
        return (has_up & (z - d >= 0)) if up_dir else (has_dn & (z + d <= line - 1))

    def src_z(up_dir, d):
        return jnp.maximum(z - d, 0) if up_dir else jnp.minimum(z + d, line - 1)

    def send(up_dir, d, sub, k):
        @pl.when(pred_send(up_dir, d))
        def _():
            zcopy(up_dir, d, sub, k, src_z(up_dir, d)).start()

    def await_send(up_dir, d, sub, k):
        @pl.when(pred_send(up_dir, d))
        def _():
            zcopy(up_dir, d, sub, k, src_z(up_dir, d)).wait_send()

    def await_recv(up_dir, d, sub, k):
        ok = (z - d - 1 >= 0) if up_dir else (z + d + 1 <= line - 1)

        @pl.when(ok)
        def _():
            zcopy(up_dir, d, sub, k, src_z(up_dir, d + 1)).wait_recv()

    def tblk(j, rr, yy, c):
        row = pl.multiple_of((2 * rr + yy) * rows + c * half, half)
        return t_out.at[j, pl.ds(row, half), :]

    def mine(j):
        src = toks if j == 0 else cots
        return src.at[pl.ds(pl.multiple_of(core * half, half), half), :]

    def tcopy(i, landing):
        j = (0, 1, 0, 1, 0, 1)[i]
        dev = xpart if i in (0, 1, 5) else ypart
        if landing:
            rr = (1 - r, 1 - r, r, r, 1 - r, 1 - r)[i]
            yy = (y, y, 1 - y, 1 - y, 1 - y, 1 - y)[i]
            src = dst = tblk(j, rr, yy, core)
        else:
            rr = (r, r, r, r, 1 - r, r)[i]
            yy = (y, y, y, y, y, 1 - y)[i]
            dst = tblk(j, rr, yy, core)
            src = mine(j) if i < 4 else dst
        return remote(src, dst, tok_s.at[i], tok_r.at[i], dev)

    def dcopy(i, c):
        j = (0, 1, 0, 1, 0, 1)[i]
        rr = (1 - r, 1 - r, r, r, 1 - r, 1 - r)[i]
        yy = (y, y, 1 - y, 1 - y, 1 - y, 1 - y)[i]
        blk = tblk(j, rr, yy, c)
        return remote(blk, blk, d2d_s.at[i], d2d_r.at[i], cpart)

    loads = [
        pltpu.make_async_copy(own(0, y), w_tmp.at[0], loc.at[0]),
        pltpu.make_async_copy(own(1, y), w_tmp.at[1], loc.at[3]),
        pltpu.make_async_copy(own(2, y), w_tmp.at[2], loc.at[4]),
        pltpu.make_async_copy(toks, t_tmp.at[0], loc.at[1]),
        pltpu.make_async_copy(cots, t_tmp.at[1], loc.at[2]),
    ]
    trow = pl.multiple_of((2 * r + y) * rows, rows)
    stores = [
        pltpu.make_async_copy(w_tmp.at[0], wblk(0, z, y), loc2.at[0]),
        pltpu.make_async_copy(w_tmp.at[1], wblk(1, z, y), loc2.at[3]),
        pltpu.make_async_copy(w_tmp.at[2], wblk(2, z, y), loc2.at[4]),
        pltpu.make_async_copy(t_tmp.at[0], t_out.at[0, pl.ds(trow, rows), :], loc2.at[1]),
        pltpu.make_async_copy(t_tmp.at[1], t_out.at[1, pl.ds(trow, rows), :], loc2.at[2]),
    ]

    for k in range(parts):
        to_y(k).start()
        send(True, 0, 0, k)
        send(False, 0, 0, k)
    for i in (0, 1, 3, 2):
        tcopy(i, False).start()
    for copy in loads:
        copy.start()
    for load, store in zip(loads, stores):
        load.wait()
        store.start()
    for k in range(parts):
        from_y(k).wait_recv()
        send(True, 0, 1, k)
        send(False, 0, 1, k)

    def event(i):
        tcopy(i, True).wait_recv()
        if i == 0:
            tcopy(4, False).start()
        if i == 3:
            tcopy(5, False).start()
        dcopy(i, core).start()

    events = [0, 3, 1, 2, 5, 4]
    for d in range(line - 1):
        for sub in range(2):
            if events:
                event(events.pop(0))
            for k in range(parts):
                for up_dir in (True, False):
                    await_recv(up_dir, d, sub, k)
                    if d + 1 < line - 1:
                        send(up_dir, d + 1, sub, k)
    for i in events:
        event(i)
    for i in range(6):
        dcopy(i, 1 - core).wait_recv()
        dcopy(i, core).wait_send()
        tcopy(i, False).wait_send()
    for k in range(parts):
        to_y(k).wait_send()
        for d in range(line - 1):
            for sub in range(2):
                await_send(True, d, sub, k)
                await_send(False, d, sub, k)
    for store in stores:
        store.wait()


def gather(gate_w, up_w, down_w, toks, cots):
    line = lax.axis_size("fs") // 2
    wrows, width = gate_w.shape[0], gate_w.shape[1] // 4
    units = [(0, 0, width), (0, width, width), (1, 0, width)]
    parts = len(units)
    depth = 2 * line * wrows
    kind = gate_w.dtype
    dma = pltpu.SemaphoreType.DMA
    zsem = dma((line - 1, 2, parts))
    anyspec = pl.BlockSpec(memory_space=pl.ANY)
    return pl.pallas_call(
        functools.partial(gather_kernel, line, units),
        out_shape=(
            jax.ShapeDtypeStruct((depth, 2 * width), kind),
            jax.ShapeDtypeStruct((depth, width), kind),
            jax.ShapeDtypeStruct((2, 4 * toks.shape[0], toks.shape[1]), toks.dtype),
        ),
        in_specs=[anyspec] * 5,
        out_specs=(anyspec,) * 3,
        scratch_shapes=[
            pltpu.VMEM((parts, wrows, width), kind),
            pltpu.VMEM((2,) + toks.shape, toks.dtype),
            zsem, zsem, zsem, zsem,
            dma((parts,)), dma((parts,)),
            dma((6,)), dma((6,)), dma((6,)), dma((6,)),
            dma((5,)), dma((5,)),
        ],
        compiler_params=pltpu.CompilerParams(collective_id=0, has_side_effects=True),
        name="gather_all",
    )(gate_w, up_w, down_w, toks, cots)


def on_device(inputs, cotangent, gate_weight, up_weight, down_weight):
    tok_rows = inputs.shape[0]
    fs_size = lax.axis_size("fs")
    rep_size = lax.axis_size("rep")
    grad_scale = 1.0 / math.sqrt(tok_rows * fs_size * rep_size)
    if lax.axis_size("tp") == 2 and rep_size == 2 and fs_size >= 8:
        return place(*fused(
            grad_scale, gate_weight, up_weight, down_weight, inputs, cotangent
        ))
    contract = (((1,), (1,)), ((), ()))
    contract_tok = (((0,), (0,)), ((), ()))
    width = gate_weight.shape[1] // 4
    gate_up, down_full, tokens = gather(
        gate_weight, up_weight, down_weight, inputs, cotangent
    )
    gate_up_val = jnp.dot(tokens[0], gate_up, preferred_element_type=jnp.float32)
    gate_val, up_val = gate_up_val[:, :width], gate_up_val[:, width:]
    grad_hidden = jnp.dot(tokens[1], down_full, preferred_element_type=jnp.float32)
    sigmoid_gate = jax.nn.sigmoid(gate_val)
    active = gate_val * sigmoid_gate
    hidden = (active * up_val).astype(jnp.bfloat16)
    grad_gate = (
        grad_hidden * up_val * sigmoid_gate * (1.0 + gate_val * (1.0 - sigmoid_gate))
    ).astype(jnp.bfloat16)
    grad_up = (grad_hidden * active).astype(jnp.bfloat16)
    pairs = [[i, i + 1] for i in range(0, fs_size, 2)]
    lines = [list(range(i, fs_size, 2)) for i in range(2)]
    grad_part = lax.dot_general(
        tokens[1], hidden, contract_tok, preferred_element_type=jnp.float32
    )
    part = lax.dot_general(
        jnp.concatenate([grad_gate, grad_up], axis=1), gate_up, contract,
        preferred_element_type=jnp.float32,
    )
    shard = lax.psum_scatter(
        grad_part.astype(jnp.bfloat16), "fs", scatter_dimension=0, tiled=True,
        axis_index_groups=lines,
    ).astype(jnp.float32) * grad_scale
    shard = lax.all_to_all(
        shard, "fs", split_axis=0, concat_axis=1, tiled=True, axis_index_groups=pairs
    )
    grad_down = lax.all_gather(shard, "rep", axis=1, tiled=True)
    part = lax.psum_scatter(
        part.astype(jnp.bfloat16), "rep", scatter_dimension=0, tiled=True
    )
    part = lax.psum_scatter(
        part, "fs", scatter_dimension=0, tiled=True, axis_index_groups=pairs
    )
    grad_input = lax.psum(part, "tp")
    return (grad_input, grad_down)


def solution(mesh):
    placed = (
        P(("rep", "fs"), None),
        P(("rep", "fs"), None),
        P("fs", "tp"),
        P("fs", "tp"),
        P("fs", "tp"),
    )
    return jax.shard_map(
        on_device,
        mesh=mesh,
        in_specs=placed,
        out_specs=(P(("rep", "fs"), None), P("fs", "tp")),
        check_vma=False,
    )
```

```python
import functools
import math

import jax
import jax.numpy as jnp
from jax import lax
from jax.experimental import pallas as pl
from jax.experimental.pallas import tpu as pltpu
from jax.sharding import PartitionSpec as P

MESH = pl.DeviceIdType.MESH


def fused_kernel(
    line, grad_scale, end_a, mid_a, gate_w, up_w, down_w, toks, cots, gi_out, gd_out,
    x, gu, dn_w, acc, hid, ggu, r1, rxa, rxb, rya, ryb, s3a, s3b, g, u_in, d_in, gfin, gl, hl,
    z_s, up_r, dn_r, wy_s, wy_r, tok_s, tok_r, d2d_s, d2d_r, loc,
    c_s, c_r, x_s, x_r, yy_s, yy_r, u_s, u_r, d_s, d_r, f_s, f_r, o_s, o_r, e_s, e_r, h_s, h_r,
):
    r = lax.axis_index("rep")
    f = lax.axis_index("fs")
    core = lax.axis_index("tp")
    z, y = f // 2, f % 2
    rows = toks.shape[0]
    half = rows // 2
    wrows = gate_w.shape[0]
    width = gate_w.shape[1] // 4
    depth = 2 * line * wrows
    zrows = 2 * wrows
    cols = depth // 2
    wide = cols // 2
    frows = wrows
    last = line - 2
    has_up, has_dn = z < line - 1, z > 0
    is_end = (z == 0) | (z == line - 1)
    up = {"fs": (f + 2) % (2 * line)}
    dn = {"fs": (f + 2 * line - 2) % (2 * line)}
    ypart = {"fs": f + 1 - 2 * y}
    xpart = {"rep": 1 - r}
    cpart = {"tp": 1 - core}

    barrier = pltpu.get_barrier_semaphore()
    for dev in (ypart, xpart, cpart, up, dn):
        pl.semaphore_signal(barrier, inc=1, device_id=dev, device_id_type=MESH)
    pl.semaphore_wait(barrier, 5)

    def remote(src, dst, s, q, dev):
        return pltpu.make_async_remote_copy(
            src_ref=src, dst_ref=dst, send_sem=s, recv_sem=q,
            device_id=dev, device_id_type=MESH,
        )

    def wblk(k, zz, yy):
        row = pl.multiple_of((2 * zz + yy) * wrows, wrows)
        if k == 2:
            return dn_w.at[pl.ds(row, wrows), :]
        return gu.at[pl.ds(row, wrows), pl.ds(k * width, width)]

    def own(k, yy):
        col = pl.multiple_of((2 * r + yy) * width, width)
        return (gate_w, up_w, down_w)[k].at[:, pl.ds(col, width)]

    def to_y(k):
        return remote(own(k, 1 - y), wblk(k, z, y), wy_s.at[k], wy_r.at[k], ypart)

    def from_y(k):
        return remote(own(k, 1 - y), wblk(k, z, 1 - y), wy_s.at[k], wy_r.at[k], ypart)

    def zcopy(up_dir, d, sub, k, zz):
        yy = y if sub == 0 else 1 - y
        src = own(k, y) if (d == 0 and sub == 0) else wblk(k, zz, yy)
        q, dev = (up_r, up) if up_dir else (dn_r, dn)
        return remote(src, wblk(k, zz, yy), z_s, q.at[d, sub, k], dev)

    def pred_send(up_dir, d):
        return (has_up & (z - d >= 0)) if up_dir else (has_dn & (z + d <= line - 1))

    def src_z(up_dir, d):
        return jnp.maximum(z - d, 0) if up_dir else jnp.minimum(z + d, line - 1)

    def send(up_dir, d, sub, k):
        @pl.when(pred_send(up_dir, d))
        def _():
            zcopy(up_dir, d, sub, k, src_z(up_dir, d)).start()

    def await_recv(up_dir, d, sub, k):
        ok = (z - d - 1 >= 0) if up_dir else (z + d + 1 <= line - 1)

        @pl.when(ok)
        def _():
            zcopy(up_dir, d, sub, k, src_z(up_dir, d + 1)).wait_recv()

    def relay(d, sub, k):
        for up_dir in (True, False):
            @pl.when(pred_send(up_dir, d + 1))
            def _():
                zcopy(up_dir, d, sub, k, src_z(up_dir, d + 1)).wait_recv()
                zcopy(up_dir, d + 1, sub, k, src_z(up_dir, d + 1)).start()

    def settle(d, sub, k):
        for up_dir in (True, False):
            ok = (z - d - 1 >= 0) if up_dir else (z + d + 1 <= line - 1)
            onward = has_up if up_dir else has_dn

            @pl.when(ok & jnp.logical_not(onward))
            def _():
                zcopy(up_dir, d, sub, k, src_z(up_dir, d + 1)).wait_recv()

    def slot(rr, yy):
        return pl.multiple_of((2 * rr + yy) * rows, rows)

    kinds = (0, 1, 1, 0, 1, 0, 1, 1)
    over_x = (True, True, True, False, False, True, False, True)
    parts = (2, 0, 1, 2, 2, 2, 0, 1)
    ntok = len(kinds)

    def span(c, p):
        if p == 2:
            return c * half, half
        return c * half + p * (half // 2), half // 2

    def tblk(i, rr, yy, c):
        at, count = span(c, parts[i])
        row = pl.multiple_of((2 * rr + yy) * rows + at, half // 2)
        return x.at[kinds[i], pl.ds(row, count), :]

    def mine(i):
        at, count = span(core, parts[i])
        src = toks if kinds[i] == 0 else cots
        return src.at[pl.ds(pl.multiple_of(at, half // 2), count), :]

    def landing(i, c):
        rr = (1 - r, 1 - r, 1 - r, r, r, 1 - r, 1 - r, 1 - r)[i]
        yy = (y, y, y, 1 - y, 1 - y, 1 - y, 1 - y, 1 - y)[i]
        return tblk(i, rr, yy, c)

    def tcopy(i, land):
        dev = xpart if over_x[i] else ypart
        if land:
            src = dst = landing(i, core)
        else:
            rr = (r, r, r, r, r, r, 1 - r, r)[i]
            yy = (y, y, y, y, y, 1 - y, y, 1 - y)[i]
            dst = tblk(i, rr, yy, core)
            src = mine(i) if i < 5 else dst
        return remote(src, dst, tok_s.at[i], tok_r.at[i], dev)

    def dcopy(i, c):
        blk = landing(i, c)
        return remote(blk, blk, d2d_s.at[i], d2d_r.at[i], cpart)

    def event(i):
        tcopy(i, True).wait_recv()
        onward = {1: 6, 3: 5, 4: 7}.get(i)
        if onward is not None:
            tcopy(onward, False).start()
        dcopy(i, core).start()

    trow = slot(r, y)
    loads = [
        pltpu.make_async_copy(own(0, y), wblk(0, z, y), loc.at[0]),
        pltpu.make_async_copy(own(1, y), wblk(1, z, y), loc.at[1]),
        pltpu.make_async_copy(own(2, y), wblk(2, z, y), loc.at[2]),
        pltpu.make_async_copy(toks, x.at[0, pl.ds(trow, rows), :], loc.at[3]),
        pltpu.make_async_copy(cots, x.at[1, pl.ds(trow, rows), :], loc.at[4]),
    ]

    tile = 256
    z_lo = jnp.maximum(z - last, 0)
    z_hi = jnp.minimum(z + last, line - 1) + 1

    def product(j, row, k0, kk, w, wcol, acol, n):
        at = pl.ds(pl.multiple_of(row, rows), rows)
        kat = pl.ds(pl.multiple_of(k0, wrows), kk)
        for c in range(0, n, tile):
            one = jnp.dot(
                x[j, at, kat], w[kat, pl.ds(wcol + c, tile)],
                preferred_element_type=jnp.float32,
            )
            acc[at, pl.ds(acol + c, tile)] += one

    def forward(j, w, acol, n, first, count):
        @pl.loop(first, first + count)
        def _(b):
            row = ((2 * r + y) + 2 * (b % 2) * (1 - 2 * r) + (b // 2) * (1 - 2 * y)) * rows

            @pl.loop(z_lo, z_hi)
            def _(zz):
                product(j, row, zz * zrows, zrows, w, 0, acol, n)

    def forward_end(j, k, sub):
        for up_dir in (True, False):
            await_recv(up_dir, last, sub, k)

        @pl.when(is_end)
        def _():
            zz = line - 1 - z
            yy = y if sub == 0 else 1 - y
            w = dn_w if k == 2 else gu

            @pl.loop(0, 4)
            def _(b):
                product(
                    j, b * rows, (2 * zz + yy) * wrows, wrows, w,
                    0 if k == 2 else k * width, k * width, width,
                )

    def total(dst, terms, count, step=64):
        @pl.loop(0, count // step)
        def _(i):
            at = pl.multiple_of(i * step, step)
            value = None
            for ref, row, col, wide in terms:
                one = ref[pl.ds(row + at, step), pl.ds(col, wide)].astype(jnp.float32)
                value = one if value is None else value + one
            ref, row, col, wide = dst
            ref[pl.ds(row + at, step), pl.ds(col, wide)] = value.astype(ref.dtype)

    for k in (0, 1):
        to_y(k).start()
        send(True, 0, 0, k)
        send(False, 0, 0, k)
    for i in (0, 1, 3):
        tcopy(i, False).start()
    to_y(2).start()
    tcopy(4, False).start()
    for copy in loads:
        copy.start()

    @pl.loop(0, 4 * rows // 64)
    def _(i):
        at = pl.ds(pl.multiple_of(i * 64, 64), 64)
        acc[at, :] = jnp.zeros((64, 3 * width), jnp.float32)

    for k in (0, 1):
        from_y(k).wait_recv()
        send(True, 0, 1, k)
        send(False, 0, 1, k)
    if last > 0:
        for sub in range(2):
            for k in (0, 1):
                relay(0, sub, k)
    event(0)
    event(3)
    tcopy(2, False).start()
    event(1)
    for d in range(1, last):
        for sub in range(2):
            for k in (0, 1):
                relay(d, sub, k)
    send(True, 0, 0, 2)
    send(False, 0, 0, 2)
    from_y(2).wait_recv()
    send(True, 0, 1, 2)
    send(False, 0, 1, 2)
    for load in loads:
        load.wait()
    for d in range(last):
        for sub in range(2):
            for k in (0, 1):
                settle(d, sub, k)
    dcopy(0, 1 - core).wait_recv()
    dcopy(3, 1 - core).wait_recv()
    forward(0, gu, 0, 2 * width, 0, 3)
    if last > 0:
        for sub in range(2):
            relay(0, sub, 2)
    event(5)
    event(4)
    dcopy(5, 1 - core).wait_recv()
    forward(0, gu, 0, 2 * width, 3, 1)
    for d in range(1, last):
        for sub in range(2):
            relay(d, sub, 2)
    for sub in range(2):
        for k in (0, 1):
            forward_end(0, k, sub)

    @pl.loop(0, 4 * rows // 32)
    def _(i):
        at = pl.ds(pl.multiple_of(i * 32, 32), 32)
        gate = acc[at, pl.ds(0, width)]
        up_val = acc[at, pl.ds(width, width)]
        sig = jax.nn.sigmoid(gate)
        active = gate * sig
        hid[at, :] = (active * up_val).astype(hid.dtype)
        acc[at, pl.ds(0, width)] = up_val * sig * (1.0 + gate * (1.0 - sig))
        acc[at, pl.ds(width, width)] = active


    zrow = pl.multiple_of(z * zrows, zrows)
    lower = z < line // 2

    def block(ref, zt):
        return ref.at[pl.ds(zt * zrows, zrows), :]

    def up_copy(zt, first):
        return remote(block(g if first else u_in, zt), block(u_in, zt), u_s.at[zt], u_r.at[zt], up)

    def dn_copy(zt, first):
        return remote(block(g if first else d_in, zt), block(d_in, zt), d_s.at[zt], d_r.at[zt], dn)

    def g_block(zt):
        at = pl.multiple_of(zt * zrows, zrows)
        one = lax.dot_general(
            x[1, :, pl.ds(at, zrows)], hid[...], (((0,), (0,)), ((), ())),
            preferred_element_type=jnp.float32,
        )
        g[pl.ds(at, zrows), :] = one.astype(g.dtype)

    def gcol(rr, yy):
        return pl.multiple_of((2 * rr + yy) * width, width)

    def gcols(ref, rr, yy):
        return ref.at[:, pl.ds(gcol(rr, yy), width)]

    def half_rows(ref, row, yy):
        return ref.at[pl.ds(pl.multiple_of(row + yy * frows, frows), frows), :]

    def f_copy(i, land, ref=gfin, row=0):
        if i == 0:
            src, dst, dev = half_rows(ref, row, 1 - y), gcols(gl, r, 1 - y if land else y), ypart
        elif i == 1:
            src, dst, dev = half_rows(ref, row, y), gcols(gl, 1 - r if land else r, y), xpart
        else:
            src, dst, dev = gcols(gl, r, 1 - y), gcols(gl, 1 - r if land else r, 1 - y), xpart
        return remote(src, dst, f_s.at[i], f_r.at[i], dev)

    def e_copy(i, land, ref=gfin, row=0):
        if i == 0:
            src, dst, dev = half_rows(ref, row, 1 - y), gcols(hl, r, 1 - y if land else y), ypart
        elif i == 1:
            src, dst, dev = half_rows(ref, row, y), gcols(hl, 1 - r if land else r, y), xpart
        else:
            src, dst, dev = gcols(hl, r, 1 - y), gcols(hl, 1 - r if land else r, 1 - y), xpart
        return remote(src, dst, e_s.at[i], e_r.at[i], dev)

    end_z = jnp.where((z == 1) | (z == line - 1), 0, line - 1)
    end_dev = {"fs": 2 * end_z + y}
    next_to_end = (z == 1) | (z == line - 2)

    def h_copy(i, ref=gfin, row=0):
        rr, yy = ((r, y), (r, 1 - y), (1 - r, y), (1 - r, 1 - y))[i]
        dst = gcols(hl, rr, yy)
        src = half_rows(ref, row, y) if i == 0 else dst
        return remote(src, dst, h_s.at[i], h_r.at[i], end_dev)

    def share(ref, row):
        h_copy(0, ref, row).start()
        e_copy(0, False, ref, row).start()
        e_copy(1, False, ref, row).start()

    def line_step(t):
        zt = line - 1 + z - t
        row_u = pl.multiple_of(zt * zrows, zrows)
        is_u = (z > 0) & (zt <= line - 1) & (zt > z)
        zd = t - (line - 1 - z)
        row_d = pl.multiple_of(zd * zrows, zrows)
        is_d = (z < line - 1) & (zd >= 0) & (zd < z)
        final = t == line - 2

        def add_u():
            up_copy(zt, False).wait_recv()
            total((u_in, row_u, 0, width), [(g, row_u, 0, width), (u_in, row_u, 0, width)], zrows)

        def add_d():
            dn_copy(zd, False).wait_recv()
            total((d_in, row_d, 0, width), [(g, row_d, 0, width), (d_in, row_d, 0, width)], zrows)

        @pl.when((is_u & (z < line - 2)) if final else is_u)
        def _():
            add_u()
            up_copy(zt, False).start()

        @pl.when((is_d & (z > 1)) if final else is_d)
        def _():
            add_d()
            dn_copy(zd, False).start()

        if final:
            @pl.when(z == line - 2)
            def _():
                add_u()
                share(u_in, (line - 1) * zrows)

            @pl.when(z == 1)
            def _():
                add_d()
                share(d_in, 0)

    order = [(1 - r, 1 - y), (1 - r, y), (r, 1 - y), (r, y)]
    my_col = pl.multiple_of(core * cols, cols)
    its_col = pl.multiple_of((1 - core) * cols, cols)
    part = x.at[0]

    def slopes(row, count):
        @pl.loop(0, count // 32)
        def _(i):
            at = pl.ds(pl.multiple_of(row + i * 32, 32), 32)
            grad = acc[at, pl.ds(2 * width, width)]
            ggu[at, pl.ds(0, width)] = (grad * acc[at, pl.ds(0, width)]).astype(ggu.dtype)
            ggu[at, pl.ds(width, width)] = (grad * acc[at, pl.ds(width, width)]).astype(ggu.dtype)

    def back(row, count, col, n):
        step = min(n, wide) if n % wide == 0 else n

        @pl.loop(0, n // step)
        def _(i):
            at = pl.multiple_of(col + i * step, 128)
            one = lax.dot_general(
                ggu[pl.ds(row, count), :], gu[pl.ds(at, step), :], (((1,), (1,)), ((), ())),
                preferred_element_type=jnp.float32,
            )
            x[0, pl.ds(row, count), pl.ds(at, step)] = one.astype(x.dtype)

    hrows = rows // 2

    def finish(b):
        @pl.when(is_end)
        def _():
            product(
                1, slot(*order[b]), (2 * (line - 1 - z) + 1 - y) * wrows, wrows,
                dn_w, 0, 2 * width, width,
            )

    here_row = slot(r, y)

    def plane_sums(pa):
        pb = cols - pa
        pieces = [
            (0, 0, hrows, 0, pa), (0, 0, hrows, pa, pb),
            (0, hrows, hrows, 0, pa), (0, hrows, hrows, pa, pb),
            (1, 0, rows, 0, cols), (2, 0, rows, 0, cols), (3, 0, rows, 0, cols),
        ]

        def place_of(i, col):
            b, at, count, c0, n = pieces[i]
            row = pl.multiple_of(slot(*order[b]) + at, hrows)
            return row, count, pl.multiple_of(col + c0, 128), c0, n

        def core_copy(i):
            row, count, col, c0, n = place_of(i, its_col)
            return remote(
                part.at[pl.ds(row, count), pl.ds(col, n)],
                r1.at[pl.ds(row, count), pl.ds(c0, n)], c_s.at[i], c_r.at[i], cpart,
            )

        def theirs(i):
            row, count, col, c0, n = place_of(i, its_col)
            if c0 == 0:
                slopes(row, count)
            back(row, count, col, n)
            core_copy(i).start()

        def summed(i):
            row, count, col, c0, n = place_of(i, my_col)
            back(row, count, col, n)
            core_copy(i).wait_recv()
            total((part, row, col, n), [(part, row, col, n), (r1, row, c0, n)], count)

        def first_block():
            theirs(0)
            theirs(1)
            theirs(2)
            summed(0)
            x_copy(0).start()
            summed(1)
            y_copy(0).start()
            theirs(3)
            summed(2)
            x_copy(1).start()
            summed(3)
            y_copy(1).start()

        def urow(u):
            return pl.multiple_of(slot(*order[0]) + u * hrows, hrows)

        second_col = pl.multiple_of(my_col + pa, 128)

        def mine_a(row, count):
            return part.at[pl.ds(row, count), pl.ds(my_col, pa)]

        def mine_b(row, count):
            return part.at[pl.ds(row, count), pl.ds(second_col, pb)]

        def x_copy(i):
            if i >= 3:
                at = pl.ds((i - 3) * hrows, hrows)
                src, dst = s3b.at[at, pl.ds(0, pb)], rxb.at[at, pl.ds(0, pb)]
            elif i == 2:
                src, dst = mine_a(slot(*order[1]), rows), rxa.at[1, :, pl.ds(0, pa)]
            else:
                src, dst = mine_a(urow(i), hrows), rxa.at[0, pl.ds(i * hrows, hrows), pl.ds(0, pa)]
            return remote(src, dst, x_s.at[i], x_r.at[i], xpart)

        def y_copy(i):
            if i == 4:
                src, dst = s3a.at[:, pl.ds(0, pa)], ryb.at[:, pl.ds(0, pa)]
            elif i in (2, 3):
                at = (i - 2) * hrows
                row = pl.multiple_of(slot(*order[2]) + at, hrows)
                src, dst = mine_b(row, hrows), rya.at[1, pl.ds(at, hrows), pl.ds(0, pb)]
            else:
                src, dst = mine_b(urow(i), hrows), rya.at[0, pl.ds(i * hrows, hrows), pl.ds(0, pb)]
            return remote(src, dst, yy_s.at[i], yy_r.at[i], ypart)

        def relay_a():
            for i in (0, 1):
                x_copy(i).wait_recv()
            total(
                (s3a, 0, 0, pa),
                [(part, slot(r, 1 - y), my_col, pa), (rxa.at[0], 0, 0, pa)], rows,
            )

        def relay_b():
            for i in (0, 1):
                y_copy(i).wait_recv()
            total(
                (s3b, 0, 0, pb),
                [(part, slot(1 - r, y), second_col, pb), (rya.at[0], 0, 0, pb)], rows,
            )
            x_copy(3).start()

        def o_copy(i, land):
            base = (1 - core if land else core) * cols
            if i == 0:
                at = gi_out.at[:, pl.ds(pl.multiple_of(base, 128), pa)]
            else:
                at = gi_out.at[
                    pl.ds((i - 1) * hrows, hrows), pl.ds(pl.multiple_of(base + pa, 128), pb)
                ]
            return remote(at, at, o_s.at[i], o_r.at[i], cpart)

        def final_a():
            x_copy(2).wait_recv()
            y_copy(4).wait_recv()
            total(
                (gi_out, 0, my_col, pa),
                [
                    (part, here_row, my_col, pa),
                    (rxa.at[1], 0, 0, pa), (ryb, 0, 0, pa),
                ], rows,
            )
            o_copy(0, False).start()

        def final_b(i):
            at = i * hrows
            x_copy(3 + i).wait_recv()
            y_copy(2 + i).wait_recv()
            total(
                (gi_out, at, second_col, pb),
                [
                    (part, here_row + at, second_col, pb),
                    (rya.at[1], at, 0, pb), (rxb, at, 0, pb),
                ], hrows,
            )
            o_copy(1 + i, False).start()

        def settled():
            for i in range(7):
                core_copy(i).wait_send()
            for i in range(5):
                y_copy(i).wait_send()
                x_copy(i).wait_send()
            for i in range(3):
                o_copy(i, True).wait_recv()
                o_copy(i, False).wait_send()

        return (
            first_block, theirs, summed, x_copy, y_copy, relay_a, relay_b,
            final_a, final_b, settled,
        )

    def scaled(terms, rr, yy):
        at_col = gcol(rr, yy)

        @pl.loop(0, frows // 64)
        def _(m):
            at = pl.multiple_of(m * 64, 64)
            value = None
            for ref, row, col in terms:
                one = ref[pl.ds(row + at, 64), pl.ds(col, width)].astype(jnp.float32)
                value = one if value is None else value + one
            gd_out[pl.ds(at, 64), pl.ds(at_col, width)] = value * grad_scale

    def inputs_sent():
        for i in (0, 3, 5):
            dcopy(i, core).wait_send()
        tcopy(5, False).wait_send()

    @pl.when(is_end)
    def _():
        (
            first_block, theirs, summed, x_copy, y_copy, relay_a, relay_b,
            final_a, final_b, settled,
        ) = plane_sums(end_a)
        for i in (2, 6, 7):
            event(i)
        for i in (1, 2, 4, 6, 7):
            dcopy(i, 1 - core).wait_recv()
        for i in range(line):
            g_block(jnp.where(lower, line - 1 - i, i))
            if i < line - 1:
                @pl.when(lower)
                def _():
                    up_copy(line - 1 - i, True).start()

                @pl.when(jnp.logical_not(lower))
                def _():
                    dn_copy(i, True).start()
        f_copy(0, False, g, zrow).start()
        f_copy(1, False, g, zrow).start()
        for d in range(last):
            for sub in range(2):
                settle(d, sub, 2)
        forward(1, dn_w, 2 * width, width, 0, 4)
        f_copy(0, True).wait_recv()
        f_copy(2, False).start()
        forward_end(1, 2, 0)
        for up_dir in (True, False):
            await_recv(up_dir, last, 1, 2)
        inputs_sent()
        finish(0)
        first_block()
        finish(1)
        theirs(4)
        summed(4)
        x_copy(2).start()
        finish(2)
        theirs(5)
        summed(5)
        y_copy(2).start()
        finish(3)
        theirs(6)
        summed(6)
        relay_a()
        y_copy(4).start()
        y_copy(3).start()
        relay_b()
        x_copy(4).start()
        h_copy(0).wait_recv()
        scaled([(g, pl.multiple_of(zrow + y * frows, frows), 0), (hl, 0, gcol(r, y))], r, y)
        final_a()
        final_b(0)
        for i, (rr, yy) in enumerate(((r, 1 - y), (1 - r, y))):
            if i == 1:
                f_copy(1, True).wait_recv()
            h_copy(1 + i).wait_recv()
            scaled([(gl, 0, gcol(rr, yy)), (hl, 0, gcol(rr, yy))], rr, yy)
        final_b(1)
        f_copy(2, True).wait_recv()
        h_copy(3).wait_recv()
        diag = gcol(1 - r, 1 - y)
        scaled([(gl, 0, diag), (hl, 0, diag)], 1 - r, 1 - y)
        settled()

    @pl.when(jnp.logical_not(is_end))
    def _():
        (
            first_block, theirs, summed, x_copy, y_copy, relay_a, relay_b,
            final_a, final_b, settled,
        ) = plane_sums(mid_a)
        event(2)
        inputs_sent()
        for i in (1, 2):
            dcopy(i, 1 - core).wait_recv()
        forward(1, dn_w, 2 * width, width, 1, 1)
        theirs(4)
        summed(4)
        x_copy(2).start()
        event(6)
        dcopy(4, 1 - core).wait_recv()
        forward(1, dn_w, 2 * width, width, 2, 1)
        theirs(5)
        event(7)
        summed(5)
        y_copy(2).start()
        y_copy(3).start()
        for i in (6, 7):
            dcopy(i, 1 - core).wait_recv()
        forward(1, dn_w, 2 * width, width, 3, 1)
        first_block()
        g_block(jnp.where(lower, line - 1, 0))
        line_step(1)
        for i in range(1, line):
            g_block(jnp.where(lower, line - 1 - i, i))
        forward(1, dn_w, 2 * width, width, 0, 1)
        theirs(6)
        summed(6)
        relay_a()
        relay_b()
        for t in range(2, line - 1):
            line_step(t)
        y_copy(4).start()
        x_copy(4).start()

        @pl.when(next_to_end)
        def _():
            e_copy(0, True).wait_recv()
            e_copy(2, False).start()
            h_copy(1).start()
            e_copy(1, True).wait_recv()
            h_copy(2).start()

        up_copy(z, False).wait_recv()
        dn_copy(z, False).wait_recv()
        total(
            (gfin, 0, 0, width),
            [(g, zrow, 0, width), (u_in, zrow, 0, width), (d_in, zrow, 0, width)], zrows,
        )
        f_copy(0, False).start()
        scaled([(gfin, pl.multiple_of(y * frows, frows), 0)], r, y)
        f_copy(1, False).start()
        final_a()
        final_b(0)

        @pl.when(next_to_end)
        def _():
            e_copy(2, True).wait_recv()
            h_copy(3).start()

        f_copy(0, True).wait_recv()
        f_copy(2, False).start()
        scaled([(gl, 0, gcol(r, 1 - y))], r, 1 - y)
        f_copy(1, True).wait_recv()
        scaled([(gl, 0, gcol(1 - r, y))], 1 - r, y)
        final_b(1)
        f_copy(2, True).wait_recv()
        scaled([(gl, 0, gcol(1 - r, 1 - y))], 1 - r, 1 - y)

        @pl.when(next_to_end)
        def _():
            for i in range(3):
                e_copy(i, False).wait_send()
            for i in range(4):
                h_copy(i).wait_send()

        settled()

    for i in range(ntok):
        if kinds[i] == 1:
            dcopy(i, core).wait_send()
        if i != 5:
            tcopy(i, False).wait_send()
    for k in range(3):
        to_y(k).wait_send()

    unit = wrows * width // (2 * x.shape[2])
    for count, here in ((6, is_end), (6 * (line + 1), jnp.logical_not(is_end))):
        @pl.when(here)
        def _(count=count):
            view = x.at[:, pl.ds(0, count * unit), :]
            pltpu.make_async_copy(view, view, z_s).wait()

    for i in range(3):
        f_copy(i, False).wait_send()
    for zt in range(line):
        if zt > 0:
            far = line - 2 if zt == line - 1 else zt
            pl.when(z < far)(lambda: up_copy(zt, True).wait_send())
        if zt < line - 1:
            near = 1 if zt == 0 else zt
            pl.when(z > near)(lambda: dn_copy(zt, True).wait_send())


def fused(grad_scale, gate_w, up_w, down_w, toks, cots):
    line = lax.axis_size("fs") // 2
    rows, full = toks.shape
    wrows, width = gate_w.shape[0], gate_w.shape[1] // 4
    depth = 2 * line * wrows
    cols = full // 2
    kind = gate_w.dtype
    dma = pltpu.SemaphoreType.DMA
    zsem = dma((line - 1, 2, 3))
    anyspec = pl.BlockSpec(memory_space=pl.ANY)
    whole = pltpu.VMEM((depth, width), kind)
    end_a, mid_a = cols // 2, cols * 3 // 8 // 128 * 128
    most_b = cols - mid_a
    return pl.pallas_call(
        functools.partial(fused_kernel, line, grad_scale, end_a, mid_a),
        out_shape=(
            pltpu.VMEM((rows, full), kind),
            pltpu.VMEM((wrows, 4 * width), jnp.float32),
        ),
        in_specs=[anyspec] * 5,
        out_specs=(pl.BlockSpec(memory_space=pltpu.VMEM),) * 2,
        scratch_shapes=[
            pltpu.VMEM((2, 4 * rows, full), kind),
            pltpu.VMEM((depth, 2 * width), kind),
            whole,
            pltpu.VMEM((4 * rows, 3 * width), jnp.float32),
            pltpu.VMEM((4 * rows, width), kind),
            pltpu.VMEM((4 * rows, 2 * width), kind),
            pltpu.VMEM((4 * rows, cols), kind),
            pltpu.VMEM((2, rows, end_a), kind), pltpu.VMEM((rows, most_b), kind),
            pltpu.VMEM((2, rows, most_b), kind), pltpu.VMEM((rows, end_a), kind),
            pltpu.VMEM((rows, end_a), kind), pltpu.VMEM((rows, most_b), kind),
            whole, whole, whole,
            pltpu.VMEM((2 * wrows, width), kind),
            pltpu.VMEM((wrows, 4 * width), kind),
            pltpu.VMEM((wrows, 4 * width), kind),
            dma, zsem, zsem,
            dma((3,)), dma((3,)),
            dma((8,)), dma((8,)), dma((8,)), dma((8,)), dma((5,)),
            dma((7,)), dma((7,)), dma((5,)), dma((5,)), dma((5,)), dma((5,)),
            dma((line,)), dma((line,)), dma((line,)), dma((line,)),
            dma((3,)), dma((3,)), dma((3,)), dma((3,)),
            dma((3,)), dma((3,)), dma((4,)), dma((4,)),
        ],
        compiler_params=pltpu.CompilerParams(
            collective_id=1, has_side_effects=True, vmem_limit_bytes=59 * 2**20
        ),
        name="fused_all",
    )(gate_w, up_w, down_w, toks, cots)


def place_kernel(a, b, a_out, b_out, sems):
    copies = [
        pltpu.make_async_copy(a, a_out, sems.at[0]),
        pltpu.make_async_copy(b, b_out, sems.at[1]),
    ]
    for copy in copies:
        copy.start()
    for copy in copies:
        copy.wait()


def place(a, b):
    anyspec = pl.BlockSpec(memory_space=pl.ANY)
    return pl.pallas_call(
        place_kernel,
        out_shape=(
            jax.ShapeDtypeStruct(a.shape, a.dtype), jax.ShapeDtypeStruct(b.shape, b.dtype),
        ),
        in_specs=[pl.BlockSpec(memory_space=pltpu.VMEM)] * 2,
        out_specs=(anyspec,) * 2,
        scratch_shapes=[pltpu.SemaphoreType.DMA((2,))],
        compiler_params=pltpu.CompilerParams(vmem_limit_bytes=16 * 2**20),
        name="place",
    )(a, b)


def gather_kernel(
    line, units, gate_w, up_w, down_w, toks, cots, gu_out, d_out, t_out, w_tmp, t_tmp,
    up_s, up_r, dn_s, dn_r, y_s, y_r, tok_s, tok_r, d2d_s, d2d_r, loc, loc2,
):
    r = lax.axis_index("rep")
    f = lax.axis_index("fs")
    t = lax.axis_index("tp")
    z, y = f // 2, f % 2
    rows = toks.shape[0]
    half = rows // 2
    wrows = gate_w.shape[0]
    width = gate_w.shape[1] // 4
    parts = len(units)
    has_up, has_dn = z < line - 1, z > 0
    up = {"fs": (f + 2) % (2 * line)}
    dn = {"fs": (f + 2 * line - 2) % (2 * line)}
    ypart = {"fs": f + 1 - 2 * y}
    xpart = {"rep": 1 - r}
    core = t % 2
    cpart = {"tp": t + 1 - 2 * core}

    barrier = pltpu.get_barrier_semaphore()

    def greet(dev):
        pl.semaphore_signal(barrier, inc=1, device_id=dev, device_id_type=MESH)

    for dev in (ypart, xpart, cpart, up, dn):
        greet(dev)
    pl.semaphore_wait(barrier, 5)

    def remote(src, dst, s, q, dev):
        return pltpu.make_async_remote_copy(
            src_ref=src, dst_ref=dst, send_sem=s, recv_sem=q,
            device_id=dev, device_id_type=MESH,
        )

    def wblk(k, zz, yy):
        row = pl.multiple_of((2 * zz + yy) * wrows, wrows)
        which, col, wide = units[k]
        return (gu_out, d_out)[which].at[pl.ds(row, wrows), pl.ds(col, wide)]

    def own(k, yy):
        col = pl.multiple_of((2 * r + yy) * width, width)
        return (gate_w, up_w, down_w)[k].at[:, pl.ds(col, width)]

    def to_y(k):
        return remote(own(k, 1 - y), wblk(k, z, y), y_s.at[k], y_r.at[k], ypart)

    def from_y(k):
        return remote(own(k, 1 - y), wblk(k, z, 1 - y), y_s.at[k], y_r.at[k], ypart)

    def zcopy(up_dir, d, sub, k, zz):
        yy = y if sub == 0 else 1 - y
        src = own(k, y) if (d == 0 and sub == 0) else wblk(k, zz, yy)
        s, q, dev = (up_s, up_r, up) if up_dir else (dn_s, dn_r, dn)
        return remote(src, wblk(k, zz, yy), s.at[d, sub, k], q.at[d, sub, k], dev)

    def pred_send(up_dir, d):
        return (has_up & (z - d >= 0)) if up_dir else (has_dn & (z + d <= line - 1))

    def src_z(up_dir, d):
        return jnp.maximum(z - d, 0) if up_dir else jnp.minimum(z + d, line - 1)

    def send(up_dir, d, sub, k):
        @pl.when(pred_send(up_dir, d))
        def _():
            zcopy(up_dir, d, sub, k, src_z(up_dir, d)).start()

    def await_send(up_dir, d, sub, k):
        @pl.when(pred_send(up_dir, d))
        def _():
            zcopy(up_dir, d, sub, k, src_z(up_dir, d)).wait_send()

    def await_recv(up_dir, d, sub, k):
        ok = (z - d - 1 >= 0) if up_dir else (z + d + 1 <= line - 1)

        @pl.when(ok)
        def _():
            zcopy(up_dir, d, sub, k, src_z(up_dir, d + 1)).wait_recv()

    def tblk(j, rr, yy, c):
        row = pl.multiple_of((2 * rr + yy) * rows + c * half, half)
        return t_out.at[j, pl.ds(row, half), :]

    def mine(j):
        src = toks if j == 0 else cots
        return src.at[pl.ds(pl.multiple_of(core * half, half), half), :]

    def tcopy(i, landing):
        j = (0, 1, 0, 1, 0, 1)[i]
        dev = xpart if i in (0, 1, 5) else ypart
        if landing:
            rr = (1 - r, 1 - r, r, r, 1 - r, 1 - r)[i]
            yy = (y, y, 1 - y, 1 - y, 1 - y, 1 - y)[i]
            src = dst = tblk(j, rr, yy, core)
        else:
            rr = (r, r, r, r, 1 - r, r)[i]
            yy = (y, y, y, y, y, 1 - y)[i]
            dst = tblk(j, rr, yy, core)
            src = mine(j) if i < 4 else dst
        return remote(src, dst, tok_s.at[i], tok_r.at[i], dev)

    def dcopy(i, c):
        j = (0, 1, 0, 1, 0, 1)[i]
        rr = (1 - r, 1 - r, r, r, 1 - r, 1 - r)[i]
        yy = (y, y, 1 - y, 1 - y, 1 - y, 1 - y)[i]
        blk = tblk(j, rr, yy, c)
        return remote(blk, blk, d2d_s.at[i], d2d_r.at[i], cpart)

    loads = [
        pltpu.make_async_copy(own(0, y), w_tmp.at[0], loc.at[0]),
        pltpu.make_async_copy(own(1, y), w_tmp.at[1], loc.at[3]),
        pltpu.make_async_copy(own(2, y), w_tmp.at[2], loc.at[4]),
        pltpu.make_async_copy(toks, t_tmp.at[0], loc.at[1]),
        pltpu.make_async_copy(cots, t_tmp.at[1], loc.at[2]),
    ]
    trow = pl.multiple_of((2 * r + y) * rows, rows)
    stores = [
        pltpu.make_async_copy(w_tmp.at[0], wblk(0, z, y), loc2.at[0]),
        pltpu.make_async_copy(w_tmp.at[1], wblk(1, z, y), loc2.at[3]),
        pltpu.make_async_copy(w_tmp.at[2], wblk(2, z, y), loc2.at[4]),
        pltpu.make_async_copy(t_tmp.at[0], t_out.at[0, pl.ds(trow, rows), :], loc2.at[1]),
        pltpu.make_async_copy(t_tmp.at[1], t_out.at[1, pl.ds(trow, rows), :], loc2.at[2]),
    ]

    for k in range(parts):
        to_y(k).start()
        send(True, 0, 0, k)
        send(False, 0, 0, k)
    for i in (0, 1, 3, 2):
        tcopy(i, False).start()
    for copy in loads:
        copy.start()
    for load, store in zip(loads, stores):
        load.wait()
        store.start()
    for k in range(parts):
        from_y(k).wait_recv()
        send(True, 0, 1, k)
        send(False, 0, 1, k)

    def event(i):
        tcopy(i, True).wait_recv()
        if i == 0:
            tcopy(4, False).start()
        if i == 3:
            tcopy(5, False).start()
        dcopy(i, core).start()

    events = [0, 3, 1, 2, 5, 4]
    for d in range(line - 1):
        for sub in range(2):
            if events:
                event(events.pop(0))
            for k in range(parts):
                for up_dir in (True, False):
                    await_recv(up_dir, d, sub, k)
                    if d + 1 < line - 1:
                        send(up_dir, d + 1, sub, k)
    for i in events:
        event(i)
    for i in range(6):
        dcopy(i, 1 - core).wait_recv()
        dcopy(i, core).wait_send()
        tcopy(i, False).wait_send()
    for k in range(parts):
        to_y(k).wait_send()
        for d in range(line - 1):
            for sub in range(2):
                await_send(True, d, sub, k)
                await_send(False, d, sub, k)
    for store in stores:
        store.wait()


def gather(gate_w, up_w, down_w, toks, cots):
    line = lax.axis_size("fs") // 2
    wrows, width = gate_w.shape[0], gate_w.shape[1] // 4
    units = [(0, 0, width), (0, width, width), (1, 0, width)]
    parts = len(units)
    depth = 2 * line * wrows
    kind = gate_w.dtype
    dma = pltpu.SemaphoreType.DMA
    zsem = dma((line - 1, 2, parts))
    anyspec = pl.BlockSpec(memory_space=pl.ANY)
    return pl.pallas_call(
        functools.partial(gather_kernel, line, units),
        out_shape=(
            jax.ShapeDtypeStruct((depth, 2 * width), kind),
            jax.ShapeDtypeStruct((depth, width), kind),
            jax.ShapeDtypeStruct((2, 4 * toks.shape[0], toks.shape[1]), toks.dtype),
        ),
        in_specs=[anyspec] * 5,
        out_specs=(anyspec,) * 3,
        scratch_shapes=[
            pltpu.VMEM((parts, wrows, width), kind),
            pltpu.VMEM((2,) + toks.shape, toks.dtype),
            zsem, zsem, zsem, zsem,
            dma((parts,)), dma((parts,)),
            dma((6,)), dma((6,)), dma((6,)), dma((6,)),
            dma((5,)), dma((5,)),
        ],
        compiler_params=pltpu.CompilerParams(collective_id=0, has_side_effects=True),
        name="gather_all",
    )(gate_w, up_w, down_w, toks, cots)


def on_device(inputs, cotangent, gate_weight, up_weight, down_weight):
    tok_rows = inputs.shape[0]
    fs_size = lax.axis_size("fs")
    rep_size = lax.axis_size("rep")
    grad_scale = 1.0 / math.sqrt(tok_rows * fs_size * rep_size)
    if lax.axis_size("tp") == 2 and rep_size == 2 and fs_size >= 8:
        return place(*fused(
            grad_scale, gate_weight, up_weight, down_weight, inputs, cotangent
        ))
    contract = (((1,), (1,)), ((), ()))
    contract_tok = (((0,), (0,)), ((), ()))
    width = gate_weight.shape[1] // 4
    gate_up, down_full, tokens = gather(
        gate_weight, up_weight, down_weight, inputs, cotangent
    )
    gate_up_val = jnp.dot(tokens[0], gate_up, preferred_element_type=jnp.float32)
    gate_val, up_val = gate_up_val[:, :width], gate_up_val[:, width:]
    grad_hidden = jnp.dot(tokens[1], down_full, preferred_element_type=jnp.float32)
    sigmoid_gate = jax.nn.sigmoid(gate_val)
    active = gate_val * sigmoid_gate
    hidden = (active * up_val).astype(jnp.bfloat16)
    grad_gate = (
        grad_hidden * up_val * sigmoid_gate * (1.0 + gate_val * (1.0 - sigmoid_gate))
    ).astype(jnp.bfloat16)
    grad_up = (grad_hidden * active).astype(jnp.bfloat16)
    pairs = [[i, i + 1] for i in range(0, fs_size, 2)]
    lines = [list(range(i, fs_size, 2)) for i in range(2)]
    grad_part = lax.dot_general(
        tokens[1], hidden, contract_tok, preferred_element_type=jnp.float32
    )
    part = lax.dot_general(
        jnp.concatenate([grad_gate, grad_up], axis=1), gate_up, contract,
        preferred_element_type=jnp.float32,
    )
    shard = lax.psum_scatter(
        grad_part.astype(jnp.bfloat16), "fs", scatter_dimension=0, tiled=True,
        axis_index_groups=lines,
    ).astype(jnp.float32) * grad_scale
    shard = lax.all_to_all(
        shard, "fs", split_axis=0, concat_axis=1, tiled=True, axis_index_groups=pairs
    )
    grad_down = lax.all_gather(shard, "rep", axis=1, tiled=True)
    part = lax.psum_scatter(
        part.astype(jnp.bfloat16), "rep", scatter_dimension=0, tiled=True
    )
    part = lax.psum_scatter(
        part, "fs", scatter_dimension=0, tiled=True, axis_index_groups=pairs
    )
    grad_input = lax.psum(part, "tp")
    return (grad_input, grad_down)


def solution(mesh):
    placed = (
        P(("rep", "fs"), None),
        P(("rep", "fs"), None),
        P("fs", "tp"),
        P("fs", "tp"),
        P("fs", "tp"),
    )
    return jax.shard_map(
        on_device,
        mesh=mesh,
        in_specs=placed,
        out_specs=(P(("rep", "fs"), None), P("fs", "tp")),
        check_vma=False,
    )
```

```python
import functools
import math

import jax
import jax.numpy as jnp
from jax import lax
from jax.experimental import pallas as pl
from jax.experimental.pallas import tpu as pltpu
from jax.sharding import PartitionSpec as P

MESH = pl.DeviceIdType.MESH


def fused_kernel(
    line, grad_scale, end_a, mid_a, gate_w, up_w, down_w, toks, cots, gi_out, gd_out,
    x, gu, dn_w, acc, hid, ggu, r1, rxa, rxb, rya, ryb, s3a, s3b, g, u_in, d_in, gfin, gl, hl,
    z_s, up_r, dn_r, wy_s, wy_r, tok_s, tok_r, d2d_s, d2d_r, loc,
    c_s, c_r, x_s, x_r, yy_s, yy_r, u_s, u_r, d_s, d_r, f_s, f_r, o_s, o_r, e_s, e_r, h_s, h_r,
):
    r = lax.axis_index("rep")
    f = lax.axis_index("fs")
    core = lax.axis_index("tp")
    z, y = f // 2, f % 2
    rows = toks.shape[0]
    half = rows // 2
    wrows = gate_w.shape[0]
    width = gate_w.shape[1] // 4
    depth = 2 * line * wrows
    zrows = 2 * wrows
    cols = depth // 2
    wide = cols // 2
    frows = wrows
    last = line - 2
    has_up, has_dn = z < line - 1, z > 0
    is_end = (z == 0) | (z == line - 1)
    up = {"fs": (f + 2) % (2 * line)}
    dn = {"fs": (f + 2 * line - 2) % (2 * line)}
    ypart = {"fs": f + 1 - 2 * y}
    xpart = {"rep": 1 - r}
    cpart = {"tp": 1 - core}

    barrier = pltpu.get_barrier_semaphore()
    for dev in (ypart, xpart, cpart, up, dn):
        pl.semaphore_signal(barrier, inc=1, device_id=dev, device_id_type=MESH)
    pl.semaphore_wait(barrier, 5)

    def remote(src, dst, s, q, dev):
        return pltpu.make_async_remote_copy(
            src_ref=src, dst_ref=dst, send_sem=s, recv_sem=q,
            device_id=dev, device_id_type=MESH,
        )

    def wblk(k, zz, yy):
        row = pl.multiple_of((2 * zz + yy) * wrows, wrows)
        if k == 2:
            return dn_w.at[pl.ds(row, wrows), :]
        return gu.at[pl.ds(row, wrows), pl.ds(k * width, width)]

    def own(k, yy):
        col = pl.multiple_of((2 * r + yy) * width, width)
        return (gate_w, up_w, down_w)[k].at[:, pl.ds(col, width)]

    def to_y(k):
        return remote(own(k, 1 - y), wblk(k, z, y), wy_s.at[k], wy_r.at[k], ypart)

    def from_y(k):
        return remote(own(k, 1 - y), wblk(k, z, 1 - y), wy_s.at[k], wy_r.at[k], ypart)

    def zcopy(up_dir, d, sub, k, zz):
        yy = y if sub == 0 else 1 - y
        src = own(k, y) if (d == 0 and sub == 0) else wblk(k, zz, yy)
        q, dev = (up_r, up) if up_dir else (dn_r, dn)
        return remote(src, wblk(k, zz, yy), z_s, q.at[d, sub, k], dev)

    def pred_send(up_dir, d):
        return (has_up & (z - d >= 0)) if up_dir else (has_dn & (z + d <= line - 1))

    def src_z(up_dir, d):
        return jnp.maximum(z - d, 0) if up_dir else jnp.minimum(z + d, line - 1)

    def send(up_dir, d, sub, k):
        @pl.when(pred_send(up_dir, d))
        def _():
            zcopy(up_dir, d, sub, k, src_z(up_dir, d)).start()

    def await_recv(up_dir, d, sub, k):
        ok = (z - d - 1 >= 0) if up_dir else (z + d + 1 <= line - 1)

        @pl.when(ok)
        def _():
            zcopy(up_dir, d, sub, k, src_z(up_dir, d + 1)).wait_recv()

    def relay(d, sub, k):
        for up_dir in (True, False):
            @pl.when(pred_send(up_dir, d + 1))
            def _():
                zcopy(up_dir, d, sub, k, src_z(up_dir, d + 1)).wait_recv()
                zcopy(up_dir, d + 1, sub, k, src_z(up_dir, d + 1)).start()

    def settle(d, sub, k):
        for up_dir in (True, False):
            ok = (z - d - 1 >= 0) if up_dir else (z + d + 1 <= line - 1)
            onward = has_up if up_dir else has_dn

            @pl.when(ok & jnp.logical_not(onward))
            def _():
                zcopy(up_dir, d, sub, k, src_z(up_dir, d + 1)).wait_recv()

    def slot(rr, yy):
        return pl.multiple_of((2 * rr + yy) * rows, rows)

    kinds = (0, 1, 1, 0, 1, 0, 1, 1)
    over_x = (True, True, True, False, False, True, False, True)
    parts = (2, 0, 1, 2, 2, 2, 0, 1)
    ntok = len(kinds)

    def span(c, p):
        if p == 2:
            return c * half, half
        return c * half + p * (half // 2), half // 2

    def tblk(i, rr, yy, c):
        at, count = span(c, parts[i])
        row = pl.multiple_of((2 * rr + yy) * rows + at, half // 2)
        return x.at[kinds[i], pl.ds(row, count), :]

    def mine(i):
        at, count = span(core, parts[i])
        src = toks if kinds[i] == 0 else cots
        return src.at[pl.ds(pl.multiple_of(at, half // 2), count), :]

    def landing(i, c):
        rr = (1 - r, 1 - r, 1 - r, r, r, 1 - r, 1 - r, 1 - r)[i]
        yy = (y, y, y, 1 - y, 1 - y, 1 - y, 1 - y, 1 - y)[i]
        return tblk(i, rr, yy, c)

    def tcopy(i, land):
        dev = xpart if over_x[i] else ypart
        if land:
            src = dst = landing(i, core)
        else:
            rr = (r, r, r, r, r, r, 1 - r, r)[i]
            yy = (y, y, y, y, y, 1 - y, y, 1 - y)[i]
            dst = tblk(i, rr, yy, core)
            src = mine(i) if i < 5 else dst
        return remote(src, dst, tok_s.at[i], tok_r.at[i], dev)

    def dcopy(i, c):
        blk = landing(i, c)
        return remote(blk, blk, d2d_s.at[i], d2d_r.at[i], cpart)

    def event(i):
        tcopy(i, True).wait_recv()
        onward = {1: 6, 3: 5, 4: 7}.get(i)
        if onward is not None:
            tcopy(onward, False).start()
        dcopy(i, core).start()

    trow = slot(r, y)
    loads = [
        pltpu.make_async_copy(own(0, y), wblk(0, z, y), loc.at[0]),
        pltpu.make_async_copy(own(1, y), wblk(1, z, y), loc.at[1]),
        pltpu.make_async_copy(own(2, y), wblk(2, z, y), loc.at[2]),
        pltpu.make_async_copy(toks, x.at[0, pl.ds(trow, rows), :], loc.at[3]),
        pltpu.make_async_copy(cots, x.at[1, pl.ds(trow, rows), :], loc.at[4]),
    ]

    tile = 256
    z_lo = jnp.maximum(z - last, 0)
    z_hi = jnp.minimum(z + last, line - 1) + 1

    def product(j, row, k0, kk, w, wcol, acol, n):
        at = pl.ds(pl.multiple_of(row, rows), rows)
        kat = pl.ds(pl.multiple_of(k0, wrows), kk)
        for c in range(0, n, tile):
            one = jnp.dot(
                x[j, at, kat], w[kat, pl.ds(wcol + c, tile)],
                preferred_element_type=jnp.float32,
            )
            acc[at, pl.ds(acol + c, tile)] += one

    def forward(j, w, acol, n, first, count):
        @pl.loop(first, first + count)
        def _(b):
            row = ((2 * r + y) + 2 * (b % 2) * (1 - 2 * r) + (b // 2) * (1 - 2 * y)) * rows

            @pl.loop(z_lo, z_hi)
            def _(zz):
                product(j, row, zz * zrows, zrows, w, 0, acol, n)

    def forward_end(j, k, sub):
        for up_dir in (True, False):
            await_recv(up_dir, last, sub, k)

        @pl.when(is_end)
        def _():
            zz = line - 1 - z
            yy = y if sub == 0 else 1 - y
            w = dn_w if k == 2 else gu

            @pl.loop(0, 4)
            def _(b):
                product(
                    j, b * rows, (2 * zz + yy) * wrows, wrows, w,
                    0 if k == 2 else k * width, k * width, width,
                )

    def total(dst, terms, count, step=64):
        @pl.loop(0, count // step)
        def _(i):
            at = pl.multiple_of(i * step, step)
            value = None
            for ref, row, col, wide in terms:
                one = ref[pl.ds(row + at, step), pl.ds(col, wide)].astype(jnp.float32)
                value = one if value is None else value + one
            ref, row, col, wide = dst
            ref[pl.ds(row + at, step), pl.ds(col, wide)] = value.astype(ref.dtype)

    for k in (0, 1):
        to_y(k).start()
        send(True, 0, 0, k)
        send(False, 0, 0, k)
    for i in (0, 1, 3):
        tcopy(i, False).start()
    to_y(2).start()
    tcopy(4, False).start()
    for copy in loads:
        copy.start()

    @pl.loop(0, 4 * rows // 64)
    def _(i):
        at = pl.ds(pl.multiple_of(i * 64, 64), 64)
        acc[at, :] = jnp.zeros((64, 3 * width), jnp.float32)

    for k in (0, 1):
        from_y(k).wait_recv()
        send(True, 0, 1, k)
        send(False, 0, 1, k)
    if last > 0:
        for sub in range(2):
            for k in (0, 1):
                relay(0, sub, k)
    event(0)
    event(3)
    tcopy(2, False).start()
    event(1)
    for d in range(1, last):
        for sub in range(2):
            for k in (0, 1):
                relay(d, sub, k)
    send(True, 0, 0, 2)
    send(False, 0, 0, 2)
    from_y(2).wait_recv()
    send(True, 0, 1, 2)
    send(False, 0, 1, 2)
    for load in loads:
        load.wait()
    for d in range(last):
        for sub in range(2):
            for k in (0, 1):
                settle(d, sub, k)
    dcopy(0, 1 - core).wait_recv()
    dcopy(3, 1 - core).wait_recv()
    forward(0, gu, 0, 2 * width, 0, 3)
    if last > 0:
        for sub in range(2):
            relay(0, sub, 2)
    event(5)
    event(4)
    dcopy(5, 1 - core).wait_recv()
    forward(0, gu, 0, 2 * width, 3, 1)
    for d in range(1, last):
        for sub in range(2):
            relay(d, sub, 2)
    for sub in range(2):
        for k in (0, 1):
            forward_end(0, k, sub)

    @pl.loop(0, 4 * rows // 32)
    def _(i):
        at = pl.ds(pl.multiple_of(i * 32, 32), 32)
        gate = acc[at, pl.ds(0, width)]
        up_val = acc[at, pl.ds(width, width)]
        sig = jax.nn.sigmoid(gate)
        active = gate * sig
        hid[at, :] = (active * up_val).astype(hid.dtype)
        acc[at, pl.ds(0, width)] = up_val * sig * (1.0 + gate * (1.0 - sig))
        acc[at, pl.ds(width, width)] = active


    zrow = pl.multiple_of(z * zrows, zrows)
    lower = z < line // 2

    def block(ref, zt):
        return ref.at[pl.ds(zt * zrows, zrows), :]

    def up_copy(zt, first):
        return remote(block(g if first else u_in, zt), block(u_in, zt), u_s.at[zt], u_r.at[zt], up)

    def dn_copy(zt, first):
        return remote(block(g if first else d_in, zt), block(d_in, zt), d_s.at[zt], d_r.at[zt], dn)

    def g_block(zt):
        at = pl.multiple_of(zt * zrows, zrows)
        one = lax.dot_general(
            x[1, :, pl.ds(at, zrows)], hid[...], (((0,), (0,)), ((), ())),
            preferred_element_type=jnp.float32,
        )
        g[pl.ds(at, zrows), :] = one.astype(g.dtype)

    def gcol(rr, yy):
        return pl.multiple_of((2 * rr + yy) * width, width)

    def gcols(ref, rr, yy):
        return ref.at[:, pl.ds(gcol(rr, yy), width)]

    def half_rows(ref, row, yy):
        return ref.at[pl.ds(pl.multiple_of(row + yy * frows, frows), frows), :]

    def f_copy(i, land, ref=gfin, row=0):
        if i == 0:
            src, dst, dev = half_rows(ref, row, 1 - y), gcols(gl, r, 1 - y if land else y), ypart
        elif i == 1:
            src, dst, dev = half_rows(ref, row, y), gcols(gl, 1 - r if land else r, y), xpart
        else:
            src, dst, dev = gcols(gl, r, 1 - y), gcols(gl, 1 - r if land else r, 1 - y), xpart
        return remote(src, dst, f_s.at[i], f_r.at[i], dev)

    def e_copy(i, land, ref=gfin, row=0):
        if i == 0:
            src, dst, dev = half_rows(ref, row, 1 - y), gcols(hl, r, 1 - y if land else y), ypart
        elif i == 1:
            src, dst, dev = half_rows(ref, row, y), gcols(hl, 1 - r if land else r, y), xpart
        else:
            src, dst, dev = gcols(hl, r, 1 - y), gcols(hl, 1 - r if land else r, 1 - y), xpart
        return remote(src, dst, e_s.at[i], e_r.at[i], dev)

    end_z = jnp.where((z == 1) | (z == line - 1), 0, line - 1)
    end_dev = {"fs": 2 * end_z + y}
    next_to_end = (z == 1) | (z == line - 2)

    def h_copy(i, ref=gfin, row=0):
        rr, yy = ((r, y), (r, 1 - y), (1 - r, y), (1 - r, 1 - y))[i]
        dst = gcols(hl, rr, yy)
        src = half_rows(ref, row, y) if i == 0 else dst
        return remote(src, dst, h_s.at[i], h_r.at[i], end_dev)

    def share(ref, row):
        h_copy(0, ref, row).start()
        e_copy(0, False, ref, row).start()
        e_copy(1, False, ref, row).start()

    def line_step(t):
        zt = line - 1 + z - t
        row_u = pl.multiple_of(zt * zrows, zrows)
        is_u = (z > 0) & (zt <= line - 1) & (zt > z)
        zd = t - (line - 1 - z)
        row_d = pl.multiple_of(zd * zrows, zrows)
        is_d = (z < line - 1) & (zd >= 0) & (zd < z)
        final = t == line - 2

        def add_u():
            up_copy(zt, False).wait_recv()
            total((u_in, row_u, 0, width), [(g, row_u, 0, width), (u_in, row_u, 0, width)], zrows)

        def add_d():
            dn_copy(zd, False).wait_recv()
            total((d_in, row_d, 0, width), [(g, row_d, 0, width), (d_in, row_d, 0, width)], zrows)

        @pl.when((is_u & (z < line - 2)) if final else is_u)
        def _():
            add_u()
            up_copy(zt, False).start()

        @pl.when((is_d & (z > 1)) if final else is_d)
        def _():
            add_d()
            dn_copy(zd, False).start()

        if final:
            @pl.when(z == line - 2)
            def _():
                add_u()
                share(u_in, (line - 1) * zrows)

            @pl.when(z == 1)
            def _():
                add_d()
                share(d_in, 0)

    order = [(1 - r, 1 - y), (1 - r, y), (r, 1 - y), (r, y)]
    my_col = pl.multiple_of(core * cols, cols)
    its_col = pl.multiple_of((1 - core) * cols, cols)
    part = x.at[0]

    def slopes(row, count):
        @pl.loop(0, count // 32)
        def _(i):
            at = pl.ds(pl.multiple_of(row + i * 32, 32), 32)
            grad = acc[at, pl.ds(2 * width, width)]
            ggu[at, pl.ds(0, width)] = (grad * acc[at, pl.ds(0, width)]).astype(ggu.dtype)
            ggu[at, pl.ds(width, width)] = (grad * acc[at, pl.ds(width, width)]).astype(ggu.dtype)

    def back(row, count, col, n):
        step = min(n, wide) if n % wide == 0 else n

        @pl.loop(0, n // step)
        def _(i):
            at = pl.multiple_of(col + i * step, 128)
            one = lax.dot_general(
                ggu[pl.ds(row, count), :], gu[pl.ds(at, step), :], (((1,), (1,)), ((), ())),
                preferred_element_type=jnp.float32,
            )
            x[0, pl.ds(row, count), pl.ds(at, step)] = one.astype(x.dtype)

    hrows = rows // 2

    def finish(b):
        @pl.when(is_end)
        def _():
            product(
                1, slot(*order[b]), (2 * (line - 1 - z) + 1 - y) * wrows, wrows,
                dn_w, 0, 2 * width, width,
            )

    here_row = slot(r, y)

    def plane_sums(pa):
        pb = cols - pa
        pieces = [
            (0, 0, hrows, 0, pa), (0, 0, hrows, pa, pb),
            (0, hrows, hrows, 0, pa), (0, hrows, hrows, pa, pb),
            (1, 0, rows, 0, cols), (2, 0, rows, 0, cols), (3, 0, rows, 0, cols),
        ]

        def place_of(i, col):
            b, at, count, c0, n = pieces[i]
            row = pl.multiple_of(slot(*order[b]) + at, hrows)
            return row, count, pl.multiple_of(col + c0, 128), c0, n

        def core_copy(i):
            row, count, col, c0, n = place_of(i, its_col)
            return remote(
                part.at[pl.ds(row, count), pl.ds(col, n)],
                r1.at[pl.ds(row, count), pl.ds(c0, n)], c_s.at[i], c_r.at[i], cpart,
            )

        def theirs(i):
            row, count, col, c0, n = place_of(i, its_col)
            if c0 == 0:
                slopes(row, count)
            back(row, count, col, n)
            core_copy(i).start()

        def summed(i):
            row, count, col, c0, n = place_of(i, my_col)
            back(row, count, col, n)
            core_copy(i).wait_recv()
            total((part, row, col, n), [(part, row, col, n), (r1, row, c0, n)], count)

        def first_block():
            theirs(0)
            theirs(1)
            theirs(2)
            summed(0)
            x_copy(0).start()
            summed(1)
            y_copy(0).start()
            theirs(3)
            summed(2)
            x_copy(1).start()
            summed(3)
            y_copy(1).start()

        def urow(u):
            return pl.multiple_of(slot(*order[0]) + u * hrows, hrows)

        second_col = pl.multiple_of(my_col + pa, 128)

        def mine_a(row, count):
            return part.at[pl.ds(row, count), pl.ds(my_col, pa)]

        def mine_b(row, count):
            return part.at[pl.ds(row, count), pl.ds(second_col, pb)]

        def x_copy(i):
            if i >= 3:
                at = pl.ds((i - 3) * hrows, hrows)
                src, dst = s3b.at[at, pl.ds(0, pb)], rxb.at[at, pl.ds(0, pb)]
            elif i == 2:
                src, dst = mine_a(slot(*order[1]), rows), rxa.at[1, :, pl.ds(0, pa)]
            else:
                src, dst = mine_a(urow(i), hrows), rxa.at[0, pl.ds(i * hrows, hrows), pl.ds(0, pa)]
            return remote(src, dst, x_s.at[i], x_r.at[i], xpart)

        def y_copy(i):
            if i == 4:
                src, dst = s3a.at[:, pl.ds(0, pa)], ryb.at[:, pl.ds(0, pa)]
            elif i in (2, 3):
                at = (i - 2) * hrows
                row = pl.multiple_of(slot(*order[2]) + at, hrows)
                src, dst = mine_b(row, hrows), rya.at[1, pl.ds(at, hrows), pl.ds(0, pb)]
            else:
                src, dst = mine_b(urow(i), hrows), rya.at[0, pl.ds(i * hrows, hrows), pl.ds(0, pb)]
            return remote(src, dst, yy_s.at[i], yy_r.at[i], ypart)

        def relay_a():
            for i in (0, 1):
                x_copy(i).wait_recv()
            total(
                (s3a, 0, 0, pa),
                [(part, slot(r, 1 - y), my_col, pa), (rxa.at[0], 0, 0, pa)], rows,
            )

        def relay_b():
            for i in (0, 1):
                y_copy(i).wait_recv()
            total(
                (s3b, 0, 0, pb),
                [(part, slot(1 - r, y), second_col, pb), (rya.at[0], 0, 0, pb)], rows,
            )
            x_copy(3).start()

        def o_copy(i, land):
            base = (1 - core if land else core) * cols
            if i == 0:
                at = gi_out.at[:, pl.ds(pl.multiple_of(base, 128), pa)]
            else:
                at = gi_out.at[
                    pl.ds((i - 1) * hrows, hrows), pl.ds(pl.multiple_of(base + pa, 128), pb)
                ]
            return remote(at, at, o_s.at[i], o_r.at[i], cpart)

        def final_a():
            x_copy(2).wait_recv()
            y_copy(4).wait_recv()
            total(
                (gi_out, 0, my_col, pa),
                [
                    (part, here_row, my_col, pa),
                    (rxa.at[1], 0, 0, pa), (ryb, 0, 0, pa),
                ], rows,
            )
            o_copy(0, False).start()

        def final_b(i):
            at = i * hrows
            x_copy(3 + i).wait_recv()
            y_copy(2 + i).wait_recv()
            total(
                (gi_out, at, second_col, pb),
                [
                    (part, here_row + at, second_col, pb),
                    (rya.at[1], at, 0, pb), (rxb, at, 0, pb),
                ], hrows,
            )
            o_copy(1 + i, False).start()

        def settled():
            for i in range(7):
                core_copy(i).wait_send()
            for i in range(5):
                y_copy(i).wait_send()
                x_copy(i).wait_send()
            for i in range(3):
                o_copy(i, True).wait_recv()
                o_copy(i, False).wait_send()

        return (
            first_block, theirs, summed, x_copy, y_copy, relay_a, relay_b,
            final_a, final_b, settled,
        )

    def scaled(terms, rr, yy):
        at_col = gcol(rr, yy)

        @pl.loop(0, frows // 64)
        def _(m):
            at = pl.multiple_of(m * 64, 64)
            value = None
            for ref, row, col in terms:
                one = ref[pl.ds(row + at, 64), pl.ds(col, width)].astype(jnp.float32)
                value = one if value is None else value + one
            gd_out[pl.ds(at, 64), pl.ds(at_col, width)] = value * grad_scale

    def inputs_sent():
        for i in (0, 3, 5):
            dcopy(i, core).wait_send()
        tcopy(5, False).wait_send()

    @pl.when(is_end)
    def _():
        (
            first_block, theirs, summed, x_copy, y_copy, relay_a, relay_b,
            final_a, final_b, settled,
        ) = plane_sums(end_a)
        for i in (2, 6, 7):
            event(i)
        for i in (1, 2, 4, 6, 7):
            dcopy(i, 1 - core).wait_recv()
        for i in range(line):
            g_block(jnp.where(lower, line - 1 - i, i))
            if i < line - 1:
                @pl.when(lower)
                def _():
                    up_copy(line - 1 - i, True).start()

                @pl.when(jnp.logical_not(lower))
                def _():
                    dn_copy(i, True).start()
        f_copy(0, False, g, zrow).start()
        f_copy(1, False, g, zrow).start()
        for d in range(last):
            for sub in range(2):
                settle(d, sub, 2)
        forward(1, dn_w, 2 * width, width, 0, 4)
        f_copy(0, True).wait_recv()
        f_copy(2, False).start()
        forward_end(1, 2, 0)
        for up_dir in (True, False):
            await_recv(up_dir, last, 1, 2)
        inputs_sent()
        finish(0)
        first_block()
        finish(1)
        theirs(4)
        summed(4)
        x_copy(2).start()
        finish(2)
        theirs(5)
        summed(5)
        y_copy(2).start()
        finish(3)
        theirs(6)
        summed(6)
        relay_a()
        y_copy(4).start()
        y_copy(3).start()
        relay_b()
        x_copy(4).start()
        h_copy(0).wait_recv()
        scaled([(g, pl.multiple_of(zrow + y * frows, frows), 0), (hl, 0, gcol(r, y))], r, y)
        final_a()
        final_b(0)
        for i, (rr, yy) in enumerate(((r, 1 - y), (1 - r, y))):
            if i == 1:
                f_copy(1, True).wait_recv()
            h_copy(1 + i).wait_recv()
            scaled([(gl, 0, gcol(rr, yy)), (hl, 0, gcol(rr, yy))], rr, yy)
        final_b(1)
        f_copy(2, True).wait_recv()
        h_copy(3).wait_recv()
        diag = gcol(1 - r, 1 - y)
        scaled([(gl, 0, diag), (hl, 0, diag)], 1 - r, 1 - y)
        settled()

    @pl.when(jnp.logical_not(is_end))
    def _():
        (
            first_block, theirs, summed, x_copy, y_copy, relay_a, relay_b,
            final_a, final_b, settled,
        ) = plane_sums(mid_a)
        event(2)
        inputs_sent()
        for i in (1, 2):
            dcopy(i, 1 - core).wait_recv()
        forward(1, dn_w, 2 * width, width, 1, 1)
        theirs(4)
        summed(4)
        x_copy(2).start()
        event(6)
        dcopy(4, 1 - core).wait_recv()
        forward(1, dn_w, 2 * width, width, 2, 1)
        theirs(5)
        event(7)
        summed(5)
        for i in (6, 7):
            dcopy(i, 1 - core).wait_recv()
        forward(1, dn_w, 2 * width, width, 3, 1)
        first_block()
        y_copy(2).start()
        y_copy(3).start()
        g_block(jnp.where(lower, line - 1, 0))
        line_step(1)
        for i in range(1, line):
            g_block(jnp.where(lower, line - 1 - i, i))
        forward(1, dn_w, 2 * width, width, 0, 1)
        theirs(6)
        summed(6)
        relay_a()
        relay_b()
        for t in range(2, line - 1):
            line_step(t)
        y_copy(4).start()
        x_copy(4).start()

        @pl.when(next_to_end)
        def _():
            e_copy(0, True).wait_recv()
            e_copy(2, False).start()
            h_copy(1).start()
            e_copy(1, True).wait_recv()
            h_copy(2).start()

        up_copy(z, False).wait_recv()
        dn_copy(z, False).wait_recv()
        total(
            (gfin, 0, 0, width),
            [(g, zrow, 0, width), (u_in, zrow, 0, width), (d_in, zrow, 0, width)], zrows,
        )
        f_copy(0, False).start()
        scaled([(gfin, pl.multiple_of(y * frows, frows), 0)], r, y)
        f_copy(1, False).start()
        final_a()
        final_b(0)

        @pl.when(next_to_end)
        def _():
            e_copy(2, True).wait_recv()
            h_copy(3).start()

        f_copy(0, True).wait_recv()
        f_copy(2, False).start()
        scaled([(gl, 0, gcol(r, 1 - y))], r, 1 - y)
        f_copy(1, True).wait_recv()
        scaled([(gl, 0, gcol(1 - r, y))], 1 - r, y)
        final_b(1)
        f_copy(2, True).wait_recv()
        scaled([(gl, 0, gcol(1 - r, 1 - y))], 1 - r, 1 - y)

        @pl.when(next_to_end)
        def _():
            for i in range(3):
                e_copy(i, False).wait_send()
            for i in range(4):
                h_copy(i).wait_send()

        settled()

    for i in range(ntok):
        if kinds[i] == 1:
            dcopy(i, core).wait_send()
        if i != 5:
            tcopy(i, False).wait_send()
    for k in range(3):
        to_y(k).wait_send()

    unit = wrows * width // (2 * x.shape[2])
    for count, here in ((6, is_end), (6 * (line + 1), jnp.logical_not(is_end))):
        @pl.when(here)
        def _(count=count):
            view = x.at[:, pl.ds(0, count * unit), :]
            pltpu.make_async_copy(view, view, z_s).wait()

    for i in range(3):
        f_copy(i, False).wait_send()
    for zt in range(line):
        if zt > 0:
            far = line - 2 if zt == line - 1 else zt
            pl.when(z < far)(lambda: up_copy(zt, True).wait_send())
        if zt < line - 1:
            near = 1 if zt == 0 else zt
            pl.when(z > near)(lambda: dn_copy(zt, True).wait_send())


def fused(grad_scale, gate_w, up_w, down_w, toks, cots):
    line = lax.axis_size("fs") // 2
    rows, full = toks.shape
    wrows, width = gate_w.shape[0], gate_w.shape[1] // 4
    depth = 2 * line * wrows
    cols = full // 2
    kind = gate_w.dtype
    dma = pltpu.SemaphoreType.DMA
    zsem = dma((line - 1, 2, 3))
    anyspec = pl.BlockSpec(memory_space=pl.ANY)
    whole = pltpu.VMEM((depth, width), kind)
    end_a, mid_a = cols // 2, cols // 2
    most_b = cols - mid_a
    return pl.pallas_call(
        functools.partial(fused_kernel, line, grad_scale, end_a, mid_a),
        out_shape=(
            pltpu.VMEM((rows, full), kind),
            pltpu.VMEM((wrows, 4 * width), jnp.float32),
        ),
        in_specs=[anyspec] * 5,
        out_specs=(pl.BlockSpec(memory_space=pltpu.VMEM),) * 2,
        scratch_shapes=[
            pltpu.VMEM((2, 4 * rows, full), kind),
            pltpu.VMEM((depth, 2 * width), kind),
            whole,
            pltpu.VMEM((4 * rows, 3 * width), jnp.float32),
            pltpu.VMEM((4 * rows, width), kind),
            pltpu.VMEM((4 * rows, 2 * width), kind),
            pltpu.VMEM((4 * rows, cols), kind),
            pltpu.VMEM((2, rows, end_a), kind), pltpu.VMEM((rows, most_b), kind),
            pltpu.VMEM((2, rows, most_b), kind), pltpu.VMEM((rows, end_a), kind),
            pltpu.VMEM((rows, end_a), kind), pltpu.VMEM((rows, most_b), kind),
            whole, whole, whole,
            pltpu.VMEM((2 * wrows, width), kind),
            pltpu.VMEM((wrows, 4 * width), kind),
            pltpu.VMEM((wrows, 4 * width), kind),
            dma, zsem, zsem,
            dma((3,)), dma((3,)),
            dma((8,)), dma((8,)), dma((8,)), dma((8,)), dma((5,)),
            dma((7,)), dma((7,)), dma((5,)), dma((5,)), dma((5,)), dma((5,)),
            dma((line,)), dma((line,)), dma((line,)), dma((line,)),
            dma((3,)), dma((3,)), dma((3,)), dma((3,)),
            dma((3,)), dma((3,)), dma((4,)), dma((4,)),
        ],
        compiler_params=pltpu.CompilerParams(
            collective_id=1, has_side_effects=True, vmem_limit_bytes=59 * 2**20
        ),
        name="fused_all",
    )(gate_w, up_w, down_w, toks, cots)


def place_kernel(a, b, a_out, b_out, sems):
    copies = [
        pltpu.make_async_copy(a, a_out, sems.at[0]),
        pltpu.make_async_copy(b, b_out, sems.at[1]),
    ]
    for copy in copies:
        copy.start()
    for copy in copies:
        copy.wait()


def place(a, b):
    anyspec = pl.BlockSpec(memory_space=pl.ANY)
    return pl.pallas_call(
        place_kernel,
        out_shape=(
            jax.ShapeDtypeStruct(a.shape, a.dtype), jax.ShapeDtypeStruct(b.shape, b.dtype),
        ),
        in_specs=[pl.BlockSpec(memory_space=pltpu.VMEM)] * 2,
        out_specs=(anyspec,) * 2,
        scratch_shapes=[pltpu.SemaphoreType.DMA((2,))],
        compiler_params=pltpu.CompilerParams(vmem_limit_bytes=16 * 2**20),
        name="place",
    )(a, b)


def gather_kernel(
    line, units, gate_w, up_w, down_w, toks, cots, gu_out, d_out, t_out, w_tmp, t_tmp,
    up_s, up_r, dn_s, dn_r, y_s, y_r, tok_s, tok_r, d2d_s, d2d_r, loc, loc2,
):
    r = lax.axis_index("rep")
    f = lax.axis_index("fs")
    t = lax.axis_index("tp")
    z, y = f // 2, f % 2
    rows = toks.shape[0]
    half = rows // 2
    wrows = gate_w.shape[0]
    width = gate_w.shape[1] // 4
    parts = len(units)
    has_up, has_dn = z < line - 1, z > 0
    up = {"fs": (f + 2) % (2 * line)}
    dn = {"fs": (f + 2 * line - 2) % (2 * line)}
    ypart = {"fs": f + 1 - 2 * y}
    xpart = {"rep": 1 - r}
    core = t % 2
    cpart = {"tp": t + 1 - 2 * core}

    barrier = pltpu.get_barrier_semaphore()

    def greet(dev):
        pl.semaphore_signal(barrier, inc=1, device_id=dev, device_id_type=MESH)

    for dev in (ypart, xpart, cpart, up, dn):
        greet(dev)
    pl.semaphore_wait(barrier, 5)

    def remote(src, dst, s, q, dev):
        return pltpu.make_async_remote_copy(
            src_ref=src, dst_ref=dst, send_sem=s, recv_sem=q,
            device_id=dev, device_id_type=MESH,
        )

    def wblk(k, zz, yy):
        row = pl.multiple_of((2 * zz + yy) * wrows, wrows)
        which, col, wide = units[k]
        return (gu_out, d_out)[which].at[pl.ds(row, wrows), pl.ds(col, wide)]

    def own(k, yy):
        col = pl.multiple_of((2 * r + yy) * width, width)
        return (gate_w, up_w, down_w)[k].at[:, pl.ds(col, width)]

    def to_y(k):
        return remote(own(k, 1 - y), wblk(k, z, y), y_s.at[k], y_r.at[k], ypart)

    def from_y(k):
        return remote(own(k, 1 - y), wblk(k, z, 1 - y), y_s.at[k], y_r.at[k], ypart)

    def zcopy(up_dir, d, sub, k, zz):
        yy = y if sub == 0 else 1 - y
        src = own(k, y) if (d == 0 and sub == 0) else wblk(k, zz, yy)
        s, q, dev = (up_s, up_r, up) if up_dir else (dn_s, dn_r, dn)
        return remote(src, wblk(k, zz, yy), s.at[d, sub, k], q.at[d, sub, k], dev)

    def pred_send(up_dir, d):
        return (has_up & (z - d >= 0)) if up_dir else (has_dn & (z + d <= line - 1))

    def src_z(up_dir, d):
        return jnp.maximum(z - d, 0) if up_dir else jnp.minimum(z + d, line - 1)

    def send(up_dir, d, sub, k):
        @pl.when(pred_send(up_dir, d))
        def _():
            zcopy(up_dir, d, sub, k, src_z(up_dir, d)).start()

    def await_send(up_dir, d, sub, k):
        @pl.when(pred_send(up_dir, d))
        def _():
            zcopy(up_dir, d, sub, k, src_z(up_dir, d)).wait_send()

    def await_recv(up_dir, d, sub, k):
        ok = (z - d - 1 >= 0) if up_dir else (z + d + 1 <= line - 1)

        @pl.when(ok)
        def _():
            zcopy(up_dir, d, sub, k, src_z(up_dir, d + 1)).wait_recv()

    def tblk(j, rr, yy, c):
        row = pl.multiple_of((2 * rr + yy) * rows + c * half, half)
        return t_out.at[j, pl.ds(row, half), :]

    def mine(j):
        src = toks if j == 0 else cots
        return src.at[pl.ds(pl.multiple_of(core * half, half), half), :]

    def tcopy(i, landing):
        j = (0, 1, 0, 1, 0, 1)[i]
        dev = xpart if i in (0, 1, 5) else ypart
        if landing:
            rr = (1 - r, 1 - r, r, r, 1 - r, 1 - r)[i]
            yy = (y, y, 1 - y, 1 - y, 1 - y, 1 - y)[i]
            src = dst = tblk(j, rr, yy, core)
        else:
            rr = (r, r, r, r, 1 - r, r)[i]
            yy = (y, y, y, y, y, 1 - y)[i]
            dst = tblk(j, rr, yy, core)
            src = mine(j) if i < 4 else dst
        return remote(src, dst, tok_s.at[i], tok_r.at[i], dev)

    def dcopy(i, c):
        j = (0, 1, 0, 1, 0, 1)[i]
        rr = (1 - r, 1 - r, r, r, 1 - r, 1 - r)[i]
        yy = (y, y, 1 - y, 1 - y, 1 - y, 1 - y)[i]
        blk = tblk(j, rr, yy, c)
        return remote(blk, blk, d2d_s.at[i], d2d_r.at[i], cpart)

    loads = [
        pltpu.make_async_copy(own(0, y), w_tmp.at[0], loc.at[0]),
        pltpu.make_async_copy(own(1, y), w_tmp.at[1], loc.at[3]),
        pltpu.make_async_copy(own(2, y), w_tmp.at[2], loc.at[4]),
        pltpu.make_async_copy(toks, t_tmp.at[0], loc.at[1]),
        pltpu.make_async_copy(cots, t_tmp.at[1], loc.at[2]),
    ]
    trow = pl.multiple_of((2 * r + y) * rows, rows)
    stores = [
        pltpu.make_async_copy(w_tmp.at[0], wblk(0, z, y), loc2.at[0]),
        pltpu.make_async_copy(w_tmp.at[1], wblk(1, z, y), loc2.at[3]),
        pltpu.make_async_copy(w_tmp.at[2], wblk(2, z, y), loc2.at[4]),
        pltpu.make_async_copy(t_tmp.at[0], t_out.at[0, pl.ds(trow, rows), :], loc2.at[1]),
        pltpu.make_async_copy(t_tmp.at[1], t_out.at[1, pl.ds(trow, rows), :], loc2.at[2]),
    ]

    for k in range(parts):
        to_y(k).start()
        send(True, 0, 0, k)
        send(False, 0, 0, k)
    for i in (0, 1, 3, 2):
        tcopy(i, False).start()
    for copy in loads:
        copy.start()
    for load, store in zip(loads, stores):
        load.wait()
        store.start()
    for k in range(parts):
        from_y(k).wait_recv()
        send(True, 0, 1, k)
        send(False, 0, 1, k)

    def event(i):
        tcopy(i, True).wait_recv()
        if i == 0:
            tcopy(4, False).start()
        if i == 3:
            tcopy(5, False).start()
        dcopy(i, core).start()

    events = [0, 3, 1, 2, 5, 4]
    for d in range(line - 1):
        for sub in range(2):
            if events:
                event(events.pop(0))
            for k in range(parts):
                for up_dir in (True, False):
                    await_recv(up_dir, d, sub, k)
                    if d + 1 < line - 1:
                        send(up_dir, d + 1, sub, k)
    for i in events:
        event(i)
    for i in range(6):
        dcopy(i, 1 - core).wait_recv()
        dcopy(i, core).wait_send()
        tcopy(i, False).wait_send()
    for k in range(parts):
        to_y(k).wait_send()
        for d in range(line - 1):
            for sub in range(2):
                await_send(True, d, sub, k)
                await_send(False, d, sub, k)
    for store in stores:
        store.wait()


def gather(gate_w, up_w, down_w, toks, cots):
    line = lax.axis_size("fs") // 2
    wrows, width = gate_w.shape[0], gate_w.shape[1] // 4
    units = [(0, 0, width), (0, width, width), (1, 0, width)]
    parts = len(units)
    depth = 2 * line * wrows
    kind = gate_w.dtype
    dma = pltpu.SemaphoreType.DMA
    zsem = dma((line - 1, 2, parts))
    anyspec = pl.BlockSpec(memory_space=pl.ANY)
    return pl.pallas_call(
        functools.partial(gather_kernel, line, units),
        out_shape=(
            jax.ShapeDtypeStruct((depth, 2 * width), kind),
            jax.ShapeDtypeStruct((depth, width), kind),
            jax.ShapeDtypeStruct((2, 4 * toks.shape[0], toks.shape[1]), toks.dtype),
        ),
        in_specs=[anyspec] * 5,
        out_specs=(anyspec,) * 3,
        scratch_shapes=[
            pltpu.VMEM((parts, wrows, width), kind),
            pltpu.VMEM((2,) + toks.shape, toks.dtype),
            zsem, zsem, zsem, zsem,
            dma((parts,)), dma((parts,)),
            dma((6,)), dma((6,)), dma((6,)), dma((6,)),
            dma((5,)), dma((5,)),
        ],
        compiler_params=pltpu.CompilerParams(collective_id=0, has_side_effects=True),
        name="gather_all",
    )(gate_w, up_w, down_w, toks, cots)


def on_device(inputs, cotangent, gate_weight, up_weight, down_weight):
    tok_rows = inputs.shape[0]
    fs_size = lax.axis_size("fs")
    rep_size = lax.axis_size("rep")
    grad_scale = 1.0 / math.sqrt(tok_rows * fs_size * rep_size)
    if lax.axis_size("tp") == 2 and rep_size == 2 and fs_size >= 8:
        return place(*fused(
            grad_scale, gate_weight, up_weight, down_weight, inputs, cotangent
        ))
    contract = (((1,), (1,)), ((), ()))
    contract_tok = (((0,), (0,)), ((), ()))
    width = gate_weight.shape[1] // 4
    gate_up, down_full, tokens = gather(
        gate_weight, up_weight, down_weight, inputs, cotangent
    )
    gate_up_val = jnp.dot(tokens[0], gate_up, preferred_element_type=jnp.float32)
    gate_val, up_val = gate_up_val[:, :width], gate_up_val[:, width:]
    grad_hidden = jnp.dot(tokens[1], down_full, preferred_element_type=jnp.float32)
    sigmoid_gate = jax.nn.sigmoid(gate_val)
    active = gate_val * sigmoid_gate
    hidden = (active * up_val).astype(jnp.bfloat16)
    grad_gate = (
        grad_hidden * up_val * sigmoid_gate * (1.0 + gate_val * (1.0 - sigmoid_gate))
    ).astype(jnp.bfloat16)
    grad_up = (grad_hidden * active).astype(jnp.bfloat16)
    pairs = [[i, i + 1] for i in range(0, fs_size, 2)]
    lines = [list(range(i, fs_size, 2)) for i in range(2)]
    grad_part = lax.dot_general(
        tokens[1], hidden, contract_tok, preferred_element_type=jnp.float32
    )
    part = lax.dot_general(
        jnp.concatenate([grad_gate, grad_up], axis=1), gate_up, contract,
        preferred_element_type=jnp.float32,
    )
    shard = lax.psum_scatter(
        grad_part.astype(jnp.bfloat16), "fs", scatter_dimension=0, tiled=True,
        axis_index_groups=lines,
    ).astype(jnp.float32) * grad_scale
    shard = lax.all_to_all(
        shard, "fs", split_axis=0, concat_axis=1, tiled=True, axis_index_groups=pairs
    )
    grad_down = lax.all_gather(shard, "rep", axis=1, tiled=True)
    part = lax.psum_scatter(
        part.astype(jnp.bfloat16), "rep", scatter_dimension=0, tiled=True
    )
    part = lax.psum_scatter(
        part, "fs", scatter_dimension=0, tiled=True, axis_index_groups=pairs
    )
    grad_input = lax.psum(part, "tp")
    return (grad_input, grad_down)


def solution(mesh):
    placed = (
        P(("rep", "fs"), None),
        P(("rep", "fs"), None),
        P("fs", "tp"),
        P("fs", "tp"),
        P("fs", "tp"),
    )
    return jax.shard_map(
        on_device,
        mesh=mesh,
        in_specs=placed,
        out_specs=(P(("rep", "fs"), None), P("fs", "tp")),
        check_vma=False,
    )
```
